32 devices in a mesh: grp: 2 (over y), sp: 4 (over z), tp: 4 (over x, core).
Axes of the slice: x: 2, y: 2, z: 4, core: 2. Of those that a mesh axis runs over, the one named last changes fastest.
Arguments:
- tokens: bfloat16 [2048, 2048], P(('grp', 'sp'), 'tp'), parts along dimension 0, may hold values from -6 to 6
- norm_gain: float32 [2048], replicated, may hold values from 0.1 to 1.9
- ret_query_weight: bfloat16 [2048, 256], P('sp', 'tp'), may hold values from -0.125 to 0.125
- ret_key_weight: bfloat16 [2048, 256], P('sp', 'tp'), may hold values from -0.125 to 0.125
- ret_value_weight: bfloat16 [2048, 512], P('sp', 'tp'), may hold values from -0.125 to 0.125
- fox_query_weight: bfloat16 [2048, 512], P('sp', 'tp'), may hold values from -8 to 8
- fox_key_weight: bfloat16 [2048, 512], P('sp', 'tp'), may hold values from -0.125 to 0.125
- fox_value_weight: bfloat16 [2048, 512], P('sp', 'tp'), may hold values from -0.125 to 0.125
- ret_decay: float32 [8], P('tp'), may hold values from -1 to 0, as said below
- ret_state: float32 [16, 32, 64], P(('grp', 'tp')), parts along dimension 0, may hold values from -64 to 64
- head_norm_gain: float32 [512], P('tp'), may hold values from 0.1 to 1.9
- fox_gates: float32 [2048, 8], P('grp', 'tp'), parts along dimension 0, may hold values from -3072 to 0, as said below
- ret_out_weight: bfloat16 [512, 2048], P('tp', 'sp'), may hold values from -0.1875 to 0.1875
- fox_out_weight: bfloat16 [512, 2048], P('tp', 'sp'), may hold values from -1 to 1
Outputs:
- mixed: bfloat16 [2048, 2048], P(('grp', 'sp', 'tp')), parts along dimension 0
The draws below stay inside these ranges and needn't reach their ends.
There are 2 independent parts, one for each index of `grp`. The reference program is written for one: setup_inputs(seed, part) draws one part's arguments, and reference() takes and returns one part's arrays. A program takes and returns all parts, laid end to end along the dimension named above; an argument that names none is the same for every part. Nothing has to cross between parts.
Inputs may be any that keep to these rules, and one draw needn't show every extreme that they name: `ret_decay`: each head's log decay is negative. `fox_gates`: along the positions each head's column never rises.
All inputs are finite; a program needn't handle non-finite values.
Results may differ from the reference program's by a relative error of at most 0.015.
The reference program's roundings to bfloat16 on the way count: a program that leaves them out, or rounds other values in their place, can miss the bound.
Values may be sent and summed in bfloat16 or wider, within the bound.
A program may use at most 64 MiB of HBM per device.

```python
import jax
import jax.numpy as jnp
from jax import lax

D = 2048
RETAIN_HEADS = 8
DK = 32
RETAIN_VALUE_DIM = 64
FH = 8
FD = 64
TOK_DEV = 256
TOKENS = 1024
N_TP = 4


def draw_fox_query_weight(key, part):
    keys = jax.random.split(jax.random.fold_in(key, 11), 1)
    columns = FH * FD
    return (jnp.clip(jax.random.normal(keys[0], (D, columns), jnp.float32), -6.0, 6.0) * D ** (-0.5)).astype(jnp.bfloat16)


def draw_ret_decay(key, part):
    keys = jax.random.split(jax.random.fold_in(key, 23), 3)
    order = jax.random.permutation(keys[0], RETAIN_HEADS)
    quick = order < RETAIN_HEADS // 2
    quick_rate = -1.0 / jax.random.uniform(keys[1], (RETAIN_HEADS,), jnp.float32, 30.0, 100.0)
    slow_rate = -jax.random.uniform(keys[2], (RETAIN_HEADS,), jnp.float32, 0.3, 2.0) / TOKENS
    return jnp.where(quick, quick_rate, slow_rate)


def draw_ret_state(key, part):
    source = jax.random.fold_in(key, 37)
    scale = 0.2 * float(TOKENS) ** 0.5
    return scale * jnp.clip(jax.random.normal(source, (RETAIN_HEADS, DK, RETAIN_VALUE_DIM), jnp.float32), -6.0, 6.0)


def draw_fox_gates(key, part):
    keys = jax.random.split(jax.random.fold_in(key, 51), 7)
    order = jax.random.permutation(keys[0], FH)
    quick = order < FH // 2
    quick_rate = 1.0 / jax.random.uniform(keys[1], (FH,), jnp.float32, 30.0, 100.0)
    slow_rate = jax.random.uniform(keys[2], (FH,), jnp.float32, 0.5, 2.0) / TOKENS
    rates = jnp.where(quick, quick_rate, slow_rate)
    blocks = TOKENS // TOK_DEV
    factor = jnp.exp(jax.random.uniform(keys[3], (blocks, 1), jnp.float32, -0.7, 0.7))
    factor = jnp.repeat(factor, TOK_DEV, axis=0)
    jitter = jax.random.uniform(keys[4], (TOKENS, FH), jnp.float32, 0.3, 1.7)
    increments = -rates[None, :] * factor * jitter
    spots = jax.random.randint(keys[5], (3,), 0, TOKENS)
    struck = jnp.any(jnp.arange(TOKENS)[:, None] == spots[None, :], axis=1)
    losses = jax.random.uniform(keys[6], (TOKENS, FH), jnp.float32, 0.22, 0.69)
    increments = increments - jnp.where(struck[:, None], losses, 0.0)
    return jnp.cumsum(increments, axis=0)


def block_scale(own_key, extent, cuts, least, top_value):
    gain, own = 1.0, jax.random.fold_in(own_key, 6)
    for axis_at, blocks in cuts:
        heights = jnp.exp(jax.random.uniform(jax.random.fold_in(own, axis_at), (blocks,), jnp.float32, least / len(cuts), top_value / len(cuts)))
        gain = gain * jnp.repeat(heights, extent[axis_at] // blocks).reshape([-1 if axis == axis_at else 1 for axis in range(len(extent))])
    return gain


def noise(key, extent, scale, limit, cuts=(), held_as=jnp.bfloat16):
    gain = block_scale(key, extent, cuts, -0.22, 0.18) if cuts else 1.0
    entries = jax.random.normal(key, extent, jnp.float32) * scale * gain
    return jnp.minimum(jnp.maximum(entries, -limit), limit).astype(held_as)


def setup_inputs(seed: int = 0, part: int = 0) -> dict:
    key_list = jax.random.split(jax.random.key(seed), 15)
    own_keys = jax.random.split(jax.random.fold_in(key_list[14], part), 15)
    return {
        "tokens": noise(own_keys[0], (TOKENS, D), 1.0, 6.0, ((0, 4), (1, 4))),
        "norm_gain": jnp.clip(1.0 + 0.18 * jax.random.normal(key_list[1], (D,), jnp.float32), 0.1, 1.9),
        "ret_query_weight": noise(key_list[2], (D, RETAIN_HEADS * DK), D ** -0.5, 0.125, ((0, 4), (1, 4))),
        "ret_key_weight": noise(key_list[3], (D, RETAIN_HEADS * DK), D ** -0.5, 0.125, ((0, 4), (1, 4))),
        "ret_value_weight": noise(key_list[4], (D, RETAIN_HEADS * RETAIN_VALUE_DIM), D ** -0.5, 0.125, ((0, 4), (1, 4))),
        "fox_query_weight": draw_fox_query_weight(jax.random.fold_in(key_list[14], 71), part),
        "fox_key_weight": noise(key_list[6], (D, FH * FD), D ** -0.5, 0.125, ((0, 4), (1, 4))),
        "fox_value_weight": noise(key_list[7], (D, FH * FD), D ** -0.5, 0.125, ((0, 4), (1, 4))),
        "ret_decay": draw_ret_decay(jax.random.fold_in(key_list[14], 71), part),
        "ret_state": draw_ret_state(jax.random.fold_in(jax.random.fold_in(key_list[14], part), 71), part),
        "head_norm_gain": jnp.clip(1.0 + 0.18 * jax.random.normal(key_list[10], (RETAIN_HEADS * RETAIN_VALUE_DIM,), jnp.float32), 0.1, 1.9),
        "fox_gates": draw_fox_gates(jax.random.fold_in(jax.random.fold_in(key_list[14], part), 71), part),
        "ret_out_weight": noise(key_list[12], (RETAIN_HEADS * RETAIN_VALUE_DIM, D), (RETAIN_HEADS * RETAIN_VALUE_DIM + FH * FD) ** -0.5, 0.1875, ((0, 4), (1, 4))),
        "fox_out_weight": noise(key_list[13], (FH * FD, D), (FH * FD // 16) ** -0.5, 1.0, ((0, 4), (1, 4))),
    }


epsilon = 1e-06
highest = lax.Precision.HIGHEST

def head_group_norm(joined_output, norm_gains):
    center = joined_output - lax.optimization_barrier(jnp.mean(joined_output, axis=-1, keepdims=True))
    spread = lax.optimization_barrier(jnp.mean(center * center, axis=-1, keepdims=True))
    normal = center * lax.rsqrt(spread + epsilon) * norm_gains.reshape(joined_output.shape[1], joined_output.shape[2])
    return normal.reshape(joined_output.shape[0], -1).astype(jnp.bfloat16)

def retention(query_rows, key_rows, value_rows, log_decay, initial, norm_gains):
    sequence_length = query_rows.shape[0]
    blocks = sequence_length // TOK_DEV
    queries = query_rows.astype(jnp.float32).reshape(blocks, TOK_DEV, RETAIN_HEADS, DK)
    keys_all = key_rows.astype(jnp.float32).reshape(blocks, TOK_DEV, RETAIN_HEADS, DK) * DK ** (-0.5)
    values_all = value_rows.astype(jnp.float32).reshape(blocks, TOK_DEV, RETAIN_HEADS, RETAIN_VALUE_DIM)
    offsets = jnp.arange(TOK_DEV, dtype=jnp.float32)
    spread = offsets[:, None] - offsets[None, :]
    within = jnp.where(spread[None] >= 0, jnp.exp(jnp.maximum(spread, 0.0)[None] * log_decay[:, None, None]), 0.0)
    leading = jnp.exp((offsets + 1.0)[:, None] * log_decay[None, :])
    trailing = jnp.exp((TOK_DEV - 1.0 - offsets)[:, None] * log_decay[None, :])
    blockwise = jnp.exp(TOK_DEV * log_decay)

    def advance(memory, inputs):
        qblock, kblock, vblock = inputs
        scores = jnp.einsum('ihd,jhd->hij', qblock, kblock, precision=highest) * within
        inner_value = jnp.einsum('hij,jhe->ihe', scores, vblock, precision=highest)
        carried_state = jnp.einsum('ihd,hde->ihe', qblock, memory, precision=highest) * leading[:, :, None]
        summary = jnp.einsum('jhd,jhe->hde', kblock * trailing[:, :, None], vblock, precision=highest)
        return (memory * blockwise[:, None, None] + summary, inner_value + carried_state)
    _, output_rows = lax.scan(advance, initial, (queries, keys_all, values_all))
    return head_group_norm(output_rows.reshape(sequence_length, RETAIN_HEADS, RETAIN_VALUE_DIM), norm_gains)

def forgetting(query_rows, key_rows, value_rows, gates):
    sequence_length = query_rows.shape[0]
    queries = query_rows.astype(jnp.float32).reshape(sequence_length, FH, FD)
    keys_all = key_rows.astype(jnp.float32).reshape(sequence_length, FH, FD)
    values_all = value_rows.astype(jnp.float32).reshape(sequence_length, FH, FD)
    key_gates = gates.T
    key_pos = jnp.arange(sequence_length, dtype=jnp.int32)

    def block(number):
        first = (number * TOK_DEV).astype(jnp.int32)
        qblock = lax.dynamic_slice_in_dim(queries, first, TOK_DEV, 0)
        own_gates = lax.dynamic_slice_in_dim(key_gates, first, TOK_DEV, 1)
        scores = jnp.einsum('qhd,khd->hqk', qblock, keys_all) * FD ** (-0.5)
        scores = scores + own_gates[:, :, None] - key_gates[:, None, :]
        query_pos = first + jnp.arange(TOK_DEV, dtype=jnp.int32)
        scores = jnp.where(key_pos[None, None, :] <= query_pos[None, :, None], scores, -jnp.inf)
        highest_score = lax.optimization_barrier(jnp.max(scores, axis=-1, keepdims=True))
        weights = jnp.exp(scores - highest_score)
        totals = lax.optimization_barrier(jnp.sum(weights, axis=-1))
        rounded = lax.optimization_barrier(weights.astype(jnp.bfloat16)).astype(jnp.float32)
        weighted = jnp.einsum('hqk,khd->hqd', rounded, values_all)
        result = weighted / totals[:, :, None]
        return jnp.transpose(result, (1, 0, 2)).reshape(TOK_DEV, FH * FD).astype(jnp.bfloat16)
    pieces = lax.map(block, jnp.arange(sequence_length // TOK_DEV, dtype=jnp.int32))
    return pieces.reshape(sequence_length, FH * FD)

def reference(tokens, norm_gain, ret_query_weight, ret_key_weight, ret_value_weight, fox_query_weight, fox_key_weight, fox_value_weight, ret_decay, ret_state, head_norm_gain, fox_gates, ret_out_weight, fox_out_weight):
    widened = tokens.astype(jnp.float32)
    normed = (widened * lax.rsqrt(lax.optimization_barrier(jnp.mean(widened * widened, axis=-1, keepdims=True)) + epsilon) * norm_gain).astype(jnp.bfloat16)
    matrices = (ret_query_weight, ret_key_weight, ret_value_weight, fox_query_weight, fox_key_weight, fox_value_weight)
    ret_query, ret_key, ret_value, fox_query, fox_key, fox_value = [jnp.dot(normed, matrix, preferred_element_type=jnp.float32).astype(jnp.bfloat16) for matrix in matrices]
    retention_mixed = retention(ret_query, ret_key, ret_value, ret_decay, ret_state, head_norm_gain)
    fox_mix = forgetting(fox_query, fox_key, fox_value, fox_gates)
    ret_width = RETAIN_HEADS * RETAIN_VALUE_DIM // N_TP
    fox_width = FH * FD // N_TP
    summed = jnp.zeros((tokens.shape[0], D), jnp.float32)
    for member in range(N_TP):
        portion = jnp.dot(retention_mixed[:, member * ret_width:(member + 1) * ret_width], ret_out_weight[member * ret_width:(member + 1) * ret_width], preferred_element_type=jnp.float32)
        portion = portion + jnp.dot(fox_mix[:, member * fox_width:(member + 1) * fox_width], fox_out_weight[member * fox_width:(member + 1) * fox_width], preferred_element_type=jnp.float32)
        summed = summed + lax.optimization_barrier(portion.astype(jnp.bfloat16)).astype(jnp.float32)
    return summed.astype(jnp.bfloat16)
```

```python
import functools

import jax
import jax.numpy as jnp
from jax import lax
from jax.experimental import pallas as pl
from jax.experimental.pallas import tpu as pltpu
from jax.sharding import PartitionSpec as P

epsilon = 1e-06
highest = lax.Precision.HIGHEST
NT = (((1,), (1,)), ((), ()))
TN = (((0,), (0,)), ((), ()))


def rdma(src, dst, send_sem, recv_sem, **target):
    return pltpu.make_async_remote_copy(
        src_ref=src,
        dst_ref=dst,
        send_sem=send_sem,
        recv_sem=recv_sem,
        device_id=target,
        device_id_type=pl.DeviceIdType.MESH,
    )


class LineGather:
    def __init__(self, owns, place, sems, n, n_grp, me, g):
        self.owns, self.place, self.n, self.n_grp, self.me, self.g = owns, place, n, n_grp, me, g
        self.up, self.down, self.zr, self.ys, self.yr, self.loc = sems
        self.arrays = len(owns)
        self.rows = owns[0].shape[0]
        self.step = self.rows // n_grp

    def piece(self, part, src, c):
        return self.place(src, c, part * self.step, self.step)

    def own_piece(self, c):
        return self.owns[c].at[pl.ds(pl.multiple_of(self.g * self.step, self.step), self.step)]

    def hop(self, sems, to, src, c, first=False):
        here = self.own_piece(c) if first else self.piece(self.g, src, c)
        at = src * self.arrays + c
        return rdma(here, self.piece(self.g, src, c), sems.at[at], self.zr.at[at], sp=to)

    def side(self, d, src, c):
        at = ((d - 1) * self.n + src) * self.arrays + c
        here = self.piece(self.g, src, c)
        return rdma(here, here, self.ys.at[at], self.yr.at[at], grp=lax.rem(self.g + d, self.n_grp))

    def side_in(self, d, src, c):
        at = ((d - 1) * self.n + src) * self.arrays + c
        part = lax.rem(self.g + self.n_grp - d, self.n_grp)
        here = self.piece(part, src, c)
        return rdma(here, here, self.ys.at[at], self.yr.at[at], grp=part)

    def local(self, c):
        return pltpu.make_async_copy(self.owns[c], self.place(self.me, c, 0, self.rows), self.loc.at[c])

    def start(self):
        me, n = self.me, self.n
        for c in range(self.arrays):

            @pl.when(me + 1 < n)
            def _():
                self.hop(self.up, me + 1, me, c, True).start()

            @pl.when(me >= 1)
            def _():
                self.hop(self.down, me - 1, me, c, True).start()

        for c in range(self.arrays):
            self.local(c).start()

    def relay(self, k):
        me, n = self.me, self.n
        for c in range(self.arrays):
            for src, sems, to in ((me - k, self.up, me + 1), (me + k, self.down, me - 1)):

                @pl.when((src >= 0) & (src < n))
                def _(src=src, sems=sems, to=to):
                    self.hop(sems, me, src, c).wait_recv()

                    @pl.when((to >= 0) & (to < n))
                    def _():
                        self.hop(sems, to, src, c).start()

                    for d in range(1, self.n_grp):
                        self.side(d, src, c).start()

    def arrive_shard(self, src, arrays):
        for c in arrays:
            for d in range(1, self.n_grp):
                self.side_in(d, src, c).wait_recv()

    def arrive(self, arrays):
        for c in arrays:
            self.local(c).wait()

        def step(k, _):
            self.arrive_shard(lax.rem(self.me + k, self.n), arrays)
            return 0

        lax.fori_loop(1, self.n, step, 0)

    def finish(self):
        me, n = self.me, self.n

        def step(src, _):
            for c in range(self.arrays):

                @pl.when((src <= me) & (me + 1 < n))
                def _():
                    self.hop(self.up, me, src, c).wait_send()

                @pl.when((src >= me) & (me >= 1))
                def _():
                    self.hop(self.down, me, src, c).wait_send()

                @pl.when(src != me)
                def _():
                    for d in range(1, self.n_grp):
                        self.side(d, src, c).wait_send()

            return 0

        lax.fori_loop(0, n, step, 0)


def kernel(
    size,
    tok_ref,
    gain_ref,
    wq_ref,
    wk_ref,
    wrv_ref,
    wfq_ref,
    wfk_ref,
    wfv_ref,
    decay_ref,
    state_ref,
    hgain_ref,
    gates_ref,
    ret_out_ref,
    fox_out_ref,
    out_ref,
    tok_buf,
    qk_own,
    w_buf,
    wout_buf,
    norm_buf,
    proj_buf,
    kv_buf,
    sum_buf,
    mix_buf,
    rs_send,
    pair_buf,
    pair_sum,
    rs_buf,
    top_buf,
    total_buf,
    weighted_buf,
    tok_s,
    tok_r,
    tok_loc,
    kv_s,
    kv_r,
    sum_s,
    sum_r,
    pair_s,
    pair_r,
    rs_s,
    rs_r,
    *gather_sems,
):
    n, n_tp, n_grp, hr, dk, vd, fh, fd, direct = size
    me, t, g = lax.axis_index("sp"), lax.axis_index("tp"), lax.axis_index("grp")
    rows, feats = tok_ref.shape
    owns = [wfk_ref, wfv_ref, wfq_ref, wrv_ref, qk_own]
    early = 2
    starts = [0]
    for own in owns:
        starts.append(starts[-1] + own.shape[1])
    shard = qk_own.shape[0]

    def weight_place(src, c, first, count):
        start = pl.multiple_of(src * shard + first, count)
        return w_buf.at[pl.ds(start, count), starts[c] : starts[c + 1]]

    depth = mix_buf.shape[1] // 2
    out_cols = ret_out_ref.shape[1] if direct else ret_out_ref.shape[0]

    def out_place(src, c, first, count):
        if direct:
            start = pl.multiple_of(c * depth + first, count)
            return wout_buf.at[pl.ds(start, count), pl.ds(pl.multiple_of(src * out_cols, out_cols), out_cols)]
        start = pl.multiple_of(src * out_cols + first, count)
        return wout_buf.at[pl.ds(start, count), c * depth : (c + 1) * depth]

    def late_place(src, c, first, count):
        return weight_place(src, c + early, first, count)

    firsts = LineGather(owns[:early], weight_place, gather_sems[:6], n, n_grp, me, g)
    lasts = LineGather(owns[early:], late_place, gather_sems[6:12], n, n_grp, me, g)
    outs = LineGather([ret_out_ref, fox_out_ref], out_place, gather_sems[12:], n, n_grp, me, g)

    barrier = pltpu.get_barrier_semaphore()

    def greet(**target):
        pl.semaphore_signal(barrier, inc=1, device_id=target, device_id_type=pl.DeviceIdType.MESH)

    has_up, has_down = me + 1 < n, me >= 1
    for d in range(1, n_tp):
        greet(tp=lax.rem(t + d, n_tp))
    for d in range(1, n_grp):
        greet(grp=lax.rem(g + d, n_grp))

    @pl.when(has_up)
    def _():
        greet(sp=me + 1)

    @pl.when(has_down)
    def _():
        greet(sp=me - 1)

    turned = jnp.concatenate((wq_ref[...], wk_ref[...]), axis=0).astype(jnp.float32)
    qk_own[...] = turned.T.astype(jnp.bfloat16)

    count = n_tp - 1 + n_grp - 1 + has_up.astype(jnp.int32) + has_down.astype(jnp.int32)
    pl.semaphore_wait(barrier, count)

    def tok_copy(d):
        return rdma(tok_ref, tok_buf.at[t], tok_s.at[d - 1], tok_r.at[d - 1], tp=lax.rem(t + d, n_tp))

    def tok_in(d):
        src = lax.rem(t + n_tp - d, n_tp)
        return rdma(tok_ref, tok_buf.at[src], tok_s.at[d - 1], tok_r.at[d - 1], tp=src)

    firsts.start()
    lasts.start()
    tok_local = pltpu.make_async_copy(tok_ref, tok_buf.at[t], tok_loc)
    for d in range(1, n_tp):
        tok_copy(d).start()
    tok_local.start()

    def first_step(k, _):
        firsts.relay(k)

        lasts.relay(k)
        return 0

    lax.fori_loop(1, n, first_step, 0)
    outs.start()

    tok_local.wait()
    for d in range(1, n_tp):
        tok_in(d).wait_recv()
    squares = jnp.zeros((rows, 1), jnp.float32)
    for i in range(n_tp):
        part = tok_buf[i].astype(jnp.float32)
        squares = squares + jnp.sum(part * part, axis=-1, keepdims=True)
    scale = lax.rsqrt(squares * (1.0 / (n_tp * feats)) + epsilon)
    for i in range(n_tp):
        part = tok_buf[i].astype(jnp.float32)
        cols = slice(i * feats, (i + 1) * feats)
        norm_buf[:, cols] = (part * scale * gain_ref[:, cols]).astype(jnp.bfloat16)

    def kv_copy(src):
        return rdma(kv_buf.at[src], kv_buf.at[src], kv_s.at[src], kv_r.at[src], sp=jnp.minimum(me + 1, n - 1))

    def sum_copy(src):
        return rdma(sum_buf.at[src], sum_buf.at[src], sum_s.at[src], sum_r.at[src], sp=jnp.minimum(me + 1, n - 1))

    firsts.arrive((0, 1))
    kv_buf[me] = jnp.dot(
        norm_buf[...], w_buf[:, : starts[2]], preferred_element_type=jnp.float32
    ).astype(jnp.bfloat16)

    def kv_forward(k):
        src = me - k

        @pl.when(src >= 0)
        def _():
            kv_copy(src).wait_recv()

            @pl.when(has_up)
            def _():
                kv_copy(src).start()

    @pl.when(has_up)
    def _():
        kv_copy(me).start()

    outs.relay(1)
    lasts.arrive((0, 1, 2))
    proj_buf[...] = jnp.dot(
        norm_buf[...], w_buf[:, starts[2] :], preferred_element_type=jnp.float32
    ).astype(jnp.bfloat16)
    rv_at, rq_at = starts[3] - starts[2], starts[4] - starts[2]

    key_scale = dk ** (-0.5)
    position = lax.broadcasted_iota(jnp.int32, (rows, 1), 0).astype(jnp.float32)
    rq, rk, rv = [], [], []
    for h in range(hr):
        rq.append(proj_buf[:, rq_at + h * dk : rq_at + (h + 1) * dk])
        rk.append(proj_buf[:, rq_at + (hr + h) * dk : rq_at + (hr + h + 1) * dk])
        rv.append(proj_buf[:, rv_at + h * vd : rv_at + (h + 1) * vd])
        keys = rk[h].astype(jnp.float32) * key_scale
        trailing = jnp.exp((rows - 1.0 - position) * decay_ref[h])
        sum_buf[me, h] = lax.dot_general(
            keys * trailing, rv[h].astype(jnp.float32), TN, precision=highest, preferred_element_type=jnp.float32
        )

    @pl.when(has_up)
    def _():
        sum_copy(me).start()

    row_id = lax.broadcasted_iota(jnp.int32, (rows, rows), 0)
    col_id = lax.broadcasted_iota(jnp.int32, (rows, rows), 1)
    causal = col_id <= row_id
    own_cols = pl.ds(pl.multiple_of(me * rows, rows), rows)
    own_gates = [
        jnp.sum(jnp.where(row_id == col_id, gates_ref[h : h + 1, own_cols], 0.0), axis=1, keepdims=True)
        for h in range(fh)
    ]

    def attend(src, diagonal):
        key_cols = pl.ds(pl.multiple_of(src * rows, rows), rows)
        for h in range(fh):
            query = proj_buf[:, h * fd : (h + 1) * fd]
            k = kv_buf[src, :, h * fd : (h + 1) * fd]
            v = kv_buf[src, :, (fh + h) * fd : (fh + h + 1) * fd]
            logits = lax.dot_general(query, k, NT, preferred_element_type=jnp.float32) * fd ** (-0.5)
            logits = logits + own_gates[h] - gates_ref[h : h + 1, key_cols]
            if diagonal:
                logits = jnp.where(causal, logits, -jnp.inf)
            top_new = jnp.max(logits, axis=-1, keepdims=True)
            if not diagonal:
                top = top_buf[h]
                top_new = jnp.maximum(top, top_new)
            p = jnp.exp(logits - top_new)
            total = jnp.sum(p, axis=-1, keepdims=True)
            weighted = jnp.dot(p.astype(jnp.bfloat16), v, preferred_element_type=jnp.float32)
            if not diagonal:
                rescale = jnp.exp(top - top_new)
                total = total_buf[h] * rescale + total
                weighted = weighted_buf[h] * rescale + weighted
            top_buf[h] = top_new
            total_buf[h] = total
            weighted_buf[h] = weighted

    def forward(k):
        src = me - k

        @pl.when(src >= 0)
        def _():
            sum_copy(src).wait_recv()

            @pl.when(has_up)
            def _():
                sum_copy(src).start()

    attend(me, True)

    offset = (me * rows).astype(jnp.float32)
    lone = jnp.zeros((dk, vd), jnp.float32)

    def step(k, entering):
        src = me - k
        kv_forward(k)
        forward(k)

        @pl.when(k + 1 < n)
        def _():
            outs.relay(k + 1)


        @pl.when(src >= 0)
        def _():
            attend(src, False)

        gap = ((k - 1) * rows).astype(jnp.float32)
        there = jnp.maximum(src, 0)
        return tuple(
            entering[h]
            + jnp.where(src >= 0, jnp.exp(lone + gap * decay_ref[h]) * sum_buf[there, h], 0.0)
            for h in range(hr)
        )

    entering = tuple(jnp.exp(lone + offset * decay_ref[h]) * state_ref[h] for h in range(hr))
    entering = lax.fori_loop(1, n, step, entering)

    distance = jnp.maximum(row_id - col_id, 0).astype(jnp.float32)
    for h in range(hr):
        scores = lax.dot_general(rq[h], rk[h], NT, preferred_element_type=jnp.float32) * key_scale
        scores = jnp.where(causal, scores * jnp.exp(distance * decay_ref[h]), 0.0)
        inner = jnp.dot(scores, rv[h].astype(jnp.float32), precision=highest, preferred_element_type=jnp.float32)
        leading = jnp.exp((position + 1.0) * decay_ref[h])
        carried = jnp.dot(
            rq[h].astype(jnp.float32), entering[h], precision=highest, preferred_element_type=jnp.float32
        )
        raw = inner + carried * leading
        center = raw - jnp.mean(raw, axis=-1, keepdims=True)
        variance = jnp.mean(center * center, axis=-1, keepdims=True)
        cols = slice(h * vd, (h + 1) * vd)
        mix_buf[:, cols] = (center * lax.rsqrt(variance + epsilon) * hgain_ref[:, cols]).astype(jnp.bfloat16)
    for h in range(fh):
        cols = slice(hr * vd + h * fd, hr * vd + (h + 1) * fd)
        mix_buf[:, cols] = (weighted_buf[h] / total_buf[h]).astype(jnp.bfloat16)

    block = rows // n_tp
    columns = pair_buf.shape[1]
    wide = out_cols if direct else columns
    pieces = columns // wide
    half = n_tp // 2
    parity, pair = lax.rem(t, 2), lax.div(t, 2)

    def piece_cols(piece):
        return pl.ds(pl.multiple_of(piece * wide, wide), wide)

    def slot(at):
        return pl.ds(pl.multiple_of(at * block, block), block)

    def pair_copy(piece):
        cols = piece_cols(piece)
        return rdma(
            rs_send.at[1 - parity, :, cols],
            pair_buf.at[:, cols],
            pair_s.at[piece],
            pair_r.at[piece],
            tp=t + 1 - 2 * parity,
        )

    def rs_copy(d, piece):
        to = lax.rem(pair + d, half)
        cols = piece_cols(piece)
        at = (d - 1) * pieces + piece
        return rdma(
            pair_sum.at[slot(to), cols], rs_buf.at[d - 1, :, cols], rs_s.at[at], rs_r.at[at], tp=2 * to + parity
        )

    def project(piece):
        cols = piece_cols(piece)
        if direct:
            value = jnp.dot(mix_buf[...], wout_buf[:, cols], preferred_element_type=jnp.float32)
        else:
            value = lax.dot_general(mix_buf[...], wout_buf[...], NT, preferred_element_type=jnp.float32)
        value = value.astype(jnp.bfloat16)
        for b in range(n_tp):
            at = slice(b // 2 * block, (b // 2 + 1) * block)
            rs_send[b % 2, at, cols] = value[b * block : (b + 1) * block]
        pair_copy(piece).start()

    def reduce(piece):
        cols = piece_cols(piece)
        pair_copy(piece).wait_recv()
        both = rs_send[parity, :, cols].astype(jnp.float32) + pair_buf[:, cols].astype(jnp.float32)
        pair_sum[:, cols] = both.astype(jnp.bfloat16)
        for d in range(1, half):
            rs_copy(d, piece).start()

    def order(i):
        falling = jnp.where(i <= me, me - i, i)
        rising = jnp.where(i <= n - 1 - me, me + i, n - 1 - i)
        return jnp.where(2 * me >= n, falling, rising)

    if direct:
        for c in range(2):
            outs.local(c).wait()
        project(me)

        def out_step(i, _):
            outs.arrive_shard(order(i), (0, 1))
            project(order(i))
            reduce(order(i - 1))
            return 0

        lax.fori_loop(1, n, out_step, 0)
        reduce(order(jnp.int32(n - 1)))
    else:
        outs.arrive((0, 1))
        project(0)
        reduce(0)

    own = slot(pair)
    summed = rs_send[parity, own, :].astype(jnp.float32) + pair_buf[own, :].astype(jnp.float32)
    for d in range(1, half):
        for piece in range(pieces):
            rs_copy(d, piece).wait_recv()
        summed = summed + rs_buf[d - 1].astype(jnp.float32)
    out_ref[...] = summed.astype(jnp.bfloat16)

    for d in range(1, n_tp):
        tok_copy(d).wait_send()
    for piece in range(pieces):
        pair_copy(piece).wait_send()
        for d in range(1, half):
            rs_copy(d, piece).wait_send()
    firsts.finish()
    lasts.finish()
    outs.finish()

    @pl.when(has_up)
    def _():
        def step(src, _):
            kv_copy(src).wait_send()
            sum_copy(src).wait_send()
            return 0

        lax.fori_loop(0, me + 1, step, 0)


def pair_kernel(
    size,
    tok_ref,
    gain_ref,
    wq_ref,
    wk_ref,
    wrv_ref,
    wfq_ref,
    wfk_ref,
    wfv_ref,
    decay_ref,
    state_ref,
    hgain_ref,
    gates_ref,
    ret_out_ref,
    fox_out_ref,
    out_ref,
    tok_buf,
    qk_own,
    w_buf,
    wout_buf,
    norm_buf,
    proj_buf,
    kv_buf,
    sum_buf,
    mix_pair,
    mix_buf,
    rs_send,
    pair_buf,
    pair_sum,
    rs_buf,
    top_buf,
    total_buf,
    weighted_buf,
    tz_s,
    tz_r,
    tx_s,
    tx_r,
    tc_s,
    tc_r,
    t_loc,
    w_s,
    w_r,
    wy_s,
    wy_r,
    w_loc,
    kv_s,
    kv_r,
    sum_s,
    sum_r,
    mix_s,
    mix_r,
    pair_s,
    pair_r,
    rs_s,
    rs_r,
    *out_sems,
):
    n, n_tp, n_grp, hr, dk, vd, fh, fd, chunks = size
    me, t, g = lax.axis_index("sp"), lax.axis_index("tp"), lax.axis_index("grp")
    rows, feats = tok_ref.shape
    shard = qk_own.shape[0]
    couples = n // 2
    couple, mine = lax.div(me, 2), lax.rem(me, 2)
    other = 1 - mine
    partner = me + 1 - 2 * mine
    fox_mine = 1 - lax.rem(couple, 2)
    is_fox = mine == fox_mine
    is_ret = mine != fox_mine
    lower = 2 * me < n
    half = n_tp // 2
    parity, pair = lax.rem(t, 2), lax.div(t, 2)

    def fox_of(q):
        return 2 * q + 1 - lax.rem(q, 2)

    def ret_of(q):
        return 2 * q + lax.rem(q, 2)

    def toward(k):
        return lax.rem(jnp.where(lower, me + k, me + n - k), n)

    barrier = pltpu.get_barrier_semaphore()

    def greet(**target):
        pl.semaphore_signal(barrier, inc=1, device_id=target, device_id_type=pl.DeviceIdType.MESH)

    greet(tp=2 * pair + 1 - parity)
    for d in range(1, half):
        greet(tp=2 * lax.rem(pair + d, half) + parity)
    for d in range(1, n_grp):
        greet(grp=lax.rem(g + d, n_grp))
    for k in range(1, n):
        greet(sp=lax.rem(me + k, n))

    turned = jnp.concatenate((wq_ref[...], wk_ref[...]), axis=0).astype(jnp.float32)
    qk_own[...] = turned.T.astype(jnp.bfloat16)

    pl.semaphore_wait(barrier, half + n_grp - 1 + n - 1)

    slab = rows // chunks

    def own_tok(m):
        return tok_ref.at[pl.ds(m * slab, slab)]

    def tok_at(h, m, src):
        return tok_buf.at[h, src, pl.ds(m * slab, slab)]

    def tok_z(m):
        return rdma(own_tok(m), tok_at(mine, m, t), tz_s.at[m], tz_r.at[m], sp=partner)

    def tok_z_in(m):
        here = tok_at(other, m, t)
        return rdma(here, here, tz_s.at[m], tz_r.at[m], sp=partner)

    def x_sem(own, m, d):
        return ((0 if own else 1) * chunks + m) * max(half - 1, 1) + d - 1

    def tok_x(own, m, d):
        at = x_sem(own, m, d)
        h = mine if own else other
        src = own_tok(m) if own else tok_at(h, m, t)
        return rdma(src, tok_at(h, m, t), tx_s.at[at], tx_r.at[at], tp=2 * lax.rem(pair + d, half) + parity)

    def tok_x_in(own, m, d):
        at = x_sem(own, m, d)
        src = 2 * lax.rem(pair + half - d, half) + parity
        here = tok_at(mine if own else other, m, src)
        return rdma(here, here, tx_s.at[at], tx_r.at[at], tp=src)

    def c_sem(own, m, d):
        return ((0 if own else 1) * chunks + m) * half + d

    def tok_c(own, m, d):
        at = c_sem(own, m, d)
        h = mine if own else other
        src = 2 * lax.rem(pair + half - d, half) + parity
        there = tok_at(h, m, src)
        here = own_tok(m) if own and d == 0 else there
        return rdma(here, there, tc_s.at[at], tc_r.at[at], tp=2 * pair + 1 - parity)

    def tok_c_in(own, m, d):
        at = c_sem(own, m, d)
        src = 2 * lax.rem(pair + half - d, half) + 1 - parity
        here = tok_at(mine if own else other, m, src)
        return rdma(here, here, tc_s.at[at], tc_r.at[at], tp=2 * pair + 1 - parity)

    tok_local = pltpu.make_async_copy(tok_ref, tok_buf.at[mine, t], t_loc)

    for m in range(chunks):
        tok_z(m).start()
        for d in range(1, half):
            tok_x(True, m, d).start()
        tok_c(True, m, 0).start()

    owns = [wfk_ref, wfv_ref, wfq_ref, wrv_ref, qk_own]
    fox_arrays, ret_arrays = (0, 1, 2), (3, 4)
    starts = {}
    for group in (fox_arrays, ret_arrays):
        at = 0
        for c in group:
            starts[c] = (at, at + owns[c].shape[1])
            at = starts[c][1]
    fox_wide, ret_wide = starts[2][1], starts[4][1]
    q_at = starts[2][0]
    step = shard // n_grp
    count = len(owns)

    def w_at(c, src, part):
        start = pl.multiple_of(src * shard + part * step, step)
        return w_buf.at[pl.ds(start, step), starts[c][0] : starts[c][1]]

    def w_send(c, to):
        here = owns[c].at[pl.ds(pl.multiple_of(g * step, step), step)]
        return rdma(here, w_at(c, me, g), w_s.at[to * count + c], w_r.at[me * count + c], sp=to)

    def w_in(c, src):
        here = w_at(c, src, g)
        return rdma(here, here, w_s.at[src * count + c], w_r.at[src * count + c], sp=src)

    def w_side(c, src, d):
        at = ((d - 1) * n + src) * count + c
        here = w_at(c, src, g)
        return rdma(here, here, wy_s.at[at], wy_r.at[at], grp=lax.rem(g + d, n_grp))

    def w_side_in(c, src, d):
        at = ((d - 1) * n + src) * count + c
        part = lax.rem(g + n_grp - d, n_grp)
        here = w_at(c, src, part)
        return rdma(here, here, wy_s.at[at], wy_r.at[at], grp=part)

    def w_local(c):
        start = pl.multiple_of(me * shard, shard)
        return pltpu.make_async_copy(
            owns[c], w_buf.at[pl.ds(start, shard), starts[c][0] : starts[c][1]], w_loc.at[c]
        )

    def each_target(arrays, whose, act):
        for c in arrays:
            for i in range(couples):
                to = whose(jnp.where(lower, i, couples - 1 - i))

                @pl.when(to != me)
                def _(c=c, to=to):
                    act(w_send(c, to))

    def send_weights(act):
        each_target((0, 1), fox_of, act)
        each_target((2,), fox_of, act)
        each_target(ret_arrays, ret_of, act)

    send_weights(lambda copy: copy.start())
    tok_local.start()

    @pl.when(is_fox)
    def _():
        for c in fox_arrays:
            w_local(c).start()

    @pl.when(is_ret)
    def _():
        for c in ret_arrays:
            w_local(c).start()

    depth = mix_buf.shape[1] // 2
    out_cols = ret_out_ref.shape[1]

    def out_place(src, c, first, rows_):
        start = pl.multiple_of(c * depth + first, rows_)
        return wout_buf.at[pl.ds(start, rows_), pl.ds(pl.multiple_of(src * out_cols, out_cols), out_cols)]

    outs = LineGather([ret_out_ref, fox_out_ref], out_place, out_sems, n, n_grp, me, g)
    outs.start()

    def w_relay(arrays, ks):
        for k in ks:
            for c in arrays:
                w_in(c, toward(k)).wait_recv()
                for d in range(1, n_grp):
                    w_side(c, toward(k), d).start()

    def w_arrive(arrays):
        for c in arrays:
            w_local(c).wait()
            for k in range(1, n):
                for d in range(1, n_grp):
                    w_side_in(c, toward(k), d).wait_recv()

    def normalize(h):
        squares = jnp.zeros((rows, 1), jnp.float32)
        for i in range(n_tp):
            part = tok_buf[h, i].astype(jnp.float32)
            squares = squares + jnp.sum(part * part, axis=-1, keepdims=True)
        scale = lax.rsqrt(squares * (1.0 / (n_tp * feats)) + epsilon)
        at = pl.ds(pl.multiple_of(h * rows, rows), rows)
        for i in range(n_tp):
            part = tok_buf[h, i].astype(jnp.float32)
            cols = slice(i * feats, (i + 1) * feats)
            norm_buf[at, cols] = (part * scale * gain_ref[:, cols]).astype(jnp.bfloat16)

    far = list(range(2, n - 1))

    @pl.when(is_fox)
    def _():
        w_relay(fox_arrays, [1])

    for m in range(chunks):
        for d in range(1, half):
            tok_x_in(True, m, d).wait_recv()
            tok_c(True, m, d).start()
        tok_z_in(m).wait_recv()
        for d in range(1, half):
            tok_x(False, m, d).start()
        tok_c(False, m, 0).start()

    @pl.when(is_fox)
    def _():
        w_relay((0, 1), [n - 1])

    @pl.when(is_ret)
    def _():
        w_relay(ret_arrays, [1])

    tok_local.wait()
    for m in range(chunks):
        for d in range(half):
            tok_c_in(True, m, d).wait_recv()
    normalize(mine)

    for m in range(chunks):
        for d in range(1, half):
            tok_x_in(False, m, d).wait_recv()
            tok_c(False, m, d).start()

    @pl.when(is_fox)
    def _():
        w_relay((0, 1), far)

    @pl.when(is_ret)
    def _():
        w_relay(ret_arrays, far)

    for m in range(chunks):
        for d in range(half):
            tok_c_in(False, m, d).wait_recv()
    normalize(other)
    outs.relay(1)

    row_id = lax.broadcasted_iota(jnp.int32, (rows, rows), 0)
    col_id = lax.broadcasted_iota(jnp.int32, (rows, rows), 1)
    causal = col_id <= row_id

    def norm_rows(h):
        return norm_buf[pl.ds(pl.multiple_of(h * rows, rows), rows), :]

    def mix_copy(first):
        return rdma(
            mix_pair.at[other], mix_buf.at[:, first : first + depth], mix_s.at[0], mix_r.at[0], sp=partner
        )

    def mix_own(first):
        mix_buf[:, first : first + depth] = mix_pair[mine]

    def mix_in(first):
        here = mix_buf.at[:, first : first + depth]
        return rdma(here, here, mix_s.at[0], mix_r.at[0], sp=partner)

    def kv_copy(b, q):
        at = 2 * couple + b
        return rdma(kv_buf.at[at], kv_buf.at[at], kv_s.at[2 * q + b], kv_r.at[at], sp=fox_of(q))

    def kv_in(at):
        return rdma(kv_buf.at[at], kv_buf.at[at], kv_s.at[at], kv_r.at[at], sp=partner)

    def sum_copy(q):
        return rdma(sum_buf.at[couple], sum_buf.at[couple], sum_s.at[q], sum_r.at[couple], sp=ret_of(q))

    def sum_in(q):
        return rdma(sum_buf.at[q], sum_buf.at[q], sum_s.at[q], sum_r.at[q], sp=partner)

    def later(act):
        for q in range(1, couples):

            @pl.when(q > couple)
            def _(q=q):
                act(jnp.int32(q))

    @pl.when(is_fox)
    def _():
        w_arrive((0, 1))

        def kv_step(i, _):
            b = jnp.where(i == 0, mine, other)
            kv_buf[2 * couple + b] = jnp.dot(
                norm_rows(b), w_buf[:, :q_at], preferred_element_type=jnp.float32
            ).astype(jnp.bfloat16)
            later(lambda q: kv_copy(b, q).start())
            return 0

        lax.fori_loop(0, 2, kv_step, 0)
        w_relay((2,), [n - 1] + far)
        w_arrive((2,))
        proj_buf[:, : fh * fd] = jnp.dot(
            norm_buf[...], w_buf[:, q_at:fox_wide], preferred_element_type=jnp.float32
        ).astype(jnp.bfloat16)

        def block_cols(at):
            return pl.ds(pl.multiple_of(at * rows, rows), rows)

        def attend(b, at, first):
            q_rows = pl.ds(pl.multiple_of(b * rows, rows), rows)
            for h in range(fh):
                query = proj_buf[q_rows, h * fd : (h + 1) * fd]
                k = kv_buf[at, :, h * fd : (h + 1) * fd]
                v = kv_buf[at, :, (fh + h) * fd : (fh + h + 1) * fd]
                own = jnp.sum(
                    jnp.where(row_id == col_id, gates_ref[h : h + 1, block_cols(2 * couple + b)], 0.0),
                    axis=1,
                    keepdims=True,
                )
                logits = lax.dot_general(query, k, NT, preferred_element_type=jnp.float32) * fd ** (-0.5)
                logits = logits + own - gates_ref[h : h + 1, block_cols(at)]
                if first:
                    logits = jnp.where(causal, logits, -jnp.inf)
                top_new = jnp.max(logits, axis=-1, keepdims=True)
                if not first:
                    top = top_buf[b, h]
                    top_new = jnp.maximum(top, top_new)
                p = jnp.exp(logits - top_new)
                total = jnp.sum(p, axis=-1, keepdims=True)
                weighted = jnp.dot(p.astype(jnp.bfloat16), v, preferred_element_type=jnp.float32)
                if not first:
                    rescale = jnp.exp(top - top_new)
                    total = total_buf[b, h] * rescale + total
                    weighted = weighted_buf[b, h] * rescale + weighted
                top_buf[b, h] = top_new
                total_buf[b, h] = total
                weighted_buf[b, h] = weighted

        def settle(b):
            for h in range(fh):
                mix_pair[b, :, h * fd : (h + 1) * fd] = (weighted_buf[b, h] / total_buf[b, h]).astype(jnp.bfloat16)

        def diagonal(b, _):
            attend(b, 2 * couple + b, True)
            return 0

        lax.fori_loop(0, 2, diagonal, 0)
        attend(1, 2 * couple, False)

        @pl.when(couple == 0)
        def _():
            settle(other)
            mix_copy(depth).start()

        outs.relay(2)

        def past(i, _):
            q = lax.div(i, 2)
            b = jnp.where(lax.rem(i, 2) == 0, fox_of(q) - 2 * q, 1 - (fox_of(q) - 2 * q))
            at = 2 * q + b
            kv_in(at).wait_recv()

            def both(j, _):
                row_half = jnp.where(j == 0, other, mine)
                attend(row_half, at, False)

                @pl.when((j == 0) & (i == 2 * couple - 1))
                def _():
                    settle(other)
                    mix_copy(depth).start()

                return 0

            lax.fori_loop(0, 2, both, 0)
            return 0

        lax.fori_loop(0, 2 * couple, past, 0)
        settle(mine)
        mix_own(depth)
        for k in range(3, n):
            outs.relay(k)
        mix_in(0).wait_recv()
        mix_copy(depth).wait_send()
        later(lambda q: kv_copy(0, q).wait_send())
        later(lambda q: kv_copy(1, q).wait_send())

    @pl.when(is_ret)
    def _():
        w_relay(ret_arrays, [n - 1])
        w_arrive(ret_arrays)
        proj_buf[:, :ret_wide] = jnp.dot(
            norm_buf[...], w_buf[:, :ret_wide], preferred_element_type=jnp.float32
        ).astype(jnp.bfloat16)
        rv_at, rq_at = starts[3][0], starts[4][0]
        key_scale = dk ** (-0.5)
        position = lax.broadcasted_iota(jnp.int32, (rows, 1), 0).astype(jnp.float32)
        distance = jnp.maximum(row_id - col_id, 0).astype(jnp.float32)
        lone = jnp.zeros((dk, vd), jnp.float32)

        def part(b, first, wide):
            return proj_buf[pl.ds(pl.multiple_of(b * rows, rows), rows), first : first + wide]

        def summary(b, h):
            keys = part(b, rq_at + (hr + h) * dk, dk).astype(jnp.float32) * key_scale
            trailing = jnp.exp((rows - 1.0 - position) * decay_ref[h])
            return lax.dot_general(
                keys * trailing,
                part(b, rv_at + h * vd, vd).astype(jnp.float32),
                TN,
                precision=highest,
                preferred_element_type=jnp.float32,
            )

        early = [summary(0, h) for h in range(hr)]
        for h in range(hr):
            sum_buf[couple, h] = jnp.exp(lone + float(rows) * decay_ref[h]) * early[h] + summary(1, h)
        later(lambda q: sum_copy(q).start())
        outs.relay(2)

        offset = (couple * 2 * rows).astype(jnp.float32)

        def gather(q, entering):
            sum_in(q).wait_recv()
            gap = ((couple - 1 - q) * 2 * rows).astype(jnp.float32)
            return tuple(entering[h] + jnp.exp(lone + gap * decay_ref[h]) * sum_buf[q, h] for h in range(hr))

        entering = tuple(jnp.exp(lone + offset * decay_ref[h]) * state_ref[h] for h in range(hr))
        entering = lax.fori_loop(0, couple, gather, entering)
        second = tuple(jnp.exp(lone + float(rows) * decay_ref[h]) * entering[h] + early[h] for h in range(hr))

        def block(i, _):
            b = jnp.where(i == 0, other, mine)
            for h in range(hr):
                rq = part(b, rq_at + h * dk, dk)
                rk = part(b, rq_at + (hr + h) * dk, dk)
                rv = part(b, rv_at + h * vd, vd)
                scores = lax.dot_general(rq, rk, NT, preferred_element_type=jnp.float32) * key_scale
                scores = jnp.where(causal, scores * jnp.exp(distance * decay_ref[h]), 0.0)
                inner = jnp.dot(
                    scores, rv.astype(jnp.float32), precision=highest, preferred_element_type=jnp.float32
                )
                leading = jnp.exp((position + 1.0) * decay_ref[h])
                carried = jnp.dot(
                    rq.astype(jnp.float32),
                    jnp.where(b == 0, entering[h], second[h]),
                    precision=highest,
                    preferred_element_type=jnp.float32,
                )
                raw = inner + carried * leading
                center = raw - jnp.mean(raw, axis=-1, keepdims=True)
                variance = jnp.mean(center * center, axis=-1, keepdims=True)
                cols = slice(h * vd, (h + 1) * vd)
                mix_pair[b, :, cols] = (center * lax.rsqrt(variance + epsilon) * hgain_ref[:, cols]).astype(
                    jnp.bfloat16
                )

            @pl.when(i == 0)
            def _():
                mix_copy(0).start()

            return 0

        lax.fori_loop(0, 2, block, 0)
        mix_own(0)
        for k in range(3, n):
            outs.relay(k)
        mix_in(depth).wait_recv()
        mix_copy(0).wait_send()
        later(lambda q: sum_copy(q).wait_send())

    block = rows // n_tp
    wide, pieces = out_cols, n

    def piece_cols(piece):
        return pl.ds(pl.multiple_of(piece * wide, wide), wide)

    def slot(at):
        return pl.ds(pl.multiple_of(at * block, block), block)

    def pair_copy(piece):
        cols = piece_cols(piece)
        return rdma(
            rs_send.at[1 - parity, :, cols],
            pair_buf.at[:, cols],
            pair_s.at[piece],
            pair_r.at[piece],
            tp=t + 1 - 2 * parity,
        )

    def rs_copy(d, piece):
        to = lax.rem(pair + d, half)
        cols = piece_cols(piece)
        at = (d - 1) * pieces + piece
        return rdma(
            pair_sum.at[slot(to), cols], rs_buf.at[d - 1, :, cols], rs_s.at[at], rs_r.at[at], tp=2 * to + parity
        )

    def project(piece):
        cols = piece_cols(piece)
        value = jnp.dot(mix_buf[...], wout_buf[:, cols], preferred_element_type=jnp.float32).astype(jnp.bfloat16)
        for b in range(n_tp):
            at = slice(b // 2 * block, (b // 2 + 1) * block)
            rs_send[b % 2, at, cols] = value[b * block : (b + 1) * block]
        pair_copy(piece).start()

    def reduce(piece):
        cols = piece_cols(piece)
        pair_copy(piece).wait_recv()
        both = rs_send[parity, :, cols].astype(jnp.float32) + pair_buf[:, cols].astype(jnp.float32)
        pair_sum[:, cols] = both.astype(jnp.bfloat16)
        for d in range(1, half):
            rs_copy(d, piece).start()

    def order(i):
        falling = jnp.where(i <= me, me - i, i)
        rising = jnp.where(i <= n - 1 - me, me + i, n - 1 - i)
        return jnp.where(lower, rising, falling)

    for c in range(2):
        outs.local(c).wait()
    project(me)

    def out_step(i, _):
        outs.arrive_shard(order(i), (0, 1))
        project(order(i))
        reduce(order(i - 1))
        return 0

    lax.fori_loop(1, n, out_step, 0)
    reduce(order(jnp.int32(n - 1)))

    own = slot(pair)
    summed = rs_send[parity, own, :].astype(jnp.float32) + pair_buf[own, :].astype(jnp.float32)
    for d in range(1, half):
        for piece in range(pieces):
            rs_copy(d, piece).wait_recv()
        summed = summed + rs_buf[d - 1].astype(jnp.float32)
    out_ref[...] = summed.astype(jnp.bfloat16)

    for m in range(chunks):
        tok_z(m).wait_send()
        for own_half in (True, False):
            for d in range(1, half):
                tok_x(own_half, m, d).wait_send()
            for d in range(half):
                tok_c(own_half, m, d).wait_send()
    send_weights(lambda copy: copy.wait_send())

    def sides(arrays):
        for c in arrays:
            for k in range(1, n):
                for d in range(1, n_grp):
                    w_side(c, toward(k), d).wait_send()

    @pl.when(is_fox)
    def _():
        sides(fox_arrays)

    @pl.when(is_ret)
    def _():
        sides(ret_arrays)

    for piece in range(pieces):
        pair_copy(piece).wait_send()
        for d in range(1, half):
            rs_copy(d, piece).wait_send()
    outs.finish()


def paired(n, n_tp, n_grp, inputs):
    tokens, ret_query_weight, ret_state, fox_gates = inputs[0], inputs[2], inputs[9], inputs[11]
    fox_query_weight, ret_out_weight = inputs[5], inputs[12]
    rows, feats = tokens.shape
    hr, dk, vd = ret_state.shape
    fh = fox_gates.shape[1]
    fd = fox_query_weight.shape[1] // fh
    shard = ret_query_weight.shape[0]
    depth, out_cols = ret_out_weight.shape
    columns = out_cols * n
    wide = max(3 * fh * fd, 2 * hr * dk + hr * vd)
    half = n_tp // 2
    block = rows // n_tp
    chunks = 2
    count = 5
    couples = n // 2
    dma = pltpu.SemaphoreType.DMA
    far = max(half - 1, 1)
    side = max(n_grp - 1, 1) * n
    vmem = pl.BlockSpec(memory_space=pltpu.VMEM)
    smem = pl.BlockSpec(memory_space=pltpu.SMEM)
    hbm = pl.BlockSpec(memory_space=pl.ANY)
    bf16, f32 = jnp.bfloat16, jnp.float32
    size = (n, n_tp, n_grp, hr, dk, vd, fh, fd, chunks)
    return pl.pallas_call(
        functools.partial(pair_kernel, size),
        out_shape=jax.ShapeDtypeStruct((block, columns), bf16),
        in_specs=[hbm, vmem, vmem, vmem, hbm, hbm, hbm, hbm, smem, vmem, vmem, vmem, hbm, hbm],
        out_specs=vmem,
        scratch_shapes=[
            pltpu.VMEM((2, n_tp, rows, feats), bf16),
            pltpu.VMEM((shard, 2 * hr * dk), bf16),
            pltpu.VMEM((n * shard, wide), bf16),
            pltpu.VMEM((2 * depth, columns), bf16),
            pltpu.VMEM((2 * rows, n_tp * feats), bf16),
            pltpu.VMEM((2 * rows, wide), bf16),
            pltpu.VMEM((n, rows, 2 * fh * fd), bf16),
            pltpu.VMEM((couples, hr, dk, vd), f32),
            pltpu.VMEM((2, rows, depth), bf16),
            pltpu.VMEM((rows, 2 * depth), bf16),
            pltpu.VMEM((2, rows // 2, columns), bf16),
            pltpu.VMEM((rows // 2, columns), bf16),
            pltpu.VMEM((rows // 2, columns), bf16),
            pltpu.VMEM((far, block, columns), bf16),
            pltpu.VMEM((2, fh, rows, 1), f32),
            pltpu.VMEM((2, fh, rows, 1), f32),
            pltpu.VMEM((2, fh, rows, fd), f32),
            dma((chunks,)),
            dma((chunks,)),
            dma((2 * chunks * far,)),
            dma((2 * chunks * far,)),
            dma((2 * chunks * half,)),
            dma((2 * chunks * half,)),
            dma,
            dma((n * count,)),
            dma((n * count,)),
            dma((side * count,)),
            dma((side * count,)),
            dma((count,)),
            dma((2 * couples,)),
            dma((n,)),
            dma((couples,)),
            dma((couples,)),
            dma((1,)),
            dma((1,)),
            dma((n,)),
            dma((n,)),
            dma((far * n,)),
            dma((far * n,)),
            dma((n * 2,)),
            dma((n * 2,)),
            dma((n * 2,)),
            dma((side * 2,)),
            dma((side * 2,)),
            dma((2,)),
        ],
        compiler_params=pltpu.CompilerParams(
            collective_id=0, has_side_effects=True, vmem_limit_bytes=56 * 1024 * 1024
        ),
        name="layer",
    )(
        tokens,
        inputs[1][None, :],
        inputs[2].T,
        inputs[3].T,
        inputs[4],
        inputs[5],
        inputs[6],
        inputs[7],
        inputs[8],
        inputs[9],
        inputs[10][None, :],
        inputs[11].T,
        inputs[12],
        inputs[13],
    )


def pairs_fit(n, n_tp, n_grp, inputs):
    rows, feats = inputs[0].shape
    hr, dk, vd = inputs[9].shape
    shard = inputs[2].shape[0]
    depth, out_cols = inputs[12].shape
    wide = inputs[5].shape[1]
    lanes = all(w % 128 == 0 for w in (out_cols, wide, 2 * hr * dk, hr * vd, feats, depth))
    even = n % 2 == 0 and n > 2 and n_tp % 2 == 0
    tiles = rows % (16 * n_tp) == 0 and rows % 32 == 0 and shard % (16 * n_grp) == 0 and depth % (16 * n_grp) == 0
    columns = n * out_cols
    held = 8 * rows * n_tp * feats + 2 * n * shard * 3 * wide + 4 * depth * columns + 4 * n * rows * wide + 6 * rows * columns
    return lanes and even and tiles and depth == wide == hr * vd and held < 40 * 1024 * 1024


def local(
    n,
    n_tp,
    n_grp,
    tokens,
    norm_gain,
    ret_query_weight,
    ret_key_weight,
    ret_value_weight,
    fox_query_weight,
    fox_key_weight,
    fox_value_weight,
    ret_decay,
    ret_state,
    head_norm_gain,
    fox_gates,
    ret_out_weight,
    fox_out_weight,
):
    inputs = (
        tokens,
        norm_gain,
        ret_query_weight,
        ret_key_weight,
        ret_value_weight,
        fox_query_weight,
        fox_key_weight,
        fox_value_weight,
        ret_decay,
        ret_state,
        head_norm_gain,
        fox_gates,
        ret_out_weight,
        fox_out_weight,
    )
    if pairs_fit(n, n_tp, n_grp, inputs):
        return paired(n, n_tp, n_grp, inputs)
    rows, feats = tokens.shape
    hr, dk, vd = ret_state.shape
    fh = fox_gates.shape[1]
    fd = fox_query_weight.shape[1] // fh
    shard = ret_query_weight.shape[0]
    width = 2 * hr * dk + hr * vd + 3 * fh * fd
    depth, out_cols = ret_out_weight.shape
    columns = out_cols * n
    direct = out_cols % 128 == 0
    if not direct:
        ret_out_weight, fox_out_weight = ret_out_weight.T, fox_out_weight.T
    dma = pltpu.SemaphoreType.DMA

    def gather_sems(arrays):
        side = max(n_grp - 1, 1) * n * arrays
        return [
            dma((n * arrays,)),
            dma((n * arrays,)),
            dma((n * arrays,)),
            dma((side,)),
            dma((side,)),
            dma((arrays,)),
        ]

    vmem = pl.BlockSpec(memory_space=pltpu.VMEM)
    smem = pl.BlockSpec(memory_space=pltpu.SMEM)
    hbm = pl.BlockSpec(memory_space=pl.ANY)
    size = (n, n_tp, n_grp, hr, dk, vd, fh, fd, direct)
    block = rows // n_tp
    peers = max(n_tp - 1, 1)
    far = max(n_tp // 2 - 1, 1)
    pieces = n if direct else 1
    return pl.pallas_call(
        functools.partial(kernel, size),
        out_shape=jax.ShapeDtypeStruct((block, columns), jnp.bfloat16),
        in_specs=[hbm, vmem, vmem, vmem, hbm, hbm, hbm, hbm, smem, vmem, vmem, vmem, hbm, hbm],
        out_specs=vmem,
        scratch_shapes=[
            pltpu.VMEM((n_tp, rows, feats), jnp.bfloat16),
            pltpu.VMEM((shard, 2 * hr * dk), jnp.bfloat16),
            pltpu.VMEM((n * shard, width), jnp.bfloat16),
            pltpu.VMEM((2 * depth, columns) if direct else (columns, 2 * depth), jnp.bfloat16),
            pltpu.VMEM((rows, n_tp * feats), jnp.bfloat16),
            pltpu.VMEM((rows, width - 2 * fh * fd), jnp.bfloat16),
            pltpu.VMEM((n, rows, 2 * fh * fd), jnp.bfloat16),
            pltpu.VMEM((n, hr, dk, vd), jnp.float32),
            pltpu.VMEM((rows, 2 * depth), jnp.bfloat16),
            pltpu.VMEM((2, rows // 2, columns), jnp.bfloat16),
            pltpu.VMEM((rows // 2, columns), jnp.bfloat16),
            pltpu.VMEM((rows // 2, columns), jnp.bfloat16),
            pltpu.VMEM((far, block, columns), jnp.bfloat16),
            pltpu.VMEM((fh, rows, 1), jnp.float32),
            pltpu.VMEM((fh, rows, 1), jnp.float32),
            pltpu.VMEM((fh, rows, fd), jnp.float32),
            dma((peers,)),
            dma((peers,)),
            dma,
            dma((n,)),
            dma((n,)),
            dma((n,)),
            dma((n,)),
            dma((pieces,)),
            dma((pieces,)),
            dma((far * pieces,)),
            dma((far * pieces,)),
        ]
        + gather_sems(2)
        + gather_sems(3)
        + gather_sems(2),
        compiler_params=pltpu.CompilerParams(
            collective_id=0, has_side_effects=True, vmem_limit_bytes=56 * 1024 * 1024
        ),
        name="layer",
    )(
        tokens,
        norm_gain[None, :],
        ret_query_weight.T,
        ret_key_weight.T,
        ret_value_weight,
        fox_query_weight,
        fox_key_weight,
        fox_value_weight,
        ret_decay,
        ret_state,
        head_norm_gain[None, :],
        fox_gates.T,
        ret_out_weight,
        fox_out_weight,
    )


def solution(mesh):
    placed = (
        P(("grp", "sp"), "tp"),
        P(),
        P("sp", "tp"),
        P("sp", "tp"),
        P("sp", "tp"),
        P("sp", "tp"),
        P("sp", "tp"),
        P("sp", "tp"),
        P("tp"),
        P(("grp", "tp"), None, None),
        P("tp"),
        P("grp", "tp"),
        P("tp", "sp"),
        P("tp", "sp"),
    )
    body = functools.partial(local, mesh.shape["sp"], mesh.shape["tp"], mesh.shape["grp"])
    return jax.shard_map(
        body, mesh=mesh, in_specs=placed, out_specs=P(("grp", "sp", "tp"), None), check_vma=False
    )
```

```python
import functools

import jax
import jax.numpy as jnp
from jax import lax
from jax.experimental import pallas as pl
from jax.experimental.pallas import tpu as pltpu
from jax.sharding import PartitionSpec as P

epsilon = 1e-06
highest = lax.Precision.HIGHEST
NT = (((1,), (1,)), ((), ()))
TN = (((0,), (0,)), ((), ()))


def rdma(src, dst, send_sem, recv_sem, **target):
    return pltpu.make_async_remote_copy(
        src_ref=src,
        dst_ref=dst,
        send_sem=send_sem,
        recv_sem=recv_sem,
        device_id=target,
        device_id_type=pl.DeviceIdType.MESH,
    )


class LineGather:
    def __init__(self, owns, place, sems, n, n_grp, me, g):
        self.owns, self.place, self.n, self.n_grp, self.me, self.g = owns, place, n, n_grp, me, g
        self.up, self.down, self.zr, self.ys, self.yr, self.loc = sems
        self.arrays = len(owns)
        self.rows = owns[0].shape[0]
        self.step = self.rows // n_grp

    def piece(self, part, src, c):
        return self.place(src, c, part * self.step, self.step)

    def own_piece(self, c):
        return self.owns[c].at[pl.ds(pl.multiple_of(self.g * self.step, self.step), self.step)]

    def hop(self, sems, to, src, c, first=False):
        here = self.own_piece(c) if first else self.piece(self.g, src, c)
        at = src * self.arrays + c
        return rdma(here, self.piece(self.g, src, c), sems.at[at], self.zr.at[at], sp=to)

    def side(self, d, src, c):
        at = ((d - 1) * self.n + src) * self.arrays + c
        here = self.piece(self.g, src, c)
        return rdma(here, here, self.ys.at[at], self.yr.at[at], grp=lax.rem(self.g + d, self.n_grp))

    def side_in(self, d, src, c):
        at = ((d - 1) * self.n + src) * self.arrays + c
        part = lax.rem(self.g + self.n_grp - d, self.n_grp)
        here = self.piece(part, src, c)
        return rdma(here, here, self.ys.at[at], self.yr.at[at], grp=part)

    def local(self, c):
        return pltpu.make_async_copy(self.owns[c], self.place(self.me, c, 0, self.rows), self.loc.at[c])

    def start(self):
        me, n = self.me, self.n
        for c in range(self.arrays):

            @pl.when(me + 1 < n)
            def _():
                self.hop(self.up, me + 1, me, c, True).start()

            @pl.when(me >= 1)
            def _():
                self.hop(self.down, me - 1, me, c, True).start()

        for c in range(self.arrays):
            self.local(c).start()

    def relay(self, k):
        me, n = self.me, self.n
        for c in range(self.arrays):
            for src, sems, to in ((me - k, self.up, me + 1), (me + k, self.down, me - 1)):

                @pl.when((src >= 0) & (src < n))
                def _(src=src, sems=sems, to=to):
                    self.hop(sems, me, src, c).wait_recv()

                    @pl.when((to >= 0) & (to < n))
                    def _():
                        self.hop(sems, to, src, c).start()

                    for d in range(1, self.n_grp):
                        self.side(d, src, c).start()

    def arrive_shard(self, src, arrays):
        for c in arrays:
            for d in range(1, self.n_grp):
                self.side_in(d, src, c).wait_recv()

    def arrive(self, arrays):
        for c in arrays:
            self.local(c).wait()

        def step(k, _):
            self.arrive_shard(lax.rem(self.me + k, self.n), arrays)
            return 0

        lax.fori_loop(1, self.n, step, 0)

    def finish(self):
        me, n = self.me, self.n

        def step(src, _):
            for c in range(self.arrays):

                @pl.when((src <= me) & (me + 1 < n))
                def _():
                    self.hop(self.up, me, src, c).wait_send()

                @pl.when((src >= me) & (me >= 1))
                def _():
                    self.hop(self.down, me, src, c).wait_send()

                @pl.when(src != me)
                def _():
                    for d in range(1, self.n_grp):
                        self.side(d, src, c).wait_send()

            return 0

        lax.fori_loop(0, n, step, 0)


def kernel(
    size,
    tok_ref,
    gain_ref,
    wq_ref,
    wk_ref,
    wrv_ref,
    wfq_ref,
    wfk_ref,
    wfv_ref,
    decay_ref,
    state_ref,
    hgain_ref,
    gates_ref,
    ret_out_ref,
    fox_out_ref,
    out_ref,
    tok_buf,
    qk_own,
    w_buf,
    wout_buf,
    norm_buf,
    proj_buf,
    kv_buf,
    sum_buf,
    mix_buf,
    rs_send,
    pair_buf,
    pair_sum,
    rs_buf,
    top_buf,
    total_buf,
    weighted_buf,
    tok_s,
    tok_r,
    tok_loc,
    kv_s,
    kv_r,
    sum_s,
    sum_r,
    pair_s,
    pair_r,
    rs_s,
    rs_r,
    *gather_sems,
):
    n, n_tp, n_grp, hr, dk, vd, fh, fd, direct = size
    me, t, g = lax.axis_index("sp"), lax.axis_index("tp"), lax.axis_index("grp")
    rows, feats = tok_ref.shape
    owns = [wfk_ref, wfv_ref, wfq_ref, wrv_ref, qk_own]
    early = 2
    starts = [0]
    for own in owns:
        starts.append(starts[-1] + own.shape[1])
    shard = qk_own.shape[0]

    def weight_place(src, c, first, count):
        start = pl.multiple_of(src * shard + first, count)
        return w_buf.at[pl.ds(start, count), starts[c] : starts[c + 1]]

    depth = mix_buf.shape[1] // 2
    out_cols = ret_out_ref.shape[1] if direct else ret_out_ref.shape[0]

    def out_place(src, c, first, count):
        if direct:
            start = pl.multiple_of(c * depth + first, count)
            return wout_buf.at[pl.ds(start, count), pl.ds(pl.multiple_of(src * out_cols, out_cols), out_cols)]
        start = pl.multiple_of(src * out_cols + first, count)
        return wout_buf.at[pl.ds(start, count), c * depth : (c + 1) * depth]

    def late_place(src, c, first, count):
        return weight_place(src, c + early, first, count)

    firsts = LineGather(owns[:early], weight_place, gather_sems[:6], n, n_grp, me, g)
    lasts = LineGather(owns[early:], late_place, gather_sems[6:12], n, n_grp, me, g)
    outs = LineGather([ret_out_ref, fox_out_ref], out_place, gather_sems[12:], n, n_grp, me, g)

    barrier = pltpu.get_barrier_semaphore()

    def greet(**target):
        pl.semaphore_signal(barrier, inc=1, device_id=target, device_id_type=pl.DeviceIdType.MESH)

    has_up, has_down = me + 1 < n, me >= 1
    for d in range(1, n_tp):
        greet(tp=lax.rem(t + d, n_tp))
    for d in range(1, n_grp):
        greet(grp=lax.rem(g + d, n_grp))

    @pl.when(has_up)
    def _():
        greet(sp=me + 1)

    @pl.when(has_down)
    def _():
        greet(sp=me - 1)

    turned = jnp.concatenate((wq_ref[...], wk_ref[...]), axis=0).astype(jnp.float32)
    qk_own[...] = turned.T.astype(jnp.bfloat16)

    count = n_tp - 1 + n_grp - 1 + has_up.astype(jnp.int32) + has_down.astype(jnp.int32)
    pl.semaphore_wait(barrier, count)

    def tok_copy(d):
        return rdma(tok_ref, tok_buf.at[t], tok_s.at[d - 1], tok_r.at[d - 1], tp=lax.rem(t + d, n_tp))

    def tok_in(d):
        src = lax.rem(t + n_tp - d, n_tp)
        return rdma(tok_ref, tok_buf.at[src], tok_s.at[d - 1], tok_r.at[d - 1], tp=src)

    firsts.start()
    lasts.start()
    tok_local = pltpu.make_async_copy(tok_ref, tok_buf.at[t], tok_loc)
    for d in range(1, n_tp):
        tok_copy(d).start()
    tok_local.start()

    def first_step(k, _):
        firsts.relay(k)

        lasts.relay(k)
        return 0

    lax.fori_loop(1, n, first_step, 0)
    outs.start()

    tok_local.wait()
    for d in range(1, n_tp):
        tok_in(d).wait_recv()
    squares = jnp.zeros((rows, 1), jnp.float32)
    for i in range(n_tp):
        part = tok_buf[i].astype(jnp.float32)
        squares = squares + jnp.sum(part * part, axis=-1, keepdims=True)
    scale = lax.rsqrt(squares * (1.0 / (n_tp * feats)) + epsilon)
    for i in range(n_tp):
        part = tok_buf[i].astype(jnp.float32)
        cols = slice(i * feats, (i + 1) * feats)
        norm_buf[:, cols] = (part * scale * gain_ref[:, cols]).astype(jnp.bfloat16)

    def kv_copy(src):
        return rdma(kv_buf.at[src], kv_buf.at[src], kv_s.at[src], kv_r.at[src], sp=jnp.minimum(me + 1, n - 1))

    def sum_copy(src):
        return rdma(sum_buf.at[src], sum_buf.at[src], sum_s.at[src], sum_r.at[src], sp=jnp.minimum(me + 1, n - 1))

    firsts.arrive((0, 1))
    kv_buf[me] = jnp.dot(
        norm_buf[...], w_buf[:, : starts[2]], preferred_element_type=jnp.float32
    ).astype(jnp.bfloat16)

    def kv_forward(k):
        src = me - k

        @pl.when(src >= 0)
        def _():
            kv_copy(src).wait_recv()

            @pl.when(has_up)
            def _():
                kv_copy(src).start()

    @pl.when(has_up)
    def _():
        kv_copy(me).start()

    outs.relay(1)
    lasts.arrive((0, 1, 2))
    proj_buf[...] = jnp.dot(
        norm_buf[...], w_buf[:, starts[2] :], preferred_element_type=jnp.float32
    ).astype(jnp.bfloat16)
    rv_at, rq_at = starts[3] - starts[2], starts[4] - starts[2]

    key_scale = dk ** (-0.5)
    position = lax.broadcasted_iota(jnp.int32, (rows, 1), 0).astype(jnp.float32)
    rq, rk, rv = [], [], []
    for h in range(hr):
        rq.append(proj_buf[:, rq_at + h * dk : rq_at + (h + 1) * dk])
        rk.append(proj_buf[:, rq_at + (hr + h) * dk : rq_at + (hr + h + 1) * dk])
        rv.append(proj_buf[:, rv_at + h * vd : rv_at + (h + 1) * vd])
        keys = rk[h].astype(jnp.float32) * key_scale
        trailing = jnp.exp((rows - 1.0 - position) * decay_ref[h])
        sum_buf[me, h] = lax.dot_general(
            keys * trailing, rv[h].astype(jnp.float32), TN, precision=highest, preferred_element_type=jnp.float32
        )

    @pl.when(has_up)
    def _():
        sum_copy(me).start()

    row_id = lax.broadcasted_iota(jnp.int32, (rows, rows), 0)
    col_id = lax.broadcasted_iota(jnp.int32, (rows, rows), 1)
    causal = col_id <= row_id
    own_cols = pl.ds(pl.multiple_of(me * rows, rows), rows)
    own_gates = [
        jnp.sum(jnp.where(row_id == col_id, gates_ref[h : h + 1, own_cols], 0.0), axis=1, keepdims=True)
        for h in range(fh)
    ]

    def attend(src, diagonal):
        key_cols = pl.ds(pl.multiple_of(src * rows, rows), rows)
        for h in range(fh):
            query = proj_buf[:, h * fd : (h + 1) * fd]
            k = kv_buf[src, :, h * fd : (h + 1) * fd]
            v = kv_buf[src, :, (fh + h) * fd : (fh + h + 1) * fd]
            logits = lax.dot_general(query, k, NT, preferred_element_type=jnp.float32) * fd ** (-0.5)
            logits = logits + own_gates[h] - gates_ref[h : h + 1, key_cols]
            if diagonal:
                logits = jnp.where(causal, logits, -jnp.inf)
            top_new = jnp.max(logits, axis=-1, keepdims=True)
            if not diagonal:
                top = top_buf[h]
                top_new = jnp.maximum(top, top_new)
            p = jnp.exp(logits - top_new)
            total = jnp.sum(p, axis=-1, keepdims=True)
            weighted = jnp.dot(p.astype(jnp.bfloat16), v, preferred_element_type=jnp.float32)
            if not diagonal:
                rescale = jnp.exp(top - top_new)
                total = total_buf[h] * rescale + total
                weighted = weighted_buf[h] * rescale + weighted
            top_buf[h] = top_new
            total_buf[h] = total
            weighted_buf[h] = weighted

    def forward(k):
        src = me - k

        @pl.when(src >= 0)
        def _():
            sum_copy(src).wait_recv()

            @pl.when(has_up)
            def _():
                sum_copy(src).start()

    attend(me, True)

    offset = (me * rows).astype(jnp.float32)
    lone = jnp.zeros((dk, vd), jnp.float32)

    def step(k, entering):
        src = me - k
        kv_forward(k)
        forward(k)

        @pl.when(k + 1 < n)
        def _():
            outs.relay(k + 1)


        @pl.when(src >= 0)
        def _():
            attend(src, False)

        gap = ((k - 1) * rows).astype(jnp.float32)
        there = jnp.maximum(src, 0)
        return tuple(
            entering[h]
            + jnp.where(src >= 0, jnp.exp(lone + gap * decay_ref[h]) * sum_buf[there, h], 0.0)
            for h in range(hr)
        )

    entering = tuple(jnp.exp(lone + offset * decay_ref[h]) * state_ref[h] for h in range(hr))
    entering = lax.fori_loop(1, n, step, entering)

    distance = jnp.maximum(row_id - col_id, 0).astype(jnp.float32)
    for h in range(hr):
        scores = lax.dot_general(rq[h], rk[h], NT, preferred_element_type=jnp.float32) * key_scale
        scores = jnp.where(causal, scores * jnp.exp(distance * decay_ref[h]), 0.0)
        inner = jnp.dot(scores, rv[h].astype(jnp.float32), precision=highest, preferred_element_type=jnp.float32)
        leading = jnp.exp((position + 1.0) * decay_ref[h])
        carried = jnp.dot(
            rq[h].astype(jnp.float32), entering[h], precision=highest, preferred_element_type=jnp.float32
        )
        raw = inner + carried * leading
        center = raw - jnp.mean(raw, axis=-1, keepdims=True)
        variance = jnp.mean(center * center, axis=-1, keepdims=True)
        cols = slice(h * vd, (h + 1) * vd)
        mix_buf[:, cols] = (center * lax.rsqrt(variance + epsilon) * hgain_ref[:, cols]).astype(jnp.bfloat16)
    for h in range(fh):
        cols = slice(hr * vd + h * fd, hr * vd + (h + 1) * fd)
        mix_buf[:, cols] = (weighted_buf[h] / total_buf[h]).astype(jnp.bfloat16)

    block = rows // n_tp
    columns = pair_buf.shape[1]
    wide = out_cols if direct else columns
    pieces = columns // wide
    half = n_tp // 2
    parity, pair = lax.rem(t, 2), lax.div(t, 2)

    def piece_cols(piece):
        return pl.ds(pl.multiple_of(piece * wide, wide), wide)

    def slot(at):
        return pl.ds(pl.multiple_of(at * block, block), block)

    def pair_copy(piece):
        cols = piece_cols(piece)
        return rdma(
            rs_send.at[1 - parity, :, cols],
            pair_buf.at[:, cols],
            pair_s.at[piece],
            pair_r.at[piece],
            tp=t + 1 - 2 * parity,
        )

    def rs_copy(d, piece):
        to = lax.rem(pair + d, half)
        cols = piece_cols(piece)
        at = (d - 1) * pieces + piece
        return rdma(
            pair_sum.at[slot(to), cols], rs_buf.at[d - 1, :, cols], rs_s.at[at], rs_r.at[at], tp=2 * to + parity
        )

    def project(piece):
        cols = piece_cols(piece)
        if direct:
            value = jnp.dot(mix_buf[...], wout_buf[:, cols], preferred_element_type=jnp.float32)
        else:
            value = lax.dot_general(mix_buf[...], wout_buf[...], NT, preferred_element_type=jnp.float32)
        value = value.astype(jnp.bfloat16)
        for b in range(n_tp):
            at = slice(b // 2 * block, (b // 2 + 1) * block)
            rs_send[b % 2, at, cols] = value[b * block : (b + 1) * block]
        pair_copy(piece).start()

    def reduce(piece):
        cols = piece_cols(piece)
        pair_copy(piece).wait_recv()
        both = rs_send[parity, :, cols].astype(jnp.float32) + pair_buf[:, cols].astype(jnp.float32)
        pair_sum[:, cols] = both.astype(jnp.bfloat16)
        for d in range(1, half):
            rs_copy(d, piece).start()

    def order(i):
        falling = jnp.where(i <= me, me - i, i)
        rising = jnp.where(i <= n - 1 - me, me + i, n - 1 - i)
        return jnp.where(2 * me >= n, falling, rising)

    if direct:
        for c in range(2):
            outs.local(c).wait()
        project(me)

        def out_step(i, _):
            outs.arrive_shard(order(i), (0, 1))
            project(order(i))
            reduce(order(i - 1))
            return 0

        lax.fori_loop(1, n, out_step, 0)
        reduce(order(jnp.int32(n - 1)))
    else:
        outs.arrive((0, 1))
        project(0)
        reduce(0)

    own = slot(pair)
    summed = rs_send[parity, own, :].astype(jnp.float32) + pair_buf[own, :].astype(jnp.float32)
    for d in range(1, half):
        for piece in range(pieces):
            rs_copy(d, piece).wait_recv()
        summed = summed + rs_buf[d - 1].astype(jnp.float32)
    out_ref[...] = summed.astype(jnp.bfloat16)

    for d in range(1, n_tp):
        tok_copy(d).wait_send()
    for piece in range(pieces):
        pair_copy(piece).wait_send()
        for d in range(1, half):
            rs_copy(d, piece).wait_send()
    firsts.finish()
    lasts.finish()
    outs.finish()

    @pl.when(has_up)
    def _():
        def step(src, _):
            kv_copy(src).wait_send()
            sum_copy(src).wait_send()
            return 0

        lax.fori_loop(0, me + 1, step, 0)


def pair_kernel(
    size,
    tok_ref,
    gain_ref,
    wq_ref,
    wk_ref,
    wrv_ref,
    wfq_ref,
    wfk_ref,
    wfv_ref,
    decay_ref,
    state_ref,
    hgain_ref,
    gates_ref,
    ret_out_ref,
    fox_out_ref,
    near_ref,
    far_ref,
    gain_buf,
    wq_buf,
    wk_buf,
    state_buf,
    hgain_buf,
    gates_buf,
    gate_col,
    tok_buf,
    qk_own,
    w_buf,
    wout_buf,
    norm_buf,
    proj_buf,
    kv_buf,
    sum_buf,
    mix_pair,
    mix_buf,
    rs_send,
    pair_buf,
    pair_sum,
    near_buf,
    top_buf,
    total_buf,
    weighted_buf,
    in_sem,
    near_sem,
    above_sem,
    below_sem,
    tz_s,
    tz_r,
    tx_s,
    tx_r,
    tc_s,
    tc_r,
    t_loc,
    w_s,
    w_r,
    wy_s,
    wy_r,
    w_loc,
    kv_s,
    kv_r,
    sum_s,
    sum_r,
    mix_s,
    mix_r,
    pair_s,
    pair_r,
    rs_s,
    rs_r,
    *out_sems,
):
    n, n_tp, n_grp, hr, dk, vd, fh, fd, chunks = size
    me, t, g = lax.axis_index("sp"), lax.axis_index("tp"), lax.axis_index("grp")
    rows, feats = tok_ref.shape
    shard = qk_own.shape[0]
    couples = n // 2
    couple, mine = lax.div(me, 2), lax.rem(me, 2)
    other = 1 - mine
    partner = me + 1 - 2 * mine
    fox_mine = 1 - lax.rem(couple, 2)
    is_fox = mine == fox_mine
    is_ret = mine != fox_mine
    lower = 2 * me < n
    half = n_tp // 2
    parity, pair = lax.rem(t, 2), lax.div(t, 2)

    def fox_of(q):
        return 2 * q + 1 - lax.rem(q, 2)

    def ret_of(q):
        return 2 * q + lax.rem(q, 2)

    def toward(k):
        return lax.rem(jnp.where(lower, me + k, me + n - k), n)

    barrier = pltpu.get_barrier_semaphore()

    def greet(**target):
        pl.semaphore_signal(barrier, inc=1, device_id=target, device_id_type=pl.DeviceIdType.MESH)

    greet(tp=2 * pair + 1 - parity)
    for d in range(1, half):
        greet(tp=2 * lax.rem(pair + d, half) + parity)
    for d in range(1, n_grp):
        greet(grp=lax.rem(g + d, n_grp))
    has_up, has_down = me + 1 < n, me >= 1

    @pl.when(has_up)
    def _():
        greet(sp=me + 1)

    @pl.when(has_down)
    def _():
        greet(sp=me - 1)

    brought = [
        pltpu.make_async_copy(src, dst, in_sem.at[i])
        for i, (src, dst) in enumerate(
            (
                (wq_ref, wq_buf),
                (wk_ref, wk_buf),
                (gain_ref, gain_buf),
                (state_ref, state_buf),
                (hgain_ref, hgain_buf),
                (gates_ref, gates_buf),
            )
        )
    ]
    for copy in brought:
        copy.start()
    for copy in brought[:2]:
        copy.wait()
    turned = jnp.concatenate((wq_buf[...], wk_buf[...]), axis=0).astype(jnp.float32)
    qk_own[...] = turned.T.astype(jnp.bfloat16)

    pl.semaphore_wait(barrier, half + n_grp - 1 + has_up.astype(jnp.int32) + has_down.astype(jnp.int32))

    def tell(sem, to):
        pl.semaphore_signal(sem, inc=1, device_id={"sp": to}, device_id_type=pl.DeviceIdType.MESH)

    @pl.when(has_up & has_down)
    def _():
        tell(above_sem, me - 1)
        tell(below_sem, me + 1)

    def meet_far():
        def from_above(i, _):
            pl.semaphore_wait(above_sem, 1)

            @pl.when(has_down)
            def _():
                tell(above_sem, me - 1)

            return 0

        def from_below(i, _):
            pl.semaphore_wait(below_sem, 1)

            @pl.when(has_up)
            def _():
                tell(below_sem, me + 1)

            return 0

        lax.fori_loop(0, jnp.maximum(n - 2 - me, 0), from_above, 0)
        lax.fori_loop(0, jnp.maximum(me - 1, 0), from_below, 0)

    slab = rows // chunks

    def own_tok(m):
        return tok_ref.at[pl.ds(m * slab, slab)]

    def tok_at(h, m, src):
        return tok_buf.at[h, src, pl.ds(m * slab, slab)]

    def tok_z(m):
        return rdma(own_tok(m), tok_at(mine, m, t), tz_s.at[m], tz_r.at[m], sp=partner)

    def tok_z_in(m):
        here = tok_at(other, m, t)
        return rdma(here, here, tz_s.at[m], tz_r.at[m], sp=partner)

    def x_sem(own, m, d):
        return ((0 if own else 1) * chunks + m) * max(half - 1, 1) + d - 1

    def tok_x(own, m, d):
        at = x_sem(own, m, d)
        h = mine if own else other
        src = own_tok(m) if own else tok_at(h, m, t)
        return rdma(src, tok_at(h, m, t), tx_s.at[at], tx_r.at[at], tp=2 * lax.rem(pair + d, half) + parity)

    def tok_x_in(own, m, d):
        at = x_sem(own, m, d)
        src = 2 * lax.rem(pair + half - d, half) + parity
        here = tok_at(mine if own else other, m, src)
        return rdma(here, here, tx_s.at[at], tx_r.at[at], tp=src)

    def c_sem(own, m, d):
        return ((0 if own else 1) * chunks + m) * half + d

    def tok_c(own, m, d):
        at = c_sem(own, m, d)
        h = mine if own else other
        src = 2 * lax.rem(pair + half - d, half) + parity
        there = tok_at(h, m, src)
        here = own_tok(m) if own and d == 0 else there
        return rdma(here, there, tc_s.at[at], tc_r.at[at], tp=2 * pair + 1 - parity)

    def tok_c_in(own, m, d):
        at = c_sem(own, m, d)
        src = 2 * lax.rem(pair + half - d, half) + 1 - parity
        here = tok_at(mine if own else other, m, src)
        return rdma(here, here, tc_s.at[at], tc_r.at[at], tp=2 * pair + 1 - parity)

    tok_local = pltpu.make_async_copy(tok_ref, tok_buf.at[mine, t], t_loc)

    for m in range(chunks):
        for d in range(1, half):
            tok_x(True, m, d).start()

    owns = [wfk_ref, wfv_ref, wfq_ref, wrv_ref, qk_own]
    fox_arrays, ret_arrays = (0, 1, 2), (3, 4)
    starts = {}
    for group in (fox_arrays, ret_arrays):
        at = 0
        for c in group:
            starts[c] = (at, at + owns[c].shape[1])
            at = starts[c][1]
    fox_wide, ret_wide = starts[2][1], starts[4][1]
    q_at = starts[2][0]
    step = shard // n_grp
    count = len(owns)

    def w_at(c, src, part):
        start = pl.multiple_of(src * shard + part * step, step)
        return w_buf.at[pl.ds(start, step), starts[c][0] : starts[c][1]]

    def w_sem(c, src, up):
        return ((0 if up else n) + src) * count + c

    def w_send(c, to, up):
        here = owns[c].at[pl.ds(pl.multiple_of(g * step, step), step)]
        return rdma(here, w_at(c, me, g), w_s.at[w_sem(c, me, up)], w_r.at[me * count + c], sp=to)

    def w_on(c, src, to, up):
        here = w_at(c, src, g)
        return rdma(here, here, w_s.at[w_sem(c, src, up)], w_r.at[src * count + c], sp=to)

    def w_in(c, src):
        here = w_at(c, src, g)
        return rdma(here, here, w_s.at[src * count + c], w_r.at[src * count + c], sp=src)

    def w_side(c, src, d):
        at = ((d - 1) * n + src) * count + c
        here = w_at(c, src, g)
        return rdma(here, here, wy_s.at[at], wy_r.at[at], grp=lax.rem(g + d, n_grp))

    def w_side_in(c, src, d):
        at = ((d - 1) * n + src) * count + c
        part = lax.rem(g + n_grp - d, n_grp)
        here = w_at(c, src, part)
        return rdma(here, here, wy_s.at[at], wy_r.at[at], grp=part)

    def w_local(c):
        start = pl.multiple_of(me * shard, shard)
        return pltpu.make_async_copy(
            owns[c], w_buf.at[pl.ds(start, shard), starts[c][0] : starts[c][1]], w_loc.at[c]
        )

    fox_up = jnp.where(is_ret & (mine == 0), partner, fox_of(couple + 1))
    fox_down = jnp.where(is_ret & (mine == 1), partner, jnp.where(couple >= 1, fox_of(jnp.maximum(couple - 1, 0)), -1))
    ret_up = jnp.where(is_fox & (mine == 0), partner, ret_of(couple + 1))
    ret_down = jnp.where(is_fox & (mine == 1), partner, jnp.where(couple >= 1, ret_of(jnp.maximum(couple - 1, 0)), -1))

    def send_weights(arrays, act):
        up, down = (fox_up, fox_down) if arrays[0] in fox_arrays else (ret_up, ret_down)
        for c in arrays:

            @pl.when(up < n)
            def _(c=c):
                act(w_send(c, up, True))

            @pl.when(down >= 0)
            def _(c=c):
                act(w_send(c, down, False))

    def start(copy):
        copy.start()

    send_weights((0, 1), start)
    for m in range(chunks):
        tok_z(m).start()
        tok_c(True, m, 0).start()
    send_weights((2,), start)
    tok_local.start()

    @pl.when(is_fox)
    def _():
        for c in fox_arrays:
            w_local(c).start()

    @pl.when(is_ret)
    def _():
        for c in ret_arrays:
            w_local(c).start()

    depth = mix_buf.shape[1] // 2
    out_cols = ret_out_ref.shape[1]

    def out_place(src, c, first, rows_):
        start = pl.multiple_of(c * depth + first, rows_)
        return wout_buf.at[pl.ds(start, rows_), pl.ds(pl.multiple_of(src * out_cols, out_cols), out_cols)]

    outs = LineGather([ret_out_ref, fox_out_ref], out_place, out_sems, n, n_grp, me, g)

    def w_pass(c, src, act):
        up, down = (fox_up, fox_down) if c in fox_arrays else (ret_up, ret_down)

        @pl.when((src < me) & (up < n))
        def _():
            act(w_on(c, src, up, True))

        @pl.when((src > me) & (down >= 0))
        def _():
            act(w_on(c, src, down, False))

    def w_relay(arrays, ks):
        for k in ks:
            for c in arrays:
                w_in(c, toward(k)).wait_recv()
                w_pass(c, toward(k), start)
                for d in range(1, n_grp):
                    w_side(c, toward(k), d).start()

    def w_arrive(arrays):
        for c in arrays:
            w_local(c).wait()
            for k in range(1, n):
                for d in range(1, n_grp):
                    w_side_in(c, toward(k), d).wait_recv()

    def normalize(h):
        squares = jnp.zeros((rows, 1), jnp.float32)
        for i in range(n_tp):
            part = tok_buf[h, i].astype(jnp.float32)
            squares = squares + jnp.sum(part * part, axis=-1, keepdims=True)
        scale = lax.rsqrt(squares * (1.0 / (n_tp * feats)) + epsilon)
        at = pl.ds(pl.multiple_of(h * rows, rows), rows)
        for i in range(n_tp):
            part = tok_buf[h, i].astype(jnp.float32)
            cols = slice(i * feats, (i + 1) * feats)
            norm_buf[at, cols] = (part * scale * gain_buf[:, cols]).astype(jnp.bfloat16)

    far = list(range(2, n - 1))

    def tok_own(m):
        for d in range(1, half):
            tok_x_in(True, m, d).wait_recv()
            tok_c(True, m, d).start()

    def tok_swap(m):
        tok_z_in(m).wait_recv()
        for d in range(1, half):
            tok_x(False, m, d).start()
        tok_c(False, m, 0).start()

    def tok_last(m):
        for d in range(1, half):
            tok_x_in(False, m, d).wait_recv()
            tok_c(False, m, d).start()

    def tok_ready(own):
        if own:
            tok_local.wait()
        for m in range(chunks):
            for d in range(half):
                tok_c_in(own, m, d).wait_recv()

    for copy in brought[2:]:
        copy.wait()

    @pl.when(is_fox)
    def _():
        w_relay((0, 1), [1, n - 1])

    meet_far()
    send_weights(ret_arrays, start)
    outs.start()

    for m in range(chunks):
        tok_own(m)
        tok_swap(m)

    @pl.when(is_fox)
    def _():
        w_relay((0, 1), far)
        w_relay((2,), [1])

    tok_ready(True)
    normalize(mine)

    row_id = lax.broadcasted_iota(jnp.int32, (rows, rows), 0)
    col_id = lax.broadcasted_iota(jnp.int32, (rows, rows), 1)
    causal = col_id <= row_id

    def norm_rows(h):
        return norm_buf[pl.ds(pl.multiple_of(h * rows, rows), rows), :]

    def mix_copy(first):
        return rdma(
            mix_pair.at[other], mix_buf.at[:, first : first + depth], mix_s.at[0], mix_r.at[0], sp=partner
        )

    def mix_own(first):
        mix_buf[:, first : first + depth] = mix_pair[mine]

    def mix_in(first):
        here = mix_buf.at[:, first : first + depth]
        return rdma(here, here, mix_s.at[0], mix_r.at[0], sp=partner)

    def kv_copy(b, q):
        at = 2 * couple + b
        return rdma(kv_buf.at[at], kv_buf.at[at], kv_s.at[2 * q + b], kv_r.at[at], sp=fox_of(q))

    def kv_in(at):
        return rdma(kv_buf.at[at], kv_buf.at[at], kv_s.at[at], kv_r.at[at], sp=partner)

    def sum_copy(q):
        return rdma(sum_buf.at[couple], sum_buf.at[couple], sum_s.at[q], sum_r.at[couple], sp=ret_of(q))

    def sum_in(q):
        return rdma(sum_buf.at[q], sum_buf.at[q], sum_s.at[q], sum_r.at[q], sp=partner)

    def later(act):
        for q in range(1, couples):

            @pl.when(q > couple)
            def _(q=q):
                act(jnp.int32(q))

    def after_tokens():
        for m in range(chunks):
            tok_last(m)

    @pl.when(is_fox)
    def _():
        def project_kv(b):
            kv_buf[2 * couple + b] = jnp.dot(
                norm_rows(b), w_buf[:, :q_at], preferred_element_type=jnp.float32
            ).astype(jnp.bfloat16)
            later(lambda q: kv_copy(b, q).start())

        after_tokens()
        w_arrive((0, 1))
        project_kv(mine)
        w_relay((2,), [n - 1] + far)
        tok_ready(False)
        normalize(other)
        project_kv(other)
        outs.relay(1)
        w_arrive((2,))
        proj_buf[:, : fh * fd] = jnp.dot(
            norm_buf[...], w_buf[:, q_at:fox_wide], preferred_element_type=jnp.float32
        ).astype(jnp.bfloat16)

        def block_cols(at):
            return pl.ds(pl.multiple_of(at * rows, rows), rows)

        for b in range(2):
            for h in range(fh):
                own = jnp.where(row_id == col_id, gates_buf[h : h + 1, block_cols(2 * couple + b)], 0.0)
                gate_col[b, h] = jnp.sum(own, axis=1, keepdims=True)

        def attend(b, at, first):
            q_rows = pl.ds(pl.multiple_of(b * rows, rows), rows)
            for h in range(fh):
                query = proj_buf[q_rows, h * fd : (h + 1) * fd]
                k = kv_buf[at, :, h * fd : (h + 1) * fd]
                v = kv_buf[at, :, (fh + h) * fd : (fh + h + 1) * fd]
                logits = lax.dot_general(query, k, NT, preferred_element_type=jnp.float32) * fd ** (-0.5)
                logits = logits + gate_col[b, h] - gates_buf[h : h + 1, block_cols(at)]
                if first:
                    logits = jnp.where(causal, logits, -jnp.inf)
                top_new = jnp.max(logits, axis=-1, keepdims=True)
                if not first:
                    top = top_buf[b, h]
                    top_new = jnp.maximum(top, top_new)
                p = jnp.exp(logits - top_new)
                total = jnp.sum(p, axis=-1, keepdims=True)
                weighted = jnp.dot(p.astype(jnp.bfloat16), v, preferred_element_type=jnp.float32)
                if not first:
                    rescale = jnp.exp(top - top_new)
                    total = total_buf[b, h] * rescale + total
                    weighted = weighted_buf[b, h] * rescale + weighted
                top_buf[b, h] = top_new
                total_buf[b, h] = total
                weighted_buf[b, h] = weighted

        def settle(b):
            for h in range(fh):
                mix_pair[b, :, h * fd : (h + 1) * fd] = (weighted_buf[b, h] / total_buf[b, h]).astype(jnp.bfloat16)

        def diagonal(b, _):
            attend(b, 2 * couple + b, True)
            return 0

        lax.fori_loop(0, 2, diagonal, 0)
        attend(1, 2 * couple, False)

        @pl.when(couple == 0)
        def _():
            settle(other)
            mix_copy(depth).start()

        def past(i, _):
            q = lax.div(i, 2)
            b = jnp.where(lax.rem(i, 2) == 0, fox_of(q) - 2 * q, 1 - (fox_of(q) - 2 * q))
            at = 2 * q + b
            kv_in(at).wait_recv()

            def both(j, _):
                row_half = jnp.where(j == 0, other, mine)
                attend(row_half, at, False)

                @pl.when((j == 0) & (i == 2 * couple - 1))
                def _():
                    settle(other)
                    mix_copy(depth).start()

                return 0

            lax.fori_loop(0, 2, both, 0)
            return 0

        lax.fori_loop(0, 2 * couple, past, 0)
        settle(mine)
        mix_own(depth)
        for k in range(2, n):
            outs.relay(k)
        mix_in(0).wait_recv()
        mix_copy(depth).wait_send()
        later(lambda q: kv_copy(0, q).wait_send())
        later(lambda q: kv_copy(1, q).wait_send())

    @pl.when(is_ret)
    def _():
        w_relay(ret_arrays, [1] + far)
        after_tokens()
        tok_ready(False)
        normalize(other)
        w_relay(ret_arrays, [n - 1])
        outs.relay(1)
        w_arrive(ret_arrays)
        proj_buf[:, :ret_wide] = jnp.dot(
            norm_buf[...], w_buf[:, :ret_wide], preferred_element_type=jnp.float32
        ).astype(jnp.bfloat16)
        rv_at, rq_at = starts[3][0], starts[4][0]
        key_scale = dk ** (-0.5)
        position = lax.broadcasted_iota(jnp.int32, (rows, 1), 0).astype(jnp.float32)
        distance = jnp.maximum(row_id - col_id, 0).astype(jnp.float32)
        lone = jnp.zeros((dk, vd), jnp.float32)

        def part(b, first, wide):
            return proj_buf[pl.ds(pl.multiple_of(b * rows, rows), rows), first : first + wide]

        def summary(b, h):
            keys = part(b, rq_at + (hr + h) * dk, dk).astype(jnp.float32) * key_scale
            trailing = jnp.exp((rows - 1.0 - position) * decay_ref[h])
            return lax.dot_general(
                keys * trailing,
                part(b, rv_at + h * vd, vd).astype(jnp.float32),
                TN,
                precision=highest,
                preferred_element_type=jnp.float32,
            )

        early = [summary(0, h) for h in range(hr)]
        for h in range(hr):
            sum_buf[couple, h] = jnp.exp(lone + float(rows) * decay_ref[h]) * early[h] + summary(1, h)
        later(lambda q: sum_copy(q).start())
        outs.relay(2)

        offset = (couple * 2 * rows).astype(jnp.float32)

        def gather(q, entering):
            sum_in(q).wait_recv()
            gap = ((couple - 1 - q) * 2 * rows).astype(jnp.float32)
            return tuple(entering[h] + jnp.exp(lone + gap * decay_ref[h]) * sum_buf[q, h] for h in range(hr))

        entering = tuple(jnp.exp(lone + offset * decay_ref[h]) * state_buf[h] for h in range(hr))
        entering = lax.fori_loop(0, couple, gather, entering)
        second = tuple(jnp.exp(lone + float(rows) * decay_ref[h]) * entering[h] + early[h] for h in range(hr))

        def block(i, _):
            b = jnp.where(i == 0, other, mine)
            for h in range(hr):
                rq = part(b, rq_at + h * dk, dk)
                rk = part(b, rq_at + (hr + h) * dk, dk)
                rv = part(b, rv_at + h * vd, vd)
                scores = lax.dot_general(rq, rk, NT, preferred_element_type=jnp.float32) * key_scale
                scores = jnp.where(causal, scores * jnp.exp(distance * decay_ref[h]), 0.0)
                inner = jnp.dot(
                    scores, rv.astype(jnp.float32), precision=highest, preferred_element_type=jnp.float32
                )
                leading = jnp.exp((position + 1.0) * decay_ref[h])
                carried = jnp.dot(
                    rq.astype(jnp.float32),
                    jnp.where(b == 0, entering[h], second[h]),
                    precision=highest,
                    preferred_element_type=jnp.float32,
                )
                raw = inner + carried * leading
                center = raw - jnp.mean(raw, axis=-1, keepdims=True)
                variance = jnp.mean(center * center, axis=-1, keepdims=True)
                cols = slice(h * vd, (h + 1) * vd)
                mix_pair[b, :, cols] = (center * lax.rsqrt(variance + epsilon) * hgain_buf[:, cols]).astype(
                    jnp.bfloat16
                )

            @pl.when(i == 0)
            def _():
                mix_copy(0).start()

            return 0

        lax.fori_loop(0, 2, block, 0)
        mix_own(0)
        for k in range(3, n):
            outs.relay(k)
        mix_in(depth).wait_recv()
        mix_copy(0).wait_send()
        later(lambda q: sum_copy(q).wait_send())

    block = rows // n_tp
    wide, pieces = out_cols, n

    def piece_cols(piece):
        return pl.ds(pl.multiple_of(piece * wide, wide), wide)

    def slot(at):
        return pl.ds(pl.multiple_of(at * block, block), block)

    def pair_copy(piece):
        cols = piece_cols(piece)
        return rdma(
            rs_send.at[1 - parity, :, cols],
            pair_buf.at[:, cols],
            pair_s.at[piece],
            pair_r.at[piece],
            tp=t + 1 - 2 * parity,
        )

    def rs_copy(d, piece):
        to = lax.rem(pair + d, half)
        cols = piece_cols(piece)
        at = (d - 1) * pieces + piece
        return rdma(
            pair_sum.at[slot(to), cols], far_ref.at[d - 1, :, cols], rs_s.at[at], rs_r.at[at], tp=2 * to + parity
        )

    def project(piece):
        cols = piece_cols(piece)
        value = jnp.dot(mix_buf[...], wout_buf[:, cols], preferred_element_type=jnp.float32).astype(jnp.bfloat16)
        for b in range(n_tp):
            at = slice(b // 2 * block, (b // 2 + 1) * block)
            rs_send[b % 2, at, cols] = value[b * block : (b + 1) * block]
        pair_copy(piece).start()

    def reduce(piece):
        cols = piece_cols(piece)
        pair_copy(piece).wait_recv()
        both = rs_send[parity, :, cols].astype(jnp.float32) + pair_buf[:, cols].astype(jnp.float32)
        pair_sum[:, cols] = both.astype(jnp.bfloat16)
        for d in range(1, half):
            rs_copy(d, piece).start()

    def order(i):
        falling = jnp.where(i <= me, me - i, i)
        rising = jnp.where(i <= n - 1 - me, me + i, n - 1 - i)
        return jnp.where(lower, rising, falling)

    for c in range(2):
        outs.local(c).wait()
    project(me)

    def out_step(i, _):
        outs.arrive_shard(order(i), (0, 1))
        project(order(i))
        reduce(order(i - 1))
        return 0

    lax.fori_loop(1, n, out_step, 0)
    reduce(order(jnp.int32(n - 1)))

    own = slot(pair)
    near_buf[...] = rs_send[parity, own, :].astype(jnp.float32) + pair_buf[own, :].astype(jnp.float32)
    near_copy = pltpu.make_async_copy(near_buf, near_ref, near_sem)
    near_copy.start()

    for m in range(chunks):
        tok_z(m).wait_send()
        for own_half in (True, False):
            for d in range(1, half):
                tok_x(own_half, m, d).wait_send()
            for d in range(half):
                tok_c(own_half, m, d).wait_send()

    def sent(copy):
        copy.wait_send()

    send_weights(fox_arrays, sent)
    send_weights(ret_arrays, sent)

    def sides(arrays):
        for c in arrays:
            for k in range(1, n):
                w_pass(c, toward(k), sent)
                for d in range(1, n_grp):
                    w_side(c, toward(k), d).wait_send()

    @pl.when(is_fox)
    def _():
        sides(fox_arrays)

    @pl.when(is_ret)
    def _():
        sides(ret_arrays)

    for piece in range(pieces):
        pair_copy(piece).wait_send()
        for d in range(1, half):
            rs_copy(d, piece).wait_send()
    outs.finish()
    near_copy.wait()
    for d in range(1, half):
        for piece in range(pieces):
            rs_copy(d, piece).wait_recv()


def paired(n, n_tp, n_grp, inputs):
    tokens, ret_query_weight, ret_state, fox_gates = inputs[0], inputs[2], inputs[9], inputs[11]
    fox_query_weight, ret_out_weight = inputs[5], inputs[12]
    rows, feats = tokens.shape
    hr, dk, vd = ret_state.shape
    fh = fox_gates.shape[1]
    fd = fox_query_weight.shape[1] // fh
    shard = ret_query_weight.shape[0]
    depth, out_cols = ret_out_weight.shape
    columns = out_cols * n
    wide = max(3 * fh * fd, 2 * hr * dk + hr * vd)
    half = n_tp // 2
    block = rows // n_tp
    chunks = 4
    count = 5
    couples = n // 2
    dma = pltpu.SemaphoreType.DMA
    far = max(half - 1, 1)
    side = max(n_grp - 1, 1) * n
    smem = pl.BlockSpec(memory_space=pltpu.SMEM)
    hbm = pl.BlockSpec(memory_space=pl.ANY)
    bf16, f32 = jnp.bfloat16, jnp.float32
    size = (n, n_tp, n_grp, hr, dk, vd, fh, fd, chunks)
    near, other = pl.pallas_call(
        functools.partial(pair_kernel, size),
        out_shape=(
            jax.ShapeDtypeStruct((block, columns), f32),
            jax.ShapeDtypeStruct((far, block, columns), bf16),
        ),
        in_specs=[hbm] * 8 + [smem] + [hbm] * 5,
        out_specs=(hbm, hbm),
        scratch_shapes=[
            pltpu.VMEM((1, n_tp * feats), f32),
            pltpu.VMEM((hr * dk, shard), bf16),
            pltpu.VMEM((hr * dk, shard), bf16),
            pltpu.VMEM((hr, dk, vd), f32),
            pltpu.VMEM((1, hr * vd), f32),
            pltpu.VMEM((fh, n * rows), f32),
            pltpu.VMEM((2, fh, rows, 1), f32),
            pltpu.VMEM((2, n_tp, rows, feats), bf16),
            pltpu.VMEM((shard, 2 * hr * dk), bf16),
            pltpu.VMEM((n * shard, wide), bf16),
            pltpu.VMEM((2 * depth, columns), bf16),
            pltpu.VMEM((2 * rows, n_tp * feats), bf16),
            pltpu.VMEM((2 * rows, wide), bf16),
            pltpu.VMEM((n, rows, 2 * fh * fd), bf16),
            pltpu.VMEM((couples, hr, dk, vd), f32),
            pltpu.VMEM((2, rows, depth), bf16),
            pltpu.VMEM((rows, 2 * depth), bf16),
            pltpu.VMEM((2, rows // 2, columns), bf16),
            pltpu.VMEM((rows // 2, columns), bf16),
            pltpu.VMEM((rows // 2, columns), bf16),
            pltpu.VMEM((block, columns), f32),
            pltpu.VMEM((2, fh, rows, 1), f32),
            pltpu.VMEM((2, fh, rows, 1), f32),
            pltpu.VMEM((2, fh, rows, fd), f32),
            dma((6,)),
            dma,
            pltpu.SemaphoreType.REGULAR,
            pltpu.SemaphoreType.REGULAR,
            dma((chunks,)),
            dma((chunks,)),
            dma((2 * chunks * far,)),
            dma((2 * chunks * far,)),
            dma((2 * chunks * half,)),
            dma((2 * chunks * half,)),
            dma,
            dma((2 * n * count,)),
            dma((n * count,)),
            dma((side * count,)),
            dma((side * count,)),
            dma((count,)),
            dma((2 * couples,)),
            dma((n,)),
            dma((couples,)),
            dma((couples,)),
            dma((1,)),
            dma((1,)),
            dma((n,)),
            dma((n,)),
            dma((far * n,)),
            dma((far * n,)),
            dma((n * 2,)),
            dma((n * 2,)),
            dma((n * 2,)),
            dma((side * 2,)),
            dma((side * 2,)),
            dma((2,)),
        ],
        compiler_params=pltpu.CompilerParams(
            collective_id=0, has_side_effects=True, vmem_limit_bytes=56 * 1024 * 1024
        ),
        name="layer",
    )(
        tokens,
        inputs[1][None, :],
        inputs[2].T,
        inputs[3].T,
        inputs[4],
        inputs[5],
        inputs[6],
        inputs[7],
        inputs[8],
        inputs[9],
        inputs[10][None, :],
        inputs[11].T,
        inputs[12],
        inputs[13],
    )
    for d in range(half - 1):
        near = near + other[d].astype(f32)
    return near.astype(bf16)


def pairs_fit(n, n_tp, n_grp, inputs):
    rows, feats = inputs[0].shape
    hr, dk, vd = inputs[9].shape
    shard = inputs[2].shape[0]
    depth, out_cols = inputs[12].shape
    wide = inputs[5].shape[1]
    lanes = all(w % 128 == 0 for w in (out_cols, wide, 2 * hr * dk, hr * vd, feats, depth))
    even = n % 2 == 0 and n > 2 and n_tp % 2 == 0
    tiles = rows % (16 * n_tp) == 0 and rows % 32 == 0 and shard % (16 * n_grp) == 0 and depth % (16 * n_grp) == 0
    columns = n * out_cols
    held = 8 * rows * n_tp * feats + 2 * n * shard * 3 * wide + 4 * depth * columns + 4 * n * rows * wide + 6 * rows * columns
    return lanes and even and tiles and depth == wide == hr * vd and held < 40 * 1024 * 1024


def local(
    n,
    n_tp,
    n_grp,
    tokens,
    norm_gain,
    ret_query_weight,
    ret_key_weight,
    ret_value_weight,
    fox_query_weight,
    fox_key_weight,
    fox_value_weight,
    ret_decay,
    ret_state,
    head_norm_gain,
    fox_gates,
    ret_out_weight,
    fox_out_weight,
):
    inputs = (
        tokens,
        norm_gain,
        ret_query_weight,
        ret_key_weight,
        ret_value_weight,
        fox_query_weight,
        fox_key_weight,
        fox_value_weight,
        ret_decay,
        ret_state,
        head_norm_gain,
        fox_gates,
        ret_out_weight,
        fox_out_weight,
    )
    if pairs_fit(n, n_tp, n_grp, inputs):
        return paired(n, n_tp, n_grp, inputs)
    rows, feats = tokens.shape
    hr, dk, vd = ret_state.shape
    fh = fox_gates.shape[1]
    fd = fox_query_weight.shape[1] // fh
    shard = ret_query_weight.shape[0]
    width = 2 * hr * dk + hr * vd + 3 * fh * fd
    depth, out_cols = ret_out_weight.shape
    columns = out_cols * n
    direct = out_cols % 128 == 0
    if not direct:
        ret_out_weight, fox_out_weight = ret_out_weight.T, fox_out_weight.T
    dma = pltpu.SemaphoreType.DMA

    def gather_sems(arrays):
        side = max(n_grp - 1, 1) * n * arrays
        return [
            dma((n * arrays,)),
            dma((n * arrays,)),
            dma((n * arrays,)),
            dma((side,)),
            dma((side,)),
            dma((arrays,)),
        ]

    vmem = pl.BlockSpec(memory_space=pltpu.VMEM)
    smem = pl.BlockSpec(memory_space=pltpu.SMEM)
    hbm = pl.BlockSpec(memory_space=pl.ANY)
    size = (n, n_tp, n_grp, hr, dk, vd, fh, fd, direct)
    block = rows // n_tp
    peers = max(n_tp - 1, 1)
    far = max(n_tp // 2 - 1, 1)
    pieces = n if direct else 1
    return pl.pallas_call(
        functools.partial(kernel, size),
        out_shape=jax.ShapeDtypeStruct((block, columns), jnp.bfloat16),
        in_specs=[hbm, vmem, vmem, vmem, hbm, hbm, hbm, hbm, smem, vmem, vmem, vmem, hbm, hbm],
        out_specs=vmem,
        scratch_shapes=[
            pltpu.VMEM((n_tp, rows, feats), jnp.bfloat16),
            pltpu.VMEM((shard, 2 * hr * dk), jnp.bfloat16),
            pltpu.VMEM((n * shard, width), jnp.bfloat16),
            pltpu.VMEM((2 * depth, columns) if direct else (columns, 2 * depth), jnp.bfloat16),
            pltpu.VMEM((rows, n_tp * feats), jnp.bfloat16),
            pltpu.VMEM((rows, width - 2 * fh * fd), jnp.bfloat16),
            pltpu.VMEM((n, rows, 2 * fh * fd), jnp.bfloat16),
            pltpu.VMEM((n, hr, dk, vd), jnp.float32),
            pltpu.VMEM((rows, 2 * depth), jnp.bfloat16),
            pltpu.VMEM((2, rows // 2, columns), jnp.bfloat16),
            pltpu.VMEM((rows // 2, columns), jnp.bfloat16),
            pltpu.VMEM((rows // 2, columns), jnp.bfloat16),
            pltpu.VMEM((far, block, columns), jnp.bfloat16),
            pltpu.VMEM((fh, rows, 1), jnp.float32),
            pltpu.VMEM((fh, rows, 1), jnp.float32),
            pltpu.VMEM((fh, rows, fd), jnp.float32),
            dma((peers,)),
            dma((peers,)),
            dma,
            dma((n,)),
            dma((n,)),
            dma((n,)),
            dma((n,)),
            dma((pieces,)),
            dma((pieces,)),
            dma((far * pieces,)),
            dma((far * pieces,)),
        ]
        + gather_sems(2)
        + gather_sems(3)
        + gather_sems(2),
        compiler_params=pltpu.CompilerParams(
            collective_id=0, has_side_effects=True, vmem_limit_bytes=56 * 1024 * 1024
        ),
        name="layer",
    )(
        tokens,
        norm_gain[None, :],
        ret_query_weight.T,
        ret_key_weight.T,
        ret_value_weight,
        fox_query_weight,
        fox_key_weight,
        fox_value_weight,
        ret_decay,
        ret_state,
        head_norm_gain[None, :],
        fox_gates.T,
        ret_out_weight,
        fox_out_weight,
    )


def solution(mesh):
    placed = (
        P(("grp", "sp"), "tp"),
        P(),
        P("sp", "tp"),
        P("sp", "tp"),
        P("sp", "tp"),
        P("sp", "tp"),
        P("sp", "tp"),
        P("sp", "tp"),
        P("tp"),
        P(("grp", "tp"), None, None),
        P("tp"),
        P("grp", "tp"),
        P("tp", "sp"),
        P("tp", "sp"),
    )
    body = functools.partial(local, mesh.shape["sp"], mesh.shape["tp"], mesh.shape["grp"])
    return jax.shard_map(
        body, mesh=mesh, in_specs=placed, out_specs=P(("grp", "sp", "tp"), None), check_vma=False
    )
```

```python
import functools

import jax
import jax.numpy as jnp
from jax import lax
from jax.experimental import pallas as pl
from jax.experimental.pallas import tpu as pltpu
from jax.sharding import PartitionSpec as P

epsilon = 1e-06
lanes = 128
highest = lax.Precision.HIGHEST
NT = (((1,), (1,)), ((), ()))
TN = (((0,), (0,)), ((), ()))


def rdma(src, dst, send_sem, recv_sem, **target):
    return pltpu.make_async_remote_copy(
        src_ref=src,
        dst_ref=dst,
        send_sem=send_sem,
        recv_sem=recv_sem,
        device_id=target,
        device_id_type=pl.DeviceIdType.MESH,
    )


class LineGather:
    def __init__(self, owns, place, sems, n, n_grp, me, g):
        self.owns, self.place, self.n, self.n_grp, self.me, self.g = owns, place, n, n_grp, me, g
        self.up, self.down, self.zr, self.ys, self.yr, self.loc = sems
        self.arrays = len(owns)
        self.rows = owns[0].shape[0]
        self.step = self.rows // n_grp

    def piece(self, part, src, c):
        return self.place(src, c, part * self.step, self.step)

    def own_piece(self, c):
        return self.owns[c].at[pl.ds(pl.multiple_of(self.g * self.step, self.step), self.step)]

    def hop(self, sems, to, src, c, first=False):
        here = self.own_piece(c) if first else self.piece(self.g, src, c)
        at = src * self.arrays + c
        return rdma(here, self.piece(self.g, src, c), sems.at[at], self.zr.at[at], sp=to)

    def side(self, d, src, c):
        at = ((d - 1) * self.n + src) * self.arrays + c
        here = self.piece(self.g, src, c)
        return rdma(here, here, self.ys.at[at], self.yr.at[at], grp=lax.rem(self.g + d, self.n_grp))

    def side_in(self, d, src, c):
        at = ((d - 1) * self.n + src) * self.arrays + c
        part = lax.rem(self.g + self.n_grp - d, self.n_grp)
        here = self.piece(part, src, c)
        return rdma(here, here, self.ys.at[at], self.yr.at[at], grp=part)

    def local(self, c):
        return pltpu.make_async_copy(self.owns[c], self.place(self.me, c, 0, self.rows), self.loc.at[c])

    def start(self):
        me, n = self.me, self.n
        for c in range(self.arrays):

            @pl.when(me + 1 < n)
            def _():
                self.hop(self.up, me + 1, me, c, True).start()

            @pl.when(me >= 1)
            def _():
                self.hop(self.down, me - 1, me, c, True).start()

        for c in range(self.arrays):
            self.local(c).start()

    def relay(self, k):
        me, n = self.me, self.n
        for c in range(self.arrays):
            for src, sems, to in ((me - k, self.up, me + 1), (me + k, self.down, me - 1)):

                @pl.when((src >= 0) & (src < n))
                def _(src=src, sems=sems, to=to):
                    self.hop(sems, me, src, c).wait_recv()

                    @pl.when((to >= 0) & (to < n))
                    def _():
                        self.hop(sems, to, src, c).start()

                    for d in range(1, self.n_grp):
                        self.side(d, src, c).start()

    def arrive_shard(self, src, arrays):
        for c in arrays:
            for d in range(1, self.n_grp):
                self.side_in(d, src, c).wait_recv()

    def arrive(self, arrays):
        for c in arrays:
            self.local(c).wait()

        def step(k, _):
            self.arrive_shard(lax.rem(self.me + k, self.n), arrays)
            return 0

        lax.fori_loop(1, self.n, step, 0)

    def finish(self):
        me, n = self.me, self.n

        def step(src, _):
            for c in range(self.arrays):

                @pl.when((src <= me) & (me + 1 < n))
                def _():
                    self.hop(self.up, me, src, c).wait_send()

                @pl.when((src >= me) & (me >= 1))
                def _():
                    self.hop(self.down, me, src, c).wait_send()

                @pl.when(src != me)
                def _():
                    for d in range(1, self.n_grp):
                        self.side(d, src, c).wait_send()

            return 0

        lax.fori_loop(0, n, step, 0)


def kernel(
    size,
    tok_ref,
    gain_ref,
    wq_ref,
    wk_ref,
    wrv_ref,
    wfq_ref,
    wfk_ref,
    wfv_ref,
    decay_ref,
    state_ref,
    hgain_ref,
    gates_ref,
    ret_out_ref,
    fox_out_ref,
    out_ref,
    tok_buf,
    qk_own,
    w_buf,
    wout_buf,
    norm_buf,
    proj_buf,
    kv_buf,
    sum_buf,
    mix_buf,
    rs_send,
    pair_buf,
    pair_sum,
    rs_buf,
    top_buf,
    total_buf,
    weighted_buf,
    tok_s,
    tok_r,
    tok_loc,
    kv_s,
    kv_r,
    sum_s,
    sum_r,
    pair_s,
    pair_r,
    rs_s,
    rs_r,
    *gather_sems,
):
    n, n_tp, n_grp, hr, dk, vd, fh, fd, direct = size
    me, t, g = lax.axis_index("sp"), lax.axis_index("tp"), lax.axis_index("grp")
    rows, feats = tok_ref.shape
    owns = [wfk_ref, wfv_ref, wfq_ref, wrv_ref, qk_own]
    early = 2
    starts = [0]
    for own in owns:
        starts.append(starts[-1] + own.shape[1])
    shard = qk_own.shape[0]

    def weight_place(src, c, first, count):
        start = pl.multiple_of(src * shard + first, count)
        return w_buf.at[pl.ds(start, count), starts[c] : starts[c + 1]]

    depth = mix_buf.shape[1] // 2
    out_cols = ret_out_ref.shape[1] if direct else ret_out_ref.shape[0]

    def out_place(src, c, first, count):
        if direct:
            start = pl.multiple_of(c * depth + first, count)
            return wout_buf.at[pl.ds(start, count), pl.ds(pl.multiple_of(src * out_cols, out_cols), out_cols)]
        start = pl.multiple_of(src * out_cols + first, count)
        return wout_buf.at[pl.ds(start, count), c * depth : (c + 1) * depth]

    def late_place(src, c, first, count):
        return weight_place(src, c + early, first, count)

    firsts = LineGather(owns[:early], weight_place, gather_sems[:6], n, n_grp, me, g)
    lasts = LineGather(owns[early:], late_place, gather_sems[6:12], n, n_grp, me, g)
    outs = LineGather([ret_out_ref, fox_out_ref], out_place, gather_sems[12:], n, n_grp, me, g)

    barrier = pltpu.get_barrier_semaphore()

    def greet(**target):
        pl.semaphore_signal(barrier, inc=1, device_id=target, device_id_type=pl.DeviceIdType.MESH)

    has_up, has_down = me + 1 < n, me >= 1
    for d in range(1, n_tp):
        greet(tp=lax.rem(t + d, n_tp))
    for d in range(1, n_grp):
        greet(grp=lax.rem(g + d, n_grp))

    @pl.when(has_up)
    def _():
        greet(sp=me + 1)

    @pl.when(has_down)
    def _():
        greet(sp=me - 1)

    turned = jnp.concatenate((wq_ref[...], wk_ref[...]), axis=0).astype(jnp.float32)
    qk_own[...] = turned.T.astype(jnp.bfloat16)

    count = n_tp - 1 + n_grp - 1 + has_up.astype(jnp.int32) + has_down.astype(jnp.int32)
    pl.semaphore_wait(barrier, count)

    def tok_copy(d):
        return rdma(tok_ref, tok_buf.at[t], tok_s.at[d - 1], tok_r.at[d - 1], tp=lax.rem(t + d, n_tp))

    def tok_in(d):
        src = lax.rem(t + n_tp - d, n_tp)
        return rdma(tok_ref, tok_buf.at[src], tok_s.at[d - 1], tok_r.at[d - 1], tp=src)

    firsts.start()
    lasts.start()
    tok_local = pltpu.make_async_copy(tok_ref, tok_buf.at[t], tok_loc)
    for d in range(1, n_tp):
        tok_copy(d).start()
    tok_local.start()

    def first_step(k, _):
        firsts.relay(k)

        lasts.relay(k)
        return 0

    lax.fori_loop(1, n, first_step, 0)
    outs.start()

    tok_local.wait()
    for d in range(1, n_tp):
        tok_in(d).wait_recv()
    squares = jnp.zeros((rows, 1), jnp.float32)
    for i in range(n_tp):
        part = tok_buf[i].astype(jnp.float32)
        squares = squares + jnp.sum(part * part, axis=-1, keepdims=True)
    scale = lax.rsqrt(squares * (1.0 / (n_tp * feats)) + epsilon)
    for i in range(n_tp):
        part = tok_buf[i].astype(jnp.float32)
        cols = slice(i * feats, (i + 1) * feats)
        norm_buf[:, cols] = (part * scale * gain_ref[:, cols]).astype(jnp.bfloat16)

    def kv_copy(src):
        return rdma(kv_buf.at[src], kv_buf.at[src], kv_s.at[src], kv_r.at[src], sp=jnp.minimum(me + 1, n - 1))

    def sum_copy(src):
        return rdma(sum_buf.at[src], sum_buf.at[src], sum_s.at[src], sum_r.at[src], sp=jnp.minimum(me + 1, n - 1))

    firsts.arrive((0, 1))
    kv_buf[me] = jnp.dot(
        norm_buf[...], w_buf[:, : starts[2]], preferred_element_type=jnp.float32
    ).astype(jnp.bfloat16)

    def kv_forward(k):
        src = me - k

        @pl.when(src >= 0)
        def _():
            kv_copy(src).wait_recv()

            @pl.when(has_up)
            def _():
                kv_copy(src).start()

    @pl.when(has_up)
    def _():
        kv_copy(me).start()

    outs.relay(1)
    lasts.arrive((0, 1, 2))
    proj_buf[...] = jnp.dot(
        norm_buf[...], w_buf[:, starts[2] :], preferred_element_type=jnp.float32
    ).astype(jnp.bfloat16)
    rv_at, rq_at = starts[3] - starts[2], starts[4] - starts[2]

    key_scale = dk ** (-0.5)
    position = lax.broadcasted_iota(jnp.int32, (rows, 1), 0).astype(jnp.float32)
    rq, rk, rv = [], [], []
    for h in range(hr):
        rq.append(proj_buf[:, rq_at + h * dk : rq_at + (h + 1) * dk])
        rk.append(proj_buf[:, rq_at + (hr + h) * dk : rq_at + (hr + h + 1) * dk])
        rv.append(proj_buf[:, rv_at + h * vd : rv_at + (h + 1) * vd])
        keys = rk[h].astype(jnp.float32) * key_scale
        trailing = jnp.exp((rows - 1.0 - position) * decay_ref[h])
        sum_buf[me, h] = lax.dot_general(
            keys * trailing, rv[h].astype(jnp.float32), TN, precision=highest, preferred_element_type=jnp.float32
        )

    @pl.when(has_up)
    def _():
        sum_copy(me).start()

    row_id = lax.broadcasted_iota(jnp.int32, (rows, rows), 0)
    col_id = lax.broadcasted_iota(jnp.int32, (rows, rows), 1)
    causal = col_id <= row_id
    own_cols = pl.ds(pl.multiple_of(me * rows, rows), rows)
    own_gates = [
        jnp.sum(jnp.where(row_id == col_id, gates_ref[h : h + 1, own_cols], 0.0), axis=1, keepdims=True)
        for h in range(fh)
    ]

    def attend(src, diagonal):
        key_cols = pl.ds(pl.multiple_of(src * rows, rows), rows)
        for h in range(fh):
            query = proj_buf[:, h * fd : (h + 1) * fd]
            k = kv_buf[src, :, h * fd : (h + 1) * fd]
            v = kv_buf[src, :, (fh + h) * fd : (fh + h + 1) * fd]
            logits = lax.dot_general(query, k, NT, preferred_element_type=jnp.float32) * fd ** (-0.5)
            logits = logits + own_gates[h] - gates_ref[h : h + 1, key_cols]
            if diagonal:
                logits = jnp.where(causal, logits, -jnp.inf)
            top_new = jnp.max(logits, axis=-1, keepdims=True)
            if not diagonal:
                top = top_buf[h]
                top_new = jnp.maximum(top, top_new)
            p = jnp.exp(logits - top_new)
            total = jnp.sum(p, axis=-1, keepdims=True)
            weighted = jnp.dot(p.astype(jnp.bfloat16), v, preferred_element_type=jnp.float32)
            if not diagonal:
                rescale = jnp.exp(top - top_new)
                total = total_buf[h] * rescale + total
                weighted = weighted_buf[h] * rescale + weighted
            top_buf[h] = top_new
            total_buf[h] = total
            weighted_buf[h] = weighted

    def forward(k):
        src = me - k

        @pl.when(src >= 0)
        def _():
            sum_copy(src).wait_recv()

            @pl.when(has_up)
            def _():
                sum_copy(src).start()

    attend(me, True)

    offset = (me * rows).astype(jnp.float32)
    lone = jnp.zeros((dk, vd), jnp.float32)

    def step(k, entering):
        src = me - k
        kv_forward(k)
        forward(k)

        @pl.when(k + 1 < n)
        def _():
            outs.relay(k + 1)


        @pl.when(src >= 0)
        def _():
            attend(src, False)

        gap = ((k - 1) * rows).astype(jnp.float32)
        there = jnp.maximum(src, 0)
        return tuple(
            entering[h]
            + jnp.where(src >= 0, jnp.exp(lone + gap * decay_ref[h]) * sum_buf[there, h], 0.0)
            for h in range(hr)
        )

    entering = tuple(jnp.exp(lone + offset * decay_ref[h]) * state_ref[h] for h in range(hr))
    entering = lax.fori_loop(1, n, step, entering)

    distance = jnp.maximum(row_id - col_id, 0).astype(jnp.float32)
    for h in range(hr):
        scores = lax.dot_general(rq[h], rk[h], NT, preferred_element_type=jnp.float32) * key_scale
        scores = jnp.where(causal, scores * jnp.exp(distance * decay_ref[h]), 0.0)
        inner = jnp.dot(scores, rv[h].astype(jnp.float32), precision=highest, preferred_element_type=jnp.float32)
        leading = jnp.exp((position + 1.0) * decay_ref[h])
        carried = jnp.dot(
            rq[h].astype(jnp.float32), entering[h], precision=highest, preferred_element_type=jnp.float32
        )
        raw = inner + carried * leading
        center = raw - jnp.mean(raw, axis=-1, keepdims=True)
        variance = jnp.mean(center * center, axis=-1, keepdims=True)
        cols = slice(h * vd, (h + 1) * vd)
        mix_buf[:, cols] = (center * lax.rsqrt(variance + epsilon) * hgain_ref[:, cols]).astype(jnp.bfloat16)
    for h in range(fh):
        cols = slice(hr * vd + h * fd, hr * vd + (h + 1) * fd)
        mix_buf[:, cols] = (weighted_buf[h] / total_buf[h]).astype(jnp.bfloat16)

    block = rows // n_tp
    columns = pair_buf.shape[1]
    wide = out_cols if direct else columns
    pieces = columns // wide
    half = n_tp // 2
    parity, pair = lax.rem(t, 2), lax.div(t, 2)

    def piece_cols(piece):
        return pl.ds(pl.multiple_of(piece * wide, wide), wide)

    def slot(at):
        return pl.ds(pl.multiple_of(at * block, block), block)

    def pair_copy(piece):
        cols = piece_cols(piece)
        return rdma(
            rs_send.at[1 - parity, :, cols],
            pair_buf.at[:, cols],
            pair_s.at[piece],
            pair_r.at[piece],
            tp=t + 1 - 2 * parity,
        )

    def rs_copy(d, piece):
        to = lax.rem(pair + d, half)
        cols = piece_cols(piece)
        at = (d - 1) * pieces + piece
        return rdma(
            pair_sum.at[slot(to), cols], rs_buf.at[d - 1, :, cols], rs_s.at[at], rs_r.at[at], tp=2 * to + parity
        )

    def project(piece):
        cols = piece_cols(piece)
        if direct:
            value = jnp.dot(mix_buf[...], wout_buf[:, cols], preferred_element_type=jnp.float32)
        else:
            value = lax.dot_general(mix_buf[...], wout_buf[...], NT, preferred_element_type=jnp.float32)
        value = value.astype(jnp.bfloat16)
        for b in range(n_tp):
            at = slice(b // 2 * block, (b // 2 + 1) * block)
            rs_send[b % 2, at, cols] = value[b * block : (b + 1) * block]
        pair_copy(piece).start()

    def reduce(piece):
        cols = piece_cols(piece)
        pair_copy(piece).wait_recv()
        both = rs_send[parity, :, cols].astype(jnp.float32) + pair_buf[:, cols].astype(jnp.float32)
        pair_sum[:, cols] = both.astype(jnp.bfloat16)
        for d in range(1, half):
            rs_copy(d, piece).start()

    def order(i):
        falling = jnp.where(i <= me, me - i, i)
        rising = jnp.where(i <= n - 1 - me, me + i, n - 1 - i)
        return jnp.where(2 * me >= n, falling, rising)

    if direct:
        for c in range(2):
            outs.local(c).wait()
        project(me)

        def out_step(i, _):
            outs.arrive_shard(order(i), (0, 1))
            project(order(i))
            reduce(order(i - 1))
            return 0

        lax.fori_loop(1, n, out_step, 0)
        reduce(order(jnp.int32(n - 1)))
    else:
        outs.arrive((0, 1))
        project(0)
        reduce(0)

    own = slot(pair)
    summed = rs_send[parity, own, :].astype(jnp.float32) + pair_buf[own, :].astype(jnp.float32)
    for d in range(1, half):
        for piece in range(pieces):
            rs_copy(d, piece).wait_recv()
        summed = summed + rs_buf[d - 1].astype(jnp.float32)
    out_ref[...] = summed.astype(jnp.bfloat16)

    for d in range(1, n_tp):
        tok_copy(d).wait_send()
    for piece in range(pieces):
        pair_copy(piece).wait_send()
        for d in range(1, half):
            rs_copy(d, piece).wait_send()
    firsts.finish()
    lasts.finish()
    outs.finish()

    @pl.when(has_up)
    def _():
        def step(src, _):
            kv_copy(src).wait_send()
            sum_copy(src).wait_send()
            return 0

        lax.fori_loop(0, me + 1, step, 0)


def pair_kernel(
    size,
    tok_ref,
    gain_ref,
    wq_ref,
    wk_ref,
    wrv_ref,
    wfq_ref,
    wfk_ref,
    wfv_ref,
    decay_ref,
    state_ref,
    hgain_ref,
    gates_ref,
    ret_out_ref,
    fox_out_ref,
    near_ref,
    far_ref,
    gain_buf,
    wqk_buf,
    state_buf,
    hgain_buf,
    gates_buf,
    gate_buf,
    tok_buf,
    qk_own,
    w_buf,
    wout_buf,
    norm_buf,
    proj_buf,
    kv_buf,
    sum_buf,
    mix_pair,
    mix_buf,
    rs_send,
    pair_buf,
    pair_sum,
    top_buf,
    total_buf,
    weighted_buf,
    in_sem,
    above_sem,
    below_sem,
    t_s,
    tz_r,
    tx_r,
    tc_r,
    t_loc,
    w_s,
    w_r,
    wy_s,
    wy_r,
    w_loc,
    o_s,
    o_r,
    oy_s,
    oy_r,
    o_loc,
    kv_s,
    kv_r,
    sum_s,
    sum_r,
    mix_s,
    mix_r,
    pair_s,
    pair_r,
    rs_s,
    rs_r,
):
    n, n_tp, n_grp, hr, dk, vd, fh, fd, chunks = size
    me, t, g = lax.axis_index("sp"), lax.axis_index("tp"), lax.axis_index("grp")
    rows, feats = tok_ref.shape
    shard = qk_own.shape[0]
    couples = n // 2
    couple, mine = lax.div(me, 2), lax.rem(me, 2)
    other = 1 - mine
    partner = me + 1 - 2 * mine
    fox_mine = 1 - lax.rem(couple, 2)
    is_fox = mine == fox_mine
    is_ret = mine != fox_mine
    lower = 2 * me < n
    half = n_tp // 2
    parity, pair = lax.rem(t, 2), lax.div(t, 2)

    def fox_of(q):
        return 2 * q + 1 - lax.rem(q, 2)

    def ret_of(q):
        return 2 * q + lax.rem(q, 2)

    def toward(k):
        return lax.rem(jnp.where(lower, me + k, me + n - k), n)

    barrier = pltpu.get_barrier_semaphore()

    def greet(**target):
        pl.semaphore_signal(barrier, inc=1, device_id=target, device_id_type=pl.DeviceIdType.MESH)

    greet(tp=2 * pair + 1 - parity)
    for d in range(1, half):
        greet(tp=2 * lax.rem(pair + d, half) + parity)
    for d in range(1, n_grp):
        greet(grp=lax.rem(g + d, n_grp))
    has_up, has_down = me + 1 < n, me >= 1

    @pl.when(has_up)
    def _():
        greet(sp=me + 1)

    @pl.when(has_down)
    def _():
        greet(sp=me - 1)

    def drained(sem, ref):
        pltpu.make_async_copy(ref, ref, sem).wait()

    width = hr * dk
    pltpu.make_async_copy(wq_ref, wqk_buf.at[:width], in_sem.at[0]).start()
    pltpu.make_async_copy(wk_ref, wqk_buf.at[width:], in_sem.at[0]).start()
    brought = [
        pltpu.make_async_copy(src, dst, in_sem.at[i + 1])
        for i, (src, dst) in enumerate(
            ((gain_ref, gain_buf), (state_ref, state_buf), (hgain_ref, hgain_buf), (gates_ref, gates_buf))
        )
    ]
    for copy in brought:
        copy.start()

    pl.semaphore_wait(barrier, half + n_grp - 1 + has_up.astype(jnp.int32) + has_down.astype(jnp.int32))

    def tell(sem, to):
        pl.semaphore_signal(sem, inc=1, device_id={"sp": to}, device_id_type=pl.DeviceIdType.MESH)

    @pl.when(has_up & has_down)
    def _():
        tell(above_sem, me - 1)
        tell(below_sem, me + 1)

    def meet_far():
        def from_above(i, _):
            pl.semaphore_wait(above_sem, 1)

            @pl.when(has_down)
            def _():
                tell(above_sem, me - 1)

            return 0

        def from_below(i, _):
            pl.semaphore_wait(below_sem, 1)

            @pl.when(has_up)
            def _():
                tell(below_sem, me + 1)

            return 0

        lax.fori_loop(0, jnp.maximum(n - 2 - me, 0), from_above, 0)
        lax.fori_loop(0, jnp.maximum(me - 1, 0), from_below, 0)

    slab = rows // chunks

    def own_tok(m):
        return tok_ref.at[pl.ds(m * slab, slab)]

    def tok_at(h, m, src):
        return tok_buf.at[h, src, pl.ds(m * slab, slab)]

    def tok_z(m):
        return rdma(own_tok(m), tok_at(mine, m, t), t_s, tz_r.at[m], sp=partner)

    def tok_z_in(m):
        here = tok_at(other, m, t)
        return rdma(here, here, t_s, tz_r.at[m], sp=partner)

    def x_sem(own, m, d):
        return (0 if own else 1 + m) * max(half - 1, 1) + d - 1

    def tok_x(own, m, d):
        h = mine if own else other
        src = own_tok(m) if own else tok_at(h, m, t)
        return rdma(src, tok_at(h, m, t), t_s, tx_r.at[x_sem(own, m, d)], tp=2 * lax.rem(pair + d, half) + parity)

    def tok_x_in(own, m, d):
        src = 2 * lax.rem(pair + half - d, half) + parity
        here = tok_buf.at[mine, src] if own else tok_at(other, m, src)
        return rdma(here, here, t_s, tx_r.at[x_sem(own, m, d)], tp=src)

    def tok_c(own, m, d):
        h = mine if own else other
        src = 2 * lax.rem(pair + half - d, half) + parity
        there = tok_at(h, m, src)
        here = own_tok(m) if own and d == 0 else there
        return rdma(here, there, t_s, tc_r.at[0 if own else 1], tp=2 * pair + 1 - parity)

    tok_local = pltpu.make_async_copy(tok_ref, tok_buf.at[mine, t], t_loc)

    for d in range(1, half):
        for m in range(chunks):
            tok_x(True, m, d).start()

    owns = [wfk_ref, wfv_ref, wfq_ref, wrv_ref, qk_own]
    fox_arrays, ret_arrays = (0, 1, 2), (3, 4)
    starts = {}
    for group in (fox_arrays, ret_arrays):
        at = 0
        for c in group:
            starts[c] = (at, at + owns[c].shape[1])
            at = starts[c][1]
    fox_wide, ret_wide = starts[2][1], starts[4][1]
    q_at = starts[2][0]
    step = shard // n_grp
    count = len(owns)

    def w_at(c, src, part):
        start = pl.multiple_of(src * shard + part * step, step)
        return w_buf.at[pl.ds(start, step), starts[c][0] : starts[c][1]]

    local_at = {c: c - group[0] for group in (fox_arrays, ret_arrays) for c in group}

    def w_recv(c, src):
        return w_r.at[src * len(fox_arrays) + local_at[c]]

    def w_send(c, to):
        here = owns[c].at[pl.ds(pl.multiple_of(g * step, step), step)]
        return rdma(here, w_at(c, me, g), w_s.at[c], w_recv(c, me), sp=to)

    def w_on(c, src, to):
        here = w_at(c, src, g)
        return rdma(here, here, w_s.at[c], w_recv(c, src), sp=to)

    def w_in(c, src):
        here = w_at(c, src, g)
        return rdma(here, here, w_s.at[c], w_recv(c, src), sp=src)

    def w_side(c, src, d):
        here = w_at(c, src, g)
        return rdma(here, here, wy_s.at[local_at[c]], wy_r.at[local_at[c]], grp=lax.rem(g + d, n_grp))

    def w_several(c, pieces):
        return w_buf.at[: pieces * step, starts[c][0] : starts[c][1]]

    def w_local(c):
        start = pl.multiple_of(me * shard, shard)
        return pltpu.make_async_copy(
            owns[c], w_buf.at[pl.ds(start, shard), starts[c][0] : starts[c][1]], w_loc.at[local_at[c]]
        )

    fox_up = jnp.where(is_ret & (mine == 0), partner, fox_of(couple + 1))
    fox_down = jnp.where(is_ret & (mine == 1), partner, jnp.where(couple >= 1, fox_of(jnp.maximum(couple - 1, 0)), -1))
    ret_up = jnp.where(is_fox & (mine == 0), partner, ret_of(couple + 1))
    ret_down = jnp.where(is_fox & (mine == 1), partner, jnp.where(couple >= 1, ret_of(jnp.maximum(couple - 1, 0)), -1))

    def send_weights(arrays):
        up, down = (fox_up, fox_down) if arrays[0] in fox_arrays else (ret_up, ret_down)
        for c in arrays:

            @pl.when(up < n)
            def _(c=c):
                w_send(c, up).start()

            @pl.when(down >= 0)
            def _(c=c):
                w_send(c, down).start()

    def sends_from(p, arrays):
        q, b = p // 2, p % 2
        plane = (lambda i: 2 * i + 1 - i % 2) if arrays[0] in fox_arrays else (lambda i: 2 * i + i % 2)
        uses = plane(q) == p
        up = p + 1 if not uses and b == 0 else plane(q + 1)
        down = p - 1 if not uses and b == 1 else (plane(q - 1) if q else -1)
        passes = ((p if up < n else 0) + (n - 1 - p if down >= 0 else 0)) if uses else 0
        return (up < n) + (down >= 0) + passes

    send_weights((0, 1))
    for m in range(chunks):
        tok_z(m).start()
        tok_c(True, m, 0).start()
    send_weights((2,))
    meet_far()
    send_weights((3,))
    drained(in_sem.at[0], wqk_buf)
    qk_own[...] = wqk_buf[...].astype(jnp.float32).T.astype(jnp.bfloat16)
    tok_local.start()

    @pl.when(is_fox)
    def _():
        for c in fox_arrays:
            w_local(c).start()

    @pl.when(is_ret)
    def _():
        w_local(3).start()

    depth = mix_buf.shape[1] // 2
    out_cols = ret_out_ref.shape[1]

    out_step = depth // n_grp
    out_refs = [ret_out_ref, fox_out_ref]

    def out_cols_of(src):
        return pl.ds(pl.multiple_of(src * out_cols, out_cols), out_cols)

    def out_at(c, src):
        return wout_buf.at[pl.ds(pl.multiple_of(c * depth + g * out_step, out_step), out_step), out_cols_of(src)]

    def out_both(src):
        return wout_buf.at[: 2 * out_step, out_cols_of(src)]

    def out_hop(c, src, to, first):
        here = out_refs[c].at[pl.ds(pl.multiple_of(g * out_step, out_step), out_step)] if first else out_at(c, src)
        return rdma(here, out_at(c, src), o_s, o_r.at[src], sp=to)

    def out_local(c):
        return pltpu.make_async_copy(out_refs[c], wout_buf.at[c * depth : (c + 1) * depth, out_cols_of(me)], o_loc)

    def out_begin():
        for c in range(2):

            @pl.when(has_up)
            def _(c=c):
                out_hop(c, me, me + 1, True).start()

            @pl.when(has_down)
            def _(c=c):
                out_hop(c, me, me - 1, True).start()

            out_local(c).start()

    def out_relay(i):
        for src, to in ((me - i, me + 1), (me + i, me - 1)):

            @pl.when((src >= 0) & (src < n))
            def _(src=src, to=to):
                both = out_both(src)
                rdma(both, both, o_s, o_r.at[src], sp=src).wait_recv()
                for c in range(2):

                    @pl.when((to >= 0) & (to < n))
                    def _(c=c):
                        out_hop(c, src, to, False).start()

                    for d in range(1, n_grp):
                        here = out_at(c, src)
                        at = (d - 1) * n + src
                        rdma(here, here, oy_s, oy_r.at[at], grp=lax.rem(g + d, n_grp)).start()

    def out_arrive(src):
        for d in range(1, n_grp):
            drained(oy_r.at[(d - 1) * n + src], out_both(src))

    def w_pass(c, src):
        up, down = (fox_up, fox_down) if c in fox_arrays else (ret_up, ret_down)

        @pl.when((src < me) & (up < n))
        def _():
            w_on(c, src, up).start()

        @pl.when((src > me) & (down >= 0))
        def _():
            w_on(c, src, down).start()

    def w_relay(arrays, ks):
        for i in ks:
            for c in arrays:
                w_in(c, toward(i)).wait_recv()
                w_pass(c, toward(i))
                for d in range(1, n_grp):
                    w_side(c, toward(i), d).start()

    def w_arrive(arrays):
        for c in arrays:
            w_local(c).wait()
            drained(wy_r.at[local_at[c]], w_several(c, (n - 1) * (n_grp - 1)))

    def normalize(h):
        squares = jnp.zeros((rows, 1), jnp.float32)
        for i in range(n_tp):
            part = tok_buf[h, i].astype(jnp.float32)
            squares = squares + jnp.sum(part * part, axis=-1, keepdims=True)
        scale = lax.rsqrt(squares * (1.0 / (n_tp * feats)) + epsilon)
        at = pl.ds(pl.multiple_of(h * rows, rows), rows)
        for i in range(n_tp):
            part = tok_buf[h, i].astype(jnp.float32)
            cols = slice(i * feats, (i + 1) * feats)
            norm_buf[at, cols] = (part * scale * gain_buf[:, cols]).astype(jnp.bfloat16)

    far = list(range(2, n - 1))

    def tok_own():
        for d in range(1, half):
            tok_x_in(True, 0, d).wait_recv()
            for m in range(chunks):
                tok_c(True, m, d).start()

    def tok_swap(m):
        tok_z_in(m).wait_recv()
        for d in range(1, half):
            tok_x(False, m, d).start()
        tok_c(False, m, 0).start()

    def tok_last(m):
        for d in range(1, half):
            tok_x_in(False, m, d).wait_recv()
            tok_c(False, m, d).start()

    def tok_ready(own):
        if own:
            tok_local.wait()
        drained(tc_r.at[0 if own else 1], tok_buf.at[mine if own else other, :half])

    for copy in brought:
        copy.wait()

    @pl.when(is_fox)
    def _():
        w_relay((0, 1), [1, n - 1])

    send_weights((4,))
    out_begin()

    @pl.when(is_ret)
    def _():
        w_local(4).start()

    tok_swap(0)
    tok_own()
    for m in range(1, chunks):
        tok_swap(m)

    @pl.when(is_fox)
    def _():
        w_relay((0, 1), far)
        w_relay((2,), [1, n - 1])

    tok_ready(True)
    normalize(mine)

    row_id = lax.broadcasted_iota(jnp.int32, (rows, rows), 0)
    col_id = lax.broadcasted_iota(jnp.int32, (rows, rows), 1)
    causal = col_id <= row_id

    def norm_rows(h):
        return norm_buf[pl.ds(pl.multiple_of(h * rows, rows), rows), :]

    def mix_copy(first):
        return rdma(
            mix_pair.at[other], mix_buf.at[:, first : first + depth], mix_s, mix_r, sp=partner
        )

    def mix_own(first):
        mix_buf[:, first : first + depth] = mix_pair[mine]

    def mix_in(first):
        here = mix_buf.at[:, first : first + depth]
        return rdma(here, here, mix_s, mix_r, sp=partner)

    def kv_copy(b, q):
        at = 2 * couple + b
        return rdma(kv_buf.at[at], kv_buf.at[at], kv_s.at[2 * q + b], kv_r.at[at], sp=fox_of(q))

    def kv_in(at):
        return rdma(kv_buf.at[at], kv_buf.at[at], kv_s.at[at], kv_r.at[at], sp=partner)

    def sum_copy(q):
        return rdma(sum_buf.at[couple], sum_buf.at[couple], sum_s.at[q], sum_r.at[couple], sp=ret_of(q))

    def sum_in(q):
        return rdma(sum_buf.at[q], sum_buf.at[q], sum_s.at[q], sum_r.at[q], sp=partner)

    def later(act):
        for q in range(1, couples):

            @pl.when(q > couple)
            def _(q=q):
                act(jnp.int32(q))

    def after_tokens():
        for m in range(chunks):
            tok_last(m)

    @pl.when(is_fox)
    def _():
        def project_kv(b):
            kv_buf[2 * couple + b] = jnp.dot(
                norm_rows(b), w_buf[:, :q_at], preferred_element_type=jnp.float32
            ).astype(jnp.bfloat16)
            later(lambda q: kv_copy(b, q).start())

        after_tokens()
        w_relay((2,), far)
        w_arrive((0, 1))
        project_kv(mine)
        tok_ready(False)
        normalize(other)
        project_kv(other)
        w_arrive((2,))
        proj_buf[:, : fh * fd] = jnp.dot(
            norm_buf[...], w_buf[:, q_at:fox_wide], preferred_element_type=jnp.float32
        ).astype(jnp.bfloat16)
        out_relay(1)

        def block_cols(at):
            return pl.ds(pl.multiple_of(at * rows, rows), rows)

        def rep_cols(x, wide):
            return jnp.concatenate([x] * (wide // lanes), axis=1)

        for b in range(2):
            for h in range(fh):
                own = jnp.where(row_id == col_id, gates_buf[h : h + 1, block_cols(2 * couple + b)], 0.0)
                gate_buf[h, b * rows : (b + 1) * rows] = jnp.broadcast_to(
                    jnp.sum(own, axis=1, keepdims=True), (rows, lanes)
                )

        def attend(at, top_row, first, offset):
            size_ = 2 * rows - top_row
            here = slice(top_row, 2 * rows)
            for h in range(fh):
                query = proj_buf[here, h * fd : (h + 1) * fd]
                k = kv_buf[at, :, h * fd : (h + 1) * fd]
                v = kv_buf[at, :, (fh + h) * fd : (fh + h + 1) * fd]
                logits = lax.dot_general(query, k, NT, preferred_element_type=jnp.float32) * fd ** (-0.5)
                logits = logits + rep_cols(gate_buf[h, here], rows) - gates_buf[h : h + 1, block_cols(at)]
                if offset is not None:
                    row = lax.broadcasted_iota(jnp.int32, (size_, rows), 0)
                    col = lax.broadcasted_iota(jnp.int32, (size_, rows), 1)
                    logits = jnp.where(col <= row, logits, -jnp.inf)
                top_new = jnp.broadcast_to(jnp.max(logits, axis=-1, keepdims=True), (size_, lanes))
                if not first:
                    top = top_buf[h, here]
                    top_new = jnp.maximum(top, top_new)
                p = jnp.exp(logits - rep_cols(top_new, rows))
                total = jnp.broadcast_to(jnp.sum(p, axis=-1, keepdims=True), (size_, lanes))
                weighted = jnp.dot(p.astype(jnp.bfloat16), v, preferred_element_type=jnp.float32)
                if not first:
                    rescale = jnp.exp(top - top_new)
                    total = total_buf[h, here] * rescale + total
                    weighted = weighted_buf[h, here] * rescale[:, :fd] + weighted
                top_buf[h, here] = top_new
                total_buf[h, here] = total
                weighted_buf[h, here] = weighted

        attend(2 * couple, 0, True, 0)
        attend(2 * couple + 1, rows, False, 0)

        def past(i, _):
            q = lax.div(i, 2)
            b = jnp.where(lax.rem(i, 2) == 0, fox_of(q) - 2 * q, 1 - (fox_of(q) - 2 * q))
            at = 2 * q + b
            kv_in(at).wait_recv()
            attend(at, 0, False, None)
            return 0

        lax.fori_loop(0, 2 * couple, past, 0)
        for b in range(2):
            at = slice(b * rows, (b + 1) * rows)
            for h in range(fh):
                mix_pair[b, :, h * fd : (h + 1) * fd] = (
                    weighted_buf[h, at] / total_buf[h, at, :fd]
                ).astype(jnp.bfloat16)
        mix_copy(depth).start()
        mix_own(depth)
        for k in range(2, n):
            out_relay(k)
        mix_in(0).wait_recv()
        mix_copy(depth).wait_send()
        later(lambda q: kv_copy(0, q).wait_send())
        later(lambda q: kv_copy(1, q).wait_send())

    @pl.when(is_ret)
    def _():
        w_relay(ret_arrays, [1] + far)
        after_tokens()
        tok_ready(False)
        normalize(other)
        w_relay(ret_arrays, [n - 1])
        out_relay(1)
        w_arrive(ret_arrays)
        proj_buf[:, :ret_wide] = jnp.dot(
            norm_buf[...], w_buf[:, :ret_wide], preferred_element_type=jnp.float32
        ).astype(jnp.bfloat16)
        rv_at, rq_at = starts[3][0], starts[4][0]
        key_scale = dk ** (-0.5)
        position = lax.broadcasted_iota(jnp.int32, (rows, 1), 0).astype(jnp.float32)
        distance = jnp.maximum(row_id - col_id, 0).astype(jnp.float32)
        lone = jnp.zeros((dk, vd), jnp.float32)

        def part(b, first, wide):
            return proj_buf[pl.ds(pl.multiple_of(b * rows, rows), rows), first : first + wide]

        def summary(b, h):
            keys = part(b, rq_at + (hr + h) * dk, dk).astype(jnp.float32) * key_scale
            trailing = jnp.exp((rows - 1.0 - position) * decay_ref[h])
            return lax.dot_general(
                keys * trailing,
                part(b, rv_at + h * vd, vd).astype(jnp.float32),
                TN,
                precision=highest,
                preferred_element_type=jnp.float32,
            )

        early = [summary(0, h) for h in range(hr)]
        for h in range(hr):
            sum_buf[couple, h] = jnp.exp(lone + float(rows) * decay_ref[h]) * early[h] + summary(1, h)
        later(lambda q: sum_copy(q).start())
        out_relay(2)

        offset = (couple * 2 * rows).astype(jnp.float32)

        def gather(q, entering):
            sum_in(q).wait_recv()
            gap = ((couple - 1 - q) * 2 * rows).astype(jnp.float32)
            return tuple(entering[h] + jnp.exp(lone + gap * decay_ref[h]) * sum_buf[q, h] for h in range(hr))

        entering = tuple(jnp.exp(lone + offset * decay_ref[h]) * state_buf[h] for h in range(hr))
        entering = lax.fori_loop(0, couple, gather, entering)
        second = tuple(jnp.exp(lone + float(rows) * decay_ref[h]) * entering[h] + early[h] for h in range(hr))

        def block(i, _):
            b = jnp.where(i == 0, other, mine)
            for h in range(hr):
                rq = part(b, rq_at + h * dk, dk)
                rk = part(b, rq_at + (hr + h) * dk, dk)
                rv = part(b, rv_at + h * vd, vd)
                scores = lax.dot_general(rq, rk, NT, preferred_element_type=jnp.float32) * key_scale
                scores = jnp.where(causal, scores * jnp.exp(distance * decay_ref[h]), 0.0)
                inner = jnp.dot(
                    scores, rv.astype(jnp.float32), precision=highest, preferred_element_type=jnp.float32
                )
                leading = jnp.exp((position + 1.0) * decay_ref[h])
                carried = jnp.dot(
                    rq.astype(jnp.float32),
                    jnp.where(b == 0, entering[h], second[h]),
                    precision=highest,
                    preferred_element_type=jnp.float32,
                )
                raw = inner + carried * leading
                center = raw - jnp.mean(raw, axis=-1, keepdims=True)
                variance = jnp.mean(center * center, axis=-1, keepdims=True)
                cols = slice(h * vd, (h + 1) * vd)
                mix_pair[b, :, cols] = (center * lax.rsqrt(variance + epsilon) * hgain_buf[:, cols]).astype(
                    jnp.bfloat16
                )

            @pl.when(i == 0)
            def _():
                mix_copy(0).start()

            return 0

        lax.fori_loop(0, 2, block, 0)
        mix_own(0)
        for k in range(3, n):
            out_relay(k)
        mix_in(depth).wait_recv()
        mix_copy(0).wait_send()
        later(lambda q: sum_copy(q).wait_send())

    block = rows // n_tp
    wide, pieces = out_cols, n

    def piece_cols(piece):
        return pl.ds(pl.multiple_of(piece * wide, wide), wide)

    def slot(at):
        return pl.ds(pl.multiple_of(at * block, block), block)

    def pair_copy(piece):
        cols = piece_cols(piece)
        return rdma(
            rs_send.at[1 - parity, :, cols],
            pair_buf.at[:, cols],
            pair_s,
            pair_r.at[piece],
            tp=t + 1 - 2 * parity,
        )

    def rs_copy(d, piece):
        to = lax.rem(pair + d, half)
        cols = piece_cols(piece)
        return rdma(
            pair_sum.at[slot(to), cols],
            far_ref.at[d - 1, :, cols],
            rs_s.at[d - 1],
            rs_r.at[d - 1],
            tp=2 * to + parity,
        )

    def project(piece):
        cols = piece_cols(piece)
        value = jnp.dot(mix_buf[...], wout_buf[:, cols], preferred_element_type=jnp.float32).astype(jnp.bfloat16)
        for b in range(n_tp):
            at = slice(b // 2 * block, (b // 2 + 1) * block)
            rs_send[b % 2, at, cols] = value[b * block : (b + 1) * block]
        pair_copy(piece).start()

    def reduce(piece):
        cols = piece_cols(piece)
        pair_copy(piece).wait_recv()
        both = rs_send[parity, :, cols].astype(jnp.float32) + pair_buf[:, cols].astype(jnp.float32)
        pair_sum[:, cols] = both.astype(jnp.bfloat16)
        for d in range(1, half):
            rs_copy(d, piece).start()

    def order(i):
        falling = jnp.where(i <= me, me - i, i)
        rising = jnp.where(i <= n - 1 - me, me + i, n - 1 - i)
        return jnp.where(lower, rising, falling)

    drained(o_loc, wout_buf.at[:, out_cols_of(me)])
    project(me)

    def turn(i, _):
        out_arrive(order(i))
        project(order(i))
        reduce(order(i - 1))
        return 0

    lax.fori_loop(1, n, turn, 0)
    reduce(order(jnp.int32(n - 1)))

    own = slot(pair)
    near_ref[...] = rs_send[parity, own, :].astype(jnp.float32) + pair_buf[own, :].astype(jnp.float32)

    slabs = rows * (2 * n_tp - 1) // (2 * n_tp)
    drained(t_s, tok_buf.at[:, :, :slabs])
    for p in range(n):

        @pl.when(me == p)
        def _(p=p):
            for arrays in (fox_arrays, ret_arrays):
                for c in arrays:
                    if sends_from(p, arrays):
                        drained(w_s.at[c], w_several(c, sends_from(p, arrays)))
            hops = 2 * ((p + 1 if p + 1 < n else 0) + (n - p if p else 0))
            drained(o_s, wout_buf.at[: hops * out_step // n])

    drained(oy_s, wout_buf.at[: 2 * (n - 1) * (n_grp - 1) * out_step // n])

    def sides(arrays):
        for c in arrays:
            drained(wy_s.at[local_at[c]], w_several(c, (n - 1) * (n_grp - 1)))

    @pl.when(is_fox)
    def _():
        sides(fox_arrays)

    @pl.when(is_ret)
    def _():
        sides(ret_arrays)

    drained(pair_s, pair_buf)
    for d in range(1, half):
        drained(rs_s.at[d - 1], pair_sum.at[:block])
    for d in range(1, half):
        drained(rs_r.at[d - 1], far_ref.at[d - 1])


def paired(n, n_tp, n_grp, inputs):
    tokens, ret_query_weight, ret_state, fox_gates = inputs[0], inputs[2], inputs[9], inputs[11]
    fox_query_weight, ret_out_weight = inputs[5], inputs[12]
    rows, feats = tokens.shape
    hr, dk, vd = ret_state.shape
    fh = fox_gates.shape[1]
    fd = fox_query_weight.shape[1] // fh
    shard = ret_query_weight.shape[0]
    depth, out_cols = ret_out_weight.shape
    columns = out_cols * n
    wide = max(3 * fh * fd, 2 * hr * dk + hr * vd)
    half = n_tp // 2
    block = rows // n_tp
    chunks = 4
    couples = n // 2
    dma = pltpu.SemaphoreType.DMA
    far = max(half - 1, 1)
    side = max(n_grp - 1, 1) * n
    vmem = pl.BlockSpec(memory_space=pltpu.VMEM)
    smem = pl.BlockSpec(memory_space=pltpu.SMEM)
    hbm = pl.BlockSpec(memory_space=pl.ANY)
    bf16, f32 = jnp.bfloat16, jnp.float32
    size = (n, n_tp, n_grp, hr, dk, vd, fh, fd, chunks)
    near, other = pl.pallas_call(
        functools.partial(pair_kernel, size),
        out_shape=(pltpu.VMEM((block, columns), f32), pltpu.VMEM((far, block, columns), bf16)),
        in_specs=[hbm] * 8 + [smem] + [hbm] * 5,
        out_specs=(vmem, vmem),
        scratch_shapes=[
            pltpu.VMEM((1, n_tp * feats), f32),
            pltpu.VMEM((2 * hr * dk, shard), bf16),
            pltpu.VMEM((hr, dk, vd), f32),
            pltpu.VMEM((1, hr * vd), f32),
            pltpu.VMEM((fh, n * rows), f32),
            pltpu.VMEM((fh, 2 * rows, lanes), f32),
            pltpu.VMEM((2, n_tp, rows, feats), bf16),
            pltpu.VMEM((shard, 2 * hr * dk), bf16),
            pltpu.VMEM((n * shard, wide), bf16),
            pltpu.VMEM((2 * depth, columns), bf16),
            pltpu.VMEM((2 * rows, n_tp * feats), bf16),
            pltpu.VMEM((2 * rows, wide), bf16),
            pltpu.VMEM((n, rows, 2 * fh * fd), bf16),
            pltpu.VMEM((couples, hr, dk, vd), f32),
            pltpu.VMEM((2, rows, depth), bf16),
            pltpu.VMEM((rows, 2 * depth), bf16),
            pltpu.VMEM((2, rows // 2, columns), bf16),
            pltpu.VMEM((rows // 2, columns), bf16),
            pltpu.VMEM((rows // 2, columns), bf16),
            pltpu.VMEM((fh, 2 * rows, lanes), f32),
            pltpu.VMEM((fh, 2 * rows, lanes), f32),
            pltpu.VMEM((fh, 2 * rows, fd), f32),
            dma((5,)),
            pltpu.SemaphoreType.REGULAR,
            pltpu.SemaphoreType.REGULAR,
            dma,
            dma((chunks,)),
            dma(((chunks + 1) * far,)),
            dma((2,)),
            dma,
            dma((5,)),
            dma((3 * n,)),
            dma((3,)),
            dma((3,)),
            dma((3,)),
            dma,
            dma((n,)),
            dma,
            dma((side,)),
            dma,
            dma((2 * couples,)),
            dma((n,)),
            dma((couples,)),
            dma((couples,)),
            dma,
            dma,
            dma,
            dma((n,)),
            dma((far,)),
            dma((far,)),
        ],
        compiler_params=pltpu.CompilerParams(
            collective_id=0, has_side_effects=True, vmem_limit_bytes=56 * 1024 * 1024
        ),
        name="layer",
    )(
        tokens,
        inputs[1][None, :],
        inputs[2].T,
        inputs[3].T,
        inputs[4],
        inputs[5],
        inputs[6],
        inputs[7],
        inputs[8],
        inputs[9],
        inputs[10][None, :],
        inputs[11].T,
        inputs[12],
        inputs[13],
    )
    for d in range(half - 1):
        near = near + other[d].astype(f32)
    return near.astype(bf16)


def pairs_fit(n, n_tp, n_grp, inputs):
    rows, feats = inputs[0].shape
    hr, dk, vd = inputs[9].shape
    shard = inputs[2].shape[0]
    depth, out_cols = inputs[12].shape
    wide = inputs[5].shape[1]
    full = all(w % lanes == 0 for w in (out_cols, wide, 2 * hr * dk, hr * vd, feats, depth, rows))
    even = n % 2 == 0 and n > 2 and n_tp % 2 == 0 and n_grp > 1
    tiles = rows % (32 * n_tp) == 0 and rows % 32 == 0 and shard % (16 * n_grp) == 0 and depth % (16 * n_grp * n) == 0 and vd <= lanes
    columns = n * out_cols
    held = 8 * rows * n_tp * feats + 2 * n * shard * 3 * wide + 4 * depth * columns + 4 * n * rows * wide + 6 * rows * columns
    return full and even and tiles and depth == wide == hr * vd and held < 40 * 1024 * 1024


def local(
    n,
    n_tp,
    n_grp,
    tokens,
    norm_gain,
    ret_query_weight,
    ret_key_weight,
    ret_value_weight,
    fox_query_weight,
    fox_key_weight,
    fox_value_weight,
    ret_decay,
    ret_state,
    head_norm_gain,
    fox_gates,
    ret_out_weight,
    fox_out_weight,
):
    inputs = (
        tokens,
        norm_gain,
        ret_query_weight,
        ret_key_weight,
        ret_value_weight,
        fox_query_weight,
        fox_key_weight,
        fox_value_weight,
        ret_decay,
        ret_state,
        head_norm_gain,
        fox_gates,
        ret_out_weight,
        fox_out_weight,
    )
    if pairs_fit(n, n_tp, n_grp, inputs):
        return paired(n, n_tp, n_grp, inputs)
    rows, feats = tokens.shape
    hr, dk, vd = ret_state.shape
    fh = fox_gates.shape[1]
    fd = fox_query_weight.shape[1] // fh
    shard = ret_query_weight.shape[0]
    width = 2 * hr * dk + hr * vd + 3 * fh * fd
    depth, out_cols = ret_out_weight.shape
    columns = out_cols * n
    direct = out_cols % 128 == 0
    if not direct:
        ret_out_weight, fox_out_weight = ret_out_weight.T, fox_out_weight.T
    dma = pltpu.SemaphoreType.DMA

    def gather_sems(arrays):
        side = max(n_grp - 1, 1) * n * arrays
        return [
            dma((n * arrays,)),
            dma((n * arrays,)),
            dma((n * arrays,)),
            dma((side,)),
            dma((side,)),
            dma((arrays,)),
        ]

    vmem = pl.BlockSpec(memory_space=pltpu.VMEM)
    smem = pl.BlockSpec(memory_space=pltpu.SMEM)
    hbm = pl.BlockSpec(memory_space=pl.ANY)
    size = (n, n_tp, n_grp, hr, dk, vd, fh, fd, direct)
    block = rows // n_tp
    peers = max(n_tp - 1, 1)
    far = max(n_tp // 2 - 1, 1)
    pieces = n if direct else 1
    return pl.pallas_call(
        functools.partial(kernel, size),
        out_shape=jax.ShapeDtypeStruct((block, columns), jnp.bfloat16),
        in_specs=[hbm, vmem, vmem, vmem, hbm, hbm, hbm, hbm, smem, vmem, vmem, vmem, hbm, hbm],
        out_specs=vmem,
        scratch_shapes=[
            pltpu.VMEM((n_tp, rows, feats), jnp.bfloat16),
            pltpu.VMEM((shard, 2 * hr * dk), jnp.bfloat16),
            pltpu.VMEM((n * shard, width), jnp.bfloat16),
            pltpu.VMEM((2 * depth, columns) if direct else (columns, 2 * depth), jnp.bfloat16),
            pltpu.VMEM((rows, n_tp * feats), jnp.bfloat16),
            pltpu.VMEM((rows, width - 2 * fh * fd), jnp.bfloat16),
            pltpu.VMEM((n, rows, 2 * fh * fd), jnp.bfloat16),
            pltpu.VMEM((n, hr, dk, vd), jnp.float32),
            pltpu.VMEM((rows, 2 * depth), jnp.bfloat16),
            pltpu.VMEM((2, rows // 2, columns), jnp.bfloat16),
            pltpu.VMEM((rows // 2, columns), jnp.bfloat16),
            pltpu.VMEM((rows // 2, columns), jnp.bfloat16),
            pltpu.VMEM((far, block, columns), jnp.bfloat16),
            pltpu.VMEM((fh, rows, 1), jnp.float32),
            pltpu.VMEM((fh, rows, 1), jnp.float32),
            pltpu.VMEM((fh, rows, fd), jnp.float32),
            dma((peers,)),
            dma((peers,)),
            dma,
            dma((n,)),
            dma((n,)),
            dma((n,)),
            dma((n,)),
            dma((pieces,)),
            dma((pieces,)),
            dma((far * pieces,)),
            dma((far * pieces,)),
        ]
        + gather_sems(2)
        + gather_sems(3)
        + gather_sems(2),
        compiler_params=pltpu.CompilerParams(
            collective_id=0, has_side_effects=True, vmem_limit_bytes=56 * 1024 * 1024
        ),
        name="layer",
    )(
        tokens,
        norm_gain[None, :],
        ret_query_weight.T,
        ret_key_weight.T,
        ret_value_weight,
        fox_query_weight,
        fox_key_weight,
        fox_value_weight,
        ret_decay,
        ret_state,
        head_norm_gain[None, :],
        fox_gates.T,
        ret_out_weight,
        fox_out_weight,
    )


def solution(mesh):
    placed = (
        P(("grp", "sp"), "tp"),
        P(),
        P("sp", "tp"),
        P("sp", "tp"),
        P("sp", "tp"),
        P("sp", "tp"),
        P("sp", "tp"),
        P("sp", "tp"),
        P("tp"),
        P(("grp", "tp"), None, None),
        P("tp"),
        P("grp", "tp"),
        P("tp", "sp"),
        P("tp", "sp"),
    )
    body = functools.partial(local, mesh.shape["sp"], mesh.shape["tp"], mesh.shape["grp"])
    return jax.shard_map(
        body, mesh=mesh, in_specs=placed, out_specs=P(("grp", "sp", "tp"), None), check_vma=False
    )
```

```python
import functools

import jax
import jax.numpy as jnp
from jax import lax
from jax.experimental import pallas as pl
from jax.experimental.pallas import tpu as pltpu
from jax.sharding import PartitionSpec as P

epsilon = 1e-06
lanes = 128
highest = lax.Precision.HIGHEST
NT = (((1,), (1,)), ((), ()))
TN = (((0,), (0,)), ((), ()))


def rdma(src, dst, send_sem, recv_sem, **target):
    return pltpu.make_async_remote_copy(
        src_ref=src,
        dst_ref=dst,
        send_sem=send_sem,
        recv_sem=recv_sem,
        device_id=target,
        device_id_type=pl.DeviceIdType.MESH,
    )


class LineGather:
    def __init__(self, owns, place, sems, n, n_grp, me, g):
        self.owns, self.place, self.n, self.n_grp, self.me, self.g = owns, place, n, n_grp, me, g
        self.up, self.down, self.zr, self.ys, self.yr, self.loc = sems
        self.arrays = len(owns)
        self.rows = owns[0].shape[0]
        self.step = self.rows // n_grp

    def piece(self, part, src, c):
        return self.place(src, c, part * self.step, self.step)

    def own_piece(self, c):
        return self.owns[c].at[pl.ds(pl.multiple_of(self.g * self.step, self.step), self.step)]

    def hop(self, sems, to, src, c, first=False):
        here = self.own_piece(c) if first else self.piece(self.g, src, c)
        at = src * self.arrays + c
        return rdma(here, self.piece(self.g, src, c), sems.at[at], self.zr.at[at], sp=to)

    def side(self, d, src, c):
        at = ((d - 1) * self.n + src) * self.arrays + c
        here = self.piece(self.g, src, c)
        return rdma(here, here, self.ys.at[at], self.yr.at[at], grp=lax.rem(self.g + d, self.n_grp))

    def side_in(self, d, src, c):
        at = ((d - 1) * self.n + src) * self.arrays + c
        part = lax.rem(self.g + self.n_grp - d, self.n_grp)
        here = self.piece(part, src, c)
        return rdma(here, here, self.ys.at[at], self.yr.at[at], grp=part)

    def local(self, c):
        return pltpu.make_async_copy(self.owns[c], self.place(self.me, c, 0, self.rows), self.loc.at[c])

    def start(self):
        me, n = self.me, self.n
        for c in range(self.arrays):

            @pl.when(me + 1 < n)
            def _():
                self.hop(self.up, me + 1, me, c, True).start()

            @pl.when(me >= 1)
            def _():
                self.hop(self.down, me - 1, me, c, True).start()

        for c in range(self.arrays):
            self.local(c).start()

    def relay(self, k):
        me, n = self.me, self.n
        for c in range(self.arrays):
            for src, sems, to in ((me - k, self.up, me + 1), (me + k, self.down, me - 1)):

                @pl.when((src >= 0) & (src < n))
                def _(src=src, sems=sems, to=to):
                    self.hop(sems, me, src, c).wait_recv()

                    @pl.when((to >= 0) & (to < n))
                    def _():
                        self.hop(sems, to, src, c).start()

                    for d in range(1, self.n_grp):
                        self.side(d, src, c).start()

    def arrive_shard(self, src, arrays):
        for c in arrays:
            for d in range(1, self.n_grp):
                self.side_in(d, src, c).wait_recv()

    def arrive(self, arrays):
        for c in arrays:
            self.local(c).wait()

        def step(k, _):
            self.arrive_shard(lax.rem(self.me + k, self.n), arrays)
            return 0

        lax.fori_loop(1, self.n, step, 0)

    def finish(self):
        me, n = self.me, self.n

        def step(src, _):
            for c in range(self.arrays):

                @pl.when((src <= me) & (me + 1 < n))
                def _():
                    self.hop(self.up, me, src, c).wait_send()

                @pl.when((src >= me) & (me >= 1))
                def _():
                    self.hop(self.down, me, src, c).wait_send()

                @pl.when(src != me)
                def _():
                    for d in range(1, self.n_grp):
                        self.side(d, src, c).wait_send()

            return 0

        lax.fori_loop(0, n, step, 0)


def kernel(
    size,
    tok_ref,
    gain_ref,
    wq_ref,
    wk_ref,
    wrv_ref,
    wfq_ref,
    wfk_ref,
    wfv_ref,
    decay_ref,
    state_ref,
    hgain_ref,
    gates_ref,
    ret_out_ref,
    fox_out_ref,
    out_ref,
    tok_buf,
    qk_own,
    w_buf,
    wout_buf,
    norm_buf,
    proj_buf,
    kv_buf,
    sum_buf,
    mix_buf,
    rs_send,
    pair_buf,
    pair_sum,
    rs_buf,
    top_buf,
    total_buf,
    weighted_buf,
    tok_s,
    tok_r,
    tok_loc,
    kv_s,
    kv_r,
    sum_s,
    sum_r,
    pair_s,
    pair_r,
    rs_s,
    rs_r,
    *gather_sems,
):
    n, n_tp, n_grp, hr, dk, vd, fh, fd, direct = size
    me, t, g = lax.axis_index("sp"), lax.axis_index("tp"), lax.axis_index("grp")
    rows, feats = tok_ref.shape
    owns = [wfk_ref, wfv_ref, wfq_ref, wrv_ref, qk_own]
    early = 2
    starts = [0]
    for own in owns:
        starts.append(starts[-1] + own.shape[1])
    shard = qk_own.shape[0]

    def weight_place(src, c, first, count):
        start = pl.multiple_of(src * shard + first, count)
        return w_buf.at[pl.ds(start, count), starts[c] : starts[c + 1]]

    depth = mix_buf.shape[1] // 2
    out_cols = ret_out_ref.shape[1] if direct else ret_out_ref.shape[0]

    def out_place(src, c, first, count):
        if direct:
            start = pl.multiple_of(c * depth + first, count)
            return wout_buf.at[pl.ds(start, count), pl.ds(pl.multiple_of(src * out_cols, out_cols), out_cols)]
        start = pl.multiple_of(src * out_cols + first, count)
        return wout_buf.at[pl.ds(start, count), c * depth : (c + 1) * depth]

    def late_place(src, c, first, count):
        return weight_place(src, c + early, first, count)

    firsts = LineGather(owns[:early], weight_place, gather_sems[:6], n, n_grp, me, g)
    lasts = LineGather(owns[early:], late_place, gather_sems[6:12], n, n_grp, me, g)
    outs = LineGather([ret_out_ref, fox_out_ref], out_place, gather_sems[12:], n, n_grp, me, g)

    barrier = pltpu.get_barrier_semaphore()

    def greet(**target):
        pl.semaphore_signal(barrier, inc=1, device_id=target, device_id_type=pl.DeviceIdType.MESH)

    has_up, has_down = me + 1 < n, me >= 1
    for d in range(1, n_tp):
        greet(tp=lax.rem(t + d, n_tp))
    for d in range(1, n_grp):
        greet(grp=lax.rem(g + d, n_grp))

    @pl.when(has_up)
    def _():
        greet(sp=me + 1)

    @pl.when(has_down)
    def _():
        greet(sp=me - 1)

    turned = jnp.concatenate((wq_ref[...], wk_ref[...]), axis=0).astype(jnp.float32)
    qk_own[...] = turned.T.astype(jnp.bfloat16)

    count = n_tp - 1 + n_grp - 1 + has_up.astype(jnp.int32) + has_down.astype(jnp.int32)
    pl.semaphore_wait(barrier, count)

    def tok_copy(d):
        return rdma(tok_ref, tok_buf.at[t], tok_s.at[d - 1], tok_r.at[d - 1], tp=lax.rem(t + d, n_tp))

    def tok_in(d):
        src = lax.rem(t + n_tp - d, n_tp)
        return rdma(tok_ref, tok_buf.at[src], tok_s.at[d - 1], tok_r.at[d - 1], tp=src)

    firsts.start()
    lasts.start()
    tok_local = pltpu.make_async_copy(tok_ref, tok_buf.at[t], tok_loc)
    for d in range(1, n_tp):
        tok_copy(d).start()
    tok_local.start()

    def first_step(k, _):
        firsts.relay(k)

        lasts.relay(k)
        return 0

    lax.fori_loop(1, n, first_step, 0)
    outs.start()

    tok_local.wait()
    for d in range(1, n_tp):
        tok_in(d).wait_recv()
    squares = jnp.zeros((rows, 1), jnp.float32)
    for i in range(n_tp):
        part = tok_buf[i].astype(jnp.float32)
        squares = squares + jnp.sum(part * part, axis=-1, keepdims=True)
    scale = lax.rsqrt(squares * (1.0 / (n_tp * feats)) + epsilon)
    for i in range(n_tp):
        part = tok_buf[i].astype(jnp.float32)
        cols = slice(i * feats, (i + 1) * feats)
        norm_buf[:, cols] = (part * scale * gain_ref[:, cols]).astype(jnp.bfloat16)

    def kv_copy(src):
        return rdma(kv_buf.at[src], kv_buf.at[src], kv_s.at[src], kv_r.at[src], sp=jnp.minimum(me + 1, n - 1))

    def sum_copy(src):
        return rdma(sum_buf.at[src], sum_buf.at[src], sum_s.at[src], sum_r.at[src], sp=jnp.minimum(me + 1, n - 1))

    firsts.arrive((0, 1))
    kv_buf[me] = jnp.dot(
        norm_buf[...], w_buf[:, : starts[2]], preferred_element_type=jnp.float32
    ).astype(jnp.bfloat16)

    def kv_forward(k):
        src = me - k

        @pl.when(src >= 0)
        def _():
            kv_copy(src).wait_recv()

            @pl.when(has_up)
            def _():
                kv_copy(src).start()

    @pl.when(has_up)
    def _():
        kv_copy(me).start()

    outs.relay(1)
    lasts.arrive((0, 1, 2))
    proj_buf[...] = jnp.dot(
        norm_buf[...], w_buf[:, starts[2] :], preferred_element_type=jnp.float32
    ).astype(jnp.bfloat16)
    rv_at, rq_at = starts[3] - starts[2], starts[4] - starts[2]

    key_scale = dk ** (-0.5)
    position = lax.broadcasted_iota(jnp.int32, (rows, 1), 0).astype(jnp.float32)
    rq, rk, rv = [], [], []
    for h in range(hr):
        rq.append(proj_buf[:, rq_at + h * dk : rq_at + (h + 1) * dk])
        rk.append(proj_buf[:, rq_at + (hr + h) * dk : rq_at + (hr + h + 1) * dk])
        rv.append(proj_buf[:, rv_at + h * vd : rv_at + (h + 1) * vd])
        keys = rk[h].astype(jnp.float32) * key_scale
        trailing = jnp.exp((rows - 1.0 - position) * decay_ref[h])
        sum_buf[me, h] = lax.dot_general(
            keys * trailing, rv[h].astype(jnp.float32), TN, precision=highest, preferred_element_type=jnp.float32
        )

    @pl.when(has_up)
    def _():
        sum_copy(me).start()

    row_id = lax.broadcasted_iota(jnp.int32, (rows, rows), 0)
    col_id = lax.broadcasted_iota(jnp.int32, (rows, rows), 1)
    causal = col_id <= row_id
    own_cols = pl.ds(pl.multiple_of(me * rows, rows), rows)
    own_gates = [
        jnp.sum(jnp.where(row_id == col_id, gates_ref[h : h + 1, own_cols], 0.0), axis=1, keepdims=True)
        for h in range(fh)
    ]

    def attend(src, diagonal):
        key_cols = pl.ds(pl.multiple_of(src * rows, rows), rows)
        for h in range(fh):
            query = proj_buf[:, h * fd : (h + 1) * fd]
            k = kv_buf[src, :, h * fd : (h + 1) * fd]
            v = kv_buf[src, :, (fh + h) * fd : (fh + h + 1) * fd]
            logits = lax.dot_general(query, k, NT, preferred_element_type=jnp.float32) * fd ** (-0.5)
            logits = logits + own_gates[h] - gates_ref[h : h + 1, key_cols]
            if diagonal:
                logits = jnp.where(causal, logits, -jnp.inf)
            top_new = jnp.max(logits, axis=-1, keepdims=True)
            if not diagonal:
                top = top_buf[h]
                top_new = jnp.maximum(top, top_new)
            p = jnp.exp(logits - top_new)
            total = jnp.sum(p, axis=-1, keepdims=True)
            weighted = jnp.dot(p.astype(jnp.bfloat16), v, preferred_element_type=jnp.float32)
            if not diagonal:
                rescale = jnp.exp(top - top_new)
                total = total_buf[h] * rescale + total
                weighted = weighted_buf[h] * rescale + weighted
            top_buf[h] = top_new
            total_buf[h] = total
            weighted_buf[h] = weighted

    def forward(k):
        src = me - k

        @pl.when(src >= 0)
        def _():
            sum_copy(src).wait_recv()

            @pl.when(has_up)
            def _():
                sum_copy(src).start()

    attend(me, True)

    offset = (me * rows).astype(jnp.float32)
    lone = jnp.zeros((dk, vd), jnp.float32)

    def step(k, entering):
        src = me - k
        kv_forward(k)
        forward(k)

        @pl.when(k + 1 < n)
        def _():
            outs.relay(k + 1)


        @pl.when(src >= 0)
        def _():
            attend(src, False)

        gap = ((k - 1) * rows).astype(jnp.float32)
        there = jnp.maximum(src, 0)
        return tuple(
            entering[h]
            + jnp.where(src >= 0, jnp.exp(lone + gap * decay_ref[h]) * sum_buf[there, h], 0.0)
            for h in range(hr)
        )

    entering = tuple(jnp.exp(lone + offset * decay_ref[h]) * state_ref[h] for h in range(hr))
    entering = lax.fori_loop(1, n, step, entering)

    distance = jnp.maximum(row_id - col_id, 0).astype(jnp.float32)
    for h in range(hr):
        scores = lax.dot_general(rq[h], rk[h], NT, preferred_element_type=jnp.float32) * key_scale
        scores = jnp.where(causal, scores * jnp.exp(distance * decay_ref[h]), 0.0)
        inner = jnp.dot(scores, rv[h].astype(jnp.float32), precision=highest, preferred_element_type=jnp.float32)
        leading = jnp.exp((position + 1.0) * decay_ref[h])
        carried = jnp.dot(
            rq[h].astype(jnp.float32), entering[h], precision=highest, preferred_element_type=jnp.float32
        )
        raw = inner + carried * leading
        center = raw - jnp.mean(raw, axis=-1, keepdims=True)
        variance = jnp.mean(center * center, axis=-1, keepdims=True)
        cols = slice(h * vd, (h + 1) * vd)
        mix_buf[:, cols] = (center * lax.rsqrt(variance + epsilon) * hgain_ref[:, cols]).astype(jnp.bfloat16)
    for h in range(fh):
        cols = slice(hr * vd + h * fd, hr * vd + (h + 1) * fd)
        mix_buf[:, cols] = (weighted_buf[h] / total_buf[h]).astype(jnp.bfloat16)

    block = rows // n_tp
    columns = pair_buf.shape[1]
    wide = out_cols if direct else columns
    pieces = columns // wide
    half = n_tp // 2
    parity, pair = lax.rem(t, 2), lax.div(t, 2)

    def piece_cols(piece):
        return pl.ds(pl.multiple_of(piece * wide, wide), wide)

    def slot(at):
        return pl.ds(pl.multiple_of(at * block, block), block)

    def pair_copy(piece):
        cols = piece_cols(piece)
        return rdma(
            rs_send.at[1 - parity, :, cols],
            pair_buf.at[:, cols],
            pair_s.at[piece],
            pair_r.at[piece],
            tp=t + 1 - 2 * parity,
        )

    def rs_copy(d, piece):
        to = lax.rem(pair + d, half)
        cols = piece_cols(piece)
        at = (d - 1) * pieces + piece
        return rdma(
            pair_sum.at[slot(to), cols], rs_buf.at[d - 1, :, cols], rs_s.at[at], rs_r.at[at], tp=2 * to + parity
        )

    def project(piece):
        cols = piece_cols(piece)
        if direct:
            value = jnp.dot(mix_buf[...], wout_buf[:, cols], preferred_element_type=jnp.float32)
        else:
            value = lax.dot_general(mix_buf[...], wout_buf[...], NT, preferred_element_type=jnp.float32)
        value = value.astype(jnp.bfloat16)
        for b in range(n_tp):
            at = slice(b // 2 * block, (b // 2 + 1) * block)
            rs_send[b % 2, at, cols] = value[b * block : (b + 1) * block]
        pair_copy(piece).start()

    def reduce(piece):
        cols = piece_cols(piece)
        pair_copy(piece).wait_recv()
        both = rs_send[parity, :, cols].astype(jnp.float32) + pair_buf[:, cols].astype(jnp.float32)
        pair_sum[:, cols] = both.astype(jnp.bfloat16)
        for d in range(1, half):
            rs_copy(d, piece).start()

    def order(i):
        falling = jnp.where(i <= me, me - i, i)
        rising = jnp.where(i <= n - 1 - me, me + i, n - 1 - i)
        return jnp.where(2 * me >= n, falling, rising)

    if direct:
        for c in range(2):
            outs.local(c).wait()
        project(me)

        def out_step(i, _):
            outs.arrive_shard(order(i), (0, 1))
            project(order(i))
            reduce(order(i - 1))
            return 0

        lax.fori_loop(1, n, out_step, 0)
        reduce(order(jnp.int32(n - 1)))
    else:
        outs.arrive((0, 1))
        project(0)
        reduce(0)

    own = slot(pair)
    summed = rs_send[parity, own, :].astype(jnp.float32) + pair_buf[own, :].astype(jnp.float32)
    for d in range(1, half):
        for piece in range(pieces):
            rs_copy(d, piece).wait_recv()
        summed = summed + rs_buf[d - 1].astype(jnp.float32)
    out_ref[...] = summed.astype(jnp.bfloat16)

    for d in range(1, n_tp):
        tok_copy(d).wait_send()
    for piece in range(pieces):
        pair_copy(piece).wait_send()
        for d in range(1, half):
            rs_copy(d, piece).wait_send()
    firsts.finish()
    lasts.finish()
    outs.finish()

    @pl.when(has_up)
    def _():
        def step(src, _):
            kv_copy(src).wait_send()
            sum_copy(src).wait_send()
            return 0

        lax.fori_loop(0, me + 1, step, 0)


def pair_kernel(
    size,
    tok_ref,
    gain_ref,
    wq_ref,
    wk_ref,
    wrv_ref,
    wfq_ref,
    wfk_ref,
    wfv_ref,
    decay_ref,
    state_ref,
    hgain_ref,
    gates_ref,
    ret_out_ref,
    fox_out_ref,
    near_ref,
    far_ref,
    gain_buf,
    wqk_buf,
    state_buf,
    hgain_buf,
    gates_buf,
    gate_buf,
    within_buf,
    raw_buf,
    tok_buf,
    qk_own,
    w_buf,
    wout_buf,
    norm_buf,
    proj_buf,
    kv_buf,
    sum_buf,
    mix_pair,
    mix_buf,
    rs_send,
    pair_buf,
    pair_sum,
    top_buf,
    total_buf,
    weighted_buf,
    in_sem,
    above_sem,
    below_sem,
    t_s,
    tz_r,
    tx_r,
    tc_r,
    t_loc,
    w_s,
    w_r,
    wy_s,
    wy_r,
    w_loc,
    o_s,
    o_r,
    oy_s,
    oy_r,
    o_loc,
    kv_s,
    kv_r,
    sum_s,
    sum_r,
    mix_s,
    mix_r,
    pair_s,
    pair_r,
    rs_s,
    rs_r,
):
    n, n_tp, n_grp, hr, dk, vd, fh, fd, chunks = size
    me, t, g = lax.axis_index("sp"), lax.axis_index("tp"), lax.axis_index("grp")
    rows, feats = tok_ref.shape
    shard = qk_own.shape[0]
    couples = n // 2
    couple, mine = lax.div(me, 2), lax.rem(me, 2)
    other = 1 - mine
    partner = me + 1 - 2 * mine
    fox_mine = 1 - lax.rem(couple, 2)
    is_fox = mine == fox_mine
    is_ret = mine != fox_mine
    lower = 2 * me < n
    half = n_tp // 2
    parity, pair = lax.rem(t, 2), lax.div(t, 2)

    def fox_of(q):
        return 2 * q + 1 - lax.rem(q, 2)

    def ret_of(q):
        return 2 * q + lax.rem(q, 2)

    def toward(k):
        return lax.rem(jnp.where(lower, me + k, me + n - k), n)

    barrier = pltpu.get_barrier_semaphore()

    def greet(**target):
        pl.semaphore_signal(barrier, inc=1, device_id=target, device_id_type=pl.DeviceIdType.MESH)

    greet(tp=2 * pair + 1 - parity)
    for d in range(1, half):
        greet(tp=2 * lax.rem(pair + d, half) + parity)
    for d in range(1, n_grp):
        greet(grp=lax.rem(g + d, n_grp))
    has_up, has_down = me + 1 < n, me >= 1

    @pl.when(has_up)
    def _():
        greet(sp=me + 1)

    @pl.when(has_down)
    def _():
        greet(sp=me - 1)

    def drained(sem, ref):
        pltpu.make_async_copy(ref, ref, sem).wait()

    width = hr * dk
    pltpu.make_async_copy(wq_ref, wqk_buf.at[:width], in_sem.at[0]).start()
    pltpu.make_async_copy(wk_ref, wqk_buf.at[width:], in_sem.at[0]).start()
    brought = [
        pltpu.make_async_copy(src, dst, in_sem.at[i + 1])
        for i, (src, dst) in enumerate(
            ((gain_ref, gain_buf), (state_ref, state_buf), (hgain_ref, hgain_buf), (gates_ref, gates_buf))
        )
    ]
    for copy in brought:
        copy.start()

    pl.semaphore_wait(barrier, half + n_grp - 1 + has_up.astype(jnp.int32) + has_down.astype(jnp.int32))

    def tell(sem, to):
        pl.semaphore_signal(sem, inc=1, device_id={"sp": to}, device_id_type=pl.DeviceIdType.MESH)

    @pl.when(has_up & has_down)
    def _():
        tell(above_sem, me - 1)
        tell(below_sem, me + 1)

    def meet_far():
        def from_above(i, _):
            pl.semaphore_wait(above_sem, 1)

            @pl.when(has_down)
            def _():
                tell(above_sem, me - 1)

            return 0

        def from_below(i, _):
            pl.semaphore_wait(below_sem, 1)

            @pl.when(has_up)
            def _():
                tell(below_sem, me + 1)

            return 0

        lax.fori_loop(0, jnp.maximum(n - 2 - me, 0), from_above, 0)
        lax.fori_loop(0, jnp.maximum(me - 1, 0), from_below, 0)

    slab = rows // chunks

    def own_tok(m):
        return tok_ref.at[pl.ds(m * slab, slab)]

    def tok_at(h, m, src):
        return tok_buf.at[h, src, pl.ds(m * slab, slab)]

    def tok_z(m):
        return rdma(own_tok(m), tok_at(mine, m, t), t_s, tz_r.at[m], sp=partner)

    def tok_z_in(m):
        here = tok_at(other, m, t)
        return rdma(here, here, t_s, tz_r.at[m], sp=partner)

    def x_sem(own, m, d):
        return (0 if own else 1 + m) * max(half - 1, 1) + d - 1

    def tok_x(own, m, d):
        h = mine if own else other
        src = own_tok(m) if own else tok_at(h, m, t)
        return rdma(src, tok_at(h, m, t), t_s, tx_r.at[x_sem(own, m, d)], tp=2 * lax.rem(pair + d, half) + parity)

    def tok_x_in(own, m, d):
        src = 2 * lax.rem(pair + half - d, half) + parity
        here = tok_buf.at[mine, src] if own else tok_at(other, m, src)
        return rdma(here, here, t_s, tx_r.at[x_sem(own, m, d)], tp=src)

    def tok_c(own, m, d):
        h = mine if own else other
        src = 2 * lax.rem(pair + half - d, half) + parity
        there = tok_at(h, m, src)
        here = own_tok(m) if own and d == 0 else there
        return rdma(here, there, t_s, tc_r.at[0 if own else 1], tp=2 * pair + 1 - parity)

    tok_local = pltpu.make_async_copy(tok_ref, tok_buf.at[mine, t], t_loc)

    for d in range(1, half):
        for m in range(chunks):
            tok_x(True, m, d).start()

    owns = [wfk_ref, wfv_ref, wfq_ref, wrv_ref, qk_own]
    fox_arrays, ret_arrays = (0, 1, 2), (3, 4)
    starts = {}
    for group in (fox_arrays, ret_arrays):
        at = 0
        for c in group:
            starts[c] = (at, at + owns[c].shape[1])
            at = starts[c][1]
    fox_wide, ret_wide = starts[2][1], starts[4][1]
    q_at = starts[2][0]
    step = shard // n_grp
    count = len(owns)

    def w_at(c, src, part):
        start = pl.multiple_of(src * shard + part * step, step)
        return w_buf.at[pl.ds(start, step), starts[c][0] : starts[c][1]]

    local_at = {c: c - group[0] for group in (fox_arrays, ret_arrays) for c in group}

    def w_recv(c, src):
        return w_r.at[src * len(fox_arrays) + local_at[c]]

    def w_send(c, to):
        here = owns[c].at[pl.ds(pl.multiple_of(g * step, step), step)]
        return rdma(here, w_at(c, me, g), w_s.at[c], w_recv(c, me), sp=to)

    def w_on(c, src, to):
        here = w_at(c, src, g)
        return rdma(here, here, w_s.at[c], w_recv(c, src), sp=to)

    def w_in(c, src):
        here = w_at(c, src, g)
        return rdma(here, here, w_s.at[c], w_recv(c, src), sp=src)

    def w_side(c, src, d):
        here = w_at(c, src, g)
        return rdma(here, here, wy_s.at[local_at[c]], wy_r.at[local_at[c]], grp=lax.rem(g + d, n_grp))

    def w_several(c, pieces):
        return w_buf.at[: pieces * step, starts[c][0] : starts[c][1]]

    def w_local(c):
        start = pl.multiple_of(me * shard, shard)
        return pltpu.make_async_copy(
            owns[c], w_buf.at[pl.ds(start, shard), starts[c][0] : starts[c][1]], w_loc.at[local_at[c]]
        )

    fox_up = jnp.where(is_ret & (mine == 0), partner, fox_of(couple + 1))
    fox_down = jnp.where(is_ret & (mine == 1), partner, jnp.where(couple >= 1, fox_of(jnp.maximum(couple - 1, 0)), -1))
    ret_up = jnp.where(is_fox & (mine == 0), partner, ret_of(couple + 1))
    ret_down = jnp.where(is_fox & (mine == 1), partner, jnp.where(couple >= 1, ret_of(jnp.maximum(couple - 1, 0)), -1))

    def send_weights(arrays):
        up, down = (fox_up, fox_down) if arrays[0] in fox_arrays else (ret_up, ret_down)
        for c in arrays:

            @pl.when(up < n)
            def _(c=c):
                w_send(c, up).start()

            @pl.when(down >= 0)
            def _(c=c):
                w_send(c, down).start()

    def sends_from(p, arrays):
        q, b = p // 2, p % 2
        plane = (lambda i: 2 * i + 1 - i % 2) if arrays[0] in fox_arrays else (lambda i: 2 * i + i % 2)
        uses = plane(q) == p
        up = p + 1 if not uses and b == 0 else plane(q + 1)
        down = p - 1 if not uses and b == 1 else (plane(q - 1) if q else -1)
        passes = ((p if up < n else 0) + (n - 1 - p if down >= 0 else 0)) if uses else 0
        return (up < n) + (down >= 0) + passes

    send_weights((0, 1))
    for m in range(chunks):
        tok_z(m).start()
        tok_c(True, m, 0).start()
    send_weights((2,))
    meet_far()
    send_weights((3,))
    drained(in_sem.at[0], wqk_buf)
    qk_own[...] = wqk_buf[...].astype(jnp.float32).T.astype(jnp.bfloat16)
    send_weights((4,))
    tok_local.start()

    @pl.when(is_fox)
    def _():
        for c in fox_arrays:
            w_local(c).start()

    @pl.when(is_ret)
    def _():
        w_local(3).start()

    depth = mix_buf.shape[1] // 2
    out_cols = ret_out_ref.shape[1]

    out_step = depth // n_grp
    out_refs = [ret_out_ref, fox_out_ref]

    def out_cols_of(src):
        return pl.ds(pl.multiple_of(src * out_cols, out_cols), out_cols)

    def out_at(c, src):
        return wout_buf.at[pl.ds(pl.multiple_of(c * depth + g * out_step, out_step), out_step), out_cols_of(src)]

    def out_both(src):
        return wout_buf.at[: 2 * out_step, out_cols_of(src)]

    def out_hop(c, src, to, first):
        here = out_refs[c].at[pl.ds(pl.multiple_of(g * out_step, out_step), out_step)] if first else out_at(c, src)
        return rdma(here, out_at(c, src), o_s, o_r.at[src], sp=to)

    def out_local(c):
        return pltpu.make_async_copy(out_refs[c], wout_buf.at[c * depth : (c + 1) * depth, out_cols_of(me)], o_loc)

    def out_begin():
        for c in range(2):

            @pl.when(has_up)
            def _(c=c):
                out_hop(c, me, me + 1, True).start()

            @pl.when(has_down)
            def _(c=c):
                out_hop(c, me, me - 1, True).start()

            out_local(c).start()

    def out_relay(i):
        for src, to in ((me - i, me + 1), (me + i, me - 1)):

            @pl.when((src >= 0) & (src < n))
            def _(src=src, to=to):
                both = out_both(src)
                rdma(both, both, o_s, o_r.at[src], sp=src).wait_recv()
                for c in range(2):

                    @pl.when((to >= 0) & (to < n))
                    def _(c=c):
                        out_hop(c, src, to, False).start()

                    for d in range(1, n_grp):
                        here = out_at(c, src)
                        at = (d - 1) * n + src
                        rdma(here, here, oy_s, oy_r.at[at], grp=lax.rem(g + d, n_grp)).start()

    def out_arrive(src):
        for d in range(1, n_grp):
            drained(oy_r.at[(d - 1) * n + src], out_both(src))

    def w_pass(c, src):
        up, down = (fox_up, fox_down) if c in fox_arrays else (ret_up, ret_down)

        @pl.when((src < me) & (up < n))
        def _():
            w_on(c, src, up).start()

        @pl.when((src > me) & (down >= 0))
        def _():
            w_on(c, src, down).start()

    def w_relay(arrays, ks):
        for i in ks:
            for c in arrays:
                w_in(c, toward(i)).wait_recv()
                w_pass(c, toward(i))
                for d in range(1, n_grp):
                    w_side(c, toward(i), d).start()

    def w_arrive(arrays):
        for c in arrays:
            w_local(c).wait()
            drained(wy_r.at[local_at[c]], w_several(c, (n - 1) * (n_grp - 1)))

    def normalize(h):
        squares = jnp.zeros((rows, 1), jnp.float32)
        for i in range(n_tp):
            part = tok_buf[h, i].astype(jnp.float32)
            squares = squares + jnp.sum(part * part, axis=-1, keepdims=True)
        scale = lax.rsqrt(squares * (1.0 / (n_tp * feats)) + epsilon)
        at = pl.ds(pl.multiple_of(h * rows, rows), rows)
        for i in range(n_tp):
            part = tok_buf[h, i].astype(jnp.float32)
            cols = slice(i * feats, (i + 1) * feats)
            norm_buf[at, cols] = (part * scale * gain_buf[:, cols]).astype(jnp.bfloat16)

    far = list(range(2, n - 1))

    def tok_own():
        for d in range(1, half):
            tok_x_in(True, 0, d).wait_recv()
            for m in range(chunks):
                tok_c(True, m, d).start()

    def tok_swap(m):
        tok_z_in(m).wait_recv()
        for d in range(1, half):
            tok_x(False, m, d).start()
        tok_c(False, m, 0).start()

    def tok_last(m):
        for d in range(1, half):
            tok_x_in(False, m, d).wait_recv()
            tok_c(False, m, d).start()

    def tok_ready(own):
        if own:
            tok_local.wait()
        drained(tc_r.at[0 if own else 1], tok_buf.at[mine if own else other, :half])

    for copy in brought:
        copy.wait()

    @pl.when(is_fox)
    def _():
        w_relay((0, 1), [1, n - 1])

    @pl.when(is_ret)
    def _():
        w_local(4).start()

    tok_swap(0)
    tok_own()
    for m in range(1, chunks):
        tok_swap(m)

    @pl.when(is_fox)
    def _():
        w_relay((0, 1), far)
        w_relay((2,), [1, n - 1])

    @pl.when(is_ret)
    def _():
        w_relay(ret_arrays, [1])

    out_begin()
    tok_ready(True)
    normalize(mine)

    row_id = lax.broadcasted_iota(jnp.int32, (rows, rows), 0)
    col_id = lax.broadcasted_iota(jnp.int32, (rows, rows), 1)
    causal = col_id <= row_id

    def norm_rows(h):
        return norm_buf[pl.ds(pl.multiple_of(h * rows, rows), rows), :]

    def mix_copy(first):
        return rdma(
            mix_pair.at[other], mix_buf.at[:, first : first + depth], mix_s, mix_r, sp=partner
        )

    def mix_own(first):
        mix_buf[:, first : first + depth] = mix_pair[mine]

    def mix_in(first):
        here = mix_buf.at[:, first : first + depth]
        return rdma(here, here, mix_s, mix_r, sp=partner)

    def kv_copy(b, q):
        at = 2 * couple + b
        return rdma(kv_buf.at[at], kv_buf.at[at], kv_s.at[2 * q + b], kv_r.at[at], sp=fox_of(q))

    def kv_in(at):
        return rdma(kv_buf.at[at], kv_buf.at[at], kv_s.at[at], kv_r.at[at], sp=partner)

    def sum_copy(q):
        return rdma(sum_buf.at[couple], sum_buf.at[couple], sum_s.at[q], sum_r.at[couple], sp=ret_of(q))

    def sum_in(q):
        return rdma(sum_buf.at[q], sum_buf.at[q], sum_s.at[q], sum_r.at[q], sp=partner)

    def later(act):
        for q in range(1, couples):

            @pl.when(q > couple)
            def _(q=q):
                act(jnp.int32(q))

    def after_tokens():
        for m in range(chunks):
            tok_last(m)

    @pl.when(is_fox)
    def _():
        def project_kv(b):
            kv_buf[2 * couple + b] = jnp.dot(
                norm_rows(b), w_buf[:, :q_at], preferred_element_type=jnp.float32
            ).astype(jnp.bfloat16)
            later(lambda q: kv_copy(b, q).start())

        after_tokens()
        w_arrive((0, 1))
        project_kv(mine)
        tok_ready(False)
        normalize(other)
        project_kv(other)
        w_relay((2,), far)
        out_relay(1)
        w_arrive((2,))
        proj_buf[:, : fh * fd] = jnp.dot(
            norm_buf[...], w_buf[:, q_at:fox_wide], preferred_element_type=jnp.float32
        ).astype(jnp.bfloat16)

        def block_cols(at):
            return pl.ds(pl.multiple_of(at * rows, rows), rows)

        def rep_cols(x, wide):
            return jnp.concatenate([x] * (wide // lanes), axis=1)

        for b in range(2):
            for h in range(fh):
                own = jnp.where(row_id == col_id, gates_buf[h : h + 1, block_cols(2 * couple + b)], 0.0)
                gate_buf[h, b * rows : (b + 1) * rows] = jnp.broadcast_to(
                    jnp.sum(own, axis=1, keepdims=True), (rows, lanes)
                )

        def attend(at, top_row, first, offset):
            size_ = 2 * rows - top_row
            here = slice(top_row, 2 * rows)
            for h in range(fh):
                query = proj_buf[here, h * fd : (h + 1) * fd]
                k = kv_buf[at, :, h * fd : (h + 1) * fd]
                v = kv_buf[at, :, (fh + h) * fd : (fh + h + 1) * fd]
                logits = lax.dot_general(query, k, NT, preferred_element_type=jnp.float32) * fd ** (-0.5)
                logits = logits + rep_cols(gate_buf[h, here], rows) - gates_buf[h : h + 1, block_cols(at)]
                if offset is not None:
                    row = lax.broadcasted_iota(jnp.int32, (size_, rows), 0)
                    col = lax.broadcasted_iota(jnp.int32, (size_, rows), 1)
                    logits = jnp.where(col <= row, logits, -jnp.inf)
                top_new = jnp.broadcast_to(jnp.max(logits, axis=-1, keepdims=True), (size_, lanes))
                if not first:
                    top = top_buf[h, here]
                    top_new = jnp.maximum(top, top_new)
                p = jnp.exp(logits - rep_cols(top_new, rows))
                total = jnp.broadcast_to(jnp.sum(p, axis=-1, keepdims=True), (size_, lanes))
                weighted = jnp.dot(p.astype(jnp.bfloat16), v, preferred_element_type=jnp.float32)
                if not first:
                    rescale = jnp.exp(top - top_new)
                    total = total_buf[h, here] * rescale + total
                    weighted = weighted_buf[h, here] * rescale[:, :fd] + weighted
                top_buf[h, here] = top_new
                total_buf[h, here] = total
                weighted_buf[h, here] = weighted

        attend(2 * couple, 0, True, 0)
        attend(2 * couple + 1, rows, False, 0)

        def past(i, _):
            q = lax.div(i, 2)
            b = jnp.where(lax.rem(i, 2) == 0, fox_of(q) - 2 * q, 1 - (fox_of(q) - 2 * q))
            at = 2 * q + b
            kv_in(at).wait_recv()
            attend(at, 0, False, None)
            return 0

        lax.fori_loop(0, 2 * couple, past, 0)
        for b in range(2):
            at = slice(b * rows, (b + 1) * rows)
            for h in range(fh):
                mix_pair[b, :, h * fd : (h + 1) * fd] = (
                    weighted_buf[h, at] / total_buf[h, at, :fd]
                ).astype(jnp.bfloat16)
        mix_copy(depth).start()
        mix_own(depth)
        for k in range(2, n):
            out_relay(k)
        mix_in(0).wait_recv()
        mix_copy(depth).wait_send()
        later(lambda q: kv_copy(0, q).wait_send())
        later(lambda q: kv_copy(1, q).wait_send())

    @pl.when(is_ret)
    def _():
        distance = jnp.maximum(row_id - col_id, 0).astype(jnp.float32)
        key_scale = dk ** (-0.5)
        for h in range(hr):
            within_buf[h] = jnp.where(causal, jnp.exp(distance * decay_ref[h]) * key_scale, 0.0)
        after_tokens()
        w_relay(ret_arrays, far)
        tok_ready(False)
        normalize(other)
        w_relay(ret_arrays, [n - 1])
        out_relay(1)
        w_arrive(ret_arrays)
        proj_buf[:, :ret_wide] = jnp.dot(
            norm_buf[...], w_buf[:, :ret_wide], preferred_element_type=jnp.float32
        ).astype(jnp.bfloat16)
        rv_at, rq_at = starts[3][0], starts[4][0]
        lone = jnp.zeros((dk, vd), jnp.float32)

        def part(b, first, wide):
            return proj_buf[b * rows : (b + 1) * rows, first : first + wide]

        def split(x, axis):
            top = x.astype(jnp.bfloat16)
            rest = x - top.astype(jnp.float32)
            middle = rest.astype(jnp.bfloat16)
            low = (rest - middle.astype(jnp.float32)).astype(jnp.bfloat16)
            return jnp.concatenate((top, middle, low), axis=axis)

        def summary(b, h):
            past_end = rows - 1.0 - lax.broadcasted_iota(jnp.int32, (rows, dk), 0).astype(jnp.float32)
            keys = part(b, rq_at + (hr + h) * dk, dk).astype(jnp.float32) * key_scale
            parts = lax.dot_general(
                split(keys * jnp.exp(past_end * decay_ref[h]), 1),
                part(b, rv_at + h * vd, vd),
                TN,
                preferred_element_type=jnp.float32,
            )
            return parts[:dk] + parts[dk : 2 * dk] + parts[2 * dk :]

        early = [summary(0, h) for h in range(hr)]
        for h in range(hr):
            sum_buf[couple, h] = jnp.exp(lone + float(rows) * decay_ref[h]) * early[h] + summary(1, h)
        later(lambda q: sum_copy(q).start())

        for b in range(2):
            for h in range(hr):
                rk = part(b, rq_at + (hr + h) * dk, dk)
                rv = part(b, rv_at + h * vd, vd)
                scores = lax.dot_general(
                    part(b, rq_at + h * dk, dk), rk, NT, preferred_element_type=jnp.float32
                )
                raw_buf[b, h] = jnp.dot(
                    split(scores * within_buf[h], 1),
                    jnp.concatenate((rv, rv, rv), axis=0),
                    preferred_element_type=jnp.float32,
                )
        out_relay(2)

        offset = (couple * 2 * rows).astype(jnp.float32)

        def gather(q, entering):
            sum_in(q).wait_recv()
            gap = ((couple - 1 - q) * 2 * rows).astype(jnp.float32)
            return tuple(entering[h] + jnp.exp(lone + gap * decay_ref[h]) * sum_buf[q, h] for h in range(hr))

        entering = tuple(jnp.exp(lone + offset * decay_ref[h]) * state_buf[h] for h in range(hr))
        entering = lax.fori_loop(0, couple, gather, entering)
        second = tuple(jnp.exp(lone + float(rows) * decay_ref[h]) * entering[h] + early[h] for h in range(hr))
        since = lax.broadcasted_iota(jnp.int32, (rows, vd), 0).astype(jnp.float32) + 1.0

        for b in range(2):
            for h in range(hr):
                rq = part(b, rq_at + h * dk, dk)
                carried = jnp.dot(
                    jnp.concatenate((rq, rq, rq), axis=1),
                    split((entering, second)[b][h], 0),
                    preferred_element_type=jnp.float32,
                )
                raw = raw_buf[b, h] + carried * jnp.exp(since * decay_ref[h])
                center = raw - jnp.mean(raw, axis=-1, keepdims=True)
                variance = jnp.mean(center * center, axis=-1, keepdims=True)
                cols = slice(h * vd, (h + 1) * vd)
                mix_pair[b, :, cols] = (center * lax.rsqrt(variance + epsilon) * hgain_buf[:, cols]).astype(
                    jnp.bfloat16
                )
        mix_copy(0).start()
        mix_own(0)
        for k in range(3, n):
            out_relay(k)
        mix_in(depth).wait_recv()
        mix_copy(0).wait_send()
        later(lambda q: sum_copy(q).wait_send())

    block = rows // n_tp
    wide, pieces = out_cols, n

    def piece_cols(piece):
        return pl.ds(pl.multiple_of(piece * wide, wide), wide)

    def slot(at):
        return pl.ds(pl.multiple_of(at * block, block), block)

    def pair_copy(piece):
        cols = piece_cols(piece)
        return rdma(
            rs_send.at[1 - parity, :, cols],
            pair_buf.at[:, cols],
            pair_s,
            pair_r.at[piece],
            tp=t + 1 - 2 * parity,
        )

    def rs_copy(d, piece):
        to = lax.rem(pair + d, half)
        cols = piece_cols(piece)
        return rdma(
            pair_sum.at[slot(to), cols],
            far_ref.at[d - 1, :, cols],
            rs_s.at[d - 1],
            rs_r.at[d - 1],
            tp=2 * to + parity,
        )

    def project(piece):
        cols = piece_cols(piece)
        value = jnp.dot(mix_buf[...], wout_buf[:, cols], preferred_element_type=jnp.float32).astype(jnp.bfloat16)
        for b in range(n_tp):
            at = slice(b // 2 * block, (b // 2 + 1) * block)
            rs_send[b % 2, at, cols] = value[b * block : (b + 1) * block]
        pair_copy(piece).start()

    def reduce(piece):
        cols = piece_cols(piece)
        pair_copy(piece).wait_recv()
        both = rs_send[parity, :, cols].astype(jnp.float32) + pair_buf[:, cols].astype(jnp.float32)
        pair_sum[:, cols] = both.astype(jnp.bfloat16)
        for d in range(1, half):
            rs_copy(d, piece).start()

    def order(i):
        falling = jnp.where(i <= me, me - i, i)
        rising = jnp.where(i <= n - 1 - me, me + i, n - 1 - i)
        return jnp.where(lower, rising, falling)

    drained(o_loc, wout_buf.at[:, out_cols_of(me)])
    project(me)

    def turn(i, _):
        out_arrive(order(i))
        project(order(i))
        reduce(order(i - 1))
        return 0

    lax.fori_loop(1, n, turn, 0)
    reduce(order(jnp.int32(n - 1)))

    own = slot(pair)
    near_ref[...] = rs_send[parity, own, :].astype(jnp.float32) + pair_buf[own, :].astype(jnp.float32)

    slabs = rows * (2 * n_tp - 1) // (2 * n_tp)
    drained(t_s, tok_buf.at[:, :, :slabs])
    for p in range(n):

        @pl.when(me == p)
        def _(p=p):
            for arrays in (fox_arrays, ret_arrays):
                for c in arrays:
                    if sends_from(p, arrays):
                        drained(w_s.at[c], w_several(c, sends_from(p, arrays)))
            hops = 2 * ((p + 1 if p + 1 < n else 0) + (n - p if p else 0))
            drained(o_s, wout_buf.at[: hops * out_step // n])

    drained(oy_s, wout_buf.at[: 2 * (n - 1) * (n_grp - 1) * out_step // n])

    def sides(arrays):
        for c in arrays:
            drained(wy_s.at[local_at[c]], w_several(c, (n - 1) * (n_grp - 1)))

    @pl.when(is_fox)
    def _():
        sides(fox_arrays)

    @pl.when(is_ret)
    def _():
        sides(ret_arrays)

    drained(pair_s, pair_buf)
    for d in range(1, half):
        drained(rs_s.at[d - 1], pair_sum.at[:block])
    for d in range(1, half):
        drained(rs_r.at[d - 1], far_ref.at[d - 1])


def paired(n, n_tp, n_grp, inputs):
    tokens, ret_query_weight, ret_state, fox_gates = inputs[0], inputs[2], inputs[9], inputs[11]
    fox_query_weight, ret_out_weight = inputs[5], inputs[12]
    rows, feats = tokens.shape
    hr, dk, vd = ret_state.shape
    fh = fox_gates.shape[1]
    fd = fox_query_weight.shape[1] // fh
    shard = ret_query_weight.shape[0]
    depth, out_cols = ret_out_weight.shape
    columns = out_cols * n
    wide = max(3 * fh * fd, 2 * hr * dk + hr * vd)
    half = n_tp // 2
    block = rows // n_tp
    chunks = 4
    couples = n // 2
    dma = pltpu.SemaphoreType.DMA
    far = max(half - 1, 1)
    side = max(n_grp - 1, 1) * n
    vmem = pl.BlockSpec(memory_space=pltpu.VMEM)
    smem = pl.BlockSpec(memory_space=pltpu.SMEM)
    hbm = pl.BlockSpec(memory_space=pl.ANY)
    bf16, f32 = jnp.bfloat16, jnp.float32
    size = (n, n_tp, n_grp, hr, dk, vd, fh, fd, chunks)
    near, other = pl.pallas_call(
        functools.partial(pair_kernel, size),
        out_shape=(pltpu.VMEM((block, columns), f32), pltpu.VMEM((far, block, columns), bf16)),
        in_specs=[hbm] * 8 + [smem] + [hbm] * 5,
        out_specs=(vmem, vmem),
        scratch_shapes=[
            pltpu.VMEM((1, n_tp * feats), f32),
            pltpu.VMEM((2 * hr * dk, shard), bf16),
            pltpu.VMEM((hr, dk, vd), f32),
            pltpu.VMEM((1, hr * vd), f32),
            pltpu.VMEM((fh, n * rows), f32),
            pltpu.VMEM((fh, 2 * rows, lanes), f32),
            pltpu.VMEM((hr, rows, rows), f32),
            pltpu.VMEM((2, hr, rows, vd), f32),
            pltpu.VMEM((2, n_tp, rows, feats), bf16),
            pltpu.VMEM((shard, 2 * hr * dk), bf16),
            pltpu.VMEM((n * shard, wide), bf16),
            pltpu.VMEM((2 * depth, columns), bf16),
            pltpu.VMEM((2 * rows, n_tp * feats), bf16),
            pltpu.VMEM((2 * rows, wide), bf16),
            pltpu.VMEM((n, rows, 2 * fh * fd), bf16),
            pltpu.VMEM((couples, hr, dk, vd), f32),
            pltpu.VMEM((2, rows, depth), bf16),
            pltpu.VMEM((rows, 2 * depth), bf16),
            pltpu.VMEM((2, rows // 2, columns), bf16),
            pltpu.VMEM((rows // 2, columns), bf16),
            pltpu.VMEM((rows // 2, columns), bf16),
            pltpu.VMEM((fh, 2 * rows, lanes), f32),
            pltpu.VMEM((fh, 2 * rows, lanes), f32),
            pltpu.VMEM((fh, 2 * rows, fd), f32),
            dma((5,)),
            pltpu.SemaphoreType.REGULAR,
            pltpu.SemaphoreType.REGULAR,
            dma,
            dma((chunks,)),
            dma(((chunks + 1) * far,)),
            dma((2,)),
            dma,
            dma((5,)),
            dma((3 * n,)),
            dma((3,)),
            dma((3,)),
            dma((3,)),
            dma,
            dma((n,)),
            dma,
            dma((side,)),
            dma,
            dma((2 * couples,)),
            dma((n,)),
            dma((couples,)),
            dma((couples,)),
            dma,
            dma,
            dma,
            dma((n,)),
            dma((far,)),
            dma((far,)),
        ],
        compiler_params=pltpu.CompilerParams(
            collective_id=0, has_side_effects=True, vmem_limit_bytes=56 * 1024 * 1024
        ),
        name="layer",
    )(
        tokens,
        inputs[1][None, :],
        inputs[2].T,
        inputs[3].T,
        inputs[4],
        inputs[5],
        inputs[6],
        inputs[7],
        inputs[8],
        inputs[9],
        inputs[10][None, :],
        inputs[11].T,
        inputs[12],
        inputs[13],
    )
    for d in range(half - 1):
        near = near + other[d].astype(f32)
    return near.astype(bf16)


def pairs_fit(n, n_tp, n_grp, inputs):
    rows, feats = inputs[0].shape
    hr, dk, vd = inputs[9].shape
    shard = inputs[2].shape[0]
    depth, out_cols = inputs[12].shape
    wide = inputs[5].shape[1]
    full = all(w % lanes == 0 for w in (out_cols, wide, 2 * hr * dk, hr * vd, feats, depth, rows))
    even = n % 2 == 0 and n > 2 and n_tp % 2 == 0 and n_grp > 1
    tiles = rows % (32 * n_tp) == 0 and rows % 32 == 0 and shard % (16 * n_grp) == 0 and depth % (16 * n_grp * n) == 0 and vd <= lanes
    columns = n * out_cols
    held = 8 * rows * n_tp * feats + 2 * n * shard * 3 * wide + 4 * depth * columns + 4 * n * rows * wide + 6 * rows * columns
    return full and even and tiles and depth == wide == hr * vd and held < 40 * 1024 * 1024


def local(
    n,
    n_tp,
    n_grp,
    tokens,
    norm_gain,
    ret_query_weight,
    ret_key_weight,
    ret_value_weight,
    fox_query_weight,
    fox_key_weight,
    fox_value_weight,
    ret_decay,
    ret_state,
    head_norm_gain,
    fox_gates,
    ret_out_weight,
    fox_out_weight,
):
    inputs = (
        tokens,
        norm_gain,
        ret_query_weight,
        ret_key_weight,
        ret_value_weight,
        fox_query_weight,
        fox_key_weight,
        fox_value_weight,
        ret_decay,
        ret_state,
        head_norm_gain,
        fox_gates,
        ret_out_weight,
        fox_out_weight,
    )
    if pairs_fit(n, n_tp, n_grp, inputs):
        return paired(n, n_tp, n_grp, inputs)
    rows, feats = tokens.shape
    hr, dk, vd = ret_state.shape
    fh = fox_gates.shape[1]
    fd = fox_query_weight.shape[1] // fh
    shard = ret_query_weight.shape[0]
    width = 2 * hr * dk + hr * vd + 3 * fh * fd
    depth, out_cols = ret_out_weight.shape
    columns = out_cols * n
    direct = out_cols % 128 == 0
    if not direct:
        ret_out_weight, fox_out_weight = ret_out_weight.T, fox_out_weight.T
    dma = pltpu.SemaphoreType.DMA

    def gather_sems(arrays):
        side = max(n_grp - 1, 1) * n * arrays
        return [
            dma((n * arrays,)),
            dma((n * arrays,)),
            dma((n * arrays,)),
            dma((side,)),
            dma((side,)),
            dma((arrays,)),
        ]

    vmem = pl.BlockSpec(memory_space=pltpu.VMEM)
    smem = pl.BlockSpec(memory_space=pltpu.SMEM)
    hbm = pl.BlockSpec(memory_space=pl.ANY)
    size = (n, n_tp, n_grp, hr, dk, vd, fh, fd, direct)
    block = rows // n_tp
    peers = max(n_tp - 1, 1)
    far = max(n_tp // 2 - 1, 1)
    pieces = n if direct else 1
    return pl.pallas_call(
        functools.partial(kernel, size),
        out_shape=jax.ShapeDtypeStruct((block, columns), jnp.bfloat16),
        in_specs=[hbm, vmem, vmem, vmem, hbm, hbm, hbm, hbm, smem, vmem, vmem, vmem, hbm, hbm],
        out_specs=vmem,
        scratch_shapes=[
            pltpu.VMEM((n_tp, rows, feats), jnp.bfloat16),
            pltpu.VMEM((shard, 2 * hr * dk), jnp.bfloat16),
            pltpu.VMEM((n * shard, width), jnp.bfloat16),
            pltpu.VMEM((2 * depth, columns) if direct else (columns, 2 * depth), jnp.bfloat16),
            pltpu.VMEM((rows, n_tp * feats), jnp.bfloat16),
            pltpu.VMEM((rows, width - 2 * fh * fd), jnp.bfloat16),
            pltpu.VMEM((n, rows, 2 * fh * fd), jnp.bfloat16),
            pltpu.VMEM((n, hr, dk, vd), jnp.float32),
            pltpu.VMEM((rows, 2 * depth), jnp.bfloat16),
            pltpu.VMEM((2, rows // 2, columns), jnp.bfloat16),
            pltpu.VMEM((rows // 2, columns), jnp.bfloat16),
            pltpu.VMEM((rows // 2, columns), jnp.bfloat16),
            pltpu.VMEM((far, block, columns), jnp.bfloat16),
            pltpu.VMEM((fh, rows, 1), jnp.float32),
            pltpu.VMEM((fh, rows, 1), jnp.float32),
            pltpu.VMEM((fh, rows, fd), jnp.float32),
            dma((peers,)),
            dma((peers,)),
            dma,
            dma((n,)),
            dma((n,)),
            dma((n,)),
            dma((n,)),
            dma((pieces,)),
            dma((pieces,)),
            dma((far * pieces,)),
            dma((far * pieces,)),
        ]
        + gather_sems(2)
        + gather_sems(3)
        + gather_sems(2),
        compiler_params=pltpu.CompilerParams(
            collective_id=0, has_side_effects=True, vmem_limit_bytes=56 * 1024 * 1024
        ),
        name="layer",
    )(
        tokens,
        norm_gain[None, :],
        ret_query_weight.T,
        ret_key_weight.T,
        ret_value_weight,
        fox_query_weight,
        fox_key_weight,
        fox_value_weight,
        ret_decay,
        ret_state,
        head_norm_gain[None, :],
        fox_gates.T,
        ret_out_weight,
        fox_out_weight,
    )


def solution(mesh):
    placed = (
        P(("grp", "sp"), "tp"),
        P(),
        P("sp", "tp"),
        P("sp", "tp"),
        P("sp", "tp"),
        P("sp", "tp"),
        P("sp", "tp"),
        P("sp", "tp"),
        P("tp"),
        P(("grp", "tp"), None, None),
        P("tp"),
        P("grp", "tp"),
        P("tp", "sp"),
        P("tp", "sp"),
    )
    body = functools.partial(local, mesh.shape["sp"], mesh.shape["tp"], mesh.shape["grp"])
    return jax.shard_map(
        body, mesh=mesh, in_specs=placed, out_specs=P(("grp", "sp", "tp"), None), check_vma=False
    )
```

```python
import functools

import jax
import jax.numpy as jnp
from jax import lax
from jax.experimental import pallas as pl
from jax.experimental.pallas import tpu as pltpu
from jax.sharding import PartitionSpec as P

epsilon = 1e-06
lanes = 128
highest = lax.Precision.HIGHEST
NT = (((1,), (1,)), ((), ()))
TN = (((0,), (0,)), ((), ()))


def rdma(src, dst, send_sem, recv_sem, **target):
    return pltpu.make_async_remote_copy(
        src_ref=src,
        dst_ref=dst,
        send_sem=send_sem,
        recv_sem=recv_sem,
        device_id=target,
        device_id_type=pl.DeviceIdType.MESH,
    )


class LineGather:
    def __init__(self, owns, place, sems, n, n_grp, me, g):
        self.owns, self.place, self.n, self.n_grp, self.me, self.g = owns, place, n, n_grp, me, g
        self.up, self.down, self.zr, self.ys, self.yr, self.loc = sems
        self.arrays = len(owns)
        self.rows = owns[0].shape[0]
        self.step = self.rows // n_grp

    def piece(self, part, src, c):
        return self.place(src, c, part * self.step, self.step)

    def own_piece(self, c):
        return self.owns[c].at[pl.ds(pl.multiple_of(self.g * self.step, self.step), self.step)]

    def hop(self, sems, to, src, c, first=False):
        here = self.own_piece(c) if first else self.piece(self.g, src, c)
        at = src * self.arrays + c
        return rdma(here, self.piece(self.g, src, c), sems.at[at], self.zr.at[at], sp=to)

    def side(self, d, src, c):
        at = ((d - 1) * self.n + src) * self.arrays + c
        here = self.piece(self.g, src, c)
        return rdma(here, here, self.ys.at[at], self.yr.at[at], grp=lax.rem(self.g + d, self.n_grp))

    def side_in(self, d, src, c):
        at = ((d - 1) * self.n + src) * self.arrays + c
        part = lax.rem(self.g + self.n_grp - d, self.n_grp)
        here = self.piece(part, src, c)
        return rdma(here, here, self.ys.at[at], self.yr.at[at], grp=part)

    def local(self, c):
        return pltpu.make_async_copy(self.owns[c], self.place(self.me, c, 0, self.rows), self.loc.at[c])

    def start(self):
        me, n = self.me, self.n
        for c in range(self.arrays):

            @pl.when(me + 1 < n)
            def _():
                self.hop(self.up, me + 1, me, c, True).start()

            @pl.when(me >= 1)
            def _():
                self.hop(self.down, me - 1, me, c, True).start()

        for c in range(self.arrays):
            self.local(c).start()

    def relay(self, k):
        me, n = self.me, self.n
        for c in range(self.arrays):
            for src, sems, to in ((me - k, self.up, me + 1), (me + k, self.down, me - 1)):

                @pl.when((src >= 0) & (src < n))
                def _(src=src, sems=sems, to=to):
                    self.hop(sems, me, src, c).wait_recv()

                    @pl.when((to >= 0) & (to < n))
                    def _():
                        self.hop(sems, to, src, c).start()

                    for d in range(1, self.n_grp):
                        self.side(d, src, c).start()

    def arrive_shard(self, src, arrays):
        for c in arrays:
            for d in range(1, self.n_grp):
                self.side_in(d, src, c).wait_recv()

    def arrive(self, arrays):
        for c in arrays:
            self.local(c).wait()

        def step(k, _):
            self.arrive_shard(lax.rem(self.me + k, self.n), arrays)
            return 0

        lax.fori_loop(1, self.n, step, 0)

    def finish(self):
        me, n = self.me, self.n

        def step(src, _):
            for c in range(self.arrays):

                @pl.when((src <= me) & (me + 1 < n))
                def _():
                    self.hop(self.up, me, src, c).wait_send()

                @pl.when((src >= me) & (me >= 1))
                def _():
                    self.hop(self.down, me, src, c).wait_send()

                @pl.when(src != me)
                def _():
                    for d in range(1, self.n_grp):
                        self.side(d, src, c).wait_send()

            return 0

        lax.fori_loop(0, n, step, 0)


def kernel(
    size,
    tok_ref,
    gain_ref,
    wq_ref,
    wk_ref,
    wrv_ref,
    wfq_ref,
    wfk_ref,
    wfv_ref,
    decay_ref,
    state_ref,
    hgain_ref,
    gates_ref,
    ret_out_ref,
    fox_out_ref,
    out_ref,
    tok_buf,
    qk_own,
    w_buf,
    wout_buf,
    norm_buf,
    proj_buf,
    kv_buf,
    sum_buf,
    mix_buf,
    rs_send,
    pair_buf,
    pair_sum,
    rs_buf,
    top_buf,
    total_buf,
    weighted_buf,
    tok_s,
    tok_r,
    tok_loc,
    kv_s,
    kv_r,
    sum_s,
    sum_r,
    pair_s,
    pair_r,
    rs_s,
    rs_r,
    *gather_sems,
):
    n, n_tp, n_grp, hr, dk, vd, fh, fd, direct = size
    me, t, g = lax.axis_index("sp"), lax.axis_index("tp"), lax.axis_index("grp")
    rows, feats = tok_ref.shape
    owns = [wfk_ref, wfv_ref, wfq_ref, wrv_ref, qk_own]
    early = 2
    starts = [0]
    for own in owns:
        starts.append(starts[-1] + own.shape[1])
    shard = qk_own.shape[0]

    def weight_place(src, c, first, count):
        start = pl.multiple_of(src * shard + first, count)
        return w_buf.at[pl.ds(start, count), starts[c] : starts[c + 1]]

    depth = mix_buf.shape[1] // 2
    out_cols = ret_out_ref.shape[1] if direct else ret_out_ref.shape[0]

    def out_place(src, c, first, count):
        if direct:
            start = pl.multiple_of(c * depth + first, count)
            return wout_buf.at[pl.ds(start, count), pl.ds(pl.multiple_of(src * out_cols, out_cols), out_cols)]
        start = pl.multiple_of(src * out_cols + first, count)
        return wout_buf.at[pl.ds(start, count), c * depth : (c + 1) * depth]

    def late_place(src, c, first, count):
        return weight_place(src, c + early, first, count)

    firsts = LineGather(owns[:early], weight_place, gather_sems[:6], n, n_grp, me, g)
    lasts = LineGather(owns[early:], late_place, gather_sems[6:12], n, n_grp, me, g)
    outs = LineGather([ret_out_ref, fox_out_ref], out_place, gather_sems[12:], n, n_grp, me, g)

    barrier = pltpu.get_barrier_semaphore()

    def greet(**target):
        pl.semaphore_signal(barrier, inc=1, device_id=target, device_id_type=pl.DeviceIdType.MESH)

    has_up, has_down = me + 1 < n, me >= 1
    for d in range(1, n_tp):
        greet(tp=lax.rem(t + d, n_tp))
    for d in range(1, n_grp):
        greet(grp=lax.rem(g + d, n_grp))

    @pl.when(has_up)
    def _():
        greet(sp=me + 1)

    @pl.when(has_down)
    def _():
        greet(sp=me - 1)

    turned = jnp.concatenate((wq_ref[...], wk_ref[...]), axis=0).astype(jnp.float32)
    qk_own[...] = turned.T.astype(jnp.bfloat16)

    count = n_tp - 1 + n_grp - 1 + has_up.astype(jnp.int32) + has_down.astype(jnp.int32)
    pl.semaphore_wait(barrier, count)

    def tok_copy(d):
        return rdma(tok_ref, tok_buf.at[t], tok_s.at[d - 1], tok_r.at[d - 1], tp=lax.rem(t + d, n_tp))

    def tok_in(d):
        src = lax.rem(t + n_tp - d, n_tp)
        return rdma(tok_ref, tok_buf.at[src], tok_s.at[d - 1], tok_r.at[d - 1], tp=src)

    firsts.start()
    lasts.start()
    tok_local = pltpu.make_async_copy(tok_ref, tok_buf.at[t], tok_loc)
    for d in range(1, n_tp):
        tok_copy(d).start()
    tok_local.start()

    def first_step(k, _):
        firsts.relay(k)

        lasts.relay(k)
        return 0

    lax.fori_loop(1, n, first_step, 0)
    outs.start()

    tok_local.wait()
    for d in range(1, n_tp):
        tok_in(d).wait_recv()
    squares = jnp.zeros((rows, 1), jnp.float32)
    for i in range(n_tp):
        part = tok_buf[i].astype(jnp.float32)
        squares = squares + jnp.sum(part * part, axis=-1, keepdims=True)
    scale = lax.rsqrt(squares * (1.0 / (n_tp * feats)) + epsilon)
    for i in range(n_tp):
        part = tok_buf[i].astype(jnp.float32)
        cols = slice(i * feats, (i + 1) * feats)
        norm_buf[:, cols] = (part * scale * gain_ref[:, cols]).astype(jnp.bfloat16)

    def kv_copy(src):
        return rdma(kv_buf.at[src], kv_buf.at[src], kv_s.at[src], kv_r.at[src], sp=jnp.minimum(me + 1, n - 1))

    def sum_copy(src):
        return rdma(sum_buf.at[src], sum_buf.at[src], sum_s.at[src], sum_r.at[src], sp=jnp.minimum(me + 1, n - 1))

    firsts.arrive((0, 1))
    kv_buf[me] = jnp.dot(
        norm_buf[...], w_buf[:, : starts[2]], preferred_element_type=jnp.float32
    ).astype(jnp.bfloat16)

    def kv_forward(k):
        src = me - k

        @pl.when(src >= 0)
        def _():
            kv_copy(src).wait_recv()

            @pl.when(has_up)
            def _():
                kv_copy(src).start()

    @pl.when(has_up)
    def _():
        kv_copy(me).start()

    outs.relay(1)
    lasts.arrive((0, 1, 2))
    proj_buf[...] = jnp.dot(
        norm_buf[...], w_buf[:, starts[2] :], preferred_element_type=jnp.float32
    ).astype(jnp.bfloat16)
    rv_at, rq_at = starts[3] - starts[2], starts[4] - starts[2]

    key_scale = dk ** (-0.5)
    position = lax.broadcasted_iota(jnp.int32, (rows, 1), 0).astype(jnp.float32)
    rq, rk, rv = [], [], []
    for h in range(hr):
        rq.append(proj_buf[:, rq_at + h * dk : rq_at + (h + 1) * dk])
        rk.append(proj_buf[:, rq_at + (hr + h) * dk : rq_at + (hr + h + 1) * dk])
        rv.append(proj_buf[:, rv_at + h * vd : rv_at + (h + 1) * vd])
        keys = rk[h].astype(jnp.float32) * key_scale
        trailing = jnp.exp((rows - 1.0 - position) * decay_ref[h])
        sum_buf[me, h] = lax.dot_general(
            keys * trailing, rv[h].astype(jnp.float32), TN, precision=highest, preferred_element_type=jnp.float32
        )

    @pl.when(has_up)
    def _():
        sum_copy(me).start()

    row_id = lax.broadcasted_iota(jnp.int32, (rows, rows), 0)
    col_id = lax.broadcasted_iota(jnp.int32, (rows, rows), 1)
    causal = col_id <= row_id
    own_cols = pl.ds(pl.multiple_of(me * rows, rows), rows)
    own_gates = [
        jnp.sum(jnp.where(row_id == col_id, gates_ref[h : h + 1, own_cols], 0.0), axis=1, keepdims=True)
        for h in range(fh)
    ]

    def attend(src, diagonal):
        key_cols = pl.ds(pl.multiple_of(src * rows, rows), rows)
        for h in range(fh):
            query = proj_buf[:, h * fd : (h + 1) * fd]
            k = kv_buf[src, :, h * fd : (h + 1) * fd]
            v = kv_buf[src, :, (fh + h) * fd : (fh + h + 1) * fd]
            logits = lax.dot_general(query, k, NT, preferred_element_type=jnp.float32) * fd ** (-0.5)
            logits = logits + own_gates[h] - gates_ref[h : h + 1, key_cols]
            if diagonal:
                logits = jnp.where(causal, logits, -jnp.inf)
            top_new = jnp.max(logits, axis=-1, keepdims=True)
            if not diagonal:
                top = top_buf[h]
                top_new = jnp.maximum(top, top_new)
            p = jnp.exp(logits - top_new)
            total = jnp.sum(p, axis=-1, keepdims=True)
            weighted = jnp.dot(p.astype(jnp.bfloat16), v, preferred_element_type=jnp.float32)
            if not diagonal:
                rescale = jnp.exp(top - top_new)
                total = total_buf[h] * rescale + total
                weighted = weighted_buf[h] * rescale + weighted
            top_buf[h] = top_new
            total_buf[h] = total
            weighted_buf[h] = weighted

    def forward(k):
        src = me - k

        @pl.when(src >= 0)
        def _():
            sum_copy(src).wait_recv()

            @pl.when(has_up)
            def _():
                sum_copy(src).start()

    attend(me, True)

    offset = (me * rows).astype(jnp.float32)
    lone = jnp.zeros((dk, vd), jnp.float32)

    def step(k, entering):
        src = me - k
        kv_forward(k)
        forward(k)

        @pl.when(k + 1 < n)
        def _():
            outs.relay(k + 1)


        @pl.when(src >= 0)
        def _():
            attend(src, False)

        gap = ((k - 1) * rows).astype(jnp.float32)
        there = jnp.maximum(src, 0)
        return tuple(
            entering[h]
            + jnp.where(src >= 0, jnp.exp(lone + gap * decay_ref[h]) * sum_buf[there, h], 0.0)
            for h in range(hr)
        )

    entering = tuple(jnp.exp(lone + offset * decay_ref[h]) * state_ref[h] for h in range(hr))
    entering = lax.fori_loop(1, n, step, entering)

    distance = jnp.maximum(row_id - col_id, 0).astype(jnp.float32)
    for h in range(hr):
        scores = lax.dot_general(rq[h], rk[h], NT, preferred_element_type=jnp.float32) * key_scale
        scores = jnp.where(causal, scores * jnp.exp(distance * decay_ref[h]), 0.0)
        inner = jnp.dot(scores, rv[h].astype(jnp.float32), precision=highest, preferred_element_type=jnp.float32)
        leading = jnp.exp((position + 1.0) * decay_ref[h])
        carried = jnp.dot(
            rq[h].astype(jnp.float32), entering[h], precision=highest, preferred_element_type=jnp.float32
        )
        raw = inner + carried * leading
        center = raw - jnp.mean(raw, axis=-1, keepdims=True)
        variance = jnp.mean(center * center, axis=-1, keepdims=True)
        cols = slice(h * vd, (h + 1) * vd)
        mix_buf[:, cols] = (center * lax.rsqrt(variance + epsilon) * hgain_ref[:, cols]).astype(jnp.bfloat16)
    for h in range(fh):
        cols = slice(hr * vd + h * fd, hr * vd + (h + 1) * fd)
        mix_buf[:, cols] = (weighted_buf[h] / total_buf[h]).astype(jnp.bfloat16)

    block = rows // n_tp
    columns = pair_buf.shape[1]
    wide = out_cols if direct else columns
    pieces = columns // wide
    half = n_tp // 2
    parity, pair = lax.rem(t, 2), lax.div(t, 2)

    def piece_cols(piece):
        return pl.ds(pl.multiple_of(piece * wide, wide), wide)

    def slot(at):
        return pl.ds(pl.multiple_of(at * block, block), block)

    def pair_copy(piece):
        cols = piece_cols(piece)
        return rdma(
            rs_send.at[1 - parity, :, cols],
            pair_buf.at[:, cols],
            pair_s.at[piece],
            pair_r.at[piece],
            tp=t + 1 - 2 * parity,
        )

    def rs_copy(d, piece):
        to = lax.rem(pair + d, half)
        cols = piece_cols(piece)
        at = (d - 1) * pieces + piece
        return rdma(
            pair_sum.at[slot(to), cols], rs_buf.at[d - 1, :, cols], rs_s.at[at], rs_r.at[at], tp=2 * to + parity
        )

    def project(piece):
        cols = piece_cols(piece)
        if direct:
            value = jnp.dot(mix_buf[...], wout_buf[:, cols], preferred_element_type=jnp.float32)
        else:
            value = lax.dot_general(mix_buf[...], wout_buf[...], NT, preferred_element_type=jnp.float32)
        value = value.astype(jnp.bfloat16)
        for b in range(n_tp):
            at = slice(b // 2 * block, (b // 2 + 1) * block)
            rs_send[b % 2, at, cols] = value[b * block : (b + 1) * block]
        pair_copy(piece).start()

    def reduce(piece):
        cols = piece_cols(piece)
        pair_copy(piece).wait_recv()
        both = rs_send[parity, :, cols].astype(jnp.float32) + pair_buf[:, cols].astype(jnp.float32)
        pair_sum[:, cols] = both.astype(jnp.bfloat16)
        for d in range(1, half):
            rs_copy(d, piece).start()

    def order(i):
        falling = jnp.where(i <= me, me - i, i)
        rising = jnp.where(i <= n - 1 - me, me + i, n - 1 - i)
        return jnp.where(2 * me >= n, falling, rising)

    if direct:
        for c in range(2):
            outs.local(c).wait()
        project(me)

        def out_step(i, _):
            outs.arrive_shard(order(i), (0, 1))
            project(order(i))
            reduce(order(i - 1))
            return 0

        lax.fori_loop(1, n, out_step, 0)
        reduce(order(jnp.int32(n - 1)))
    else:
        outs.arrive((0, 1))
        project(0)
        reduce(0)

    own = slot(pair)
    summed = rs_send[parity, own, :].astype(jnp.float32) + pair_buf[own, :].astype(jnp.float32)
    for d in range(1, half):
        for piece in range(pieces):
            rs_copy(d, piece).wait_recv()
        summed = summed + rs_buf[d - 1].astype(jnp.float32)
    out_ref[...] = summed.astype(jnp.bfloat16)

    for d in range(1, n_tp):
        tok_copy(d).wait_send()
    for piece in range(pieces):
        pair_copy(piece).wait_send()
        for d in range(1, half):
            rs_copy(d, piece).wait_send()
    firsts.finish()
    lasts.finish()
    outs.finish()

    @pl.when(has_up)
    def _():
        def step(src, _):
            kv_copy(src).wait_send()
            sum_copy(src).wait_send()
            return 0

        lax.fori_loop(0, me + 1, step, 0)


def pair_kernel(
    size,
    tok_ref,
    gain_ref,
    wq_ref,
    wk_ref,
    wrv_ref,
    wfq_ref,
    wfk_ref,
    wfv_ref,
    decay_ref,
    state_ref,
    hgain_ref,
    gates_ref,
    ret_out_ref,
    fox_out_ref,
    near_ref,
    far_ref,
    gain_buf,
    wqk_buf,
    state_buf,
    hgain_buf,
    gates_buf,
    gate_buf,
    within_buf,
    raw_buf,
    sums_buf,
    tok_buf,
    qk_own,
    w_buf,
    wout_buf,
    norm_buf,
    proj_buf,
    kv_buf,
    sum_buf,
    mix_pair,
    mix_buf,
    rs_send,
    pair_buf,
    pair_sum,
    top_buf,
    total_buf,
    weighted_buf,
    in_sem,
    above_sem,
    below_sem,
    t_s,
    tz_r,
    tx_r,
    tc_r,
    t_loc,
    w_s,
    w_r,
    wy_s,
    wy_r,
    w_loc,
    o_s,
    o_r,
    oy_s,
    oy_r,
    o_loc,
    kv_s,
    kv_r,
    sum_s,
    sum_r,
    mix_s,
    mix_r,
    pair_s,
    pair_r,
    rs_s,
    rs_r,
):
    n, n_tp, n_grp, hr, dk, vd, fh, fd, chunks = size
    me, t, g = lax.axis_index("sp"), lax.axis_index("tp"), lax.axis_index("grp")
    rows, feats = tok_ref.shape
    shard = qk_own.shape[0]
    couples = n // 2
    couple, mine = lax.div(me, 2), lax.rem(me, 2)
    other = 1 - mine
    partner = me + 1 - 2 * mine
    fox_mine = 1 - lax.rem(couple, 2)
    is_fox = mine == fox_mine
    is_ret = mine != fox_mine
    lower = 2 * me < n
    half = n_tp // 2
    parity, pair = lax.rem(t, 2), lax.div(t, 2)

    def fox_of(q):
        return 2 * q + 1 - lax.rem(q, 2)

    def ret_of(q):
        return 2 * q + lax.rem(q, 2)

    def toward(k):
        return lax.rem(jnp.where(lower, me + k, me + n - k), n)

    barrier = pltpu.get_barrier_semaphore()

    def greet(**target):
        pl.semaphore_signal(barrier, inc=1, device_id=target, device_id_type=pl.DeviceIdType.MESH)

    greet(tp=2 * pair + 1 - parity)
    for d in range(1, half):
        greet(tp=2 * lax.rem(pair + d, half) + parity)
    for d in range(1, n_grp):
        greet(grp=lax.rem(g + d, n_grp))
    has_up, has_down = me + 1 < n, me >= 1

    @pl.when(has_up)
    def _():
        greet(sp=me + 1)

    @pl.when(has_down)
    def _():
        greet(sp=me - 1)

    def drained(sem, ref):
        pltpu.make_async_copy(ref, ref, sem).wait()

    width = hr * dk
    pltpu.make_async_copy(wq_ref, wqk_buf.at[:width], in_sem.at[0]).start()
    pltpu.make_async_copy(wk_ref, wqk_buf.at[width:], in_sem.at[0]).start()
    brought = [
        pltpu.make_async_copy(src, dst, in_sem.at[i + 1])
        for i, (src, dst) in enumerate(
            ((gain_ref, gain_buf), (state_ref, state_buf), (hgain_ref, hgain_buf), (gates_ref, gates_buf))
        )
    ]
    for copy in brought:
        copy.start()

    pl.semaphore_wait(barrier, half + n_grp - 1 + has_up.astype(jnp.int32) + has_down.astype(jnp.int32))

    def tell(sem, to):
        pl.semaphore_signal(sem, inc=1, device_id={"sp": to}, device_id_type=pl.DeviceIdType.MESH)

    @pl.when(has_up & has_down)
    def _():
        tell(above_sem, me - 1)
        tell(below_sem, me + 1)

    def meet_far():
        def from_above(i, _):
            pl.semaphore_wait(above_sem, 1)

            @pl.when(has_down)
            def _():
                tell(above_sem, me - 1)

            return 0

        def from_below(i, _):
            pl.semaphore_wait(below_sem, 1)

            @pl.when(has_up)
            def _():
                tell(below_sem, me + 1)

            return 0

        lax.fori_loop(0, jnp.maximum(n - 2 - me, 0), from_above, 0)
        lax.fori_loop(0, jnp.maximum(me - 1, 0), from_below, 0)

    slab = rows // chunks

    def own_tok(m):
        return tok_ref.at[pl.ds(m * slab, slab)]

    def tok_at(h, m, src):
        return tok_buf.at[h, src, pl.ds(m * slab, slab)]

    def tok_z(m):
        return rdma(own_tok(m), tok_at(mine, m, t), t_s, tz_r.at[m], sp=partner)

    def tok_z_in(m):
        here = tok_at(other, m, t)
        return rdma(here, here, t_s, tz_r.at[m], sp=partner)

    def x_sem(own, m, d):
        return (0 if own else 1 + m) * max(half - 1, 1) + d - 1

    def tok_x(own, m, d):
        h = mine if own else other
        src = own_tok(m) if own else tok_at(h, m, t)
        return rdma(src, tok_at(h, m, t), t_s, tx_r.at[x_sem(own, m, d)], tp=2 * lax.rem(pair + d, half) + parity)

    def tok_x_in(own, m, d):
        src = 2 * lax.rem(pair + half - d, half) + parity
        here = tok_buf.at[mine, src] if own else tok_at(other, m, src)
        return rdma(here, here, t_s, tx_r.at[x_sem(own, m, d)], tp=src)

    def tok_c(own, m, d):
        h = mine if own else other
        src = 2 * lax.rem(pair + half - d, half) + parity
        there = tok_at(h, m, src)
        here = own_tok(m) if own and d == 0 else there
        return rdma(here, there, t_s, tc_r.at[0 if own else 1], tp=2 * pair + 1 - parity)

    tok_local = pltpu.make_async_copy(tok_ref, tok_buf.at[mine, t], t_loc)

    for d in range(1, half):
        for m in range(chunks):
            tok_x(True, m, d).start()

    owns = [wfk_ref, wfv_ref, wfq_ref, wrv_ref, qk_own]
    fox_arrays, ret_arrays = (0, 1, 2), (3, 4)
    starts = {}
    for group in (fox_arrays, ret_arrays):
        at = 0
        for c in group:
            starts[c] = (at, at + owns[c].shape[1])
            at = starts[c][1]
    fox_wide, ret_wide = starts[2][1], starts[4][1]
    q_at = starts[2][0]
    step = shard // n_grp
    count = len(owns)

    def w_at(c, src, part):
        start = pl.multiple_of(src * shard + part * step, step)
        return w_buf.at[pl.ds(start, step), starts[c][0] : starts[c][1]]

    far = list(range(2, n - 1))
    local_at = {c: c - group[0] for group in (fox_arrays, ret_arrays) for c in group}

    def w_recv(c, src):
        return w_r.at[src * len(fox_arrays) + local_at[c]]

    def w_send(c, to):
        here = owns[c].at[pl.ds(pl.multiple_of(g * step, step), step)]
        return rdma(here, w_at(c, me, g), w_s.at[c], w_recv(c, me), sp=to)

    def w_on(c, src, to):
        here = w_at(c, src, g)
        return rdma(here, here, w_s.at[c], w_recv(c, src), sp=to)

    def w_in(c, src):
        here = w_at(c, src, g)
        return rdma(here, here, w_s.at[c], w_recv(c, src), sp=src)

    def w_side(c, k, d):
        here = w_at(c, toward(k), g)
        return rdma(here, here, wy_s.at[local_at[c]], wy_r.at[wy_at(c, k in late_of(c))], grp=lax.rem(g + d, n_grp))

    def late_of(c):
        return far if c in fox_arrays else [n - 1]

    def wy_at(c, late):
        return local_at[c] + (len(fox_arrays) if late and c not in (0, 1) else 0)

    def w_late(c):
        drained(wy_r.at[wy_at(c, True)], w_several(c, len(late_of(c)) * (n_grp - 1)))

    def w_early(c):
        w_local(c).wait()
        drained(wy_r.at[wy_at(c, False)], w_several(c, (n - 1 - len(late_of(c))) * (n_grp - 1)))

    def w_several(c, pieces):
        return w_buf.at[: pieces * step, starts[c][0] : starts[c][1]]

    def w_local(c):
        start = pl.multiple_of(me * shard, shard)
        return pltpu.make_async_copy(
            owns[c], w_buf.at[pl.ds(start, shard), starts[c][0] : starts[c][1]], w_loc.at[local_at[c]]
        )

    fox_up = jnp.where(is_ret & (mine == 0), partner, fox_of(couple + 1))
    fox_down = jnp.where(is_ret & (mine == 1), partner, jnp.where(couple >= 1, fox_of(jnp.maximum(couple - 1, 0)), -1))
    ret_up = jnp.where(is_fox & (mine == 0), partner, ret_of(couple + 1))
    ret_down = jnp.where(is_fox & (mine == 1), partner, jnp.where(couple >= 1, ret_of(jnp.maximum(couple - 1, 0)), -1))

    def send_weights(arrays):
        up, down = (fox_up, fox_down) if arrays[0] in fox_arrays else (ret_up, ret_down)
        for c in arrays:

            @pl.when(up < n)
            def _(c=c):
                w_send(c, up).start()

            @pl.when(down >= 0)
            def _(c=c):
                w_send(c, down).start()

    def sends_from(p, arrays):
        q, b = p // 2, p % 2
        plane = (lambda i: 2 * i + 1 - i % 2) if arrays[0] in fox_arrays else (lambda i: 2 * i + i % 2)
        uses = plane(q) == p
        up = p + 1 if not uses and b == 0 else plane(q + 1)
        down = p - 1 if not uses and b == 1 else (plane(q - 1) if q else -1)
        passes = ((p if up < n else 0) + (n - 1 - p if down >= 0 else 0)) if uses else 0
        return (up < n) + (down >= 0) + passes

    def swap_tokens():
        for m in range(chunks):
            tok_z(m).start()

    send_weights((0, 1))
    for m in range(chunks):
        tok_c(True, m, 0).start()

    swap_tokens()
    meet_far()
    send_weights((3,))
    drained(in_sem.at[0], wqk_buf)
    qk_own[...] = wqk_buf[...].astype(jnp.float32).T.astype(jnp.bfloat16)
    send_weights((4,))

    send_weights((2,))
    tok_local.start()

    @pl.when(is_fox)
    def _():
        for c in fox_arrays:
            w_local(c).start()

    @pl.when(is_ret)
    def _():
        for c in ret_arrays:
            w_local(c).start()

    depth = mix_buf.shape[1] // 2
    out_cols = ret_out_ref.shape[1]

    out_step = depth // n_grp
    out_refs = [ret_out_ref, fox_out_ref]

    def out_cols_of(src):
        return pl.ds(pl.multiple_of(src * out_cols, out_cols), out_cols)

    def out_at(c, src):
        return wout_buf.at[pl.ds(pl.multiple_of(c * depth + g * out_step, out_step), out_step), out_cols_of(src)]

    def out_both(src):
        return wout_buf.at[: 2 * out_step, out_cols_of(src)]

    def out_hop(c, src, to, first):
        here = out_refs[c].at[pl.ds(pl.multiple_of(g * out_step, out_step), out_step)] if first else out_at(c, src)
        return rdma(here, out_at(c, src), o_s, o_r.at[src], sp=to)

    def out_local(c):
        return pltpu.make_async_copy(out_refs[c], wout_buf.at[c * depth : (c + 1) * depth, out_cols_of(me)], o_loc)

    def out_begin():
        for c in range(2):

            @pl.when(has_up)
            def _(c=c):
                out_hop(c, me, me + 1, True).start()

            @pl.when(has_down)
            def _(c=c):
                out_hop(c, me, me - 1, True).start()

            out_local(c).start()

    def out_relay(i):
        for src, to in ((me - i, me + 1), (me + i, me - 1)):

            @pl.when((src >= 0) & (src < n))
            def _(src=src, to=to):
                both = out_both(src)
                rdma(both, both, o_s, o_r.at[src], sp=src).wait_recv()
                for c in range(2):

                    @pl.when((to >= 0) & (to < n))
                    def _(c=c):
                        out_hop(c, src, to, False).start()

                    for d in range(1, n_grp):
                        here = out_at(c, src)
                        at = (d - 1) * n + src
                        rdma(here, here, oy_s, oy_r.at[at], grp=lax.rem(g + d, n_grp)).start()

    def out_arrive(src):
        for d in range(1, n_grp):
            drained(oy_r.at[(d - 1) * n + src], out_both(src))

    def w_pass(c, src):
        up, down = (fox_up, fox_down) if c in fox_arrays else (ret_up, ret_down)

        @pl.when((src < me) & (up < n))
        def _():
            w_on(c, src, up).start()

        @pl.when((src > me) & (down >= 0))
        def _():
            w_on(c, src, down).start()

    def w_relay(arrays, ks):
        for i in ks:
            for c in arrays:
                w_in(c, toward(i)).wait_recv()
                w_pass(c, toward(i))
                for d in range(1, n_grp):
                    w_side(c, i, d).start()

    def w_arrive(arrays):
        for c in arrays:
            w_local(c).wait()
            drained(wy_r.at[local_at[c]], w_several(c, (n - 1) * (n_grp - 1)))

    def normalize(h):
        squares = jnp.zeros((rows, 1), jnp.float32)
        for i in range(n_tp):
            part = tok_buf[h, i].astype(jnp.float32)
            squares = squares + jnp.sum(part * part, axis=-1, keepdims=True)
        scale = lax.rsqrt(squares * (1.0 / (n_tp * feats)) + epsilon)
        at = pl.ds(pl.multiple_of(h * rows, rows), rows)
        for i in range(n_tp):
            part = tok_buf[h, i].astype(jnp.float32)
            cols = slice(i * feats, (i + 1) * feats)
            norm_buf[at, cols] = (part * scale * gain_buf[:, cols]).astype(jnp.bfloat16)


    def tok_own():
        for d in range(1, half):
            tok_x_in(True, 0, d).wait_recv()
            for m in range(chunks):
                tok_c(True, m, d).start()

    def tok_swap(m):
        tok_z_in(m).wait_recv()
        for d in range(1, half):
            tok_x(False, m, d).start()
        tok_c(False, m, 0).start()

    def tok_last(m):
        for d in range(1, half):
            tok_x_in(False, m, d).wait_recv()
            tok_c(False, m, d).start()

    def tok_ready(own):
        if own:
            tok_local.wait()
        drained(tc_r.at[0 if own else 1], tok_buf.at[mine if own else other, :half])

    for copy in brought:
        copy.wait()

    @pl.when(is_fox)
    def _():
        w_relay((0, 1), [1, n - 1])

    @pl.when(is_fox)
    def _():
        tok_swap(0)
        tok_own()
        for m in range(1, chunks):
            tok_swap(m)
        w_relay((0, 1), far)
        w_relay((2,), [1, n - 1])

    @pl.when(is_ret)
    def _():
        tok_own()
        for m in range(chunks):
            tok_swap(m)
            if m == 1:
                w_relay((3,), far)
            if m == 2:
                w_relay((4,), far)
        w_relay(ret_arrays, [1])

    out_begin()
    tok_ready(True)
    normalize(mine)

    row_id = lax.broadcasted_iota(jnp.int32, (rows, rows), 0)
    col_id = lax.broadcasted_iota(jnp.int32, (rows, rows), 1)
    causal = col_id <= row_id

    def norm_rows(h):
        return norm_buf[pl.ds(pl.multiple_of(h * rows, rows), rows), :]

    def mix_copy(first):
        return rdma(
            mix_pair.at[other], mix_buf.at[:, first : first + depth], mix_s, mix_r, sp=partner
        )

    def mix_own(first):
        mix_buf[:, first : first + depth] = mix_pair[mine]

    def mix_in(first):
        here = mix_buf.at[:, first : first + depth]
        return rdma(here, here, mix_s, mix_r, sp=partner)

    def kv_copy(b, q):
        at = 2 * couple + b
        return rdma(kv_buf.at[at], kv_buf.at[at], kv_s.at[2 * q + b], kv_r.at[at], sp=fox_of(q))

    def kv_in(at):
        return rdma(kv_buf.at[at], kv_buf.at[at], kv_s.at[at], kv_r.at[at], sp=partner)

    def sum_copy(q):
        return rdma(sum_buf.at[couple], sum_buf.at[couple], sum_s.at[q], sum_r.at[couple], sp=ret_of(q))

    def sum_in(q):
        return rdma(sum_buf.at[q], sum_buf.at[q], sum_s.at[q], sum_r.at[q], sp=partner)

    def later(act):
        for q in range(1, couples):

            @pl.when(q > couple)
            def _(q=q):
                act(jnp.int32(q))

    def after_tokens():
        for m in range(chunks):
            tok_last(m)

    @pl.when(is_fox)
    def _():
        def project_kv(b):
            kv_buf[2 * couple + b] = jnp.dot(
                norm_rows(b), w_buf[:, :q_at], preferred_element_type=jnp.float32
            ).astype(jnp.bfloat16)
            later(lambda q: kv_copy(b, q).start())

        def q_part(srcs):
            total = 0.0
            for src in srcs:
                cols = pl.ds(pl.multiple_of(src * shard, shard), shard)
                total = total + jnp.dot(
                    norm_buf[:, cols], w_buf[cols, q_at:fox_wide], preferred_element_type=jnp.float32
                )
            return total

        for b in range(2):
            for h in range(fh):
                own_cols = pl.ds(pl.multiple_of((2 * couple + b) * rows, rows), rows)
                own = jnp.where(row_id == col_id, gates_buf[h : h + 1, own_cols], 0.0)
                gate_buf[h, b * rows : (b + 1) * rows] = jnp.broadcast_to(
                    jnp.sum(own, axis=1, keepdims=True), (rows, lanes)
                )
        after_tokens()
        w_arrive((0, 1))
        project_kv(mine)
        w_relay((2,), far)
        out_relay(1)
        tok_ready(False)
        normalize(other)
        project_kv(other)
        w_early(2)
        sums_buf[:, : fh * fd] = q_part([me, toward(1), toward(n - 1)])
        w_late(2)
        proj_buf[:, : fh * fd] = (sums_buf[:, : fh * fd] + q_part([toward(k) for k in far])).astype(jnp.bfloat16)

        def block_cols(at):
            return pl.ds(pl.multiple_of(at * rows, rows), rows)

        def rep_cols(x, wide):
            return jnp.concatenate([x] * (wide // lanes), axis=1)

        def attend(at, top_row, first, offset):
            size_ = 2 * rows - top_row
            here = slice(top_row, 2 * rows)
            for h in range(fh):
                query = proj_buf[here, h * fd : (h + 1) * fd]
                k = kv_buf[at, :, h * fd : (h + 1) * fd]
                v = kv_buf[at, :, (fh + h) * fd : (fh + h + 1) * fd]
                logits = lax.dot_general(query, k, NT, preferred_element_type=jnp.float32) * fd ** (-0.5)
                logits = logits + rep_cols(gate_buf[h, here], rows) - gates_buf[h : h + 1, block_cols(at)]
                if offset is not None:
                    row = lax.broadcasted_iota(jnp.int32, (size_, rows), 0)
                    col = lax.broadcasted_iota(jnp.int32, (size_, rows), 1)
                    logits = jnp.where(col <= row, logits, -jnp.inf)
                top_new = jnp.broadcast_to(jnp.max(logits, axis=-1, keepdims=True), (size_, lanes))
                if not first:
                    top = top_buf[h, here]
                    top_new = jnp.maximum(top, top_new)
                p = jnp.exp(logits - rep_cols(top_new, rows))
                total = jnp.broadcast_to(jnp.sum(p, axis=-1, keepdims=True), (size_, lanes))
                weighted = jnp.dot(p.astype(jnp.bfloat16), v, preferred_element_type=jnp.float32)
                if not first:
                    rescale = jnp.exp(top - top_new)
                    total = total_buf[h, here] * rescale + total
                    weighted = weighted_buf[h, here] * rescale[:, :fd] + weighted
                top_buf[h, here] = top_new
                total_buf[h, here] = total
                weighted_buf[h, here] = weighted

        attend(2 * couple, 0, True, 0)
        attend(2 * couple + 1, rows, False, 0)
        out_relay(2)

        def past(i, _):
            q = lax.div(i, 2)
            b = jnp.where(lax.rem(i, 2) == 0, fox_of(q) - 2 * q, 1 - (fox_of(q) - 2 * q))
            at = 2 * q + b
            kv_in(at).wait_recv()
            attend(at, 0, False, None)
            return 0

        lax.fori_loop(0, 2 * couple, past, 0)
        for b in range(2):
            at = slice(b * rows, (b + 1) * rows)
            for h in range(fh):
                mix_pair[b, :, h * fd : (h + 1) * fd] = (
                    weighted_buf[h, at] / total_buf[h, at, :fd]
                ).astype(jnp.bfloat16)
        mix_copy(depth).start()
        mix_own(depth)
        for k in range(3, n):
            out_relay(k)
        mix_in(0).wait_recv()
        mix_copy(depth).wait_send()
        later(lambda q: kv_copy(0, q).wait_send())
        later(lambda q: kv_copy(1, q).wait_send())

    @pl.when(is_ret)
    def _():
        distance = jnp.maximum(row_id - col_id, 0).astype(jnp.float32)
        key_scale = dk ** (-0.5)
        for h in range(hr):
            within_buf[h] = jnp.where(causal, jnp.exp(distance * decay_ref[h]) * key_scale, 0.0)
        w_relay(ret_arrays, [n - 1])
        after_tokens()
        tok_ready(False)
        normalize(other)
        out_relay(1)

        def ret_part(srcs):
            total = 0.0
            for src in srcs:
                cols = pl.ds(pl.multiple_of(src * shard, shard), shard)
                total = total + jnp.dot(
                    norm_buf[:, cols], w_buf[cols, :ret_wide], preferred_element_type=jnp.float32
                )
            return total

        for c in ret_arrays:
            w_early(c)
        sums_buf[:, :ret_wide] = ret_part([me] + [toward(k) for k in range(1, n - 1)])
        for c in ret_arrays:
            w_late(c)
        proj_buf[:, :ret_wide] = (sums_buf[:, :ret_wide] + ret_part([toward(n - 1)])).astype(jnp.bfloat16)
        rv_at, rq_at = starts[3][0], starts[4][0]
        lone = jnp.zeros((dk, vd), jnp.float32)

        def part(b, first, wide):
            return proj_buf[b * rows : (b + 1) * rows, first : first + wide]

        def split(x, axis):
            top = x.astype(jnp.bfloat16)
            rest = x - top.astype(jnp.float32)
            middle = rest.astype(jnp.bfloat16)
            low = (rest - middle.astype(jnp.float32)).astype(jnp.bfloat16)
            return jnp.concatenate((top, middle, low), axis=axis)

        def summary(b, h):
            past_end = rows - 1.0 - lax.broadcasted_iota(jnp.int32, (rows, dk), 0).astype(jnp.float32)
            keys = part(b, rq_at + (hr + h) * dk, dk).astype(jnp.float32) * key_scale
            parts = lax.dot_general(
                split(keys * jnp.exp(past_end * decay_ref[h]), 1),
                part(b, rv_at + h * vd, vd),
                TN,
                preferred_element_type=jnp.float32,
            )
            return parts[:dk] + parts[dk : 2 * dk] + parts[2 * dk :]

        early = [summary(0, h) for h in range(hr)]
        for h in range(hr):
            sum_buf[couple, h] = jnp.exp(lone + float(rows) * decay_ref[h]) * early[h] + summary(1, h)
        later(lambda q: sum_copy(q).start())

        for b in range(2):
            for h in range(hr):
                rk = part(b, rq_at + (hr + h) * dk, dk)
                rv = part(b, rv_at + h * vd, vd)
                scores = lax.dot_general(
                    part(b, rq_at + h * dk, dk), rk, NT, preferred_element_type=jnp.float32
                )
                raw_buf[b, h] = jnp.dot(
                    split(scores * within_buf[h], 1),
                    jnp.concatenate((rv, rv, rv), axis=0),
                    preferred_element_type=jnp.float32,
                )
        out_relay(2)

        offset = (couple * 2 * rows).astype(jnp.float32)

        def gather(q, entering):
            sum_in(q).wait_recv()
            gap = ((couple - 1 - q) * 2 * rows).astype(jnp.float32)
            return tuple(entering[h] + jnp.exp(lone + gap * decay_ref[h]) * sum_buf[q, h] for h in range(hr))

        entering = tuple(jnp.exp(lone + offset * decay_ref[h]) * state_buf[h] for h in range(hr))
        entering = lax.fori_loop(0, couple, gather, entering)
        second = tuple(jnp.exp(lone + float(rows) * decay_ref[h]) * entering[h] + early[h] for h in range(hr))
        since = lax.broadcasted_iota(jnp.int32, (rows, vd), 0).astype(jnp.float32) + 1.0

        for b in range(2):
            for h in range(hr):
                rq = part(b, rq_at + h * dk, dk)
                carried = jnp.dot(
                    jnp.concatenate((rq, rq, rq), axis=1),
                    split((entering, second)[b][h], 0),
                    preferred_element_type=jnp.float32,
                )
                raw = raw_buf[b, h] + carried * jnp.exp(since * decay_ref[h])
                center = raw - jnp.mean(raw, axis=-1, keepdims=True)
                variance = jnp.mean(center * center, axis=-1, keepdims=True)
                cols = slice(h * vd, (h + 1) * vd)
                mix_pair[b, :, cols] = (center * lax.rsqrt(variance + epsilon) * hgain_buf[:, cols]).astype(
                    jnp.bfloat16
                )
        mix_copy(0).start()
        mix_own(0)
        for k in range(3, n):
            out_relay(k)
        mix_in(depth).wait_recv()
        mix_copy(0).wait_send()
        later(lambda q: sum_copy(q).wait_send())

    block = rows // n_tp
    wide, pieces = out_cols, n

    def piece_cols(piece):
        return pl.ds(pl.multiple_of(piece * wide, wide), wide)

    def slot(at):
        return pl.ds(pl.multiple_of(at * block, block), block)

    def pair_copy(piece):
        cols = piece_cols(piece)
        return rdma(
            rs_send.at[1 - parity, :, cols],
            pair_buf.at[:, cols],
            pair_s,
            pair_r.at[piece],
            tp=t + 1 - 2 * parity,
        )

    def rs_copy(d, piece):
        to = lax.rem(pair + d, half)
        cols = piece_cols(piece)
        return rdma(
            pair_sum.at[slot(to), cols],
            far_ref.at[d - 1, :, cols],
            rs_s.at[d - 1],
            rs_r.at[d - 1],
            tp=2 * to + parity,
        )

    def project(piece):
        cols = piece_cols(piece)
        value = jnp.dot(mix_buf[...], wout_buf[:, cols], preferred_element_type=jnp.float32).astype(jnp.bfloat16)
        for b in range(n_tp):
            at = slice(b // 2 * block, (b // 2 + 1) * block)
            rs_send[b % 2, at, cols] = value[b * block : (b + 1) * block]
        pair_copy(piece).start()

    def reduce(piece):
        cols = piece_cols(piece)
        pair_copy(piece).wait_recv()
        both = rs_send[parity, :, cols].astype(jnp.float32) + pair_buf[:, cols].astype(jnp.float32)
        pair_sum[:, cols] = both.astype(jnp.bfloat16)
        for d in range(1, half):
            rs_copy(d, piece).start()

    def order(i):
        falling = jnp.where(i <= me, me - i, i)
        rising = jnp.where(i <= n - 1 - me, me + i, n - 1 - i)
        return jnp.where(lower, rising, falling)

    drained(o_loc, wout_buf.at[:, out_cols_of(me)])
    project(me)

    def turn(i, _):
        out_arrive(order(i))
        project(order(i))
        reduce(order(i - 1))
        return 0

    lax.fori_loop(1, n, turn, 0)
    reduce(order(jnp.int32(n - 1)))

    own = slot(pair)
    near_ref[...] = rs_send[parity, own, :].astype(jnp.float32) + pair_buf[own, :].astype(jnp.float32)

    slabs = rows * (2 * n_tp - 1) // (2 * n_tp)
    drained(t_s, tok_buf.at[:, :, :slabs])
    for p in range(n):

        @pl.when(me == p)
        def _(p=p):
            for arrays in (fox_arrays, ret_arrays):
                for c in arrays:
                    if sends_from(p, arrays):
                        drained(w_s.at[c], w_several(c, sends_from(p, arrays)))
            hops = 2 * ((p + 1 if p + 1 < n else 0) + (n - p if p else 0))
            drained(o_s, wout_buf.at[: hops * out_step // n])

    drained(oy_s, wout_buf.at[: 2 * (n - 1) * (n_grp - 1) * out_step // n])

    def sides(arrays):
        for c in arrays:
            drained(wy_s.at[local_at[c]], w_several(c, (n - 1) * (n_grp - 1)))

    @pl.when(is_fox)
    def _():
        sides(fox_arrays)

    @pl.when(is_ret)
    def _():
        sides(ret_arrays)

    drained(pair_s, pair_buf)
    for d in range(1, half):
        drained(rs_s.at[d - 1], pair_sum.at[:block])
    for d in range(1, half):
        drained(rs_r.at[d - 1], far_ref.at[d - 1])


def paired(n, n_tp, n_grp, inputs):
    tokens, ret_query_weight, ret_state, fox_gates = inputs[0], inputs[2], inputs[9], inputs[11]
    fox_query_weight, ret_out_weight = inputs[5], inputs[12]
    rows, feats = tokens.shape
    hr, dk, vd = ret_state.shape
    fh = fox_gates.shape[1]
    fd = fox_query_weight.shape[1] // fh
    shard = ret_query_weight.shape[0]
    depth, out_cols = ret_out_weight.shape
    columns = out_cols * n
    wide = max(3 * fh * fd, 2 * hr * dk + hr * vd)
    half = n_tp // 2
    block = rows // n_tp
    chunks = 4
    couples = n // 2
    dma = pltpu.SemaphoreType.DMA
    far = max(half - 1, 1)
    side = max(n_grp - 1, 1) * n
    vmem = pl.BlockSpec(memory_space=pltpu.VMEM)
    smem = pl.BlockSpec(memory_space=pltpu.SMEM)
    hbm = pl.BlockSpec(memory_space=pl.ANY)
    bf16, f32 = jnp.bfloat16, jnp.float32
    size = (n, n_tp, n_grp, hr, dk, vd, fh, fd, chunks)
    near, other = pl.pallas_call(
        functools.partial(pair_kernel, size),
        out_shape=(pltpu.VMEM((block, columns), f32), pltpu.VMEM((far, block, columns), bf16)),
        in_specs=[hbm] * 8 + [smem] + [hbm] * 5,
        out_specs=(vmem, vmem),
        scratch_shapes=[
            pltpu.VMEM((1, n_tp * feats), f32),
            pltpu.VMEM((2 * hr * dk, shard), bf16),
            pltpu.VMEM((hr, dk, vd), f32),
            pltpu.VMEM((1, hr * vd), f32),
            pltpu.VMEM((fh, n * rows), f32),
            pltpu.VMEM((fh, 2 * rows, lanes), f32),
            pltpu.VMEM((hr, rows, rows), f32),
            pltpu.VMEM((2, hr, rows, vd), f32),
            pltpu.VMEM((2 * rows, wide), f32),
            pltpu.VMEM((2, n_tp, rows, feats), bf16),
            pltpu.VMEM((shard, 2 * hr * dk), bf16),
            pltpu.VMEM((n * shard, wide), bf16),
            pltpu.VMEM((2 * depth, columns), bf16),
            pltpu.VMEM((2 * rows, n_tp * feats), bf16),
            pltpu.VMEM((2 * rows, wide), bf16),
            pltpu.VMEM((n, rows, 2 * fh * fd), bf16),
            pltpu.VMEM((couples, hr, dk, vd), f32),
            pltpu.VMEM((2, rows, depth), bf16),
            pltpu.VMEM((rows, 2 * depth), bf16),
            pltpu.VMEM((2, rows // 2, columns), bf16),
            pltpu.VMEM((rows // 2, columns), bf16),
            pltpu.VMEM((rows // 2, columns), bf16),
            pltpu.VMEM((fh, 2 * rows, lanes), f32),
            pltpu.VMEM((fh, 2 * rows, lanes), f32),
            pltpu.VMEM((fh, 2 * rows, fd), f32),
            dma((5,)),
            pltpu.SemaphoreType.REGULAR,
            pltpu.SemaphoreType.REGULAR,
            dma,
            dma((chunks,)),
            dma(((chunks + 1) * far,)),
            dma((2,)),
            dma,
            dma((5,)),
            dma((3 * n,)),
            dma((3,)),
            dma((6,)),
            dma((3,)),
            dma,
            dma((n,)),
            dma,
            dma((side,)),
            dma,
            dma((2 * couples,)),
            dma((n,)),
            dma((couples,)),
            dma((couples,)),
            dma,
            dma,
            dma,
            dma((n,)),
            dma((far,)),
            dma((far,)),
        ],
        compiler_params=pltpu.CompilerParams(
            collective_id=0, has_side_effects=True, vmem_limit_bytes=56 * 1024 * 1024
        ),
        name="layer",
    )(
        tokens,
        inputs[1][None, :],
        inputs[2].T,
        inputs[3].T,
        inputs[4],
        inputs[5],
        inputs[6],
        inputs[7],
        inputs[8],
        inputs[9],
        inputs[10][None, :],
        inputs[11].T,
        inputs[12],
        inputs[13],
    )
    for d in range(half - 1):
        near = near + other[d].astype(f32)
    return near.astype(bf16)


def pairs_fit(n, n_tp, n_grp, inputs):
    rows, feats = inputs[0].shape
    hr, dk, vd = inputs[9].shape
    shard = inputs[2].shape[0]
    depth, out_cols = inputs[12].shape
    wide = inputs[5].shape[1]
    full = all(w % lanes == 0 for w in (out_cols, wide, 2 * hr * dk, hr * vd, feats, depth, rows))
    even = n % 2 == 0 and n > 2 and n_tp % 2 == 0 and n_grp > 1
    tiles = rows % (32 * n_tp) == 0 and rows % 32 == 0 and shard % (16 * n_grp) == 0 and depth % (16 * n_grp * n) == 0 and vd <= lanes
    columns = n * out_cols
    held = 8 * rows * n_tp * feats + 2 * n * shard * 3 * wide + 4 * depth * columns + 4 * n * rows * wide + 6 * rows * columns
    return full and even and tiles and depth == wide == hr * vd and held < 40 * 1024 * 1024


def local(
    n,
    n_tp,
    n_grp,
    tokens,
    norm_gain,
    ret_query_weight,
    ret_key_weight,
    ret_value_weight,
    fox_query_weight,
    fox_key_weight,
    fox_value_weight,
    ret_decay,
    ret_state,
    head_norm_gain,
    fox_gates,
    ret_out_weight,
    fox_out_weight,
):
    inputs = (
        tokens,
        norm_gain,
        ret_query_weight,
        ret_key_weight,
        ret_value_weight,
        fox_query_weight,
        fox_key_weight,
        fox_value_weight,
        ret_decay,
        ret_state,
        head_norm_gain,
        fox_gates,
        ret_out_weight,
        fox_out_weight,
    )
    if pairs_fit(n, n_tp, n_grp, inputs):
        return paired(n, n_tp, n_grp, inputs)
    rows, feats = tokens.shape
    hr, dk, vd = ret_state.shape
    fh = fox_gates.shape[1]
    fd = fox_query_weight.shape[1] // fh
    shard = ret_query_weight.shape[0]
    width = 2 * hr * dk + hr * vd + 3 * fh * fd
    depth, out_cols = ret_out_weight.shape
    columns = out_cols * n
    direct = out_cols % 128 == 0
    if not direct:
        ret_out_weight, fox_out_weight = ret_out_weight.T, fox_out_weight.T
    dma = pltpu.SemaphoreType.DMA

    def gather_sems(arrays):
        side = max(n_grp - 1, 1) * n * arrays
        return [
            dma((n * arrays,)),
            dma((n * arrays,)),
            dma((n * arrays,)),
            dma((side,)),
            dma((side,)),
            dma((arrays,)),
        ]

    vmem = pl.BlockSpec(memory_space=pltpu.VMEM)
    smem = pl.BlockSpec(memory_space=pltpu.SMEM)
    hbm = pl.BlockSpec(memory_space=pl.ANY)
    size = (n, n_tp, n_grp, hr, dk, vd, fh, fd, direct)
    block = rows // n_tp
    peers = max(n_tp - 1, 1)
    far = max(n_tp // 2 - 1, 1)
    pieces = n if direct else 1
    return pl.pallas_call(
        functools.partial(kernel, size),
        out_shape=jax.ShapeDtypeStruct((block, columns), jnp.bfloat16),
        in_specs=[hbm, vmem, vmem, vmem, hbm, hbm, hbm, hbm, smem, vmem, vmem, vmem, hbm, hbm],
        out_specs=vmem,
        scratch_shapes=[
            pltpu.VMEM((n_tp, rows, feats), jnp.bfloat16),
            pltpu.VMEM((shard, 2 * hr * dk), jnp.bfloat16),
            pltpu.VMEM((n * shard, width), jnp.bfloat16),
            pltpu.VMEM((2 * depth, columns) if direct else (columns, 2 * depth), jnp.bfloat16),
            pltpu.VMEM((rows, n_tp * feats), jnp.bfloat16),
            pltpu.VMEM((rows, width - 2 * fh * fd), jnp.bfloat16),
            pltpu.VMEM((n, rows, 2 * fh * fd), jnp.bfloat16),
            pltpu.VMEM((n, hr, dk, vd), jnp.float32),
            pltpu.VMEM((rows, 2 * depth), jnp.bfloat16),
            pltpu.VMEM((2, rows // 2, columns), jnp.bfloat16),
            pltpu.VMEM((rows // 2, columns), jnp.bfloat16),
            pltpu.VMEM((rows // 2, columns), jnp.bfloat16),
            pltpu.VMEM((far, block, columns), jnp.bfloat16),
            pltpu.VMEM((fh, rows, 1), jnp.float32),
            pltpu.VMEM((fh, rows, 1), jnp.float32),
            pltpu.VMEM((fh, rows, fd), jnp.float32),
            dma((peers,)),
            dma((peers,)),
            dma,
            dma((n,)),
            dma((n,)),
            dma((n,)),
            dma((n,)),
            dma((pieces,)),
            dma((pieces,)),
            dma((far * pieces,)),
            dma((far * pieces,)),
        ]
        + gather_sems(2)
        + gather_sems(3)
        + gather_sems(2),
        compiler_params=pltpu.CompilerParams(
            collective_id=0, has_side_effects=True, vmem_limit_bytes=56 * 1024 * 1024
        ),
        name="layer",
    )(
        tokens,
        norm_gain[None, :],
        ret_query_weight.T,
        ret_key_weight.T,
        ret_value_weight,
        fox_query_weight,
        fox_key_weight,
        fox_value_weight,
        ret_decay,
        ret_state,
        head_norm_gain[None, :],
        fox_gates.T,
        ret_out_weight,
        fox_out_weight,
    )


def solution(mesh):
    placed = (
        P(("grp", "sp"), "tp"),
        P(),
        P("sp", "tp"),
        P("sp", "tp"),
        P("sp", "tp"),
        P("sp", "tp"),
        P("sp", "tp"),
        P("sp", "tp"),
        P("tp"),
        P(("grp", "tp"), None, None),
        P("tp"),
        P("grp", "tp"),
        P("tp", "sp"),
        P("tp", "sp"),
    )
    body = functools.partial(local, mesh.shape["sp"], mesh.shape["tp"], mesh.shape["grp"])
    return jax.shard_map(
        body, mesh=mesh, in_specs=placed, out_specs=P(("grp", "sp", "tp"), None), check_vma=False
    )
```

```python
import functools

import jax
import jax.numpy as jnp
from jax import lax
from jax.experimental import pallas as pl
from jax.experimental.pallas import tpu as pltpu
from jax.sharding import PartitionSpec as P

epsilon = 1e-06
lanes = 128
highest = lax.Precision.HIGHEST
NT = (((1,), (1,)), ((), ()))
TN = (((0,), (0,)), ((), ()))


def rdma(src, dst, send_sem, recv_sem, **target):
    return pltpu.make_async_remote_copy(
        src_ref=src,
        dst_ref=dst,
        send_sem=send_sem,
        recv_sem=recv_sem,
        device_id=target,
        device_id_type=pl.DeviceIdType.MESH,
    )


class LineGather:
    def __init__(self, owns, place, sems, n, n_grp, me, g):
        self.owns, self.place, self.n, self.n_grp, self.me, self.g = owns, place, n, n_grp, me, g
        self.up, self.down, self.zr, self.ys, self.yr, self.loc = sems
        self.arrays = len(owns)
        self.rows = owns[0].shape[0]
        self.step = self.rows // n_grp

    def piece(self, part, src, c):
        return self.place(src, c, part * self.step, self.step)

    def own_piece(self, c):
        return self.owns[c].at[pl.ds(pl.multiple_of(self.g * self.step, self.step), self.step)]

    def hop(self, sems, to, src, c, first=False):
        here = self.own_piece(c) if first else self.piece(self.g, src, c)
        at = src * self.arrays + c
        return rdma(here, self.piece(self.g, src, c), sems.at[at], self.zr.at[at], sp=to)

    def side(self, d, src, c):
        at = ((d - 1) * self.n + src) * self.arrays + c
        here = self.piece(self.g, src, c)
        return rdma(here, here, self.ys.at[at], self.yr.at[at], grp=lax.rem(self.g + d, self.n_grp))

    def side_in(self, d, src, c):
        at = ((d - 1) * self.n + src) * self.arrays + c
        part = lax.rem(self.g + self.n_grp - d, self.n_grp)
        here = self.piece(part, src, c)
        return rdma(here, here, self.ys.at[at], self.yr.at[at], grp=part)

    def local(self, c):
        return pltpu.make_async_copy(self.owns[c], self.place(self.me, c, 0, self.rows), self.loc.at[c])

    def start(self):
        me, n = self.me, self.n
        for c in range(self.arrays):

            @pl.when(me + 1 < n)
            def _():
                self.hop(self.up, me + 1, me, c, True).start()

            @pl.when(me >= 1)
            def _():
                self.hop(self.down, me - 1, me, c, True).start()

        for c in range(self.arrays):
            self.local(c).start()

    def relay(self, k):
        me, n = self.me, self.n
        for c in range(self.arrays):
            for src, sems, to in ((me - k, self.up, me + 1), (me + k, self.down, me - 1)):

                @pl.when((src >= 0) & (src < n))
                def _(src=src, sems=sems, to=to):
                    self.hop(sems, me, src, c).wait_recv()

                    @pl.when((to >= 0) & (to < n))
                    def _():
                        self.hop(sems, to, src, c).start()

                    for d in range(1, self.n_grp):
                        self.side(d, src, c).start()

    def arrive_shard(self, src, arrays):
        for c in arrays:
            for d in range(1, self.n_grp):
                self.side_in(d, src, c).wait_recv()

    def arrive(self, arrays):
        for c in arrays:
            self.local(c).wait()

        def step(k, _):
            self.arrive_shard(lax.rem(self.me + k, self.n), arrays)
            return 0

        lax.fori_loop(1, self.n, step, 0)

    def finish(self):
        me, n = self.me, self.n

        def step(src, _):
            for c in range(self.arrays):

                @pl.when((src <= me) & (me + 1 < n))
                def _():
                    self.hop(self.up, me, src, c).wait_send()

                @pl.when((src >= me) & (me >= 1))
                def _():
                    self.hop(self.down, me, src, c).wait_send()

                @pl.when(src != me)
                def _():
                    for d in range(1, self.n_grp):
                        self.side(d, src, c).wait_send()

            return 0

        lax.fori_loop(0, n, step, 0)


def kernel(
    size,
    tok_ref,
    gain_ref,
    wq_ref,
    wk_ref,
    wrv_ref,
    wfq_ref,
    wfk_ref,
    wfv_ref,
    decay_ref,
    state_ref,
    hgain_ref,
    gates_ref,
    ret_out_ref,
    fox_out_ref,
    out_ref,
    tok_buf,
    qk_own,
    w_buf,
    wout_buf,
    norm_buf,
    proj_buf,
    kv_buf,
    sum_buf,
    mix_buf,
    rs_send,
    pair_buf,
    pair_sum,
    rs_buf,
    top_buf,
    total_buf,
    weighted_buf,
    tok_s,
    tok_r,
    tok_loc,
    kv_s,
    kv_r,
    sum_s,
    sum_r,
    pair_s,
    pair_r,
    rs_s,
    rs_r,
    *gather_sems,
):
    n, n_tp, n_grp, hr, dk, vd, fh, fd, direct = size
    me, t, g = lax.axis_index("sp"), lax.axis_index("tp"), lax.axis_index("grp")
    rows, feats = tok_ref.shape
    owns = [wfk_ref, wfv_ref, wfq_ref, wrv_ref, qk_own]
    early = 2
    starts = [0]
    for own in owns:
        starts.append(starts[-1] + own.shape[1])
    shard = qk_own.shape[0]

    def weight_place(src, c, first, count):
        start = pl.multiple_of(src * shard + first, count)
        return w_buf.at[pl.ds(start, count), starts[c] : starts[c + 1]]

    depth = mix_buf.shape[1] // 2
    out_cols = ret_out_ref.shape[1] if direct else ret_out_ref.shape[0]

    def out_place(src, c, first, count):
        if direct:
            start = pl.multiple_of(c * depth + first, count)
            return wout_buf.at[pl.ds(start, count), pl.ds(pl.multiple_of(src * out_cols, out_cols), out_cols)]
        start = pl.multiple_of(src * out_cols + first, count)
        return wout_buf.at[pl.ds(start, count), c * depth : (c + 1) * depth]

    def late_place(src, c, first, count):
        return weight_place(src, c + early, first, count)

    firsts = LineGather(owns[:early], weight_place, gather_sems[:6], n, n_grp, me, g)
    lasts = LineGather(owns[early:], late_place, gather_sems[6:12], n, n_grp, me, g)
    outs = LineGather([ret_out_ref, fox_out_ref], out_place, gather_sems[12:], n, n_grp, me, g)

    barrier = pltpu.get_barrier_semaphore()

    def greet(**target):
        pl.semaphore_signal(barrier, inc=1, device_id=target, device_id_type=pl.DeviceIdType.MESH)

    has_up, has_down = me + 1 < n, me >= 1
    for d in range(1, n_tp):
        greet(tp=lax.rem(t + d, n_tp))
    for d in range(1, n_grp):
        greet(grp=lax.rem(g + d, n_grp))

    @pl.when(has_up)
    def _():
        greet(sp=me + 1)

    @pl.when(has_down)
    def _():
        greet(sp=me - 1)

    turned = jnp.concatenate((wq_ref[...], wk_ref[...]), axis=0).astype(jnp.float32)
    qk_own[...] = turned.T.astype(jnp.bfloat16)

    count = n_tp - 1 + n_grp - 1 + has_up.astype(jnp.int32) + has_down.astype(jnp.int32)
    pl.semaphore_wait(barrier, count)

    def tok_copy(d):
        return rdma(tok_ref, tok_buf.at[t], tok_s.at[d - 1], tok_r.at[d - 1], tp=lax.rem(t + d, n_tp))

    def tok_in(d):
        src = lax.rem(t + n_tp - d, n_tp)
        return rdma(tok_ref, tok_buf.at[src], tok_s.at[d - 1], tok_r.at[d - 1], tp=src)

    firsts.start()
    lasts.start()
    tok_local = pltpu.make_async_copy(tok_ref, tok_buf.at[t], tok_loc)
    for d in range(1, n_tp):
        tok_copy(d).start()
    tok_local.start()

    def first_step(k, _):
        firsts.relay(k)

        lasts.relay(k)
        return 0

    lax.fori_loop(1, n, first_step, 0)
    outs.start()

    tok_local.wait()
    for d in range(1, n_tp):
        tok_in(d).wait_recv()
    squares = jnp.zeros((rows, 1), jnp.float32)
    for i in range(n_tp):
        part = tok_buf[i].astype(jnp.float32)
        squares = squares + jnp.sum(part * part, axis=-1, keepdims=True)
    scale = lax.rsqrt(squares * (1.0 / (n_tp * feats)) + epsilon)
    for i in range(n_tp):
        part = tok_buf[i].astype(jnp.float32)
        cols = slice(i * feats, (i + 1) * feats)
        norm_buf[:, cols] = (part * scale * gain_ref[:, cols]).astype(jnp.bfloat16)

    def kv_copy(src):
        return rdma(kv_buf.at[src], kv_buf.at[src], kv_s.at[src], kv_r.at[src], sp=jnp.minimum(me + 1, n - 1))

    def sum_copy(src):
        return rdma(sum_buf.at[src], sum_buf.at[src], sum_s.at[src], sum_r.at[src], sp=jnp.minimum(me + 1, n - 1))

    firsts.arrive((0, 1))
    kv_buf[me] = jnp.dot(
        norm_buf[...], w_buf[:, : starts[2]], preferred_element_type=jnp.float32
    ).astype(jnp.bfloat16)

    def kv_forward(k):
        src = me - k

        @pl.when(src >= 0)
        def _():
            kv_copy(src).wait_recv()

            @pl.when(has_up)
            def _():
                kv_copy(src).start()

    @pl.when(has_up)
    def _():
        kv_copy(me).start()

    outs.relay(1)
    lasts.arrive((0, 1, 2))
    proj_buf[...] = jnp.dot(
        norm_buf[...], w_buf[:, starts[2] :], preferred_element_type=jnp.float32
    ).astype(jnp.bfloat16)
    rv_at, rq_at = starts[3] - starts[2], starts[4] - starts[2]

    key_scale = dk ** (-0.5)
    position = lax.broadcasted_iota(jnp.int32, (rows, 1), 0).astype(jnp.float32)
    rq, rk, rv = [], [], []
    for h in range(hr):
        rq.append(proj_buf[:, rq_at + h * dk : rq_at + (h + 1) * dk])
        rk.append(proj_buf[:, rq_at + (hr + h) * dk : rq_at + (hr + h + 1) * dk])
        rv.append(proj_buf[:, rv_at + h * vd : rv_at + (h + 1) * vd])
        keys = rk[h].astype(jnp.float32) * key_scale
        trailing = jnp.exp((rows - 1.0 - position) * decay_ref[h])
        sum_buf[me, h] = lax.dot_general(
            keys * trailing, rv[h].astype(jnp.float32), TN, precision=highest, preferred_element_type=jnp.float32
        )

    @pl.when(has_up)
    def _():
        sum_copy(me).start()

    row_id = lax.broadcasted_iota(jnp.int32, (rows, rows), 0)
    col_id = lax.broadcasted_iota(jnp.int32, (rows, rows), 1)
    causal = col_id <= row_id
    own_cols = pl.ds(pl.multiple_of(me * rows, rows), rows)
    own_gates = [
        jnp.sum(jnp.where(row_id == col_id, gates_ref[h : h + 1, own_cols], 0.0), axis=1, keepdims=True)
        for h in range(fh)
    ]

    def attend(src, diagonal):
        key_cols = pl.ds(pl.multiple_of(src * rows, rows), rows)
        for h in range(fh):
            query = proj_buf[:, h * fd : (h + 1) * fd]
            k = kv_buf[src, :, h * fd : (h + 1) * fd]
            v = kv_buf[src, :, (fh + h) * fd : (fh + h + 1) * fd]
            logits = lax.dot_general(query, k, NT, preferred_element_type=jnp.float32) * fd ** (-0.5)
            logits = logits + own_gates[h] - gates_ref[h : h + 1, key_cols]
            if diagonal:
                logits = jnp.where(causal, logits, -jnp.inf)
            top_new = jnp.max(logits, axis=-1, keepdims=True)
            if not diagonal:
                top = top_buf[h]
                top_new = jnp.maximum(top, top_new)
            p = jnp.exp(logits - top_new)
            total = jnp.sum(p, axis=-1, keepdims=True)
            weighted = jnp.dot(p.astype(jnp.bfloat16), v, preferred_element_type=jnp.float32)
            if not diagonal:
                rescale = jnp.exp(top - top_new)
                total = total_buf[h] * rescale + total
                weighted = weighted_buf[h] * rescale + weighted
            top_buf[h] = top_new
            total_buf[h] = total
            weighted_buf[h] = weighted

    def forward(k):
        src = me - k

        @pl.when(src >= 0)
        def _():
            sum_copy(src).wait_recv()

            @pl.when(has_up)
            def _():
                sum_copy(src).start()

    attend(me, True)

    offset = (me * rows).astype(jnp.float32)
    lone = jnp.zeros((dk, vd), jnp.float32)

    def step(k, entering):
        src = me - k
        kv_forward(k)
        forward(k)

        @pl.when(k + 1 < n)
        def _():
            outs.relay(k + 1)


        @pl.when(src >= 0)
        def _():
            attend(src, False)

        gap = ((k - 1) * rows).astype(jnp.float32)
        there = jnp.maximum(src, 0)
        return tuple(
            entering[h]
            + jnp.where(src >= 0, jnp.exp(lone + gap * decay_ref[h]) * sum_buf[there, h], 0.0)
            for h in range(hr)
        )

    entering = tuple(jnp.exp(lone + offset * decay_ref[h]) * state_ref[h] for h in range(hr))
    entering = lax.fori_loop(1, n, step, entering)

    distance = jnp.maximum(row_id - col_id, 0).astype(jnp.float32)
    for h in range(hr):
        scores = lax.dot_general(rq[h], rk[h], NT, preferred_element_type=jnp.float32) * key_scale
        scores = jnp.where(causal, scores * jnp.exp(distance * decay_ref[h]), 0.0)
        inner = jnp.dot(scores, rv[h].astype(jnp.float32), precision=highest, preferred_element_type=jnp.float32)
        leading = jnp.exp((position + 1.0) * decay_ref[h])
        carried = jnp.dot(
            rq[h].astype(jnp.float32), entering[h], precision=highest, preferred_element_type=jnp.float32
        )
        raw = inner + carried * leading
        center = raw - jnp.mean(raw, axis=-1, keepdims=True)
        variance = jnp.mean(center * center, axis=-1, keepdims=True)
        cols = slice(h * vd, (h + 1) * vd)
        mix_buf[:, cols] = (center * lax.rsqrt(variance + epsilon) * hgain_ref[:, cols]).astype(jnp.bfloat16)
    for h in range(fh):
        cols = slice(hr * vd + h * fd, hr * vd + (h + 1) * fd)
        mix_buf[:, cols] = (weighted_buf[h] / total_buf[h]).astype(jnp.bfloat16)

    block = rows // n_tp
    columns = pair_buf.shape[1]
    wide = out_cols if direct else columns
    pieces = columns // wide
    half = n_tp // 2
    parity, pair = lax.rem(t, 2), lax.div(t, 2)

    def piece_cols(piece):
        return pl.ds(pl.multiple_of(piece * wide, wide), wide)

    def slot(at):
        return pl.ds(pl.multiple_of(at * block, block), block)

    def pair_copy(piece):
        cols = piece_cols(piece)
        return rdma(
            rs_send.at[1 - parity, :, cols],
            pair_buf.at[:, cols],
            pair_s.at[piece],
            pair_r.at[piece],
            tp=t + 1 - 2 * parity,
        )

    def rs_copy(d, piece):
        to = lax.rem(pair + d, half)
        cols = piece_cols(piece)
        at = (d - 1) * pieces + piece
        return rdma(
            pair_sum.at[slot(to), cols], rs_buf.at[d - 1, :, cols], rs_s.at[at], rs_r.at[at], tp=2 * to + parity
        )

    def project(piece):
        cols = piece_cols(piece)
        if direct:
            value = jnp.dot(mix_buf[...], wout_buf[:, cols], preferred_element_type=jnp.float32)
        else:
            value = lax.dot_general(mix_buf[...], wout_buf[...], NT, preferred_element_type=jnp.float32)
        value = value.astype(jnp.bfloat16)
        for b in range(n_tp):
            at = slice(b // 2 * block, (b // 2 + 1) * block)
            rs_send[b % 2, at, cols] = value[b * block : (b + 1) * block]
        pair_copy(piece).start()

    def reduce(piece):
        cols = piece_cols(piece)
        pair_copy(piece).wait_recv()
        both = rs_send[parity, :, cols].astype(jnp.float32) + pair_buf[:, cols].astype(jnp.float32)
        pair_sum[:, cols] = both.astype(jnp.bfloat16)
        for d in range(1, half):
            rs_copy(d, piece).start()

    def order(i):
        falling = jnp.where(i <= me, me - i, i)
        rising = jnp.where(i <= n - 1 - me, me + i, n - 1 - i)
        return jnp.where(2 * me >= n, falling, rising)

    if direct:
        for c in range(2):
            outs.local(c).wait()
        project(me)

        def out_step(i, _):
            outs.arrive_shard(order(i), (0, 1))
            project(order(i))
            reduce(order(i - 1))
            return 0

        lax.fori_loop(1, n, out_step, 0)
        reduce(order(jnp.int32(n - 1)))
    else:
        outs.arrive((0, 1))
        project(0)
        reduce(0)

    own = slot(pair)
    summed = rs_send[parity, own, :].astype(jnp.float32) + pair_buf[own, :].astype(jnp.float32)
    for d in range(1, half):
        for piece in range(pieces):
            rs_copy(d, piece).wait_recv()
        summed = summed + rs_buf[d - 1].astype(jnp.float32)
    out_ref[...] = summed.astype(jnp.bfloat16)

    for d in range(1, n_tp):
        tok_copy(d).wait_send()
    for piece in range(pieces):
        pair_copy(piece).wait_send()
        for d in range(1, half):
            rs_copy(d, piece).wait_send()
    firsts.finish()
    lasts.finish()
    outs.finish()

    @pl.when(has_up)
    def _():
        def step(src, _):
            kv_copy(src).wait_send()
            sum_copy(src).wait_send()
            return 0

        lax.fori_loop(0, me + 1, step, 0)


def pair_kernel(
    size,
    tok_ref,
    gain_ref,
    wq_ref,
    wk_ref,
    wrv_ref,
    wfq_ref,
    wfk_ref,
    wfv_ref,
    decay_hbm,
    state_ref,
    hgain_ref,
    gates_ref,
    ret_out_ref,
    fox_out_ref,
    near_ref,
    far_ref,
    decay_ref,
    gain_buf,
    wqk_buf,
    state_buf,
    hgain_buf,
    gates_buf,
    gate_buf,
    within_buf,
    raw_buf,
    sums_buf,
    tok_buf,
    qk_own,
    w_buf,
    wout_buf,
    norm_buf,
    proj_buf,
    kv_buf,
    sum_buf,
    mix_pair,
    mix_buf,
    rs_send,
    pair_buf,
    pair_sum,
    top_buf,
    total_buf,
    weighted_buf,
    in_sem,
    above_sem,
    below_sem,
    t_s,
    tz_r,
    tx_r,
    tc_r,
    t_loc,
    w_s,
    w_r,
    wy_s,
    wy_r,
    w_loc,
    o_s,
    o_r,
    oy_s,
    oy_r,
    o_loc,
    kv_s,
    kv_r,
    sum_s,
    sum_r,
    mix_s,
    mix_r,
    pair_s,
    pair_r,
    rs_s,
    rs_r,
):
    n, n_tp, n_grp, hr, dk, vd, fh, fd, chunks = size
    me, t, g = lax.axis_index("sp"), lax.axis_index("tp"), lax.axis_index("grp")
    rows, feats = tok_ref.shape
    shard = qk_own.shape[0]
    couples = n // 2
    couple, mine = lax.div(me, 2), lax.rem(me, 2)
    other = 1 - mine
    partner = me + 1 - 2 * mine
    fox_mine = 1 - lax.rem(couple, 2)
    is_fox = mine == fox_mine
    is_ret = mine != fox_mine
    lower = 2 * me < n
    half = n_tp // 2
    parity, pair = lax.rem(t, 2), lax.div(t, 2)

    def fox_of(q):
        return 2 * q + 1 - lax.rem(q, 2)

    def ret_of(q):
        return 2 * q + lax.rem(q, 2)

    def toward(k):
        return lax.rem(jnp.where(lower, me + k, me + n - k), n)

    barrier = pltpu.get_barrier_semaphore()

    def greet(**target):
        pl.semaphore_signal(barrier, inc=1, device_id=target, device_id_type=pl.DeviceIdType.MESH)

    greet(tp=2 * pair + 1 - parity)
    for d in range(1, half):
        greet(tp=2 * lax.rem(pair + d, half) + parity)
    for d in range(1, n_grp):
        greet(grp=lax.rem(g + d, n_grp))
    has_up, has_down = me + 1 < n, me >= 1

    @pl.when(has_up)
    def _():
        greet(sp=me + 1)

    @pl.when(has_down)
    def _():
        greet(sp=me - 1)

    def drained(sem, ref):
        pltpu.make_async_copy(ref, ref, sem).wait()

    width = hr * dk
    pltpu.make_async_copy(wq_ref, wqk_buf.at[:width], in_sem.at[0]).start()
    pltpu.make_async_copy(wk_ref, wqk_buf.at[width:], in_sem.at[0]).start()
    brought = [
        pltpu.make_async_copy(src, dst, in_sem.at[i + 1])
        for i, (src, dst) in enumerate(
            ((gain_ref, gain_buf), (state_ref, state_buf), (hgain_ref, hgain_buf), (gates_ref, gates_buf), (decay_hbm, decay_ref))
        )
    ]
    for copy in brought:
        copy.start()

    pl.semaphore_wait(barrier, half + n_grp - 1 + has_up.astype(jnp.int32) + has_down.astype(jnp.int32))

    def tell(sem, to):
        pl.semaphore_signal(sem, inc=1, device_id={"sp": to}, device_id_type=pl.DeviceIdType.MESH)

    @pl.when(has_up & has_down)
    def _():
        tell(above_sem, me - 1)
        tell(below_sem, me + 1)

    def meet_far():
        def from_above(i, _):
            pl.semaphore_wait(above_sem, 1)

            @pl.when(has_down)
            def _():
                tell(above_sem, me - 1)

            return 0

        def from_below(i, _):
            pl.semaphore_wait(below_sem, 1)

            @pl.when(has_up)
            def _():
                tell(below_sem, me + 1)

            return 0

        lax.fori_loop(0, jnp.maximum(n - 2 - me, 0), from_above, 0)
        lax.fori_loop(0, jnp.maximum(me - 1, 0), from_below, 0)

    slab = rows // chunks

    def own_tok(m):
        return tok_ref.at[pl.ds(m * slab, slab)]

    def tok_at(h, m, src):
        return tok_buf.at[h, src, pl.ds(m * slab, slab)]

    def tok_z(m):
        return rdma(own_tok(m), tok_at(mine, m, t), t_s, tz_r.at[m], sp=partner)

    def tok_z_in(m):
        here = tok_at(other, m, t)
        return rdma(here, here, t_s, tz_r.at[m], sp=partner)

    def x_sem(own, m, d):
        return (0 if own else 1 + m) * max(half - 1, 1) + d - 1

    def tok_x(own, m, d):
        h = mine if own else other
        src = own_tok(m) if own else tok_at(h, m, t)
        return rdma(src, tok_at(h, m, t), t_s, tx_r.at[x_sem(own, m, d)], tp=2 * lax.rem(pair + d, half) + parity)

    def tok_x_in(own, m, d):
        src = 2 * lax.rem(pair + half - d, half) + parity
        here = tok_buf.at[mine, src] if own else tok_at(other, m, src)
        return rdma(here, here, t_s, tx_r.at[x_sem(own, m, d)], tp=src)

    def tok_c(own, m, d):
        h = mine if own else other
        src = 2 * lax.rem(pair + half - d, half) + parity
        there = tok_at(h, m, src)
        here = own_tok(m) if own and d == 0 else there
        return rdma(here, there, t_s, tc_r.at[0 if own else 1], tp=2 * pair + 1 - parity)

    tok_local = pltpu.make_async_copy(tok_ref, tok_buf.at[mine, t], t_loc)

    for d in range(1, half):
        for m in range(chunks):
            tok_x(True, m, d).start()

    owns = [wfk_ref, wfv_ref, wfq_ref, wrv_ref, qk_own]
    fox_arrays, ret_arrays = (0, 1, 2), (3, 4)
    starts = {}
    for group in (fox_arrays, ret_arrays):
        at = 0
        for c in group:
            starts[c] = (at, at + owns[c].shape[1])
            at = starts[c][1]
    fox_wide, ret_wide = starts[2][1], starts[4][1]
    q_at = starts[2][0]
    step = shard // n_grp
    count = len(owns)

    def w_at(c, src, part):
        start = pl.multiple_of(src * shard + part * step, step)
        return w_buf.at[pl.ds(start, step), starts[c][0] : starts[c][1]]

    far = list(range(2, n - 1))
    local_at = {c: c - group[0] for group in (fox_arrays, ret_arrays) for c in group}

    def w_recv(c, src):
        return w_r.at[src * len(fox_arrays) + local_at[c]]

    def w_send(c, to):
        here = owns[c].at[pl.ds(pl.multiple_of(g * step, step), step)]
        return rdma(here, w_at(c, me, g), w_s.at[c], w_recv(c, me), sp=to)

    def w_on(c, src, to):
        here = w_at(c, src, g)
        return rdma(here, here, w_s.at[c], w_recv(c, src), sp=to)

    def w_in(c, src):
        here = w_at(c, src, g)
        return rdma(here, here, w_s.at[c], w_recv(c, src), sp=src)

    def w_side(c, k, d):
        here = w_at(c, toward(k), g)
        return rdma(here, here, wy_s.at[local_at[c]], wy_r.at[wy_at(c, k in late_of(c))], grp=lax.rem(g + d, n_grp))

    def late_of(c):
        return far if c in fox_arrays else [n - 1]

    def wy_at(c, late):
        return local_at[c] + (len(fox_arrays) if late and c not in (0, 1) else 0)

    def w_late(c):
        drained(wy_r.at[wy_at(c, True)], w_several(c, len(late_of(c)) * (n_grp - 1)))

    def w_early(c):
        w_local(c).wait()
        drained(wy_r.at[wy_at(c, False)], w_several(c, (n - 1 - len(late_of(c))) * (n_grp - 1)))

    def w_several(c, pieces):
        return w_buf.at[: pieces * step, starts[c][0] : starts[c][1]]

    def w_local(c):
        start = pl.multiple_of(me * shard, shard)
        return pltpu.make_async_copy(
            owns[c], w_buf.at[pl.ds(start, shard), starts[c][0] : starts[c][1]], w_loc.at[local_at[c]]
        )

    fox_up = jnp.where(is_ret & (mine == 0), partner, fox_of(couple + 1))
    fox_down = jnp.where(is_ret & (mine == 1), partner, jnp.where(couple >= 1, fox_of(jnp.maximum(couple - 1, 0)), -1))
    ret_up = jnp.where(is_fox & (mine == 0), partner, ret_of(couple + 1))
    ret_down = jnp.where(is_fox & (mine == 1), partner, jnp.where(couple >= 1, ret_of(jnp.maximum(couple - 1, 0)), -1))

    def send_weights(arrays):
        for c in arrays:
            up, down = (fox_up, fox_down) if c in fox_arrays else (ret_up, ret_down)

            @pl.when(up < n)
            def _(c=c, up=up):
                w_send(c, up).start()

            @pl.when(down >= 0)
            def _(c=c, down=down):
                w_send(c, down).start()

    def sends_from(p, arrays):
        q, b = p // 2, p % 2
        plane = (lambda i: 2 * i + 1 - i % 2) if arrays[0] in fox_arrays else (lambda i: 2 * i + i % 2)
        uses = plane(q) == p
        up = p + 1 if not uses and b == 0 else plane(q + 1)
        down = p - 1 if not uses and b == 1 else (plane(q - 1) if q else -1)
        passes = ((p if up < n else 0) + (n - 1 - p if down >= 0 else 0)) if uses else 0
        return (up < n) + (down >= 0) + passes

    def swap_tokens():
        for m in range(chunks):
            tok_z(m).start()

    send_weights((0, 1))
    for m in range(chunks):
        tok_c(True, m, 0).start()

    swap_tokens()

    @pl.when(is_ret)
    def _():
        send_weights((2,))

    meet_far()
    send_weights((3,))
    drained(in_sem.at[0], wqk_buf)
    qk_own[...] = wqk_buf[...].astype(jnp.float32).T.astype(jnp.bfloat16)

    @pl.when(is_ret)
    def _():
        send_weights((4,))

    tok_local.start()

    @pl.when(is_fox)
    def _():
        for c in fox_arrays:
            w_local(c).start()

    @pl.when(is_ret)
    def _():
        for c in ret_arrays:
            w_local(c).start()

    depth = mix_buf.shape[1] // 2
    out_cols = ret_out_ref.shape[1]

    out_step = depth // n_grp
    out_refs = [ret_out_ref, fox_out_ref]

    def out_cols_of(src):
        return pl.ds(pl.multiple_of(src * out_cols, out_cols), out_cols)

    def out_at(c, src):
        return wout_buf.at[pl.ds(pl.multiple_of(c * depth + g * out_step, out_step), out_step), out_cols_of(src)]

    def out_both(src):
        return wout_buf.at[: 2 * out_step, out_cols_of(src)]

    def out_hop(c, src, to, first):
        here = out_refs[c].at[pl.ds(pl.multiple_of(g * out_step, out_step), out_step)] if first else out_at(c, src)
        return rdma(here, out_at(c, src), o_s, o_r.at[2 * src + c], sp=to)

    def out_local(c):
        return pltpu.make_async_copy(out_refs[c], wout_buf.at[c * depth : (c + 1) * depth, out_cols_of(me)], o_loc)

    def out_begin():
        for c in range(2):

            @pl.when(has_up)
            def _(c=c):
                out_hop(c, me, me + 1, True).start()

            @pl.when(has_down)
            def _(c=c):
                out_hop(c, me, me - 1, True).start()

            out_local(c).start()

    def out_relay(i):
        for src, to in ((me - i, me + 1), (me + i, me - 1)):

            @pl.when((src >= 0) & (src < n))
            def _(src=src, to=to):
                for c in range(2):
                    there = out_at(c, src)
                    rdma(there, there, o_s, o_r.at[2 * src + c], sp=src).wait_recv()

                    @pl.when((to >= 0) & (to < n))
                    def _(c=c):
                        out_hop(c, src, to, False).start()

                    for d in range(1, n_grp):
                        here = out_at(c, src)
                        at = (d - 1) * n + src
                        rdma(here, here, oy_s, oy_r.at[at], grp=lax.rem(g + d, n_grp)).start()

    def out_arrive(src):
        for d in range(1, n_grp):
            drained(oy_r.at[(d - 1) * n + src], out_both(src))

    def w_pass(c, src):
        up, down = (fox_up, fox_down) if c in fox_arrays else (ret_up, ret_down)

        @pl.when((src < me) & (up < n))
        def _():
            w_on(c, src, up).start()

        @pl.when((src > me) & (down >= 0))
        def _():
            w_on(c, src, down).start()

    def w_relay(arrays, ks):
        for i in ks:
            for c in arrays:
                w_in(c, toward(i)).wait_recv()
                w_pass(c, toward(i))
                for d in range(1, n_grp):
                    w_side(c, i, d).start()

    def w_arrive(arrays):
        for c in arrays:
            w_local(c).wait()
            drained(wy_r.at[local_at[c]], w_several(c, (n - 1) * (n_grp - 1)))

    def normalize(h):
        squares = jnp.zeros((rows, 1), jnp.float32)
        for i in range(n_tp):
            part = tok_buf[h, i].astype(jnp.float32)
            squares = squares + jnp.sum(part * part, axis=-1, keepdims=True)
        scale = lax.rsqrt(squares * (1.0 / (n_tp * feats)) + epsilon)
        at = pl.ds(pl.multiple_of(h * rows, rows), rows)
        for i in range(n_tp):
            part = tok_buf[h, i].astype(jnp.float32)
            cols = slice(i * feats, (i + 1) * feats)
            norm_buf[at, cols] = (part * scale * gain_buf[:, cols]).astype(jnp.bfloat16)


    def tok_own():
        for d in range(1, half):
            tok_x_in(True, 0, d).wait_recv()
            for m in range(chunks):
                tok_c(True, m, d).start()

    def tok_swap(m):
        tok_z_in(m).wait_recv()
        for d in range(1, half):
            tok_x(False, m, d).start()
        tok_c(False, m, 0).start()

    def tok_last(m):
        for d in range(1, half):
            tok_x_in(False, m, d).wait_recv()
            tok_c(False, m, d).start()

    def tok_ready(own):
        if own:
            tok_local.wait()
        drained(tc_r.at[0 if own else 1], tok_buf.at[mine if own else other, :half])

    for copy in brought:
        copy.wait()

    @pl.when(is_fox)
    def _():
        w_relay((0, 1), [1, n - 1])
        send_weights((4, 2))

    @pl.when(is_fox)
    def _():
        tok_swap(0)
        tok_own()
        for m in range(1, chunks):
            tok_swap(m)
        w_relay((0, 1), far)
        w_relay((2,), [1, n - 1])

    @pl.when(is_ret)
    def _():
        tok_own()
        for m in range(chunks):
            tok_swap(m)
            if m == 1:
                w_relay((3,), far)
            if m == 2:
                w_relay((4,), far)
        w_relay(ret_arrays, [1])

    out_begin()
    tok_ready(True)
    normalize(mine)

    row_id = lax.broadcasted_iota(jnp.int32, (rows, rows), 0)
    col_id = lax.broadcasted_iota(jnp.int32, (rows, rows), 1)
    causal = col_id <= row_id

    def norm_rows(h):
        return norm_buf[pl.ds(pl.multiple_of(h * rows, rows), rows), :]

    block = rows // n_tp
    span = 2 * block

    def mix_rows(d):
        return pl.ds(pl.multiple_of(lax.rem(pair + d, half) * span, span), span)

    away = [*range(1, half), 0]

    def mix_copy(first, d):
        here = mix_pair.at[other, mix_rows(d)]
        return rdma(here, mix_buf.at[mix_rows(d), first : first + depth], mix_s.at[d], mix_r.at[d], sp=partner)

    def mix_send(first):
        for d in away:
            mix_copy(first, d).start()

    def mix_own(first):
        mix_buf[:, first : first + depth] = mix_pair[mine]

    def mix_in(d):
        here = mix_buf.at[mix_rows(d), :depth]
        rdma(here, here, mix_s.at[d], mix_r.at[d], sp=partner).wait_recv()

    def kv_copy(b, q):
        at = 2 * couple + b
        return rdma(kv_buf.at[at], kv_buf.at[at], kv_s.at[2 * q + b], kv_r.at[at], sp=fox_of(q))

    def kv_in(at):
        return rdma(kv_buf.at[at], kv_buf.at[at], kv_s.at[at], kv_r.at[at], sp=partner)

    def sum_copy(q):
        return rdma(sum_buf.at[couple], sum_buf.at[couple], sum_s.at[q], sum_r.at[couple], sp=ret_of(q))

    def sum_in(q):
        return rdma(sum_buf.at[q], sum_buf.at[q], sum_s.at[q], sum_r.at[q], sp=partner)

    def later(act):
        for q in range(1, couples):

            @pl.when(q > couple)
            def _(q=q):
                act(jnp.int32(q))

    def after_tokens():
        for m in range(chunks):
            tok_last(m)

    @pl.when(is_fox)
    def _():
        def project_kv(b):
            kv_buf[2 * couple + b] = jnp.dot(
                norm_rows(b), w_buf[:, :q_at], preferred_element_type=jnp.float32
            ).astype(jnp.bfloat16)
            later(lambda q: kv_copy(b, q).start())

        def q_part(srcs):
            total = 0.0
            for src in srcs:
                cols = pl.ds(pl.multiple_of(src * shard, shard), shard)
                total = total + jnp.dot(
                    norm_buf[:, cols], w_buf[cols, q_at:fox_wide], preferred_element_type=jnp.float32
                )
            return total

        for b in range(2):
            for h in range(fh):
                own_cols = pl.ds(pl.multiple_of((2 * couple + b) * rows, rows), rows)
                own = jnp.where(row_id == col_id, gates_buf[h : h + 1, own_cols], 0.0)
                gate_buf[h, b * rows : (b + 1) * rows] = jnp.broadcast_to(
                    jnp.sum(own, axis=1, keepdims=True), (rows, lanes)
                )
        after_tokens()
        w_arrive((0, 1))
        project_kv(mine)
        w_relay((2,), far)
        out_relay(1)
        tok_ready(False)
        normalize(other)
        project_kv(other)
        w_early(2)
        sums_buf[:, : fh * fd] = q_part([me, toward(1), toward(n - 1)])
        w_late(2)
        proj_buf[:, : fh * fd] = (sums_buf[:, : fh * fd] + q_part([toward(k) for k in far])).astype(jnp.bfloat16)

        def block_cols(at):
            return pl.ds(pl.multiple_of(at * rows, rows), rows)

        def rep_cols(x, wide):
            return jnp.concatenate([x] * (wide // lanes), axis=1)

        def attend(at, top_row, first, offset):
            size_ = 2 * rows - top_row
            here = slice(top_row, 2 * rows)
            for h in range(fh):
                query = proj_buf[here, h * fd : (h + 1) * fd]
                k = kv_buf[at, :, h * fd : (h + 1) * fd]
                v = kv_buf[at, :, (fh + h) * fd : (fh + h + 1) * fd]
                logits = lax.dot_general(query, k, NT, preferred_element_type=jnp.float32) * fd ** (-0.5)
                logits = logits + rep_cols(gate_buf[h, here], rows) - gates_buf[h : h + 1, block_cols(at)]
                if offset is not None:
                    row = lax.broadcasted_iota(jnp.int32, (size_, rows), 0)
                    col = lax.broadcasted_iota(jnp.int32, (size_, rows), 1)
                    logits = jnp.where(col <= row, logits, -jnp.inf)
                top_new = jnp.broadcast_to(jnp.max(logits, axis=-1, keepdims=True), (size_, lanes))
                if not first:
                    top = top_buf[h, here]
                    top_new = jnp.maximum(top, top_new)
                p = jnp.exp(logits - rep_cols(top_new, rows))
                total = jnp.broadcast_to(jnp.sum(p, axis=-1, keepdims=True), (size_, lanes))
                weighted = jnp.dot(p.astype(jnp.bfloat16), v, preferred_element_type=jnp.float32)
                if not first:
                    rescale = jnp.exp(top - top_new)
                    total = total_buf[h, here] * rescale + total
                    weighted = weighted_buf[h, here] * rescale[:, :fd] + weighted
                top_buf[h, here] = top_new
                total_buf[h, here] = total
                weighted_buf[h, here] = weighted

        attend(2 * couple, 0, True, 0)
        attend(2 * couple + 1, rows, False, 0)
        out_relay(2)

        def past(i, _):
            q = lax.div(i, 2)
            b = jnp.where(lax.rem(i, 2) == 0, fox_of(q) - 2 * q, 1 - (fox_of(q) - 2 * q))
            at = 2 * q + b
            kv_in(at).wait_recv()
            attend(at, 0, False, None)
            return 0

        lax.fori_loop(0, 2 * couple, past, 0)
        for b in range(2):
            at = slice(b * rows, (b + 1) * rows)
            for h in range(fh):
                mix_pair[b, :, h * fd : (h + 1) * fd] = (
                    weighted_buf[h, at] / total_buf[h, at, :fd]
                ).astype(jnp.bfloat16)
        mix_send(depth)
        mix_own(depth)
        for k in range(3, n):
            out_relay(k)
        for d in away:
            mix_copy(depth, d).wait_send()
        later(lambda q: kv_copy(0, q).wait_send())
        later(lambda q: kv_copy(1, q).wait_send())

    @pl.when(is_ret)
    def _():
        distance = jnp.maximum(row_id - col_id, 0).astype(jnp.float32)
        key_scale = dk ** (-0.5)
        for h in range(hr):
            within_buf[h] = jnp.where(causal, jnp.exp(distance * decay_ref[h]) * key_scale, 0.0)
        w_relay(ret_arrays, [n - 1])
        after_tokens()
        tok_ready(False)
        normalize(other)
        out_relay(1)

        def ret_part(srcs):
            total = 0.0
            for src in srcs:
                cols = pl.ds(pl.multiple_of(src * shard, shard), shard)
                total = total + jnp.dot(
                    norm_buf[:, cols], w_buf[cols, :ret_wide], preferred_element_type=jnp.float32
                )
            return total

        for c in ret_arrays:
            w_early(c)
        sums_buf[:, :ret_wide] = ret_part([me] + [toward(k) for k in range(1, n - 1)])
        for c in ret_arrays:
            w_late(c)
        proj_buf[:, :ret_wide] = (sums_buf[:, :ret_wide] + ret_part([toward(n - 1)])).astype(jnp.bfloat16)
        rv_at, rq_at = starts[3][0], starts[4][0]
        lone = jnp.zeros((dk, vd), jnp.float32)

        def part(b, first, wide):
            return proj_buf[b * rows : (b + 1) * rows, first : first + wide]

        def split(x, axis):
            top = x.astype(jnp.bfloat16)
            rest = x - top.astype(jnp.float32)
            middle = rest.astype(jnp.bfloat16)
            low = (rest - middle.astype(jnp.float32)).astype(jnp.bfloat16)
            return jnp.concatenate((top, middle, low), axis=axis)

        def summary(b, h):
            past_end = rows - 1.0 - lax.broadcasted_iota(jnp.int32, (rows, dk), 0).astype(jnp.float32)
            keys = part(b, rq_at + (hr + h) * dk, dk).astype(jnp.float32) * key_scale
            parts = lax.dot_general(
                split(keys * jnp.exp(past_end * decay_ref[h]), 1),
                part(b, rv_at + h * vd, vd),
                TN,
                preferred_element_type=jnp.float32,
            )
            return parts[:dk] + parts[dk : 2 * dk] + parts[2 * dk :]

        early = [summary(0, h) for h in range(hr)]
        for h in range(hr):
            sum_buf[couple, h] = jnp.exp(lone + float(rows) * decay_ref[h]) * early[h] + summary(1, h)
        later(lambda q: sum_copy(q).start())

        for b in range(2):
            for h in range(hr):
                rk = part(b, rq_at + (hr + h) * dk, dk)
                rv = part(b, rv_at + h * vd, vd)
                scores = lax.dot_general(
                    part(b, rq_at + h * dk, dk), rk, NT, preferred_element_type=jnp.float32
                )
                raw_buf[b, h] = jnp.dot(
                    split(scores * within_buf[h], 1),
                    jnp.concatenate((rv, rv, rv), axis=0),
                    preferred_element_type=jnp.float32,
                )
        out_relay(2)

        offset = (couple * 2 * rows).astype(jnp.float32)

        def gather(q, entering):
            sum_in(q).wait_recv()
            gap = ((couple - 1 - q) * 2 * rows).astype(jnp.float32)
            return tuple(entering[h] + jnp.exp(lone + gap * decay_ref[h]) * sum_buf[q, h] for h in range(hr))

        entering = tuple(jnp.exp(lone + offset * decay_ref[h]) * state_buf[h] for h in range(hr))
        entering = lax.fori_loop(0, couple, gather, entering)
        second = tuple(jnp.exp(lone + float(rows) * decay_ref[h]) * entering[h] + early[h] for h in range(hr))
        since = lax.broadcasted_iota(jnp.int32, (rows, vd), 0).astype(jnp.float32) + 1.0

        for b in range(2):
            for h in range(hr):
                rq = part(b, rq_at + h * dk, dk)
                carried = jnp.dot(
                    jnp.concatenate((rq, rq, rq), axis=1),
                    split((entering, second)[b][h], 0),
                    preferred_element_type=jnp.float32,
                )
                raw = raw_buf[b, h] + carried * jnp.exp(since * decay_ref[h])
                center = raw - jnp.mean(raw, axis=-1, keepdims=True)
                variance = jnp.mean(center * center, axis=-1, keepdims=True)
                cols = slice(h * vd, (h + 1) * vd)
                mix_pair[b, :, cols] = (center * lax.rsqrt(variance + epsilon) * hgain_buf[:, cols]).astype(
                    jnp.bfloat16
                )
        mix_send(0)
        mix_own(0)
        for k in range(3, n):
            out_relay(k)
        for d in away:
            mix_copy(0, d).wait_send()
        later(lambda q: sum_copy(q).wait_send())

    wide, pieces = out_cols, n

    def piece_cols(piece):
        return pl.ds(pl.multiple_of(piece * wide, wide), wide)

    def slot(d):
        return pl.ds(pl.multiple_of(lax.rem(pair + d, half) * block, block), block)

    def pair_copy(piece, d):
        cols = piece_cols(piece)
        return rdma(
            rs_send.at[1 - parity, slot(d), cols],
            pair_buf.at[slot(d), cols],
            pair_s,
            pair_r.at[piece * half + d],
            tp=t + 1 - 2 * parity,
        )

    def rs_copy(d, piece):
        cols = piece_cols(piece)
        return rdma(
            pair_sum.at[slot(d), cols],
            far_ref.at[d - 1, :, cols],
            rs_s.at[d - 1],
            rs_r.at[d - 1],
            tp=2 * lax.rem(pair + d, half) + parity,
        )

    def project(piece, d):
        cols = piece_cols(piece)
        value = jnp.dot(mix_buf[mix_rows(d), :], wout_buf[:, cols], preferred_element_type=jnp.float32)
        value = value.astype(jnp.bfloat16)
        for b in range(2):
            rs_send[b, slot(d), cols] = value[b * block : (b + 1) * block]
        pair_copy(piece, d).start()

    def reduce(piece, d):
        cols = piece_cols(piece)
        pair_copy(piece, d).wait_recv()
        both = rs_send[parity, slot(d), cols].astype(jnp.float32) + pair_buf[slot(d), cols].astype(jnp.float32)
        if d:
            pair_sum[slot(d), cols] = both.astype(jnp.bfloat16)
            rs_copy(d, piece).start()
        else:
            near_ref[:, cols] = both

    def order(i):
        falling = jnp.where(i <= me, me - i, i)
        rising = jnp.where(i <= n - 1 - me, me + i, n - 1 - i)
        return jnp.where(lower, rising, falling)

    drained(o_loc, wout_buf.at[:, out_cols_of(me)])
    for d in range(1, half):
        mix_in(d)
        project(me, d)
    mix_in(0)

    def turn(i, _):
        out_arrive(order(i))
        for d in range(1, half):
            project(order(i), d)
            reduce(order(i - 1), d)
        project(order(i - 1), 0)
        return 0

    lax.fori_loop(1, n, turn, 0)
    for d in range(1, half):
        reduce(order(jnp.int32(n - 1)), d)
    project(order(jnp.int32(n - 1)), 0)
    for piece in range(pieces):
        reduce(piece, 0)

    slabs = rows * (2 * n_tp - 1) // (2 * n_tp)
    drained(t_s, tok_buf.at[:, :, :slabs])
    for p in range(n):

        @pl.when(me == p)
        def _(p=p):
            for arrays in (fox_arrays, ret_arrays):
                for c in arrays:
                    if sends_from(p, arrays):
                        drained(w_s.at[c], w_several(c, sends_from(p, arrays)))
            hops = 2 * ((p + 1 if p + 1 < n else 0) + (n - p if p else 0))
            drained(o_s, wout_buf.at[: hops * out_step // n])

    drained(oy_s, wout_buf.at[: 2 * (n - 1) * (n_grp - 1) * out_step // n])

    def sides(arrays):
        for c in arrays:
            drained(wy_s.at[local_at[c]], w_several(c, (n - 1) * (n_grp - 1)))

    @pl.when(is_fox)
    def _():
        sides(fox_arrays)

    @pl.when(is_ret)
    def _():
        sides(ret_arrays)

    drained(pair_s, pair_buf)
    for d in range(1, half):
        drained(rs_s.at[d - 1], pair_sum.at[:block])
    for d in range(1, half):
        drained(rs_r.at[d - 1], far_ref.at[d - 1])


def paired(n, n_tp, n_grp, inputs):
    tokens, ret_query_weight, ret_state, fox_gates = inputs[0], inputs[2], inputs[9], inputs[11]
    fox_query_weight, ret_out_weight = inputs[5], inputs[12]
    rows, feats = tokens.shape
    hr, dk, vd = ret_state.shape
    fh = fox_gates.shape[1]
    fd = fox_query_weight.shape[1] // fh
    shard = ret_query_weight.shape[0]
    depth, out_cols = ret_out_weight.shape
    columns = out_cols * n
    wide = max(3 * fh * fd, 2 * hr * dk + hr * vd)
    half = n_tp // 2
    block = rows // n_tp
    chunks = 4
    couples = n // 2
    dma = pltpu.SemaphoreType.DMA
    far = max(half - 1, 1)
    side = max(n_grp - 1, 1) * n
    vmem = pl.BlockSpec(memory_space=pltpu.VMEM)
    hbm = pl.BlockSpec(memory_space=pl.ANY)
    bf16, f32 = jnp.bfloat16, jnp.float32
    size = (n, n_tp, n_grp, hr, dk, vd, fh, fd, chunks)
    near, other = pl.pallas_call(
        functools.partial(pair_kernel, size),
        out_shape=(pltpu.VMEM((block, columns), f32), pltpu.VMEM((far, block, columns), bf16)),
        in_specs=[hbm] * 14,
        out_specs=(vmem, vmem),
        scratch_shapes=[
            pltpu.SMEM((hr,), f32),
            pltpu.VMEM((1, n_tp * feats), f32),
            pltpu.VMEM((2 * hr * dk, shard), bf16),
            pltpu.VMEM((hr, dk, vd), f32),
            pltpu.VMEM((1, hr * vd), f32),
            pltpu.VMEM((fh, n * rows), f32),
            pltpu.VMEM((fh, 2 * rows, lanes), f32),
            pltpu.VMEM((hr, rows, rows), f32),
            pltpu.VMEM((2, hr, rows, vd), f32),
            pltpu.VMEM((2 * rows, wide), f32),
            pltpu.VMEM((2, n_tp, rows, feats), bf16),
            pltpu.VMEM((shard, 2 * hr * dk), bf16),
            pltpu.VMEM((n * shard, wide), bf16),
            pltpu.VMEM((2 * depth, columns), bf16),
            pltpu.VMEM((2 * rows, n_tp * feats), bf16),
            pltpu.VMEM((2 * rows, wide), bf16),
            pltpu.VMEM((n, rows, 2 * fh * fd), bf16),
            pltpu.VMEM((couples, hr, dk, vd), f32),
            pltpu.VMEM((2, rows, depth), bf16),
            pltpu.VMEM((rows, 2 * depth), bf16),
            pltpu.VMEM((2, rows // 2, columns), bf16),
            pltpu.VMEM((rows // 2, columns), bf16),
            pltpu.VMEM((rows // 2, columns), bf16),
            pltpu.VMEM((fh, 2 * rows, lanes), f32),
            pltpu.VMEM((fh, 2 * rows, lanes), f32),
            pltpu.VMEM((fh, 2 * rows, fd), f32),
            dma((6,)),
            pltpu.SemaphoreType.REGULAR,
            pltpu.SemaphoreType.REGULAR,
            dma,
            dma((chunks,)),
            dma(((chunks + 1) * far,)),
            dma((2,)),
            dma,
            dma((5,)),
            dma((3 * n,)),
            dma((3,)),
            dma((6,)),
            dma((3,)),
            dma,
            dma((2 * n,)),
            dma,
            dma((side,)),
            dma,
            dma((2 * couples,)),
            dma((n,)),
            dma((couples,)),
            dma((couples,)),
            dma((half,)),
            dma((half,)),
            dma,
            dma((n * half,)),
            dma((far,)),
            dma((far,)),
        ],
        compiler_params=pltpu.CompilerParams(
            collective_id=0, has_side_effects=True, vmem_limit_bytes=56 * 1024 * 1024
        ),
        name="layer",
    )(
        tokens,
        inputs[1][None, :],
        inputs[2].T,
        inputs[3].T,
        inputs[4],
        inputs[5],
        inputs[6],
        inputs[7],
        inputs[8],
        inputs[9],
        inputs[10][None, :],
        inputs[11].T,
        inputs[12],
        inputs[13],
    )
    for d in range(half - 1):
        near = near + other[d].astype(f32)
    return near.astype(bf16)


def pairs_fit(n, n_tp, n_grp, inputs):
    rows, feats = inputs[0].shape
    hr, dk, vd = inputs[9].shape
    shard = inputs[2].shape[0]
    depth, out_cols = inputs[12].shape
    wide = inputs[5].shape[1]
    full = all(w % lanes == 0 for w in (out_cols, wide, 2 * hr * dk, hr * vd, feats, depth, rows))
    even = n % 2 == 0 and n > 2 and n_tp % 2 == 0 and n_grp > 1
    tiles = rows % (32 * n_tp) == 0 and rows % 32 == 0 and shard % (16 * n_grp) == 0 and depth % (16 * n_grp * n) == 0 and vd <= lanes
    columns = n * out_cols
    held = 8 * rows * n_tp * feats + 2 * n * shard * 3 * wide + 4 * depth * columns + 4 * n * rows * wide + 6 * rows * columns
    return full and even and tiles and depth == wide == hr * vd and held < 40 * 1024 * 1024


def local(
    n,
    n_tp,
    n_grp,
    tokens,
    norm_gain,
    ret_query_weight,
    ret_key_weight,
    ret_value_weight,
    fox_query_weight,
    fox_key_weight,
    fox_value_weight,
    ret_decay,
    ret_state,
    head_norm_gain,
    fox_gates,
    ret_out_weight,
    fox_out_weight,
):
    inputs = (
        tokens,
        norm_gain,
        ret_query_weight,
        ret_key_weight,
        ret_value_weight,
        fox_query_weight,
        fox_key_weight,
        fox_value_weight,
        ret_decay,
        ret_state,
        head_norm_gain,
        fox_gates,
        ret_out_weight,
        fox_out_weight,
    )
    if pairs_fit(n, n_tp, n_grp, inputs):
        return paired(n, n_tp, n_grp, inputs)
    rows, feats = tokens.shape
    hr, dk, vd = ret_state.shape
    fh = fox_gates.shape[1]
    fd = fox_query_weight.shape[1] // fh
    shard = ret_query_weight.shape[0]
    width = 2 * hr * dk + hr * vd + 3 * fh * fd
    depth, out_cols = ret_out_weight.shape
    columns = out_cols * n
    direct = out_cols % 128 == 0
    if not direct:
        ret_out_weight, fox_out_weight = ret_out_weight.T, fox_out_weight.T
    dma = pltpu.SemaphoreType.DMA

    def gather_sems(arrays):
        side = max(n_grp - 1, 1) * n * arrays
        return [
            dma((n * arrays,)),
            dma((n * arrays,)),
            dma((n * arrays,)),
            dma((side,)),
            dma((side,)),
            dma((arrays,)),
        ]

    vmem = pl.BlockSpec(memory_space=pltpu.VMEM)
    smem = pl.BlockSpec(memory_space=pltpu.SMEM)
    hbm = pl.BlockSpec(memory_space=pl.ANY)
    size = (n, n_tp, n_grp, hr, dk, vd, fh, fd, direct)
    block = rows // n_tp
    peers = max(n_tp - 1, 1)
    far = max(n_tp // 2 - 1, 1)
    pieces = n if direct else 1
    return pl.pallas_call(
        functools.partial(kernel, size),
        out_shape=jax.ShapeDtypeStruct((block, columns), jnp.bfloat16),
        in_specs=[hbm, vmem, vmem, vmem, hbm, hbm, hbm, hbm, smem, vmem, vmem, vmem, hbm, hbm],
        out_specs=vmem,
        scratch_shapes=[
            pltpu.VMEM((n_tp, rows, feats), jnp.bfloat16),
            pltpu.VMEM((shard, 2 * hr * dk), jnp.bfloat16),
            pltpu.VMEM((n * shard, width), jnp.bfloat16),
            pltpu.VMEM((2 * depth, columns) if direct else (columns, 2 * depth), jnp.bfloat16),
            pltpu.VMEM((rows, n_tp * feats), jnp.bfloat16),
            pltpu.VMEM((rows, width - 2 * fh * fd), jnp.bfloat16),
            pltpu.VMEM((n, rows, 2 * fh * fd), jnp.bfloat16),
            pltpu.VMEM((n, hr, dk, vd), jnp.float32),
            pltpu.VMEM((rows, 2 * depth), jnp.bfloat16),
            pltpu.VMEM((2, rows // 2, columns), jnp.bfloat16),
            pltpu.VMEM((rows // 2, columns), jnp.bfloat16),
            pltpu.VMEM((rows // 2, columns), jnp.bfloat16),
            pltpu.VMEM((far, block, columns), jnp.bfloat16),
            pltpu.VMEM((fh, rows, 1), jnp.float32),
            pltpu.VMEM((fh, rows, 1), jnp.float32),
            pltpu.VMEM((fh, rows, fd), jnp.float32),
            dma((peers,)),
            dma((peers,)),
            dma,
            dma((n,)),
            dma((n,)),
            dma((n,)),
            dma((n,)),
            dma((pieces,)),
            dma((pieces,)),
            dma((far * pieces,)),
            dma((far * pieces,)),
        ]
        + gather_sems(2)
        + gather_sems(3)
        + gather_sems(2),
        compiler_params=pltpu.CompilerParams(
            collective_id=0, has_side_effects=True, vmem_limit_bytes=56 * 1024 * 1024
        ),
        name="layer",
    )(
        tokens,
        norm_gain[None, :],
        ret_query_weight.T,
        ret_key_weight.T,
        ret_value_weight,
        fox_query_weight,
        fox_key_weight,
        fox_value_weight,
        ret_decay,
        ret_state,
        head_norm_gain[None, :],
        fox_gates.T,
        ret_out_weight,
        fox_out_weight,
    )


def solution(mesh):
    placed = (
        P(("grp", "sp"), "tp"),
        P(),
        P("sp", "tp"),
        P("sp", "tp"),
        P("sp", "tp"),
        P("sp", "tp"),
        P("sp", "tp"),
        P("sp", "tp"),
        P("tp"),
        P(("grp", "tp"), None, None),
        P("tp"),
        P("grp", "tp"),
        P("tp", "sp"),
        P("tp", "sp"),
    )
    body = functools.partial(local, mesh.shape["sp"], mesh.shape["tp"], mesh.shape["grp"])
    return jax.shard_map(
        body, mesh=mesh, in_specs=placed, out_specs=P(("grp", "sp", "tp"), None), check_vma=False
    )
```

```python
import functools

import jax
import jax.numpy as jnp
from jax import lax
from jax.experimental import pallas as pl
from jax.experimental.pallas import tpu as pltpu
from jax.sharding import PartitionSpec as P

epsilon = 1e-06
lanes = 128
highest = lax.Precision.HIGHEST
NT = (((1,), (1,)), ((), ()))
TN = (((0,), (0,)), ((), ()))


def rdma(src, dst, send_sem, recv_sem, **target):
    return pltpu.make_async_remote_copy(
        src_ref=src,
        dst_ref=dst,
        send_sem=send_sem,
        recv_sem=recv_sem,
        device_id=target,
        device_id_type=pl.DeviceIdType.MESH,
    )


class LineGather:
    def __init__(self, owns, place, sems, n, n_grp, me, g):
        self.owns, self.place, self.n, self.n_grp, self.me, self.g = owns, place, n, n_grp, me, g
        self.up, self.down, self.zr, self.ys, self.yr, self.loc = sems
        self.arrays = len(owns)
        self.rows = owns[0].shape[0]
        self.step = self.rows // n_grp

    def piece(self, part, src, c):
        return self.place(src, c, part * self.step, self.step)

    def own_piece(self, c):
        return self.owns[c].at[pl.ds(pl.multiple_of(self.g * self.step, self.step), self.step)]

    def hop(self, sems, to, src, c, first=False):
        here = self.own_piece(c) if first else self.piece(self.g, src, c)
        at = src * self.arrays + c
        return rdma(here, self.piece(self.g, src, c), sems.at[at], self.zr.at[at], sp=to)

    def side(self, d, src, c):
        at = ((d - 1) * self.n + src) * self.arrays + c
        here = self.piece(self.g, src, c)
        return rdma(here, here, self.ys.at[at], self.yr.at[at], grp=lax.rem(self.g + d, self.n_grp))

    def side_in(self, d, src, c):
        at = ((d - 1) * self.n + src) * self.arrays + c
        part = lax.rem(self.g + self.n_grp - d, self.n_grp)
        here = self.piece(part, src, c)
        return rdma(here, here, self.ys.at[at], self.yr.at[at], grp=part)

    def local(self, c):
        return pltpu.make_async_copy(self.owns[c], self.place(self.me, c, 0, self.rows), self.loc.at[c])

    def start(self):
        me, n = self.me, self.n
        for c in range(self.arrays):

            @pl.when(me + 1 < n)
            def _():
                self.hop(self.up, me + 1, me, c, True).start()

            @pl.when(me >= 1)
            def _():
                self.hop(self.down, me - 1, me, c, True).start()

        for c in range(self.arrays):
            self.local(c).start()

    def relay(self, k):
        me, n = self.me, self.n
        for c in range(self.arrays):
            for src, sems, to in ((me - k, self.up, me + 1), (me + k, self.down, me - 1)):

                @pl.when((src >= 0) & (src < n))
                def _(src=src, sems=sems, to=to):
                    self.hop(sems, me, src, c).wait_recv()

                    @pl.when((to >= 0) & (to < n))
                    def _():
                        self.hop(sems, to, src, c).start()

                    for d in range(1, self.n_grp):
                        self.side(d, src, c).start()

    def arrive_shard(self, src, arrays):
        for c in arrays:
            for d in range(1, self.n_grp):
                self.side_in(d, src, c).wait_recv()

    def arrive(self, arrays):
        for c in arrays:
            self.local(c).wait()

        def step(k, _):
            self.arrive_shard(lax.rem(self.me + k, self.n), arrays)
            return 0

        lax.fori_loop(1, self.n, step, 0)

    def finish(self):
        me, n = self.me, self.n

        def step(src, _):
            for c in range(self.arrays):

                @pl.when((src <= me) & (me + 1 < n))
                def _():
                    self.hop(self.up, me, src, c).wait_send()

                @pl.when((src >= me) & (me >= 1))
                def _():
                    self.hop(self.down, me, src, c).wait_send()

                @pl.when(src != me)
                def _():
                    for d in range(1, self.n_grp):
                        self.side(d, src, c).wait_send()

            return 0

        lax.fori_loop(0, n, step, 0)


def kernel(
    size,
    tok_ref,
    gain_ref,
    wq_ref,
    wk_ref,
    wrv_ref,
    wfq_ref,
    wfk_ref,
    wfv_ref,
    decay_ref,
    state_ref,
    hgain_ref,
    gates_ref,
    ret_out_ref,
    fox_out_ref,
    out_ref,
    tok_buf,
    qk_own,
    w_buf,
    wout_buf,
    norm_buf,
    proj_buf,
    kv_buf,
    sum_buf,
    mix_buf,
    rs_send,
    pair_buf,
    pair_sum,
    rs_buf,
    top_buf,
    total_buf,
    weighted_buf,
    tok_s,
    tok_r,
    tok_loc,
    kv_s,
    kv_r,
    sum_s,
    sum_r,
    pair_s,
    pair_r,
    rs_s,
    rs_r,
    *gather_sems,
):
    n, n_tp, n_grp, hr, dk, vd, fh, fd, direct = size
    me, t, g = lax.axis_index("sp"), lax.axis_index("tp"), lax.axis_index("grp")
    rows, feats = tok_ref.shape
    owns = [wfk_ref, wfv_ref, wfq_ref, wrv_ref, qk_own]
    early = 2
    starts = [0]
    for own in owns:
        starts.append(starts[-1] + own.shape[1])
    shard = qk_own.shape[0]

    def weight_place(src, c, first, count):
        start = pl.multiple_of(src * shard + first, count)
        return w_buf.at[pl.ds(start, count), starts[c] : starts[c + 1]]

    depth = mix_buf.shape[1] // 2
    out_cols = ret_out_ref.shape[1] if direct else ret_out_ref.shape[0]

    def out_place(src, c, first, count):
        if direct:
            start = pl.multiple_of(c * depth + first, count)
            return wout_buf.at[pl.ds(start, count), pl.ds(pl.multiple_of(src * out_cols, out_cols), out_cols)]
        start = pl.multiple_of(src * out_cols + first, count)
        return wout_buf.at[pl.ds(start, count), c * depth : (c + 1) * depth]

    def late_place(src, c, first, count):
        return weight_place(src, c + early, first, count)

    firsts = LineGather(owns[:early], weight_place, gather_sems[:6], n, n_grp, me, g)
    lasts = LineGather(owns[early:], late_place, gather_sems[6:12], n, n_grp, me, g)
    outs = LineGather([ret_out_ref, fox_out_ref], out_place, gather_sems[12:], n, n_grp, me, g)

    barrier = pltpu.get_barrier_semaphore()

    def greet(**target):
        pl.semaphore_signal(barrier, inc=1, device_id=target, device_id_type=pl.DeviceIdType.MESH)

    has_up, has_down = me + 1 < n, me >= 1
    for d in range(1, n_tp):
        greet(tp=lax.rem(t + d, n_tp))
    for d in range(1, n_grp):
        greet(grp=lax.rem(g + d, n_grp))

    @pl.when(has_up)
    def _():
        greet(sp=me + 1)

    @pl.when(has_down)
    def _():
        greet(sp=me - 1)

    turned = jnp.concatenate((wq_ref[...], wk_ref[...]), axis=0).astype(jnp.float32)
    qk_own[...] = turned.T.astype(jnp.bfloat16)

    count = n_tp - 1 + n_grp - 1 + has_up.astype(jnp.int32) + has_down.astype(jnp.int32)
    pl.semaphore_wait(barrier, count)

    def tok_copy(d):
        return rdma(tok_ref, tok_buf.at[t], tok_s.at[d - 1], tok_r.at[d - 1], tp=lax.rem(t + d, n_tp))

    def tok_in(d):
        src = lax.rem(t + n_tp - d, n_tp)
        return rdma(tok_ref, tok_buf.at[src], tok_s.at[d - 1], tok_r.at[d - 1], tp=src)

    firsts.start()
    lasts.start()
    tok_local = pltpu.make_async_copy(tok_ref, tok_buf.at[t], tok_loc)
    for d in range(1, n_tp):
        tok_copy(d).start()
    tok_local.start()

    def first_step(k, _):
        firsts.relay(k)

        lasts.relay(k)
        return 0

    lax.fori_loop(1, n, first_step, 0)
    outs.start()

    tok_local.wait()
    for d in range(1, n_tp):
        tok_in(d).wait_recv()
    squares = jnp.zeros((rows, 1), jnp.float32)
    for i in range(n_tp):
        part = tok_buf[i].astype(jnp.float32)
        squares = squares + jnp.sum(part * part, axis=-1, keepdims=True)
    scale = lax.rsqrt(squares * (1.0 / (n_tp * feats)) + epsilon)
    for i in range(n_tp):
        part = tok_buf[i].astype(jnp.float32)
        cols = slice(i * feats, (i + 1) * feats)
        norm_buf[:, cols] = (part * scale * gain_ref[:, cols]).astype(jnp.bfloat16)

    def kv_copy(src):
        return rdma(kv_buf.at[src], kv_buf.at[src], kv_s.at[src], kv_r.at[src], sp=jnp.minimum(me + 1, n - 1))

    def sum_copy(src):
        return rdma(sum_buf.at[src], sum_buf.at[src], sum_s.at[src], sum_r.at[src], sp=jnp.minimum(me + 1, n - 1))

    firsts.arrive((0, 1))
    kv_buf[me] = jnp.dot(
        norm_buf[...], w_buf[:, : starts[2]], preferred_element_type=jnp.float32
    ).astype(jnp.bfloat16)

    def kv_forward(k):
        src = me - k

        @pl.when(src >= 0)
        def _():
            kv_copy(src).wait_recv()

            @pl.when(has_up)
            def _():
                kv_copy(src).start()

    @pl.when(has_up)
    def _():
        kv_copy(me).start()

    outs.relay(1)
    lasts.arrive((0, 1, 2))
    proj_buf[...] = jnp.dot(
        norm_buf[...], w_buf[:, starts[2] :], preferred_element_type=jnp.float32
    ).astype(jnp.bfloat16)
    rv_at, rq_at = starts[3] - starts[2], starts[4] - starts[2]

    key_scale = dk ** (-0.5)
    position = lax.broadcasted_iota(jnp.int32, (rows, 1), 0).astype(jnp.float32)
    rq, rk, rv = [], [], []
    for h in range(hr):
        rq.append(proj_buf[:, rq_at + h * dk : rq_at + (h + 1) * dk])
        rk.append(proj_buf[:, rq_at + (hr + h) * dk : rq_at + (hr + h + 1) * dk])
        rv.append(proj_buf[:, rv_at + h * vd : rv_at + (h + 1) * vd])
        keys = rk[h].astype(jnp.float32) * key_scale
        trailing = jnp.exp((rows - 1.0 - position) * decay_ref[h])
        sum_buf[me, h] = lax.dot_general(
            keys * trailing, rv[h].astype(jnp.float32), TN, precision=highest, preferred_element_type=jnp.float32
        )

    @pl.when(has_up)
    def _():
        sum_copy(me).start()

    row_id = lax.broadcasted_iota(jnp.int32, (rows, rows), 0)
    col_id = lax.broadcasted_iota(jnp.int32, (rows, rows), 1)
    causal = col_id <= row_id
    own_cols = pl.ds(pl.multiple_of(me * rows, rows), rows)
    own_gates = [
        jnp.sum(jnp.where(row_id == col_id, gates_ref[h : h + 1, own_cols], 0.0), axis=1, keepdims=True)
        for h in range(fh)
    ]

    def attend(src, diagonal):
        key_cols = pl.ds(pl.multiple_of(src * rows, rows), rows)
        for h in range(fh):
            query = proj_buf[:, h * fd : (h + 1) * fd]
            k = kv_buf[src, :, h * fd : (h + 1) * fd]
            v = kv_buf[src, :, (fh + h) * fd : (fh + h + 1) * fd]
            logits = lax.dot_general(query, k, NT, preferred_element_type=jnp.float32) * fd ** (-0.5)
            logits = logits + own_gates[h] - gates_ref[h : h + 1, key_cols]
            if diagonal:
                logits = jnp.where(causal, logits, -jnp.inf)
            top_new = jnp.max(logits, axis=-1, keepdims=True)
            if not diagonal:
                top = top_buf[h]
                top_new = jnp.maximum(top, top_new)
            p = jnp.exp(logits - top_new)
            total = jnp.sum(p, axis=-1, keepdims=True)
            weighted = jnp.dot(p.astype(jnp.bfloat16), v, preferred_element_type=jnp.float32)
            if not diagonal:
                rescale = jnp.exp(top - top_new)
                total = total_buf[h] * rescale + total
                weighted = weighted_buf[h] * rescale + weighted
            top_buf[h] = top_new
            total_buf[h] = total
            weighted_buf[h] = weighted

    def forward(k):
        src = me - k

        @pl.when(src >= 0)
        def _():
            sum_copy(src).wait_recv()

            @pl.when(has_up)
            def _():
                sum_copy(src).start()

    attend(me, True)

    offset = (me * rows).astype(jnp.float32)
    lone = jnp.zeros((dk, vd), jnp.float32)

    def step(k, entering):
        src = me - k
        kv_forward(k)
        forward(k)

        @pl.when(k + 1 < n)
        def _():
            outs.relay(k + 1)


        @pl.when(src >= 0)
        def _():
            attend(src, False)

        gap = ((k - 1) * rows).astype(jnp.float32)
        there = jnp.maximum(src, 0)
        return tuple(
            entering[h]
            + jnp.where(src >= 0, jnp.exp(lone + gap * decay_ref[h]) * sum_buf[there, h], 0.0)
            for h in range(hr)
        )

    entering = tuple(jnp.exp(lone + offset * decay_ref[h]) * state_ref[h] for h in range(hr))
    entering = lax.fori_loop(1, n, step, entering)

    distance = jnp.maximum(row_id - col_id, 0).astype(jnp.float32)
    for h in range(hr):
        scores = lax.dot_general(rq[h], rk[h], NT, preferred_element_type=jnp.float32) * key_scale
        scores = jnp.where(causal, scores * jnp.exp(distance * decay_ref[h]), 0.0)
        inner = jnp.dot(scores, rv[h].astype(jnp.float32), precision=highest, preferred_element_type=jnp.float32)
        leading = jnp.exp((position + 1.0) * decay_ref[h])
        carried = jnp.dot(
            rq[h].astype(jnp.float32), entering[h], precision=highest, preferred_element_type=jnp.float32
        )
        raw = inner + carried * leading
        center = raw - jnp.mean(raw, axis=-1, keepdims=True)
        variance = jnp.mean(center * center, axis=-1, keepdims=True)
        cols = slice(h * vd, (h + 1) * vd)
        mix_buf[:, cols] = (center * lax.rsqrt(variance + epsilon) * hgain_ref[:, cols]).astype(jnp.bfloat16)
    for h in range(fh):
        cols = slice(hr * vd + h * fd, hr * vd + (h + 1) * fd)
        mix_buf[:, cols] = (weighted_buf[h] / total_buf[h]).astype(jnp.bfloat16)

    block = rows // n_tp
    columns = pair_buf.shape[1]
    wide = out_cols if direct else columns
    pieces = columns // wide
    half = n_tp // 2
    parity, pair = lax.rem(t, 2), lax.div(t, 2)

    def piece_cols(piece):
        return pl.ds(pl.multiple_of(piece * wide, wide), wide)

    def slot(at):
        return pl.ds(pl.multiple_of(at * block, block), block)

    def pair_copy(piece):
        cols = piece_cols(piece)
        return rdma(
            rs_send.at[1 - parity, :, cols],
            pair_buf.at[:, cols],
            pair_s.at[piece],
            pair_r.at[piece],
            tp=t + 1 - 2 * parity,
        )

    def rs_copy(d, piece):
        to = lax.rem(pair + d, half)
        cols = piece_cols(piece)
        at = (d - 1) * pieces + piece
        return rdma(
            pair_sum.at[slot(to), cols], rs_buf.at[d - 1, :, cols], rs_s.at[at], rs_r.at[at], tp=2 * to + parity
        )

    def project(piece):
        cols = piece_cols(piece)
        if direct:
            value = jnp.dot(mix_buf[...], wout_buf[:, cols], preferred_element_type=jnp.float32)
        else:
            value = lax.dot_general(mix_buf[...], wout_buf[...], NT, preferred_element_type=jnp.float32)
        value = value.astype(jnp.bfloat16)
        for b in range(n_tp):
            at = slice(b // 2 * block, (b // 2 + 1) * block)
            rs_send[b % 2, at, cols] = value[b * block : (b + 1) * block]
        pair_copy(piece).start()

    def reduce(piece):
        cols = piece_cols(piece)
        pair_copy(piece).wait_recv()
        both = rs_send[parity, :, cols].astype(jnp.float32) + pair_buf[:, cols].astype(jnp.float32)
        pair_sum[:, cols] = both.astype(jnp.bfloat16)
        for d in range(1, half):
            rs_copy(d, piece).start()

    def order(i):
        falling = jnp.where(i <= me, me - i, i)
        rising = jnp.where(i <= n - 1 - me, me + i, n - 1 - i)
        return jnp.where(2 * me >= n, falling, rising)

    if direct:
        for c in range(2):
            outs.local(c).wait()
        project(me)

        def out_step(i, _):
            outs.arrive_shard(order(i), (0, 1))
            project(order(i))
            reduce(order(i - 1))
            return 0

        lax.fori_loop(1, n, out_step, 0)
        reduce(order(jnp.int32(n - 1)))
    else:
        outs.arrive((0, 1))
        project(0)
        reduce(0)

    own = slot(pair)
    summed = rs_send[parity, own, :].astype(jnp.float32) + pair_buf[own, :].astype(jnp.float32)
    for d in range(1, half):
        for piece in range(pieces):
            rs_copy(d, piece).wait_recv()
        summed = summed + rs_buf[d - 1].astype(jnp.float32)
    out_ref[...] = summed.astype(jnp.bfloat16)

    for d in range(1, n_tp):
        tok_copy(d).wait_send()
    for piece in range(pieces):
        pair_copy(piece).wait_send()
        for d in range(1, half):
            rs_copy(d, piece).wait_send()
    firsts.finish()
    lasts.finish()
    outs.finish()

    @pl.when(has_up)
    def _():
        def step(src, _):
            kv_copy(src).wait_send()
            sum_copy(src).wait_send()
            return 0

        lax.fori_loop(0, me + 1, step, 0)


def pair_kernel(
    size,
    tok_ref,
    gain_ref,
    wq_ref,
    wk_ref,
    wrv_ref,
    wfq_ref,
    wfk_ref,
    wfv_ref,
    decay_hbm,
    state_ref,
    hgain_ref,
    gates_ref,
    ret_out_ref,
    fox_out_ref,
    near_ref,
    far_ref,
    decay_ref,
    gain_buf,
    wqk_buf,
    state_buf,
    hgain_buf,
    gates_buf,
    gate_buf,
    within_buf,
    raw_buf,
    sums_buf,
    tok_buf,
    qk_own,
    w_buf,
    wout_buf,
    norm_buf,
    proj_buf,
    kv_buf,
    sum_buf,
    mix_pair,
    mix_buf,
    rs_send,
    pair_buf,
    pair_sum,
    p_buf,
    top_buf,
    total_buf,
    weighted_buf,
    in_sem,
    above_sem,
    below_sem,
    t_s,
    tz_r,
    tx_r,
    tc_r,
    t_loc,
    w_s,
    w_r,
    wy_s,
    wy_r,
    w_loc,
    o_s,
    o_r,
    oy_s,
    oy_r,
    o_loc,
    kv_s,
    kv_r,
    sum_s,
    sum_r,
    mix_s,
    mix_r,
    pair_s,
    pair_r,
    rs_s,
    rs_r,
):
    n, n_tp, n_grp, hr, dk, vd, fh, fd, chunks = size
    me, t, g = lax.axis_index("sp"), lax.axis_index("tp"), lax.axis_index("grp")
    rows, feats = tok_ref.shape
    shard = qk_own.shape[0]
    couples = n // 2
    couple, mine = lax.div(me, 2), lax.rem(me, 2)
    other = 1 - mine
    partner = me + 1 - 2 * mine
    fox_mine = 1 - lax.rem(couple, 2)
    is_fox = mine == fox_mine
    is_ret = mine != fox_mine
    lower = 2 * me < n
    half = n_tp // 2
    parity, pair = lax.rem(t, 2), lax.div(t, 2)

    def fox_of(q):
        return 2 * q + 1 - lax.rem(q, 2)

    def ret_of(q):
        return 2 * q + lax.rem(q, 2)

    def toward(k):
        return lax.rem(jnp.where(lower, me + k, me + n - k), n)

    barrier = pltpu.get_barrier_semaphore()

    def greet(**target):
        pl.semaphore_signal(barrier, inc=1, device_id=target, device_id_type=pl.DeviceIdType.MESH)

    greet(tp=2 * pair + 1 - parity)
    for d in range(1, half):
        greet(tp=2 * lax.rem(pair + d, half) + parity)
    for d in range(1, n_grp):
        greet(grp=lax.rem(g + d, n_grp))
    has_up, has_down = me + 1 < n, me >= 1

    @pl.when(has_up)
    def _():
        greet(sp=me + 1)

    @pl.when(has_down)
    def _():
        greet(sp=me - 1)

    def drained(sem, ref):
        pltpu.make_async_copy(ref, ref, sem).wait()

    width = hr * dk
    pltpu.make_async_copy(wq_ref, wqk_buf.at[:width], in_sem.at[0]).start()
    pltpu.make_async_copy(wk_ref, wqk_buf.at[width:], in_sem.at[0]).start()
    brought = [
        pltpu.make_async_copy(src, dst, in_sem.at[i + 1])
        for i, (src, dst) in enumerate(
            ((gain_ref, gain_buf), (state_ref, state_buf), (hgain_ref, hgain_buf), (gates_ref, gates_buf), (decay_hbm, decay_ref))
        )
    ]
    for copy in brought:
        copy.start()

    pl.semaphore_wait(barrier, half + n_grp - 1 + has_up.astype(jnp.int32) + has_down.astype(jnp.int32))

    def tell(sem, to):
        pl.semaphore_signal(sem, inc=1, device_id={"sp": to}, device_id_type=pl.DeviceIdType.MESH)

    @pl.when(has_up & has_down)
    def _():
        tell(above_sem, me - 1)
        tell(below_sem, me + 1)

    def meet_far():
        def from_above(i, _):
            pl.semaphore_wait(above_sem, 1)

            @pl.when(has_down)
            def _():
                tell(above_sem, me - 1)

            return 0

        def from_below(i, _):
            pl.semaphore_wait(below_sem, 1)

            @pl.when(has_up)
            def _():
                tell(below_sem, me + 1)

            return 0

        lax.fori_loop(0, jnp.maximum(n - 2 - me, 0), from_above, 0)
        lax.fori_loop(0, jnp.maximum(me - 1, 0), from_below, 0)

    slab = rows // chunks

    def own_tok(m):
        return tok_ref.at[pl.ds(m * slab, slab)]

    def tok_at(h, m, src):
        return tok_buf.at[h, src, pl.ds(m * slab, slab)]

    def tok_z(m):
        return rdma(own_tok(m), tok_at(mine, m, t), t_s, tz_r.at[m], sp=partner)

    def tok_z_in(m):
        here = tok_at(other, m, t)
        return rdma(here, here, t_s, tz_r.at[m], sp=partner)

    def x_sem(own, m, d):
        return (0 if own else 1 + m) * max(half - 1, 1) + d - 1

    def tok_x(own, m, d):
        h = mine if own else other
        src = own_tok(m) if own else tok_at(h, m, t)
        return rdma(src, tok_at(h, m, t), t_s, tx_r.at[x_sem(own, m, d)], tp=2 * lax.rem(pair + d, half) + parity)

    def tok_x_in(own, m, d):
        src = 2 * lax.rem(pair + half - d, half) + parity
        here = tok_buf.at[mine, src] if own else tok_at(other, m, src)
        return rdma(here, here, t_s, tx_r.at[x_sem(own, m, d)], tp=src)

    def tok_c(own, m, d):
        h = mine if own else other
        src = 2 * lax.rem(pair + half - d, half) + parity
        there = tok_at(h, m, src)
        here = own_tok(m) if own and d == 0 else there
        return rdma(here, there, t_s, tc_r.at[0 if own else 1], tp=2 * pair + 1 - parity)

    tok_local = pltpu.make_async_copy(tok_ref, tok_buf.at[mine, t], t_loc)

    for d in range(1, half):
        for m in range(chunks):
            tok_x(True, m, d).start()

    owns = [wfk_ref, wfv_ref, wfq_ref, wrv_ref, qk_own]
    fox_arrays, ret_arrays = (0, 1, 2), (3, 4)
    starts = {}
    for group in (fox_arrays, ret_arrays):
        at = 0
        for c in group:
            starts[c] = (at, at + owns[c].shape[1])
            at = starts[c][1]
    fox_wide, ret_wide = starts[2][1], starts[4][1]
    q_at = starts[2][0]
    step = shard // n_grp
    count = len(owns)

    def w_at(c, src, part):
        start = pl.multiple_of(src * shard + part * step, step)
        return w_buf.at[pl.ds(start, step), starts[c][0] : starts[c][1]]

    far = list(range(2, n - 1))
    local_at = {c: c - group[0] for group in (fox_arrays, ret_arrays) for c in group}

    def w_recv(c, src):
        return w_r.at[src * len(fox_arrays) + local_at[c]]

    def w_send(c, to):
        here = owns[c].at[pl.ds(pl.multiple_of(g * step, step), step)]
        return rdma(here, w_at(c, me, g), w_s.at[c], w_recv(c, me), sp=to)

    def w_on(c, src, to):
        here = w_at(c, src, g)
        return rdma(here, here, w_s.at[c], w_recv(c, src), sp=to)

    def w_in(c, src):
        here = w_at(c, src, g)
        return rdma(here, here, w_s.at[c], w_recv(c, src), sp=src)

    def w_side(c, k, d):
        here = w_at(c, toward(k), g)
        return rdma(here, here, wy_s.at[local_at[c]], wy_r.at[wy_at(c, k in late_of(c))], grp=lax.rem(g + d, n_grp))

    def late_of(c):
        return far if c in fox_arrays else [n - 1]

    def wy_at(c, late):
        return local_at[c] + (len(fox_arrays) if late and c not in (0, 1) else 0)

    def w_late(c):
        drained(wy_r.at[wy_at(c, True)], w_several(c, len(late_of(c)) * (n_grp - 1)))

    def w_early(c):
        w_local(c).wait()
        drained(wy_r.at[wy_at(c, False)], w_several(c, (n - 1 - len(late_of(c))) * (n_grp - 1)))

    def w_several(c, pieces):
        return w_buf.at[: pieces * step, starts[c][0] : starts[c][1]]

    def w_local(c):
        start = pl.multiple_of(me * shard, shard)
        return pltpu.make_async_copy(
            owns[c], w_buf.at[pl.ds(start, shard), starts[c][0] : starts[c][1]], w_loc.at[local_at[c]]
        )

    fox_up = jnp.where(is_ret & (mine == 0), partner, fox_of(couple + 1))
    fox_down = jnp.where(is_ret & (mine == 1), partner, jnp.where(couple >= 1, fox_of(jnp.maximum(couple - 1, 0)), -1))
    ret_up = jnp.where(is_fox & (mine == 0), partner, ret_of(couple + 1))
    ret_down = jnp.where(is_fox & (mine == 1), partner, jnp.where(couple >= 1, ret_of(jnp.maximum(couple - 1, 0)), -1))

    def send_weights(arrays):
        for c in arrays:
            up, down = (fox_up, fox_down) if c in fox_arrays else (ret_up, ret_down)

            @pl.when(up < n)
            def _(c=c, up=up):
                w_send(c, up).start()

            @pl.when(down >= 0)
            def _(c=c, down=down):
                w_send(c, down).start()

    def sends_from(p, arrays):
        q, b = p // 2, p % 2
        plane = (lambda i: 2 * i + 1 - i % 2) if arrays[0] in fox_arrays else (lambda i: 2 * i + i % 2)
        uses = plane(q) == p
        up = p + 1 if not uses and b == 0 else plane(q + 1)
        down = p - 1 if not uses and b == 1 else (plane(q - 1) if q else -1)
        passes = ((p if up < n else 0) + (n - 1 - p if down >= 0 else 0)) if uses else 0
        return (up < n) + (down >= 0) + passes

    def swap_tokens():
        for m in range(chunks):
            tok_z(m).start()

    send_weights((0, 1))
    for m in range(chunks):
        tok_c(True, m, 0).start()

    swap_tokens()

    @pl.when(is_ret)
    def _():
        send_weights((2,))

    meet_far()
    send_weights((3,))
    drained(in_sem.at[0], wqk_buf)
    qk_own[...] = wqk_buf[...].astype(jnp.float32).T.astype(jnp.bfloat16)

    @pl.when(is_ret)
    def _():
        send_weights((4,))

    tok_local.start()

    @pl.when(is_fox)
    def _():
        for c in fox_arrays:
            w_local(c).start()

    @pl.when(is_ret)
    def _():
        for c in ret_arrays:
            w_local(c).start()

    depth = mix_buf.shape[1] // 2
    out_cols = ret_out_ref.shape[1]

    out_step = depth // n_grp
    out_refs = [ret_out_ref, fox_out_ref]

    def out_cols_of(src):
        return pl.ds(pl.multiple_of(src * out_cols, out_cols), out_cols)

    def out_at(c, src):
        return wout_buf.at[pl.ds(pl.multiple_of(c * depth + g * out_step, out_step), out_step), out_cols_of(src)]

    def out_both(src):
        return wout_buf.at[: 2 * out_step, out_cols_of(src)]

    def out_hop(c, src, to, first):
        here = out_refs[c].at[pl.ds(pl.multiple_of(g * out_step, out_step), out_step)] if first else out_at(c, src)
        return rdma(here, out_at(c, src), o_s, o_r.at[2 * src + c], sp=to)

    def out_local(c):
        return pltpu.make_async_copy(out_refs[c], wout_buf.at[c * depth : (c + 1) * depth, out_cols_of(me)], o_loc)

    def out_begin():
        for c in range(2):

            @pl.when(has_up)
            def _(c=c):
                out_hop(c, me, me + 1, True).start()

            @pl.when(has_down)
            def _(c=c):
                out_hop(c, me, me - 1, True).start()

            out_local(c).start()

    def out_relay(i):
        for src, to in ((me - i, me + 1), (me + i, me - 1)):

            @pl.when((src >= 0) & (src < n))
            def _(src=src, to=to):
                for c in range(2):
                    there = out_at(c, src)
                    rdma(there, there, o_s, o_r.at[2 * src + c], sp=src).wait_recv()

                    @pl.when((to >= 0) & (to < n))
                    def _(c=c):
                        out_hop(c, src, to, False).start()

                    for d in range(1, n_grp):
                        here = out_at(c, src)
                        at = (d - 1) * n + src
                        rdma(here, here, oy_s, oy_r.at[at], grp=lax.rem(g + d, n_grp)).start()

    def out_arrive(src):
        for d in range(1, n_grp):
            drained(oy_r.at[(d - 1) * n + src], out_both(src))

    def w_pass(c, src):
        up, down = (fox_up, fox_down) if c in fox_arrays else (ret_up, ret_down)

        @pl.when((src < me) & (up < n))
        def _():
            w_on(c, src, up).start()

        @pl.when((src > me) & (down >= 0))
        def _():
            w_on(c, src, down).start()

    def w_relay(arrays, ks):
        for i in ks:
            for c in arrays:
                w_in(c, toward(i)).wait_recv()
                w_pass(c, toward(i))
                for d in range(1, n_grp):
                    w_side(c, i, d).start()

    def w_arrive(arrays):
        for c in arrays:
            w_local(c).wait()
            drained(wy_r.at[local_at[c]], w_several(c, (n - 1) * (n_grp - 1)))

    def normalize(h):
        squares = jnp.zeros((rows, 1), jnp.float32)
        for i in range(n_tp):
            part = tok_buf[h, i].astype(jnp.float32)
            squares = squares + jnp.sum(part * part, axis=-1, keepdims=True)
        scale = lax.rsqrt(squares * (1.0 / (n_tp * feats)) + epsilon)
        at = pl.ds(pl.multiple_of(h * rows, rows), rows)
        for i in range(n_tp):
            part = tok_buf[h, i].astype(jnp.float32)
            cols = slice(i * feats, (i + 1) * feats)
            norm_buf[at, cols] = (part * scale * gain_buf[:, cols]).astype(jnp.bfloat16)


    def tok_own():
        for d in range(1, half):
            tok_x_in(True, 0, d).wait_recv()
            for m in range(chunks):
                tok_c(True, m, d).start()

    def tok_swap(m):
        tok_z_in(m).wait_recv()
        for d in range(1, half):
            tok_x(False, m, d).start()
        tok_c(False, m, 0).start()

    def tok_last(m):
        for d in range(1, half):
            tok_x_in(False, m, d).wait_recv()
            tok_c(False, m, d).start()

    def tok_ready(own):
        if own:
            tok_local.wait()
        drained(tc_r.at[0 if own else 1], tok_buf.at[mine if own else other, :half])

    for copy in brought:
        copy.wait()

    @pl.when(is_fox)
    def _():
        w_relay((0, 1), [1, n - 1])
        send_weights((4, 2))

    @pl.when(is_fox)
    def _():
        tok_swap(0)
        tok_own()
        for m in range(1, chunks):
            tok_swap(m)
        w_relay((0, 1), far)
        w_relay((2,), [1, n - 1])
        out_begin()

    @pl.when(is_ret)
    def _():
        tok_own()
        for m in range(chunks):
            tok_swap(m)
            if m == 1:
                w_relay((3,), far)
            if m == 2:
                w_relay((4,), far)
        out_begin()
        w_relay(ret_arrays, [1])

    tok_ready(True)
    normalize(mine)

    row_id = lax.broadcasted_iota(jnp.int32, (rows, rows), 0)
    col_id = lax.broadcasted_iota(jnp.int32, (rows, rows), 1)
    causal = col_id <= row_id

    def norm_rows(h):
        return norm_buf[pl.ds(pl.multiple_of(h * rows, rows), rows), :]

    block = rows // n_tp
    span = 2 * block

    def mix_rows(d):
        return pl.ds(pl.multiple_of(lax.rem(pair + d, half) * span, span), span)

    away = [*range(1, half), 0]

    def mix_copy(first, d):
        here = mix_pair.at[other, mix_rows(d)]
        return rdma(here, mix_buf.at[mix_rows(d), first : first + depth], mix_s.at[d], mix_r.at[d], sp=partner)

    def mix_send(first):
        for d in away:
            mix_copy(first, d).start()

    def mix_own(first):
        mix_buf[:, first : first + depth] = mix_pair[mine]

    def mix_in(d):
        here = mix_buf.at[mix_rows(d), :depth]
        rdma(here, here, mix_s.at[d], mix_r.at[d], sp=partner).wait_recv()

    def kv_part(at, values):
        first = fh * fd if values else 0
        return kv_buf.at[at, :, first : first + fh * fd]

    def kv_copy(b, q, values):
        here = kv_part(2 * couple + b, values)
        send = kv_s.at[2 * (2 * (q - 1) + b) + values]
        return rdma(here, here, send, kv_r.at[2 * (2 * couple + b) + values], sp=fox_of(q))

    def kv_in(at, values):
        here = kv_part(at, values)
        return rdma(here, here, kv_s.at[values], kv_r.at[2 * at + values], sp=partner)

    def sum_copy(q):
        return rdma(sum_buf.at[couple], sum_buf.at[couple], sum_s.at[q], sum_r.at[couple], sp=ret_of(q))

    def sum_in(q):
        return rdma(sum_buf.at[q], sum_buf.at[q], sum_s.at[q], sum_r.at[q], sp=partner)

    def later(act):
        for q in range(1, couples):

            @pl.when(q > couple)
            def _(q=q):
                act(jnp.int32(q))

    def after_tokens():
        for m in range(chunks):
            tok_last(m)

    @pl.when(is_fox)
    def _():
        def project_kv(b):
            kv_buf[2 * couple + b] = jnp.dot(
                norm_rows(b), w_buf[:, :q_at], preferred_element_type=jnp.float32
            ).astype(jnp.bfloat16)
            for values in range(2):
                later(lambda q, values=values: kv_copy(b, q, values).start())

        def q_part(srcs):
            total = 0.0
            for src in srcs:
                cols = pl.ds(pl.multiple_of(src * shard, shard), shard)
                total = total + jnp.dot(
                    norm_buf[:, cols], w_buf[cols, q_at:fox_wide], preferred_element_type=jnp.float32
                )
            return total

        for b in range(2):
            for h in range(fh):
                own_cols = pl.ds(pl.multiple_of((2 * couple + b) * rows, rows), rows)
                own = jnp.where(row_id == col_id, gates_buf[h : h + 1, own_cols], 0.0)
                gate_buf[h, b * rows : (b + 1) * rows] = jnp.broadcast_to(
                    jnp.sum(own, axis=1, keepdims=True), (rows, lanes)
                )
        after_tokens()
        w_arrive((0, 1))
        project_kv(mine)
        w_relay((2,), far)
        out_relay(1)
        tok_ready(False)
        normalize(other)
        project_kv(other)
        w_early(2)
        sums_buf[:, : fh * fd] = q_part([me, toward(1), toward(n - 1)])
        w_late(2)
        proj_buf[:, : fh * fd] = (sums_buf[:, : fh * fd] + q_part([toward(k) for k in far])).astype(jnp.bfloat16)

        def block_cols(at):
            return pl.ds(pl.multiple_of(at * rows, rows), rows)

        def rep_cols(x, wide):
            return jnp.concatenate([x] * (wide // lanes), axis=1)

        def attend(at, top_row, first, offset):
            size_ = 2 * rows - top_row
            here = slice(top_row, 2 * rows)
            for h in range(fh):
                query = proj_buf[here, h * fd : (h + 1) * fd]
                k = kv_buf[at, :, h * fd : (h + 1) * fd]
                v = kv_buf[at, :, (fh + h) * fd : (fh + h + 1) * fd]
                logits = lax.dot_general(query, k, NT, preferred_element_type=jnp.float32) * fd ** (-0.5)
                logits = logits + rep_cols(gate_buf[h, here], rows) - gates_buf[h : h + 1, block_cols(at)]
                if offset is not None:
                    row = lax.broadcasted_iota(jnp.int32, (size_, rows), 0)
                    col = lax.broadcasted_iota(jnp.int32, (size_, rows), 1)
                    logits = jnp.where(col <= row, logits, -jnp.inf)
                top_new = jnp.broadcast_to(jnp.max(logits, axis=-1, keepdims=True), (size_, lanes))
                if not first:
                    top = top_buf[h, here]
                    top_new = jnp.maximum(top, top_new)
                p = jnp.exp(logits - rep_cols(top_new, rows))
                total = jnp.broadcast_to(jnp.sum(p, axis=-1, keepdims=True), (size_, lanes))
                weighted = jnp.dot(p.astype(jnp.bfloat16), v, preferred_element_type=jnp.float32)
                if not first:
                    rescale = jnp.exp(top - top_new)
                    total = total_buf[h, here] * rescale + total
                    weighted = weighted_buf[h, here] * rescale[:, :fd] + weighted
                top_buf[h, here] = top_new
                total_buf[h, here] = total
                weighted_buf[h, here] = weighted

        attend(2 * couple, 0, True, 0)
        attend(2 * couple + 1, rows, False, 0)
        out_relay(2)

        def past(i, _):
            q = lax.div(i, 2)
            b = jnp.where(lax.rem(i, 2) == 0, fox_of(q) - 2 * q, 1 - (fox_of(q) - 2 * q))
            at = 2 * q + b
            kv_in(at, 0).wait_recv()
            for h in range(fh):
                k = kv_buf[at, :, h * fd : (h + 1) * fd]
                logits = lax.dot_general(
                    proj_buf[:, h * fd : (h + 1) * fd], k, NT, preferred_element_type=jnp.float32
                ) * fd ** (-0.5)
                logits = logits + rep_cols(gate_buf[h], rows) - gates_buf[h : h + 1, block_cols(at)]
                top = top_buf[h]
                top_new = jnp.maximum(
                    top, jnp.broadcast_to(jnp.max(logits, axis=-1, keepdims=True), (2 * rows, lanes))
                )
                p = jnp.exp(logits - rep_cols(top_new, rows))
                rescale = jnp.exp(top - top_new)
                top_buf[h] = top_new
                total_buf[h] = total_buf[h] * rescale + jnp.broadcast_to(
                    jnp.sum(p, axis=-1, keepdims=True), (2 * rows, lanes)
                )
                weighted_buf[h] = weighted_buf[h] * rescale[:, :fd]
                p_buf[h] = p.astype(jnp.bfloat16)
            kv_in(at, 1).wait_recv()
            for h in range(fh):
                v = kv_buf[at, :, (fh + h) * fd : (fh + h + 1) * fd]
                weighted_buf[h] = weighted_buf[h] + jnp.dot(p_buf[h], v, preferred_element_type=jnp.float32)
            return 0

        lax.fori_loop(0, 2 * couple, past, 0)
        for b in range(2):
            at = slice(b * rows, (b + 1) * rows)
            for h in range(fh):
                mix_pair[b, :, h * fd : (h + 1) * fd] = (
                    weighted_buf[h, at] / total_buf[h, at, :fd]
                ).astype(jnp.bfloat16)
        mix_send(depth)
        mix_own(depth)
        for k in range(3, n):
            out_relay(k)

    @pl.when(is_ret)
    def _():
        distance = jnp.maximum(row_id - col_id, 0).astype(jnp.float32)
        key_scale = dk ** (-0.5)
        for h in range(hr):
            within_buf[h] = jnp.where(causal, jnp.exp(distance * decay_ref[h]) * key_scale, 0.0)
        w_relay(ret_arrays, [n - 1])
        after_tokens()
        tok_ready(False)
        normalize(other)
        out_relay(1)

        def ret_part(srcs):
            total = 0.0
            for src in srcs:
                cols = pl.ds(pl.multiple_of(src * shard, shard), shard)
                total = total + jnp.dot(
                    norm_buf[:, cols], w_buf[cols, :ret_wide], preferred_element_type=jnp.float32
                )
            return total

        for c in ret_arrays:
            w_early(c)
        sums_buf[:, :ret_wide] = ret_part([me] + [toward(k) for k in range(1, n - 1)])
        for c in ret_arrays:
            w_late(c)
        proj_buf[:, :ret_wide] = (sums_buf[:, :ret_wide] + ret_part([toward(n - 1)])).astype(jnp.bfloat16)
        rv_at, rq_at = starts[3][0], starts[4][0]
        lone = jnp.zeros((dk, vd), jnp.float32)

        def part(b, first, wide):
            return proj_buf[b * rows : (b + 1) * rows, first : first + wide]

        def split(x, axis):
            top = x.astype(jnp.bfloat16)
            rest = x - top.astype(jnp.float32)
            middle = rest.astype(jnp.bfloat16)
            low = (rest - middle.astype(jnp.float32)).astype(jnp.bfloat16)
            return jnp.concatenate((top, middle, low), axis=axis)

        def summary(b, h):
            past_end = rows - 1.0 - lax.broadcasted_iota(jnp.int32, (rows, dk), 0).astype(jnp.float32)
            keys = part(b, rq_at + (hr + h) * dk, dk).astype(jnp.float32) * key_scale
            parts = lax.dot_general(
                split(keys * jnp.exp(past_end * decay_ref[h]), 1),
                part(b, rv_at + h * vd, vd),
                TN,
                preferred_element_type=jnp.float32,
            )
            return parts[:dk] + parts[dk : 2 * dk] + parts[2 * dk :]

        early = [summary(0, h) for h in range(hr)]
        for h in range(hr):
            sum_buf[couple, h] = jnp.exp(lone + float(rows) * decay_ref[h]) * early[h] + summary(1, h)
        later(lambda q: sum_copy(q).start())

        for b in range(2):
            for h in range(hr):
                rk = part(b, rq_at + (hr + h) * dk, dk)
                rv = part(b, rv_at + h * vd, vd)
                scores = lax.dot_general(
                    part(b, rq_at + h * dk, dk), rk, NT, preferred_element_type=jnp.float32
                )
                raw_buf[b, h] = jnp.dot(
                    split(scores * within_buf[h], 1),
                    jnp.concatenate((rv, rv, rv), axis=0),
                    preferred_element_type=jnp.float32,
                )
        out_relay(2)

        offset = (couple * 2 * rows).astype(jnp.float32)

        def gather(q, entering):
            sum_in(q).wait_recv()
            gap = ((couple - 1 - q) * 2 * rows).astype(jnp.float32)
            return tuple(entering[h] + jnp.exp(lone + gap * decay_ref[h]) * sum_buf[q, h] for h in range(hr))

        entering = tuple(jnp.exp(lone + offset * decay_ref[h]) * state_buf[h] for h in range(hr))
        entering = lax.fori_loop(0, couple, gather, entering)
        second = tuple(jnp.exp(lone + float(rows) * decay_ref[h]) * entering[h] + early[h] for h in range(hr))
        since = lax.broadcasted_iota(jnp.int32, (rows, vd), 0).astype(jnp.float32) + 1.0

        for b in range(2):
            for h in range(hr):
                rq = part(b, rq_at + h * dk, dk)
                carried = jnp.dot(
                    jnp.concatenate((rq, rq, rq), axis=1),
                    split((entering, second)[b][h], 0),
                    preferred_element_type=jnp.float32,
                )
                raw = raw_buf[b, h] + carried * jnp.exp(since * decay_ref[h])
                center = raw - jnp.mean(raw, axis=-1, keepdims=True)
                variance = jnp.mean(center * center, axis=-1, keepdims=True)
                cols = slice(h * vd, (h + 1) * vd)
                mix_pair[b, :, cols] = (center * lax.rsqrt(variance + epsilon) * hgain_buf[:, cols]).astype(
                    jnp.bfloat16
                )
        mix_send(0)
        mix_own(0)
        for k in range(3, n):
            out_relay(k)

    wide, pieces = out_cols, n

    def piece_cols(piece):
        return pl.ds(pl.multiple_of(piece * wide, wide), wide)

    def slot(d):
        return pl.ds(pl.multiple_of(lax.rem(pair + d, half) * block, block), block)

    def pair_copy(piece, d):
        cols = piece_cols(piece)
        return rdma(
            rs_send.at[1 - parity, slot(d), cols],
            pair_buf.at[slot(d), cols],
            pair_s,
            pair_r.at[piece * half + d],
            tp=t + 1 - 2 * parity,
        )

    def rs_copy(d, piece):
        cols = piece_cols(piece)
        return rdma(
            pair_sum.at[slot(d), cols],
            far_ref.at[d - 1, :, cols],
            rs_s.at[d - 1],
            rs_r.at[d - 1],
            tp=2 * lax.rem(pair + d, half) + parity,
        )

    def project(piece, d):
        cols = piece_cols(piece)
        value = jnp.dot(mix_buf[mix_rows(d), :], wout_buf[:, cols], preferred_element_type=jnp.float32)
        value = value.astype(jnp.bfloat16)
        for b in range(2):
            rs_send[b, slot(d), cols] = value[b * block : (b + 1) * block]
        pair_copy(piece, d).start()

    def reduce(piece, d):
        cols = piece_cols(piece)
        pair_copy(piece, d).wait_recv()
        both = rs_send[parity, slot(d), cols].astype(jnp.float32) + pair_buf[slot(d), cols].astype(jnp.float32)
        if d:
            pair_sum[slot(d), cols] = both.astype(jnp.bfloat16)
            rs_copy(d, piece).start()
        else:
            near_ref[:, cols] = both

    def order(i):
        falling = jnp.where(i <= me, me - i, i)
        rising = jnp.where(i <= n - 1 - me, me + i, n - 1 - i)
        return jnp.where(lower, rising, falling)

    drained(o_loc, wout_buf.at[:, out_cols_of(me)])
    for d in range(1, half):
        mix_in(d)
        project(me, d)
    mix_in(0)

    def turn(i, _):
        out_arrive(order(i))
        for d in range(1, half):
            project(order(i), d)
            reduce(order(i - 1), d)
        project(order(i - 1), 0)
        return 0

    lax.fori_loop(1, n, turn, 0)
    for d in range(1, half):
        reduce(order(jnp.int32(n - 1)), d)
    project(order(jnp.int32(n - 1)), 0)
    for piece in range(pieces):
        reduce(piece, 0)

    slabs = rows * (2 * n_tp - 1) // (2 * n_tp)
    drained(t_s, tok_buf.at[:, :, :slabs])
    for p in range(n):

        @pl.when(me == p)
        def _(p=p):
            for arrays in (fox_arrays, ret_arrays):
                for c in arrays:
                    if sends_from(p, arrays):
                        drained(w_s.at[c], w_several(c, sends_from(p, arrays)))
            hops = 2 * ((p + 1 if p + 1 < n else 0) + (n - p if p else 0))
            drained(o_s, wout_buf.at[: hops * out_step // n])

    drained(oy_s, wout_buf.at[: 2 * (n - 1) * (n_grp - 1) * out_step // n])

    def sides(arrays):
        for c in arrays:
            drained(wy_s.at[local_at[c]], w_several(c, (n - 1) * (n_grp - 1)))

    @pl.when(is_fox)
    def _():
        sides(fox_arrays)
        for d in away:
            mix_copy(depth, d).wait_send()
        for b in range(2):
            for values in range(2):
                later(lambda q, b=b, values=values: kv_copy(b, q, values).wait_send())

    @pl.when(is_ret)
    def _():
        sides(ret_arrays)
        for d in away:
            mix_copy(0, d).wait_send()
        later(lambda q: sum_copy(q).wait_send())

    drained(pair_s, pair_buf)
    for d in range(1, half):
        drained(rs_s.at[d - 1], pair_sum.at[:block])
    for d in range(1, half):
        drained(rs_r.at[d - 1], far_ref.at[d - 1])


def paired(n, n_tp, n_grp, inputs):
    tokens, ret_query_weight, ret_state, fox_gates = inputs[0], inputs[2], inputs[9], inputs[11]
    fox_query_weight, ret_out_weight = inputs[5], inputs[12]
    rows, feats = tokens.shape
    hr, dk, vd = ret_state.shape
    fh = fox_gates.shape[1]
    fd = fox_query_weight.shape[1] // fh
    shard = ret_query_weight.shape[0]
    depth, out_cols = ret_out_weight.shape
    columns = out_cols * n
    wide = max(3 * fh * fd, 2 * hr * dk + hr * vd)
    half = n_tp // 2
    block = rows // n_tp
    chunks = 4
    couples = n // 2
    dma = pltpu.SemaphoreType.DMA
    far = max(half - 1, 1)
    side = max(n_grp - 1, 1) * n
    vmem = pl.BlockSpec(memory_space=pltpu.VMEM)
    hbm = pl.BlockSpec(memory_space=pl.ANY)
    bf16, f32 = jnp.bfloat16, jnp.float32
    size = (n, n_tp, n_grp, hr, dk, vd, fh, fd, chunks)
    near, other = pl.pallas_call(
        functools.partial(pair_kernel, size),
        out_shape=(pltpu.VMEM((block, columns), f32), pltpu.VMEM((far, block, columns), bf16)),
        in_specs=[hbm] * 14,
        out_specs=(vmem, vmem),
        scratch_shapes=[
            pltpu.SMEM((hr,), f32),
            pltpu.VMEM((1, n_tp * feats), f32),
            pltpu.VMEM((2 * hr * dk, shard), bf16),
            pltpu.VMEM((hr, dk, vd), f32),
            pltpu.VMEM((1, hr * vd), f32),
            pltpu.VMEM((fh, n * rows), f32),
            pltpu.VMEM((fh, 2 * rows, lanes), f32),
            pltpu.VMEM((hr, rows, rows), f32),
            pltpu.VMEM((2, hr, rows, vd), f32),
            pltpu.VMEM((2 * rows, wide), f32),
            pltpu.VMEM((2, n_tp, rows, feats), bf16),
            pltpu.VMEM((shard, 2 * hr * dk), bf16),
            pltpu.VMEM((n * shard, wide), bf16),
            pltpu.VMEM((2 * depth, columns), bf16),
            pltpu.VMEM((2 * rows, n_tp * feats), bf16),
            pltpu.VMEM((2 * rows, wide), bf16),
            pltpu.VMEM((n, rows, 2 * fh * fd), bf16),
            pltpu.VMEM((couples, hr, dk, vd), f32),
            pltpu.VMEM((2, rows, depth), bf16),
            pltpu.VMEM((rows, 2 * depth), bf16),
            pltpu.VMEM((2, rows // 2, columns), bf16),
            pltpu.VMEM((rows // 2, columns), bf16),
            pltpu.VMEM((rows // 2, columns), bf16),
            pltpu.VMEM((fh, 2 * rows, rows), bf16),
            pltpu.VMEM((fh, 2 * rows, lanes), f32),
            pltpu.VMEM((fh, 2 * rows, lanes), f32),
            pltpu.VMEM((fh, 2 * rows, fd), f32),
            dma((6,)),
            pltpu.SemaphoreType.REGULAR,
            pltpu.SemaphoreType.REGULAR,
            dma,
            dma((chunks,)),
            dma(((chunks + 1) * far,)),
            dma((2,)),
            dma,
            dma((5,)),
            dma((3 * n,)),
            dma((3,)),
            dma((6,)),
            dma((3,)),
            dma,
            dma((2 * n,)),
            dma,
            dma((side,)),
            dma,
            dma((4 * (couples - 1),)),
            dma((2 * (n - 2),)),
            dma((couples,)),
            dma((couples,)),
            dma((half,)),
            dma((half,)),
            dma,
            dma((n * half,)),
            dma((far,)),
            dma((far,)),
        ],
        compiler_params=pltpu.CompilerParams(
            collective_id=0, has_side_effects=True, vmem_limit_bytes=56 * 1024 * 1024
        ),
        name="layer",
    )(
        tokens,
        inputs[1][None, :],
        inputs[2].T,
        inputs[3].T,
        inputs[4],
        inputs[5],
        inputs[6],
        inputs[7],
        inputs[8],
        inputs[9],
        inputs[10][None, :],
        inputs[11].T,
        inputs[12],
        inputs[13],
    )
    for d in range(half - 1):
        near = near + other[d].astype(f32)
    return near.astype(bf16)


def pairs_fit(n, n_tp, n_grp, inputs):
    rows, feats = inputs[0].shape
    hr, dk, vd = inputs[9].shape
    shard = inputs[2].shape[0]
    depth, out_cols = inputs[12].shape
    wide = inputs[5].shape[1]
    full = all(w % lanes == 0 for w in (out_cols, wide, 2 * hr * dk, hr * vd, feats, depth, rows))
    even = n % 2 == 0 and n > 2 and n_tp % 2 == 0 and n_grp > 1
    tiles = rows % (32 * n_tp) == 0 and rows % 32 == 0 and shard % (16 * n_grp) == 0 and depth % (16 * n_grp * n) == 0 and vd <= lanes
    columns = n * out_cols
    held = 8 * rows * n_tp * feats + 2 * n * shard * 3 * wide + 4 * depth * columns + 4 * n * rows * wide + 6 * rows * columns
    return full and even and tiles and depth == wide == hr * vd and held < 40 * 1024 * 1024


def local(
    n,
    n_tp,
    n_grp,
    tokens,
    norm_gain,
    ret_query_weight,
    ret_key_weight,
    ret_value_weight,
    fox_query_weight,
    fox_key_weight,
    fox_value_weight,
    ret_decay,
    ret_state,
    head_norm_gain,
    fox_gates,
    ret_out_weight,
    fox_out_weight,
):
    inputs = (
        tokens,
        norm_gain,
        ret_query_weight,
        ret_key_weight,
        ret_value_weight,
        fox_query_weight,
        fox_key_weight,
        fox_value_weight,
        ret_decay,
        ret_state,
        head_norm_gain,
        fox_gates,
        ret_out_weight,
        fox_out_weight,
    )
    if pairs_fit(n, n_tp, n_grp, inputs):
        return paired(n, n_tp, n_grp, inputs)
    rows, feats = tokens.shape
    hr, dk, vd = ret_state.shape
    fh = fox_gates.shape[1]
    fd = fox_query_weight.shape[1] // fh
    shard = ret_query_weight.shape[0]
    width = 2 * hr * dk + hr * vd + 3 * fh * fd
    depth, out_cols = ret_out_weight.shape
    columns = out_cols * n
    direct = out_cols % 128 == 0
    if not direct:
        ret_out_weight, fox_out_weight = ret_out_weight.T, fox_out_weight.T
    dma = pltpu.SemaphoreType.DMA

    def gather_sems(arrays):
        side = max(n_grp - 1, 1) * n * arrays
        return [
            dma((n * arrays,)),
            dma((n * arrays,)),
            dma((n * arrays,)),
            dma((side,)),
            dma((side,)),
            dma((arrays,)),
        ]

    vmem = pl.BlockSpec(memory_space=pltpu.VMEM)
    smem = pl.BlockSpec(memory_space=pltpu.SMEM)
    hbm = pl.BlockSpec(memory_space=pl.ANY)
    size = (n, n_tp, n_grp, hr, dk, vd, fh, fd, direct)
    block = rows // n_tp
    peers = max(n_tp - 1, 1)
    far = max(n_tp // 2 - 1, 1)
    pieces = n if direct else 1
    return pl.pallas_call(
        functools.partial(kernel, size),
        out_shape=jax.ShapeDtypeStruct((block, columns), jnp.bfloat16),
        in_specs=[hbm, vmem, vmem, vmem, hbm, hbm, hbm, hbm, smem, vmem, vmem, vmem, hbm, hbm],
        out_specs=vmem,
        scratch_shapes=[
            pltpu.VMEM((n_tp, rows, feats), jnp.bfloat16),
            pltpu.VMEM((shard, 2 * hr * dk), jnp.bfloat16),
            pltpu.VMEM((n * shard, width), jnp.bfloat16),
            pltpu.VMEM((2 * depth, columns) if direct else (columns, 2 * depth), jnp.bfloat16),
            pltpu.VMEM((rows, n_tp * feats), jnp.bfloat16),
            pltpu.VMEM((rows, width - 2 * fh * fd), jnp.bfloat16),
            pltpu.VMEM((n, rows, 2 * fh * fd), jnp.bfloat16),
            pltpu.VMEM((n, hr, dk, vd), jnp.float32),
            pltpu.VMEM((rows, 2 * depth), jnp.bfloat16),
            pltpu.VMEM((2, rows // 2, columns), jnp.bfloat16),
            pltpu.VMEM((rows // 2, columns), jnp.bfloat16),
            pltpu.VMEM((rows // 2, columns), jnp.bfloat16),
            pltpu.VMEM((far, block, columns), jnp.bfloat16),
            pltpu.VMEM((fh, rows, 1), jnp.float32),
            pltpu.VMEM((fh, rows, 1), jnp.float32),
            pltpu.VMEM((fh, rows, fd), jnp.float32),
            dma((peers,)),
            dma((peers,)),
            dma,
            dma((n,)),
            dma((n,)),
            dma((n,)),
            dma((n,)),
            dma((pieces,)),
            dma((pieces,)),
            dma((far * pieces,)),
            dma((far * pieces,)),
        ]
        + gather_sems(2)
        + gather_sems(3)
        + gather_sems(2),
        compiler_params=pltpu.CompilerParams(
            collective_id=0, has_side_effects=True, vmem_limit_bytes=56 * 1024 * 1024
        ),
        name="layer",
    )(
        tokens,
        norm_gain[None, :],
        ret_query_weight.T,
        ret_key_weight.T,
        ret_value_weight,
        fox_query_weight,
        fox_key_weight,
        fox_value_weight,
        ret_decay,
        ret_state,
        head_norm_gain[None, :],
        fox_gates.T,
        ret_out_weight,
        fox_out_weight,
    )


def solution(mesh):
    placed = (
        P(("grp", "sp"), "tp"),
        P(),
        P("sp", "tp"),
        P("sp", "tp"),
        P("sp", "tp"),
        P("sp", "tp"),
        P("sp", "tp"),
        P("sp", "tp"),
        P("tp"),
        P(("grp", "tp"), None, None),
        P("tp"),
        P("grp", "tp"),
        P("tp", "sp"),
        P("tp", "sp"),
    )
    body = functools.partial(local, mesh.shape["sp"], mesh.shape["tp"], mesh.shape["grp"])
    return jax.shard_map(
        body, mesh=mesh, in_specs=placed, out_specs=P(("grp", "sp", "tp"), None), check_vma=False
    )
```

```python
import functools

import jax
import jax.numpy as jnp
from jax import lax
from jax.experimental import pallas as pl
from jax.experimental.pallas import tpu as pltpu
from jax.sharding import PartitionSpec as P

epsilon = 1e-06
lanes = 128
highest = lax.Precision.HIGHEST
NT = (((1,), (1,)), ((), ()))
TN = (((0,), (0,)), ((), ()))


def rdma(src, dst, send_sem, recv_sem, **target):
    return pltpu.make_async_remote_copy(
        src_ref=src,
        dst_ref=dst,
        send_sem=send_sem,
        recv_sem=recv_sem,
        device_id=target,
        device_id_type=pl.DeviceIdType.MESH,
    )


class LineGather:
    def __init__(self, owns, place, sems, n, n_grp, me, g):
        self.owns, self.place, self.n, self.n_grp, self.me, self.g = owns, place, n, n_grp, me, g
        self.up, self.down, self.zr, self.ys, self.yr, self.loc = sems
        self.arrays = len(owns)
        self.rows = owns[0].shape[0]
        self.step = self.rows // n_grp

    def piece(self, part, src, c):
        return self.place(src, c, part * self.step, self.step)

    def own_piece(self, c):
        return self.owns[c].at[pl.ds(pl.multiple_of(self.g * self.step, self.step), self.step)]

    def hop(self, sems, to, src, c, first=False):
        here = self.own_piece(c) if first else self.piece(self.g, src, c)
        at = src * self.arrays + c
        return rdma(here, self.piece(self.g, src, c), sems.at[at], self.zr.at[at], sp=to)

    def side(self, d, src, c):
        at = ((d - 1) * self.n + src) * self.arrays + c
        here = self.piece(self.g, src, c)
        return rdma(here, here, self.ys.at[at], self.yr.at[at], grp=lax.rem(self.g + d, self.n_grp))

    def side_in(self, d, src, c):
        at = ((d - 1) * self.n + src) * self.arrays + c
        part = lax.rem(self.g + self.n_grp - d, self.n_grp)
        here = self.piece(part, src, c)
        return rdma(here, here, self.ys.at[at], self.yr.at[at], grp=part)

    def local(self, c):
        return pltpu.make_async_copy(self.owns[c], self.place(self.me, c, 0, self.rows), self.loc.at[c])

    def start(self):
        me, n = self.me, self.n
        for c in range(self.arrays):

            @pl.when(me + 1 < n)
            def _():
                self.hop(self.up, me + 1, me, c, True).start()

            @pl.when(me >= 1)
            def _():
                self.hop(self.down, me - 1, me, c, True).start()

        for c in range(self.arrays):
            self.local(c).start()

    def relay(self, k):
        me, n = self.me, self.n
        for c in range(self.arrays):
            for src, sems, to in ((me - k, self.up, me + 1), (me + k, self.down, me - 1)):

                @pl.when((src >= 0) & (src < n))
                def _(src=src, sems=sems, to=to):
                    self.hop(sems, me, src, c).wait_recv()

                    @pl.when((to >= 0) & (to < n))
                    def _():
                        self.hop(sems, to, src, c).start()

                    for d in range(1, self.n_grp):
                        self.side(d, src, c).start()

    def arrive_shard(self, src, arrays):
        for c in arrays:
            for d in range(1, self.n_grp):
                self.side_in(d, src, c).wait_recv()

    def arrive(self, arrays):
        for c in arrays:
            self.local(c).wait()

        def step(k, _):
            self.arrive_shard(lax.rem(self.me + k, self.n), arrays)
            return 0

        lax.fori_loop(1, self.n, step, 0)

    def finish(self):
        me, n = self.me, self.n

        def step(src, _):
            for c in range(self.arrays):

                @pl.when((src <= me) & (me + 1 < n))
                def _():
                    self.hop(self.up, me, src, c).wait_send()

                @pl.when((src >= me) & (me >= 1))
                def _():
                    self.hop(self.down, me, src, c).wait_send()

                @pl.when(src != me)
                def _():
                    for d in range(1, self.n_grp):
                        self.side(d, src, c).wait_send()

            return 0

        lax.fori_loop(0, n, step, 0)


def kernel(
    size,
    tok_ref,
    gain_ref,
    wq_ref,
    wk_ref,
    wrv_ref,
    wfq_ref,
    wfk_ref,
    wfv_ref,
    decay_ref,
    state_ref,
    hgain_ref,
    gates_ref,
    ret_out_ref,
    fox_out_ref,
    out_ref,
    tok_buf,
    qk_own,
    w_buf,
    wout_buf,
    norm_buf,
    proj_buf,
    kv_buf,
    sum_buf,
    mix_buf,
    rs_send,
    pair_buf,
    pair_sum,
    rs_buf,
    top_buf,
    total_buf,
    weighted_buf,
    tok_s,
    tok_r,
    tok_loc,
    kv_s,
    kv_r,
    sum_s,
    sum_r,
    pair_s,
    pair_r,
    rs_s,
    rs_r,
    *gather_sems,
):
    n, n_tp, n_grp, hr, dk, vd, fh, fd, direct = size
    me, t, g = lax.axis_index("sp"), lax.axis_index("tp"), lax.axis_index("grp")
    rows, feats = tok_ref.shape
    owns = [wfk_ref, wfv_ref, wfq_ref, wrv_ref, qk_own]
    early = 2
    starts = [0]
    for own in owns:
        starts.append(starts[-1] + own.shape[1])
    shard = qk_own.shape[0]

    def weight_place(src, c, first, count):
        start = pl.multiple_of(src * shard + first, count)
        return w_buf.at[pl.ds(start, count), starts[c] : starts[c + 1]]

    depth = mix_buf.shape[1] // 2
    out_cols = ret_out_ref.shape[1] if direct else ret_out_ref.shape[0]

    def out_place(src, c, first, count):
        if direct:
            start = pl.multiple_of(c * depth + first, count)
            return wout_buf.at[pl.ds(start, count), pl.ds(pl.multiple_of(src * out_cols, out_cols), out_cols)]
        start = pl.multiple_of(src * out_cols + first, count)
        return wout_buf.at[pl.ds(start, count), c * depth : (c + 1) * depth]

    def late_place(src, c, first, count):
        return weight_place(src, c + early, first, count)

    firsts = LineGather(owns[:early], weight_place, gather_sems[:6], n, n_grp, me, g)
    lasts = LineGather(owns[early:], late_place, gather_sems[6:12], n, n_grp, me, g)
    outs = LineGather([ret_out_ref, fox_out_ref], out_place, gather_sems[12:], n, n_grp, me, g)

    barrier = pltpu.get_barrier_semaphore()

    def greet(**target):
        pl.semaphore_signal(barrier, inc=1, device_id=target, device_id_type=pl.DeviceIdType.MESH)

    has_up, has_down = me + 1 < n, me >= 1
    for d in range(1, n_tp):
        greet(tp=lax.rem(t + d, n_tp))
    for d in range(1, n_grp):
        greet(grp=lax.rem(g + d, n_grp))

    @pl.when(has_up)
    def _():
        greet(sp=me + 1)

    @pl.when(has_down)
    def _():
        greet(sp=me - 1)

    turned = jnp.concatenate((wq_ref[...], wk_ref[...]), axis=0).astype(jnp.float32)
    qk_own[...] = turned.T.astype(jnp.bfloat16)

    count = n_tp - 1 + n_grp - 1 + has_up.astype(jnp.int32) + has_down.astype(jnp.int32)
    pl.semaphore_wait(barrier, count)

    def tok_copy(d):
        return rdma(tok_ref, tok_buf.at[t], tok_s.at[d - 1], tok_r.at[d - 1], tp=lax.rem(t + d, n_tp))

    def tok_in(d):
        src = lax.rem(t + n_tp - d, n_tp)
        return rdma(tok_ref, tok_buf.at[src], tok_s.at[d - 1], tok_r.at[d - 1], tp=src)

    firsts.start()
    lasts.start()
    tok_local = pltpu.make_async_copy(tok_ref, tok_buf.at[t], tok_loc)
    for d in range(1, n_tp):
        tok_copy(d).start()
    tok_local.start()

    def first_step(k, _):
        firsts.relay(k)

        lasts.relay(k)
        return 0

    lax.fori_loop(1, n, first_step, 0)
    outs.start()

    tok_local.wait()
    for d in range(1, n_tp):
        tok_in(d).wait_recv()
    squares = jnp.zeros((rows, 1), jnp.float32)
    for i in range(n_tp):
        part = tok_buf[i].astype(jnp.float32)
        squares = squares + jnp.sum(part * part, axis=-1, keepdims=True)
    scale = lax.rsqrt(squares * (1.0 / (n_tp * feats)) + epsilon)
    for i in range(n_tp):
        part = tok_buf[i].astype(jnp.float32)
        cols = slice(i * feats, (i + 1) * feats)
        norm_buf[:, cols] = (part * scale * gain_ref[:, cols]).astype(jnp.bfloat16)

    def kv_copy(src):
        return rdma(kv_buf.at[src], kv_buf.at[src], kv_s.at[src], kv_r.at[src], sp=jnp.minimum(me + 1, n - 1))

    def sum_copy(src):
        return rdma(sum_buf.at[src], sum_buf.at[src], sum_s.at[src], sum_r.at[src], sp=jnp.minimum(me + 1, n - 1))

    firsts.arrive((0, 1))
    kv_buf[me] = jnp.dot(
        norm_buf[...], w_buf[:, : starts[2]], preferred_element_type=jnp.float32
    ).astype(jnp.bfloat16)

    def kv_forward(k):
        src = me - k

        @pl.when(src >= 0)
        def _():
            kv_copy(src).wait_recv()

            @pl.when(has_up)
            def _():
                kv_copy(src).start()

    @pl.when(has_up)
    def _():
        kv_copy(me).start()

    outs.relay(1)
    lasts.arrive((0, 1, 2))
    proj_buf[...] = jnp.dot(
        norm_buf[...], w_buf[:, starts[2] :], preferred_element_type=jnp.float32
    ).astype(jnp.bfloat16)
    rv_at, rq_at = starts[3] - starts[2], starts[4] - starts[2]

    key_scale = dk ** (-0.5)
    position = lax.broadcasted_iota(jnp.int32, (rows, 1), 0).astype(jnp.float32)
    rq, rk, rv = [], [], []
    for h in range(hr):
        rq.append(proj_buf[:, rq_at + h * dk : rq_at + (h + 1) * dk])
        rk.append(proj_buf[:, rq_at + (hr + h) * dk : rq_at + (hr + h + 1) * dk])
        rv.append(proj_buf[:, rv_at + h * vd : rv_at + (h + 1) * vd])
        keys = rk[h].astype(jnp.float32) * key_scale
        trailing = jnp.exp((rows - 1.0 - position) * decay_ref[h])
        sum_buf[me, h] = lax.dot_general(
            keys * trailing, rv[h].astype(jnp.float32), TN, precision=highest, preferred_element_type=jnp.float32
        )

    @pl.when(has_up)
    def _():
        sum_copy(me).start()

    row_id = lax.broadcasted_iota(jnp.int32, (rows, rows), 0)
    col_id = lax.broadcasted_iota(jnp.int32, (rows, rows), 1)
    causal = col_id <= row_id
    own_cols = pl.ds(pl.multiple_of(me * rows, rows), rows)
    own_gates = [
        jnp.sum(jnp.where(row_id == col_id, gates_ref[h : h + 1, own_cols], 0.0), axis=1, keepdims=True)
        for h in range(fh)
    ]

    def attend(src, diagonal):
        key_cols = pl.ds(pl.multiple_of(src * rows, rows), rows)
        for h in range(fh):
            query = proj_buf[:, h * fd : (h + 1) * fd]
            k = kv_buf[src, :, h * fd : (h + 1) * fd]
            v = kv_buf[src, :, (fh + h) * fd : (fh + h + 1) * fd]
            logits = lax.dot_general(query, k, NT, preferred_element_type=jnp.float32) * fd ** (-0.5)
            logits = logits + own_gates[h] - gates_ref[h : h + 1, key_cols]
            if diagonal:
                logits = jnp.where(causal, logits, -jnp.inf)
            top_new = jnp.max(logits, axis=-1, keepdims=True)
            if not diagonal:
                top = top_buf[h]
                top_new = jnp.maximum(top, top_new)
            p = jnp.exp(logits - top_new)
            total = jnp.sum(p, axis=-1, keepdims=True)
            weighted = jnp.dot(p.astype(jnp.bfloat16), v, preferred_element_type=jnp.float32)
            if not diagonal:
                rescale = jnp.exp(top - top_new)
                total = total_buf[h] * rescale + total
                weighted = weighted_buf[h] * rescale + weighted
            top_buf[h] = top_new
            total_buf[h] = total
            weighted_buf[h] = weighted

    def forward(k):
        src = me - k

        @pl.when(src >= 0)
        def _():
            sum_copy(src).wait_recv()

            @pl.when(has_up)
            def _():
                sum_copy(src).start()

    attend(me, True)

    offset = (me * rows).astype(jnp.float32)
    lone = jnp.zeros((dk, vd), jnp.float32)

    def step(k, entering):
        src = me - k
        kv_forward(k)
        forward(k)

        @pl.when(k + 1 < n)
        def _():
            outs.relay(k + 1)


        @pl.when(src >= 0)
        def _():
            attend(src, False)

        gap = ((k - 1) * rows).astype(jnp.float32)
        there = jnp.maximum(src, 0)
        return tuple(
            entering[h]
            + jnp.where(src >= 0, jnp.exp(lone + gap * decay_ref[h]) * sum_buf[there, h], 0.0)
            for h in range(hr)
        )

    entering = tuple(jnp.exp(lone + offset * decay_ref[h]) * state_ref[h] for h in range(hr))
    entering = lax.fori_loop(1, n, step, entering)

    distance = jnp.maximum(row_id - col_id, 0).astype(jnp.float32)
    for h in range(hr):
        scores = lax.dot_general(rq[h], rk[h], NT, preferred_element_type=jnp.float32) * key_scale
        scores = jnp.where(causal, scores * jnp.exp(distance * decay_ref[h]), 0.0)
        inner = jnp.dot(scores, rv[h].astype(jnp.float32), precision=highest, preferred_element_type=jnp.float32)
        leading = jnp.exp((position + 1.0) * decay_ref[h])
        carried = jnp.dot(
            rq[h].astype(jnp.float32), entering[h], precision=highest, preferred_element_type=jnp.float32
        )
        raw = inner + carried * leading
        center = raw - jnp.mean(raw, axis=-1, keepdims=True)
        variance = jnp.mean(center * center, axis=-1, keepdims=True)
        cols = slice(h * vd, (h + 1) * vd)
        mix_buf[:, cols] = (center * lax.rsqrt(variance + epsilon) * hgain_ref[:, cols]).astype(jnp.bfloat16)
    for h in range(fh):
        cols = slice(hr * vd + h * fd, hr * vd + (h + 1) * fd)
        mix_buf[:, cols] = (weighted_buf[h] / total_buf[h]).astype(jnp.bfloat16)

    block = rows // n_tp
    columns = pair_buf.shape[1]
    wide = out_cols if direct else columns
    pieces = columns // wide
    half = n_tp // 2
    parity, pair = lax.rem(t, 2), lax.div(t, 2)

    def piece_cols(piece):
        return pl.ds(pl.multiple_of(piece * wide, wide), wide)

    def slot(at):
        return pl.ds(pl.multiple_of(at * block, block), block)

    def pair_copy(piece):
        cols = piece_cols(piece)
        return rdma(
            rs_send.at[1 - parity, :, cols],
            pair_buf.at[:, cols],
            pair_s.at[piece],
            pair_r.at[piece],
            tp=t + 1 - 2 * parity,
        )

    def rs_copy(d, piece):
        to = lax.rem(pair + d, half)
        cols = piece_cols(piece)
        at = (d - 1) * pieces + piece
        return rdma(
            pair_sum.at[slot(to), cols], rs_buf.at[d - 1, :, cols], rs_s.at[at], rs_r.at[at], tp=2 * to + parity
        )

    def project(piece):
        cols = piece_cols(piece)
        if direct:
            value = jnp.dot(mix_buf[...], wout_buf[:, cols], preferred_element_type=jnp.float32)
        else:
            value = lax.dot_general(mix_buf[...], wout_buf[...], NT, preferred_element_type=jnp.float32)
        value = value.astype(jnp.bfloat16)
        for b in range(n_tp):
            at = slice(b // 2 * block, (b // 2 + 1) * block)
            rs_send[b % 2, at, cols] = value[b * block : (b + 1) * block]
        pair_copy(piece).start()

    def reduce(piece):
        cols = piece_cols(piece)
        pair_copy(piece).wait_recv()
        both = rs_send[parity, :, cols].astype(jnp.float32) + pair_buf[:, cols].astype(jnp.float32)
        pair_sum[:, cols] = both.astype(jnp.bfloat16)
        for d in range(1, half):
            rs_copy(d, piece).start()

    def order(i):
        falling = jnp.where(i <= me, me - i, i)
        rising = jnp.where(i <= n - 1 - me, me + i, n - 1 - i)
        return jnp.where(2 * me >= n, falling, rising)

    if direct:
        for c in range(2):
            outs.local(c).wait()
        project(me)

        def out_step(i, _):
            outs.arrive_shard(order(i), (0, 1))
            project(order(i))
            reduce(order(i - 1))
            return 0

        lax.fori_loop(1, n, out_step, 0)
        reduce(order(jnp.int32(n - 1)))
    else:
        outs.arrive((0, 1))
        project(0)
        reduce(0)

    own = slot(pair)
    summed = rs_send[parity, own, :].astype(jnp.float32) + pair_buf[own, :].astype(jnp.float32)
    for d in range(1, half):
        for piece in range(pieces):
            rs_copy(d, piece).wait_recv()
        summed = summed + rs_buf[d - 1].astype(jnp.float32)
    out_ref[...] = summed.astype(jnp.bfloat16)

    for d in range(1, n_tp):
        tok_copy(d).wait_send()
    for piece in range(pieces):
        pair_copy(piece).wait_send()
        for d in range(1, half):
            rs_copy(d, piece).wait_send()
    firsts.finish()
    lasts.finish()
    outs.finish()

    @pl.when(has_up)
    def _():
        def step(src, _):
            kv_copy(src).wait_send()
            sum_copy(src).wait_send()
            return 0

        lax.fori_loop(0, me + 1, step, 0)


def pair_kernel(
    size,
    tok_ref,
    gain_ref,
    wq_ref,
    wk_ref,
    wrv_ref,
    wfq_ref,
    wfk_ref,
    wfv_ref,
    decay_hbm,
    state_ref,
    hgain_ref,
    gates_ref,
    ret_out_ref,
    fox_out_ref,
    near_ref,
    far_ref,
    decay_ref,
    gain_buf,
    wqk_buf,
    state_buf,
    hgain_buf,
    gates_buf,
    gate_buf,
    within_buf,
    raw_buf,
    sums_buf,
    tok_buf,
    qk_own,
    w_buf,
    wout_buf,
    norm_buf,
    proj_buf,
    kv_buf,
    sum_buf,
    mix_pair,
    mix_buf,
    rs_send,
    pair_buf,
    pair_sum,
    p_buf,
    top_buf,
    total_buf,
    weighted_buf,
    in_sem,
    above_sem,
    below_sem,
    t_s,
    tz_r,
    tx_r,
    tc_r,
    t_loc,
    w_s,
    w_r,
    wy_s,
    wy_r,
    w_loc,
    o_s,
    o_r,
    oy_s,
    oy_r,
    o_loc,
    kv_s,
    kv_r,
    sum_s,
    sum_r,
    mix_s,
    mix_r,
    pair_s,
    pair_r,
    rs_s,
    rs_r,
):
    n, n_tp, n_grp, hr, dk, vd, fh, fd, chunks = size
    me, t, g = lax.axis_index("sp"), lax.axis_index("tp"), lax.axis_index("grp")
    rows, feats = tok_ref.shape
    shard = qk_own.shape[0]
    couples = n // 2
    couple, mine = lax.div(me, 2), lax.rem(me, 2)
    other = 1 - mine
    partner = me + 1 - 2 * mine
    fox_mine = 1 - lax.rem(couple, 2)
    is_fox = mine == fox_mine
    is_ret = mine != fox_mine
    lower = 2 * me < n
    half = n_tp // 2
    parity, pair = lax.rem(t, 2), lax.div(t, 2)

    def fox_of(q):
        return 2 * q + 1 - lax.rem(q, 2)

    def ret_of(q):
        return 2 * q + lax.rem(q, 2)

    def toward(k):
        return lax.rem(jnp.where(lower, me + k, me + n - k), n)

    barrier = pltpu.get_barrier_semaphore()

    def greet(**target):
        pl.semaphore_signal(barrier, inc=1, device_id=target, device_id_type=pl.DeviceIdType.MESH)

    greet(tp=2 * pair + 1 - parity)
    for d in range(1, half):
        greet(tp=2 * lax.rem(pair + d, half) + parity)
    for d in range(1, n_grp):
        greet(grp=lax.rem(g + d, n_grp))
    has_up, has_down = me + 1 < n, me >= 1

    @pl.when(has_up)
    def _():
        greet(sp=me + 1)

    @pl.when(has_down)
    def _():
        greet(sp=me - 1)

    def drained(sem, ref):
        pltpu.make_async_copy(ref, ref, sem).wait()

    width = hr * dk
    pltpu.make_async_copy(wq_ref, wqk_buf.at[:width], in_sem.at[0]).start()
    pltpu.make_async_copy(wk_ref, wqk_buf.at[width:], in_sem.at[0]).start()
    brought = [
        pltpu.make_async_copy(src, dst, in_sem.at[i + 1])
        for i, (src, dst) in enumerate(
            ((gain_ref, gain_buf), (state_ref, state_buf), (hgain_ref, hgain_buf), (gates_ref, gates_buf), (decay_hbm, decay_ref))
        )
    ]
    for copy in brought:
        copy.start()

    pl.semaphore_wait(barrier, half + n_grp - 1 + has_up.astype(jnp.int32) + has_down.astype(jnp.int32))

    def tell(sem, to):
        pl.semaphore_signal(sem, inc=1, device_id={"sp": to}, device_id_type=pl.DeviceIdType.MESH)

    @pl.when(has_up & has_down)
    def _():
        tell(above_sem, me - 1)
        tell(below_sem, me + 1)

    def meet_far():
        def from_above(i, _):
            pl.semaphore_wait(above_sem, 1)

            @pl.when(has_down)
            def _():
                tell(above_sem, me - 1)

            return 0

        def from_below(i, _):
            pl.semaphore_wait(below_sem, 1)

            @pl.when(has_up)
            def _():
                tell(below_sem, me + 1)

            return 0

        lax.fori_loop(0, jnp.maximum(n - 2 - me, 0), from_above, 0)
        lax.fori_loop(0, jnp.maximum(me - 1, 0), from_below, 0)

    slab = rows // chunks

    def own_tok(m):
        return tok_ref.at[pl.ds(m * slab, slab)]

    def tok_at(h, m, src):
        return tok_buf.at[h, src, pl.ds(m * slab, slab)]

    def tok_z(m):
        return rdma(own_tok(m), tok_at(mine, m, t), t_s, tz_r.at[m], sp=partner)

    def tok_z_in(m):
        here = tok_at(other, m, t)
        return rdma(here, here, t_s, tz_r.at[m], sp=partner)

    def x_sem(own, m, d):
        return (0 if own else 1 + m) * max(half - 1, 1) + d - 1

    def tok_x(own, m, d):
        h = mine if own else other
        src = own_tok(m) if own else tok_at(h, m, t)
        return rdma(src, tok_at(h, m, t), t_s, tx_r.at[x_sem(own, m, d)], tp=2 * lax.rem(pair + d, half) + parity)

    def tok_x_in(own, m, d):
        src = 2 * lax.rem(pair + half - d, half) + parity
        here = tok_buf.at[mine, src] if own else tok_at(other, m, src)
        return rdma(here, here, t_s, tx_r.at[x_sem(own, m, d)], tp=src)

    def tok_c(own, m, d):
        h = mine if own else other
        src = 2 * lax.rem(pair + half - d, half) + parity
        there = tok_at(h, m, src)
        here = own_tok(m) if own and d == 0 else there
        return rdma(here, there, t_s, tc_r.at[0 if own else 1], tp=2 * pair + 1 - parity)

    tok_local = pltpu.make_async_copy(tok_ref, tok_buf.at[mine, t], t_loc)

    for d in range(1, half):
        for m in range(chunks):
            tok_x(True, m, d).start()

    owns = [wfk_ref, wfv_ref, wfq_ref, wrv_ref, qk_own]
    fox_arrays, ret_arrays = (0, 1, 2), (3, 4)
    starts = {}
    for group in (fox_arrays, ret_arrays):
        at = 0
        for c in group:
            starts[c] = (at, at + owns[c].shape[1])
            at = starts[c][1]
    fox_wide, ret_wide = starts[2][1], starts[4][1]
    q_at = starts[2][0]
    step = shard // n_grp
    count = len(owns)

    def w_at(c, src, part):
        start = pl.multiple_of(src * shard + part * step, step)
        return w_buf.at[pl.ds(start, step), starts[c][0] : starts[c][1]]

    far = list(range(2, n - 1))
    local_at = {c: c - group[0] for group in (fox_arrays, ret_arrays) for c in group}

    def w_recv(c, src):
        return w_r.at[src * len(fox_arrays) + local_at[c]]

    def w_send(c, to):
        here = owns[c].at[pl.ds(pl.multiple_of(g * step, step), step)]
        return rdma(here, w_at(c, me, g), w_s.at[c], w_recv(c, me), sp=to)

    def w_on(c, src, to):
        here = w_at(c, src, g)
        return rdma(here, here, w_s.at[c], w_recv(c, src), sp=to)

    def w_in(c, src):
        here = w_at(c, src, g)
        return rdma(here, here, w_s.at[c], w_recv(c, src), sp=src)

    def w_side(c, k, d):
        here = w_at(c, toward(k), g)
        return rdma(here, here, wy_s.at[local_at[c]], wy_r.at[wy_at(c, k in late_of(c))], grp=lax.rem(g + d, n_grp))

    def late_of(c):
        return far if c in fox_arrays else [n - 1]

    def wy_at(c, late):
        return local_at[c] + (len(fox_arrays) if late and c not in (0, 1) else 0)

    def w_late(c):
        drained(wy_r.at[wy_at(c, True)], w_several(c, len(late_of(c)) * (n_grp - 1)))

    def w_early(c):
        w_local(c).wait()
        drained(wy_r.at[wy_at(c, False)], w_several(c, (n - 1 - len(late_of(c))) * (n_grp - 1)))

    def w_several(c, pieces):
        return w_buf.at[: pieces * step, starts[c][0] : starts[c][1]]

    def w_local(c):
        start = pl.multiple_of(me * shard, shard)
        return pltpu.make_async_copy(
            owns[c], w_buf.at[pl.ds(start, shard), starts[c][0] : starts[c][1]], w_loc.at[local_at[c]]
        )

    fox_up = jnp.where(is_ret & (mine == 0), partner, fox_of(couple + 1))
    fox_down = jnp.where(is_ret & (mine == 1), partner, jnp.where(couple >= 1, fox_of(jnp.maximum(couple - 1, 0)), -1))
    ret_up = jnp.where(is_fox & (mine == 0), partner, ret_of(couple + 1))
    ret_down = jnp.where(is_fox & (mine == 1), partner, jnp.where(couple >= 1, ret_of(jnp.maximum(couple - 1, 0)), -1))

    def send_weights(arrays):
        for c in arrays:
            up, down = (fox_up, fox_down) if c in fox_arrays else (ret_up, ret_down)

            @pl.when(up < n)
            def _(c=c, up=up):
                w_send(c, up).start()

            @pl.when(down >= 0)
            def _(c=c, down=down):
                w_send(c, down).start()

    def sends_from(p, arrays):
        q, b = p // 2, p % 2
        plane = (lambda i: 2 * i + 1 - i % 2) if arrays[0] in fox_arrays else (lambda i: 2 * i + i % 2)
        uses = plane(q) == p
        up = p + 1 if not uses and b == 0 else plane(q + 1)
        down = p - 1 if not uses and b == 1 else (plane(q - 1) if q else -1)
        passes = ((p if up < n else 0) + (n - 1 - p if down >= 0 else 0)) if uses else 0
        return (up < n) + (down >= 0) + passes

    def swap_tokens():
        for m in range(chunks):
            tok_z(m).start()

    send_weights((0, 1))
    for m in range(chunks):
        tok_c(True, m, 0).start()

    swap_tokens()

    @pl.when(is_ret)
    def _():
        send_weights((2,))

    meet_far()
    send_weights((3,))
    drained(in_sem.at[0], wqk_buf)
    qk_own[...] = wqk_buf[...].astype(jnp.float32).T.astype(jnp.bfloat16)

    @pl.when(is_ret)
    def _():
        send_weights((4,))

    tok_local.start()

    @pl.when(is_fox)
    def _():
        for c in fox_arrays:
            w_local(c).start()

    @pl.when(is_ret)
    def _():
        for c in ret_arrays:
            w_local(c).start()

    depth = mix_buf.shape[1] // 2
    out_cols = ret_out_ref.shape[1]

    out_step = depth // n_grp
    out_refs = [ret_out_ref, fox_out_ref]

    def out_cols_of(src):
        return pl.ds(pl.multiple_of(src * out_cols, out_cols), out_cols)

    def out_at(c, src):
        return wout_buf.at[pl.ds(pl.multiple_of(c * depth + g * out_step, out_step), out_step), out_cols_of(src)]

    def out_both(src):
        return wout_buf.at[: 2 * out_step, out_cols_of(src)]

    def out_hop(c, src, to, first):
        here = out_refs[c].at[pl.ds(pl.multiple_of(g * out_step, out_step), out_step)] if first else out_at(c, src)
        return rdma(here, out_at(c, src), o_s, o_r.at[2 * src + c], sp=to)

    def out_local(c):
        return pltpu.make_async_copy(out_refs[c], wout_buf.at[c * depth : (c + 1) * depth, out_cols_of(me)], o_loc)

    def out_begin():
        for c in range(2):

            @pl.when(has_up)
            def _(c=c):
                out_hop(c, me, me + 1, True).start()

            @pl.when(has_down)
            def _(c=c):
                out_hop(c, me, me - 1, True).start()

            out_local(c).start()

    def out_relay(i):
        for src, to in ((me - i, me + 1), (me + i, me - 1)):

            @pl.when((src >= 0) & (src < n))
            def _(src=src, to=to):
                for c in range(2):
                    there = out_at(c, src)
                    rdma(there, there, o_s, o_r.at[2 * src + c], sp=src).wait_recv()

                    @pl.when((to >= 0) & (to < n))
                    def _(c=c):
                        out_hop(c, src, to, False).start()

                    for d in range(1, n_grp):
                        here = out_at(c, src)
                        at = (d - 1) * n + src
                        rdma(here, here, oy_s, oy_r.at[at], grp=lax.rem(g + d, n_grp)).start()

    def out_arrive(src):
        for d in range(1, n_grp):
            drained(oy_r.at[(d - 1) * n + src], out_both(src))

    def w_pass(c, src):
        up, down = (fox_up, fox_down) if c in fox_arrays else (ret_up, ret_down)

        @pl.when((src < me) & (up < n))
        def _():
            w_on(c, src, up).start()

        @pl.when((src > me) & (down >= 0))
        def _():
            w_on(c, src, down).start()

    def w_relay(arrays, ks):
        for i in ks:
            for c in arrays:
                w_in(c, toward(i)).wait_recv()
                w_pass(c, toward(i))
                for d in range(1, n_grp):
                    w_side(c, i, d).start()

    def w_arrive(arrays):
        for c in arrays:
            w_local(c).wait()
            drained(wy_r.at[local_at[c]], w_several(c, (n - 1) * (n_grp - 1)))

    def normalize(h):
        squares = jnp.zeros((rows, 1), jnp.float32)
        for i in range(n_tp):
            part = tok_buf[h, i].astype(jnp.float32)
            squares = squares + jnp.sum(part * part, axis=-1, keepdims=True)
        scale = lax.rsqrt(squares * (1.0 / (n_tp * feats)) + epsilon)
        at = pl.ds(pl.multiple_of(h * rows, rows), rows)
        for i in range(n_tp):
            part = tok_buf[h, i].astype(jnp.float32)
            cols = slice(i * feats, (i + 1) * feats)
            norm_buf[at, cols] = (part * scale * gain_buf[:, cols]).astype(jnp.bfloat16)


    def tok_own():
        for d in range(1, half):
            tok_x_in(True, 0, d).wait_recv()
            for m in range(chunks):
                tok_c(True, m, d).start()

    def tok_swap(m):
        tok_z_in(m).wait_recv()
        for d in range(1, half):
            tok_x(False, m, d).start()
        tok_c(False, m, 0).start()

    def tok_last(m):
        for d in range(1, half):
            tok_x_in(False, m, d).wait_recv()
            tok_c(False, m, d).start()

    def tok_ready(own):
        if own:
            tok_local.wait()
        drained(tc_r.at[0 if own else 1], tok_buf.at[mine if own else other, :half])

    for copy in brought:
        copy.wait()

    @pl.when(is_fox)
    def _():
        w_relay((0, 1), [1, n - 1])
        send_weights((4, 2))

    @pl.when(is_fox)
    def _():
        tok_swap(0)
        tok_own()
        for m in range(1, chunks):
            tok_swap(m)
        w_relay((0, 1), far)
        w_relay((2,), [1, n - 1])
        out_begin()

    row_id = lax.broadcasted_iota(jnp.int32, (rows, rows), 0)
    col_id = lax.broadcasted_iota(jnp.int32, (rows, rows), 1)

    @pl.when(is_ret)
    def _():
        distance = jnp.maximum(row_id - col_id, 0).astype(jnp.float32)
        for h in range(hr):
            within = jnp.exp(distance * decay_ref[h]) * dk ** (-0.5)
            within_buf[h] = jnp.where(col_id <= row_id, within, 0.0)
        tok_own()
        for m in range(chunks):
            tok_swap(m)
            if m == 1:
                w_relay((3,), far)
            if m == 2:
                w_relay((4,), far)
        out_begin()
        w_relay(ret_arrays, [1])

    tok_ready(True)
    normalize(mine)

    def norm_rows(h):
        return norm_buf[pl.ds(pl.multiple_of(h * rows, rows), rows), :]

    block = rows // n_tp
    span = 2 * block

    def mix_rows(d):
        return pl.ds(pl.multiple_of(lax.rem(pair + d, half) * span, span), span)

    away = [*range(1, half), 0]

    def mix_copy(first, d):
        here = mix_pair.at[other, mix_rows(d)]
        return rdma(here, mix_buf.at[mix_rows(d), first : first + depth], mix_s.at[d], mix_r.at[d], sp=partner)

    def mix_send(first):
        for d in away:
            mix_copy(first, d).start()

    def mix_own(first):
        mix_buf[:, first : first + depth] = mix_pair[mine]

    def mix_in(d):
        here = mix_buf.at[mix_rows(d), :depth]
        rdma(here, here, mix_s.at[d], mix_r.at[d], sp=partner).wait_recv()

    def kv_part(at, values):
        first = fh * fd if values else 0
        return kv_buf.at[at, :, first : first + fh * fd]

    def kv_copy(b, q, values):
        here = kv_part(2 * couple + b, values)
        send = kv_s.at[2 * (2 * (q - 1) + b) + values]
        return rdma(here, here, send, kv_r.at[2 * (2 * couple + b) + values], sp=fox_of(q))

    def kv_in(at, values):
        here = kv_part(at, values)
        return rdma(here, here, kv_s.at[values], kv_r.at[2 * at + values], sp=partner)

    def sum_copy(q):
        return rdma(sum_buf.at[couple], sum_buf.at[couple], sum_s.at[q], sum_r.at[couple], sp=ret_of(q))

    def sum_in(q):
        return rdma(sum_buf.at[q], sum_buf.at[q], sum_s.at[q], sum_r.at[q], sp=partner)

    def later(act):
        for q in range(1, couples):

            @pl.when(q > couple)
            def _(q=q):
                act(jnp.int32(q))

    def after_tokens():
        for m in range(chunks):
            tok_last(m)

    @pl.when(is_fox)
    def _():
        def project_kv(b):
            kv_buf[2 * couple + b] = jnp.dot(
                norm_rows(b), w_buf[:, :q_at], preferred_element_type=jnp.float32
            ).astype(jnp.bfloat16)
            for values in range(2):
                later(lambda q, values=values: kv_copy(b, q, values).start())

        def q_part(srcs):
            total = 0.0
            for src in srcs:
                cols = pl.ds(pl.multiple_of(src * shard, shard), shard)
                total = total + jnp.dot(
                    norm_buf[:, cols], w_buf[cols, q_at:fox_wide], preferred_element_type=jnp.float32
                )
            return total

        for b in range(2):
            for h in range(fh):
                own_cols = pl.ds(pl.multiple_of((2 * couple + b) * rows, rows), rows)
                own = jnp.where(row_id == col_id, gates_buf[h : h + 1, own_cols], 0.0)
                gate_buf[h, b * rows : (b + 1) * rows] = jnp.broadcast_to(
                    jnp.sum(own, axis=1, keepdims=True), (rows, lanes)
                )
        after_tokens()
        w_arrive((0, 1))
        project_kv(mine)
        w_relay((2,), far)
        out_relay(1)
        tok_ready(False)
        normalize(other)
        project_kv(other)
        w_early(2)
        sums_buf[:, : fh * fd] = q_part([me, toward(1), toward(n - 1)])
        w_late(2)
        proj_buf[:, : fh * fd] = (sums_buf[:, : fh * fd] + q_part([toward(k) for k in far])).astype(jnp.bfloat16)

        def block_cols(at):
            return pl.ds(pl.multiple_of(at * rows, rows), rows)

        def rep_cols(x, wide):
            return jnp.concatenate([x] * (wide // lanes), axis=1)

        def attend(at, top_row, first, offset):
            size_ = 2 * rows - top_row
            here = slice(top_row, 2 * rows)
            for h in range(fh):
                query = proj_buf[here, h * fd : (h + 1) * fd]
                k = kv_buf[at, :, h * fd : (h + 1) * fd]
                v = kv_buf[at, :, (fh + h) * fd : (fh + h + 1) * fd]
                logits = lax.dot_general(query, k, NT, preferred_element_type=jnp.float32) * fd ** (-0.5)
                logits = logits + rep_cols(gate_buf[h, here], rows) - gates_buf[h : h + 1, block_cols(at)]
                if offset is not None:
                    row = lax.broadcasted_iota(jnp.int32, (size_, rows), 0)
                    col = lax.broadcasted_iota(jnp.int32, (size_, rows), 1)
                    logits = jnp.where(col <= row, logits, -jnp.inf)
                top_new = jnp.broadcast_to(jnp.max(logits, axis=-1, keepdims=True), (size_, lanes))
                if not first:
                    top = top_buf[h, here]
                    top_new = jnp.maximum(top, top_new)
                p = jnp.exp(logits - rep_cols(top_new, rows))
                total = jnp.broadcast_to(jnp.sum(p, axis=-1, keepdims=True), (size_, lanes))
                weighted = jnp.dot(p.astype(jnp.bfloat16), v, preferred_element_type=jnp.float32)
                if not first:
                    rescale = jnp.exp(top - top_new)
                    total = total_buf[h, here] * rescale + total
                    weighted = weighted_buf[h, here] * rescale[:, :fd] + weighted
                top_buf[h, here] = top_new
                total_buf[h, here] = total
                weighted_buf[h, here] = weighted

        attend(2 * couple, 0, True, 0)
        attend(2 * couple + 1, rows, False, 0)
        out_relay(2)

        def past(i, _):
            q = lax.div(i, 2)
            b = jnp.where(lax.rem(i, 2) == 0, fox_of(q) - 2 * q, 1 - (fox_of(q) - 2 * q))
            at = 2 * q + b
            kv_in(at, 0).wait_recv()
            for h in range(fh):
                k = kv_buf[at, :, h * fd : (h + 1) * fd]
                logits = lax.dot_general(
                    proj_buf[:, h * fd : (h + 1) * fd], k, NT, preferred_element_type=jnp.float32
                ) * fd ** (-0.5)
                logits = logits + rep_cols(gate_buf[h], rows) - gates_buf[h : h + 1, block_cols(at)]
                top = top_buf[h]
                top_new = jnp.maximum(
                    top, jnp.broadcast_to(jnp.max(logits, axis=-1, keepdims=True), (2 * rows, lanes))
                )
                p = jnp.exp(logits - rep_cols(top_new, rows))
                rescale = jnp.exp(top - top_new)
                top_buf[h] = top_new
                total_buf[h] = total_buf[h] * rescale + jnp.broadcast_to(
                    jnp.sum(p, axis=-1, keepdims=True), (2 * rows, lanes)
                )
                weighted_buf[h] = weighted_buf[h] * rescale[:, :fd]
                p_buf[h] = p.astype(jnp.bfloat16)
            kv_in(at, 1).wait_recv()
            for h in range(fh):
                v = kv_buf[at, :, (fh + h) * fd : (fh + h + 1) * fd]
                weighted_buf[h] = weighted_buf[h] + jnp.dot(p_buf[h], v, preferred_element_type=jnp.float32)
            return 0

        lax.fori_loop(0, 2 * couple, past, 0)
        for b in range(2):
            at = slice(b * rows, (b + 1) * rows)
            for h in range(fh):
                mix_pair[b, :, h * fd : (h + 1) * fd] = (
                    weighted_buf[h, at] / total_buf[h, at, :fd]
                ).astype(jnp.bfloat16)
        mix_send(depth)
        mix_own(depth)
        for k in range(3, n):
            out_relay(k)

    @pl.when(is_ret)
    def _():
        key_scale = dk ** (-0.5)
        w_relay(ret_arrays, [n - 1])
        after_tokens()
        tok_ready(False)
        normalize(other)
        out_relay(1)

        def ret_part(srcs):
            total = 0.0
            for src in srcs:
                cols = pl.ds(pl.multiple_of(src * shard, shard), shard)
                total = total + jnp.dot(
                    norm_buf[:, cols], w_buf[cols, :ret_wide], preferred_element_type=jnp.float32
                )
            return total

        for c in ret_arrays:
            w_early(c)
        sums_buf[:, :ret_wide] = ret_part([me] + [toward(k) for k in range(1, n - 1)])
        for c in ret_arrays:
            w_late(c)
        proj_buf[:, :ret_wide] = (sums_buf[:, :ret_wide] + ret_part([toward(n - 1)])).astype(jnp.bfloat16)
        rv_at, rq_at = starts[3][0], starts[4][0]
        lone = jnp.zeros((dk, vd), jnp.float32)

        def part(b, first, wide):
            return proj_buf[b * rows : (b + 1) * rows, first : first + wide]

        def split(x, axis):
            top = x.astype(jnp.bfloat16)
            rest = x - top.astype(jnp.float32)
            middle = rest.astype(jnp.bfloat16)
            low = (rest - middle.astype(jnp.float32)).astype(jnp.bfloat16)
            return jnp.concatenate((top, middle, low), axis=axis)

        def summary(b, h):
            past_end = rows - 1.0 - lax.broadcasted_iota(jnp.int32, (rows, dk), 0).astype(jnp.float32)
            keys = part(b, rq_at + (hr + h) * dk, dk).astype(jnp.float32) * key_scale
            parts = lax.dot_general(
                split(keys * jnp.exp(past_end * decay_ref[h]), 1),
                part(b, rv_at + h * vd, vd),
                TN,
                preferred_element_type=jnp.float32,
            )
            return parts[:dk] + parts[dk : 2 * dk] + parts[2 * dk :]

        early = [summary(0, h) for h in range(hr)]
        for h in range(hr):
            sum_buf[couple, h] = jnp.exp(lone + float(rows) * decay_ref[h]) * early[h] + summary(1, h)
        later(lambda q: sum_copy(q).start())

        for b in range(2):
            for h in range(hr):
                rk = part(b, rq_at + (hr + h) * dk, dk)
                rv = part(b, rv_at + h * vd, vd)
                scores = lax.dot_general(
                    part(b, rq_at + h * dk, dk), rk, NT, preferred_element_type=jnp.float32
                )
                raw_buf[b, h] = jnp.dot(
                    split(scores * within_buf[h], 1),
                    jnp.concatenate((rv, rv, rv), axis=0),
                    preferred_element_type=jnp.float32,
                )
        out_relay(2)

        offset = (couple * 2 * rows).astype(jnp.float32)

        def gather(q, entering):
            sum_in(q).wait_recv()
            gap = ((couple - 1 - q) * 2 * rows).astype(jnp.float32)
            return tuple(entering[h] + jnp.exp(lone + gap * decay_ref[h]) * sum_buf[q, h] for h in range(hr))

        entering = tuple(jnp.exp(lone + offset * decay_ref[h]) * state_buf[h] for h in range(hr))
        entering = lax.fori_loop(0, couple, gather, entering)
        second = tuple(jnp.exp(lone + float(rows) * decay_ref[h]) * entering[h] + early[h] for h in range(hr))
        since = lax.broadcasted_iota(jnp.int32, (rows, vd), 0).astype(jnp.float32) + 1.0

        for b in range(2):
            for h in range(hr):
                rq = part(b, rq_at + h * dk, dk)
                carried = jnp.dot(
                    jnp.concatenate((rq, rq, rq), axis=1),
                    split((entering, second)[b][h], 0),
                    preferred_element_type=jnp.float32,
                )
                raw = raw_buf[b, h] + carried * jnp.exp(since * decay_ref[h])
                center = raw - jnp.mean(raw, axis=-1, keepdims=True)
                variance = jnp.mean(center * center, axis=-1, keepdims=True)
                cols = slice(h * vd, (h + 1) * vd)
                mix_pair[b, :, cols] = (center * lax.rsqrt(variance + epsilon) * hgain_buf[:, cols]).astype(
                    jnp.bfloat16
                )
        mix_send(0)
        mix_own(0)
        for k in range(3, n):
            out_relay(k)

    wide, pieces = out_cols, n

    def piece_cols(piece):
        return pl.ds(pl.multiple_of(piece * wide, wide), wide)

    def slot(d):
        return pl.ds(pl.multiple_of(lax.rem(pair + d, half) * block, block), block)

    def pair_copy(piece, d):
        cols = piece_cols(piece)
        return rdma(
            rs_send.at[1 - parity, slot(d), cols],
            pair_buf.at[slot(d), cols],
            pair_s,
            pair_r.at[pieces * (half - 1) if d == 0 else piece * (half - 1) + d - 1],
            tp=t + 1 - 2 * parity,
        )

    def rs_copy(d, piece):
        cols = piece_cols(piece)
        return rdma(
            pair_sum.at[slot(d), cols],
            far_ref.at[d - 1, :, cols],
            rs_s.at[d - 1],
            rs_r.at[d - 1],
            tp=2 * lax.rem(pair + d, half) + parity,
        )

    def project(piece, d):
        cols = piece_cols(piece)
        value = jnp.dot(mix_buf[mix_rows(d), :], wout_buf[:, cols], preferred_element_type=jnp.float32)
        value = value.astype(jnp.bfloat16)
        for b in range(2):
            rs_send[b, slot(d), cols] = value[b * block : (b + 1) * block]
        pair_copy(piece, d).start()

    def reduce(piece, d):
        cols = piece_cols(piece)
        if d:
            pair_copy(piece, d).wait_recv()
        both = rs_send[parity, slot(d), cols].astype(jnp.float32) + pair_buf[slot(d), cols].astype(jnp.float32)
        if d:
            pair_sum[slot(d), cols] = both.astype(jnp.bfloat16)
            rs_copy(d, piece).start()
        else:
            near_ref[:, cols] = both

    def order(i):
        falling = jnp.where(i <= me, me - i, i)
        rising = jnp.where(i <= n - 1 - me, me + i, n - 1 - i)
        return jnp.where(lower, rising, falling)

    drained(o_loc, wout_buf.at[:, out_cols_of(me)])
    for d in range(1, half):
        mix_in(d)
        project(me, d)
    mix_in(0)

    def turn(i, _):
        out_arrive(order(i))
        for d in range(1, half):
            project(order(i), d)
            reduce(order(i - 1), d)
        project(order(i - 1), 0)
        return 0

    lax.fori_loop(1, n, turn, 0)
    for d in range(1, half):
        reduce(order(jnp.int32(n - 1)), d)
    project(order(jnp.int32(n - 1)), 0)
    drained(pair_r.at[pieces * (half - 1)], pair_buf.at[slot(0)])
    for piece in range(pieces):
        reduce(piece, 0)

    slabs = rows * (2 * n_tp - 1) // (2 * n_tp)
    drained(t_s, tok_buf.at[:, :, :slabs])
    for p in range(n):

        @pl.when(me == p)
        def _(p=p):
            for arrays in (fox_arrays, ret_arrays):
                for c in arrays:
                    if sends_from(p, arrays):
                        drained(w_s.at[c], w_several(c, sends_from(p, arrays)))
            hops = 2 * ((p + 1 if p + 1 < n else 0) + (n - p if p else 0))
            drained(o_s, wout_buf.at[: hops * out_step // n])

    drained(oy_s, wout_buf.at[: 2 * (n - 1) * (n_grp - 1) * out_step // n])

    def sides(arrays):
        for c in arrays:
            drained(wy_s.at[local_at[c]], w_several(c, (n - 1) * (n_grp - 1)))

    @pl.when(is_fox)
    def _():
        sides(fox_arrays)
        for d in away:
            mix_copy(depth, d).wait_send()
        for b in range(2):
            for values in range(2):
                later(lambda q, b=b, values=values: kv_copy(b, q, values).wait_send())

    @pl.when(is_ret)
    def _():
        sides(ret_arrays)
        for d in away:
            mix_copy(0, d).wait_send()
        later(lambda q: sum_copy(q).wait_send())

    drained(pair_s, pair_buf)
    for d in range(1, half):
        drained(rs_s.at[d - 1], pair_sum.at[:block])
    for d in range(1, half):
        drained(rs_r.at[d - 1], far_ref.at[d - 1])


def paired(n, n_tp, n_grp, inputs):
    tokens, ret_query_weight, ret_state, fox_gates = inputs[0], inputs[2], inputs[9], inputs[11]
    fox_query_weight, ret_out_weight = inputs[5], inputs[12]
    rows, feats = tokens.shape
    hr, dk, vd = ret_state.shape
    fh = fox_gates.shape[1]
    fd = fox_query_weight.shape[1] // fh
    shard = ret_query_weight.shape[0]
    depth, out_cols = ret_out_weight.shape
    columns = out_cols * n
    wide = max(3 * fh * fd, 2 * hr * dk + hr * vd)
    half = n_tp // 2
    block = rows // n_tp
    chunks = 4
    couples = n // 2
    dma = pltpu.SemaphoreType.DMA
    far = max(half - 1, 1)
    side = max(n_grp - 1, 1) * n
    vmem = pl.BlockSpec(memory_space=pltpu.VMEM)
    hbm = pl.BlockSpec(memory_space=pl.ANY)
    bf16, f32 = jnp.bfloat16, jnp.float32
    size = (n, n_tp, n_grp, hr, dk, vd, fh, fd, chunks)
    near, other = pl.pallas_call(
        functools.partial(pair_kernel, size),
        out_shape=(pltpu.VMEM((block, columns), f32), pltpu.VMEM((far, block, columns), bf16)),
        in_specs=[hbm] * 14,
        out_specs=(vmem, vmem),
        scratch_shapes=[
            pltpu.SMEM((hr,), f32),
            pltpu.VMEM((1, n_tp * feats), f32),
            pltpu.VMEM((2 * hr * dk, shard), bf16),
            pltpu.VMEM((hr, dk, vd), f32),
            pltpu.VMEM((1, hr * vd), f32),
            pltpu.VMEM((fh, n * rows), f32),
            pltpu.VMEM((fh, 2 * rows, lanes), f32),
            pltpu.VMEM((hr, rows, rows), f32),
            pltpu.VMEM((2, hr, rows, vd), f32),
            pltpu.VMEM((2 * rows, wide), f32),
            pltpu.VMEM((2, n_tp, rows, feats), bf16),
            pltpu.VMEM((shard, 2 * hr * dk), bf16),
            pltpu.VMEM((n * shard, wide), bf16),
            pltpu.VMEM((2 * depth, columns), bf16),
            pltpu.VMEM((2 * rows, n_tp * feats), bf16),
            pltpu.VMEM((2 * rows, wide), bf16),
            pltpu.VMEM((n, rows, 2 * fh * fd), bf16),
            pltpu.VMEM((couples, hr, dk, vd), f32),
            pltpu.VMEM((2, rows, depth), bf16),
            pltpu.VMEM((rows, 2 * depth), bf16),
            pltpu.VMEM((2, rows // 2, columns), bf16),
            pltpu.VMEM((rows // 2, columns), bf16),
            pltpu.VMEM((rows // 2, columns), bf16),
            pltpu.VMEM((fh, 2 * rows, rows), bf16),
            pltpu.VMEM((fh, 2 * rows, lanes), f32),
            pltpu.VMEM((fh, 2 * rows, lanes), f32),
            pltpu.VMEM((fh, 2 * rows, fd), f32),
            dma((6,)),
            pltpu.SemaphoreType.REGULAR,
            pltpu.SemaphoreType.REGULAR,
            dma,
            dma((chunks,)),
            dma(((chunks + 1) * far,)),
            dma((2,)),
            dma,
            dma((5,)),
            dma((3 * n,)),
            dma((3,)),
            dma((6,)),
            dma((3,)),
            dma,
            dma((2 * n,)),
            dma,
            dma((side,)),
            dma,
            dma((4 * (couples - 1),)),
            dma((2 * (n - 2),)),
            dma((couples,)),
            dma((couples,)),
            dma((half,)),
            dma((half,)),
            dma,
            dma((n * (half - 1) + 1,)),
            dma((far,)),
            dma((far,)),
        ],
        compiler_params=pltpu.CompilerParams(
            collective_id=0, has_side_effects=True, vmem_limit_bytes=56 * 1024 * 1024
        ),
        name="layer",
    )(
        tokens,
        inputs[1][None, :],
        inputs[2].T,
        inputs[3].T,
        inputs[4],
        inputs[5],
        inputs[6],
        inputs[7],
        inputs[8],
        inputs[9],
        inputs[10][None, :],
        inputs[11].T,
        inputs[12],
        inputs[13],
    )
    for d in range(half - 1):
        near = near + other[d].astype(f32)
    return near.astype(bf16)


def pairs_fit(n, n_tp, n_grp, inputs):
    rows, feats = inputs[0].shape
    hr, dk, vd = inputs[9].shape
    shard = inputs[2].shape[0]
    depth, out_cols = inputs[12].shape
    wide = inputs[5].shape[1]
    full = all(w % lanes == 0 for w in (out_cols, wide, 2 * hr * dk, hr * vd, feats, depth, rows))
    even = n % 2 == 0 and n > 2 and n_tp % 2 == 0 and n_grp > 1
    tiles = rows % (32 * n_tp) == 0 and rows % 32 == 0 and shard % (16 * n_grp) == 0 and depth % (16 * n_grp * n) == 0 and vd <= lanes
    columns = n * out_cols
    held = 8 * rows * n_tp * feats + 2 * n * shard * 3 * wide + 4 * depth * columns + 4 * n * rows * wide + 6 * rows * columns
    return full and even and tiles and depth == wide == hr * vd and held < 40 * 1024 * 1024


def local(
    n,
    n_tp,
    n_grp,
    tokens,
    norm_gain,
    ret_query_weight,
    ret_key_weight,
    ret_value_weight,
    fox_query_weight,
    fox_key_weight,
    fox_value_weight,
    ret_decay,
    ret_state,
    head_norm_gain,
    fox_gates,
    ret_out_weight,
    fox_out_weight,
):
    inputs = (
        tokens,
        norm_gain,
        ret_query_weight,
        ret_key_weight,
        ret_value_weight,
        fox_query_weight,
        fox_key_weight,
        fox_value_weight,
        ret_decay,
        ret_state,
        head_norm_gain,
        fox_gates,
        ret_out_weight,
        fox_out_weight,
    )
    if pairs_fit(n, n_tp, n_grp, inputs):
        return paired(n, n_tp, n_grp, inputs)
    rows, feats = tokens.shape
    hr, dk, vd = ret_state.shape
    fh = fox_gates.shape[1]
    fd = fox_query_weight.shape[1] // fh
    shard = ret_query_weight.shape[0]
    width = 2 * hr * dk + hr * vd + 3 * fh * fd
    depth, out_cols = ret_out_weight.shape
    columns = out_cols * n
    direct = out_cols % 128 == 0
    if not direct:
        ret_out_weight, fox_out_weight = ret_out_weight.T, fox_out_weight.T
    dma = pltpu.SemaphoreType.DMA

    def gather_sems(arrays):
        side = max(n_grp - 1, 1) * n * arrays
        return [
            dma((n * arrays,)),
            dma((n * arrays,)),
            dma((n * arrays,)),
            dma((side,)),
            dma((side,)),
            dma((arrays,)),
        ]

    vmem = pl.BlockSpec(memory_space=pltpu.VMEM)
    smem = pl.BlockSpec(memory_space=pltpu.SMEM)
    hbm = pl.BlockSpec(memory_space=pl.ANY)
    size = (n, n_tp, n_grp, hr, dk, vd, fh, fd, direct)
    block = rows // n_tp
    peers = max(n_tp - 1, 1)
    far = max(n_tp // 2 - 1, 1)
    pieces = n if direct else 1
    return pl.pallas_call(
        functools.partial(kernel, size),
        out_shape=jax.ShapeDtypeStruct((block, columns), jnp.bfloat16),
        in_specs=[hbm, vmem, vmem, vmem, hbm, hbm, hbm, hbm, smem, vmem, vmem, vmem, hbm, hbm],
        out_specs=vmem,
        scratch_shapes=[
            pltpu.VMEM((n_tp, rows, feats), jnp.bfloat16),
            pltpu.VMEM((shard, 2 * hr * dk), jnp.bfloat16),
            pltpu.VMEM((n * shard, width), jnp.bfloat16),
            pltpu.VMEM((2 * depth, columns) if direct else (columns, 2 * depth), jnp.bfloat16),
            pltpu.VMEM((rows, n_tp * feats), jnp.bfloat16),
            pltpu.VMEM((rows, width - 2 * fh * fd), jnp.bfloat16),
            pltpu.VMEM((n, rows, 2 * fh * fd), jnp.bfloat16),
            pltpu.VMEM((n, hr, dk, vd), jnp.float32),
            pltpu.VMEM((rows, 2 * depth), jnp.bfloat16),
            pltpu.VMEM((2, rows // 2, columns), jnp.bfloat16),
            pltpu.VMEM((rows // 2, columns), jnp.bfloat16),
            pltpu.VMEM((rows // 2, columns), jnp.bfloat16),
            pltpu.VMEM((far, block, columns), jnp.bfloat16),
            pltpu.VMEM((fh, rows, 1), jnp.float32),
            pltpu.VMEM((fh, rows, 1), jnp.float32),
            pltpu.VMEM((fh, rows, fd), jnp.float32),
            dma((peers,)),
            dma((peers,)),
            dma,
            dma((n,)),
            dma((n,)),
            dma((n,)),
            dma((n,)),
            dma((pieces,)),
            dma((pieces,)),
            dma((far * pieces,)),
            dma((far * pieces,)),
        ]
        + gather_sems(2)
        + gather_sems(3)
        + gather_sems(2),
        compiler_params=pltpu.CompilerParams(
            collective_id=0, has_side_effects=True, vmem_limit_bytes=56 * 1024 * 1024
        ),
        name="layer",
    )(
        tokens,
        norm_gain[None, :],
        ret_query_weight.T,
        ret_key_weight.T,
        ret_value_weight,
        fox_query_weight,
        fox_key_weight,
        fox_value_weight,
        ret_decay,
        ret_state,
        head_norm_gain[None, :],
        fox_gates.T,
        ret_out_weight,
        fox_out_weight,
    )


def solution(mesh):
    placed = (
        P(("grp", "sp"), "tp"),
        P(),
        P("sp", "tp"),
        P("sp", "tp"),
        P("sp", "tp"),
        P("sp", "tp"),
        P("sp", "tp"),
        P("sp", "tp"),
        P("tp"),
        P(("grp", "tp"), None, None),
        P("tp"),
        P("grp", "tp"),
        P("tp", "sp"),
        P("tp", "sp"),
    )
    body = functools.partial(local, mesh.shape["sp"], mesh.shape["tp"], mesh.shape["grp"])
    return jax.shard_map(
        body, mesh=mesh, in_specs=placed, out_specs=P(("grp", "sp", "tp"), None), check_vma=False
    )
```
